32 devices in a mesh: rep: 2 (over x), fs: 4 (over z), tp: 4 (over y, core).
Axes of the slice: x: 2, y: 2, z: 4, core: 2. Of those that a mesh axis runs over, the one named last changes fastest.
Arguments:
- tokens: bfloat16 [3072, 2048], P(('rep', 'fs'), 'tp'), may hold values from -6 to 6
- norm_gain: bfloat16 [2048], replicated, may hold values from 0.099609375 to 1.8984375
- w_gate: bfloat16 [2048, 5120], P('fs', 'tp'), may hold values from -0.125 to 0.125
- w_up: bfloat16 [2048, 5120], P('fs', 'tp'), may hold values from -0.125 to 0.125
- w_down: bfloat16 [5120, 2048], P('tp', 'fs'), may hold values from -0.078125 to 0.078125
- cotangent: bfloat16 [3072, 2048], P(('rep', 'fs'), 'tp'), may hold values from -6 to 6
Outputs:
- grad_tokens: bfloat16 [3072, 2048], P(('rep', 'fs'), 'tp')
- grad_gain: float32 [2048], P('tp')
- grad_gate: float32 [2048, 5120], P('fs', 'tp')
- grad_up: float32 [2048, 5120], P('fs', 'tp')
- grad_down: float32 [5120, 2048], P('tp', 'fs')
- gate_up_sq: float32 [2, 2048], P(None, 'fs')
- down_sq: float32 [5120], P('tp')
The draws below stay inside these ranges and needn't reach their ends.
All inputs are finite; a program needn't handle non-finite values.
Results may differ from the reference program's by a relative error of at most 0.018.
Values may be sent and summed in bfloat16 or wider, within the bound.
A program may use at most 128 MiB of HBM per device.

```python
import jax
import jax.numpy as jnp
from jax import lax

D = 2048
FF = 5120
TOKENS = 3072


def raised(array, own_key, source, target, shards_of, factor):
    def block_of(position):
        return (jnp.arange(array.shape[position]) // (array.shape[position] // shards_of)).reshape((-1,) + (1,) * (array.ndim - 1 - position))

    first = jax.random.permutation(own_key, shards_of)[block_of(target)]
    far = (block_of(target) + shards_of // 2) % shards_of
    return jnp.where((block_of(source) == first) | (block_of(source) == far), factor * array, array)


def block_scale(rng, extent, pieces, smallest, top_value):
    factor_of = 1.0
    for position, shards_of in pieces:
        draws = jax.random.uniform(jax.random.fold_in(jax.random.fold_in(rng, 6), position), (shards_of,), jnp.float32, smallest / len(pieces), top_value / len(pieces))
        factor_of = factor_of * jnp.repeat(jnp.exp(draws), extent[position] // shards_of).reshape((-1,) + (1,) * (len(extent) - 1 - position))
    return factor_of


def scatter_about(stream_key, shape, scale, reach, split=(), held_as=jnp.bfloat16):
    gain = block_scale(stream_key, shape, split, -0.22, 0.18) if split else 1.0
    drawn = jax.random.normal(stream_key, shape, jnp.float32) * scale * gain
    return jnp.minimum(jnp.maximum(drawn, -reach), reach).astype(held_as)


def heavy_noise(own_key, extent, scale, limit, split, heavy, held_as=jnp.bfloat16):
    entries = scale * jax.random.normal(own_key, extent, jnp.float32)
    if split:
        entries = entries * block_scale(own_key, extent, split, -0.22, 0.18)
    return jnp.clip(raised(entries, jax.random.fold_in(own_key, 3), *heavy), -limit, limit).astype(held_as)


def setup_inputs(seed: int = 0) -> dict:
    splits = jax.random.split(jax.random.key(seed), 7)
    tokens = scatter_about(splits[0], (TOKENS, D), 1.0, 6.0, ((0, 8), (1, 4)))
    norm_gain = jnp.clip(1.0 + 0.18 * jax.random.normal(splits[1], (D,), jnp.float32), 0.099609375, 1.8984375).astype(jnp.bfloat16)
    w_gate = scatter_about(splits[2], (D, FF), D ** -0.5, 0.125, ((0, 4), (1, 4)))
    w_up = scatter_about(splits[3], (D, FF), D ** -0.5, 0.125, ((0, 4), (1, 4)))
    w_down = scatter_about(splits[4], (FF, D), FF ** -0.5, 0.078125, ((0, 4), (1, 4)))
    cotangent = heavy_noise(splits[5], (TOKENS, D), 1.0, 6.0, ((0, 8), (1, 4)), (0, 1, 8, 2.0))
    return {"tokens": tokens, "norm_gain": norm_gain, "w_gate": w_gate, "w_up": w_up, "w_down": w_down, "cotangent": cotangent}


def reference(tokens, norm_gain, w_gate, w_up, w_down, cotangent):
    wide_tokens = tokens.astype(jnp.float32)
    gain_f = norm_gain.astype(jnp.float32)
    inverse = jax.lax.rsqrt(lax.optimization_barrier(jnp.mean(wide_tokens * wide_tokens, axis=-1, keepdims=True)) + 1e-06)
    normed = (wide_tokens * inverse * gain_f).astype(jnp.bfloat16)
    gate = jnp.dot(normed, w_gate, preferred_element_type=jnp.float32)
    up_proj = jnp.dot(normed, w_up, preferred_element_type=jnp.float32)
    sigma = jax.nn.sigmoid(gate)
    active = gate * sigma
    hidden = (active * up_proj).astype(jnp.bfloat16)
    back = 0.5 * jnp.dot(cotangent, w_down.T, preferred_element_type=jnp.float32)
    d_up = (back * active).astype(jnp.bfloat16)
    d_gate = (back * up_proj * sigma * (1.0 + gate * (1.0 - sigma))).astype(jnp.bfloat16)
    d_normed = jnp.dot(d_gate, w_gate.T, preferred_element_type=jnp.float32) + jnp.dot(d_up, w_up.T, preferred_element_type=jnp.float32)
    grad_gain = lax.optimization_barrier(jnp.sum(d_normed * wide_tokens * inverse, axis=0))
    scaled_grad = d_normed * gain_f
    rowdot = lax.optimization_barrier(jnp.sum(scaled_grad * wide_tokens, axis=-1, keepdims=True))
    grad_tokens = (cotangent.astype(jnp.float32) + inverse * scaled_grad - wide_tokens * inverse ** 3 * rowdot / D).astype(jnp.bfloat16)
    grad_gate = jnp.einsum('td,tf->df', normed, d_gate, preferred_element_type=jnp.float32)
    grad_up = jnp.einsum('td,tf->df', normed, d_up, preferred_element_type=jnp.float32)
    grad_down = 0.5 * jnp.einsum('tf,td->fd', hidden, cotangent, preferred_element_type=jnp.float32)
    gate_up_sq = jnp.stack([lax.optimization_barrier(jnp.sum(grad_gate * grad_gate, axis=1)), lax.optimization_barrier(jnp.sum(grad_up * grad_up, axis=1))])
    down_sq = lax.optimization_barrier(jnp.sum(grad_down * grad_down, axis=1))
    return (grad_tokens, grad_gain, grad_gate, grad_up, grad_down, gate_up_sq, down_sq)
```

```python
import functools

import jax
import jax.numpy as jnp
from jax import lax
from jax.experimental import pallas as pl
from jax.experimental.pallas import tpu as pltpu
from jax.sharding import PartitionSpec as P

MESH = pl.DeviceIdType.MESH


def contract_last(left, right):
    return lax.dot_general(
        left, right, (((1,), (1,)), ((), ())), preferred_element_type=jnp.float32
    )


def contract_first(left, right):
    return lax.dot_general(
        left, right, (((0,), (0,)), ((), ())), preferred_element_type=jnp.float32
    )


def remote(source, target, send_sem, recv_sem, where):
    return pltpu.make_async_remote_copy(
        src_ref=source,
        dst_ref=target,
        send_sem=send_sem,
        recv_sem=recv_sem,
        device_id=where,
        device_id_type=MESH,
    )


def line_sends(z, n_fs, side, d):
    if side == 0:
        return jnp.logical_and(z >= d - 1, z <= n_fs - 2)
    return jnp.logical_and(z + d <= n_fs, z >= 1)


def line_receives(z, n_fs, side, d):
    return z >= d if side == 0 else z + d <= n_fs - 1


def greet(peers):
    barrier = pltpu.get_barrier_semaphore()
    for peer in peers:
        pl.semaphore_signal(barrier, inc=1, device_id=peer, device_id_type=MESH)
    pl.semaphore_wait(barrier, len(peers))


def keep_own(sources, holders, targets, sems):
    count = len(sources)
    loads = [
        pltpu.make_async_copy(sources[i], holders[i], sems.at[0, i]) for i in range(count)
    ]
    stores = [
        pltpu.make_async_copy(holders[i], targets[i], sems.at[1, i]) for i in range(count)
    ]
    for load in loads:
        load.start()

    def finish():
        for load, store in zip(loads, stores):
            load.wait()
            store.start()
        for store in stores:
            store.wait()

    return finish


def weights_kernel(n_fs, n_tp, *refs):
    tokens, cot, w_gate, w_up, w_down = refs[:5]
    whole_x, whole_dy, full_gate, full_up, full_down = refs[5:10]
    holders = refs[10:15]
    own_sem, ring_send, ring_recv, rep_send, rep_recv, tp_send, tp_recv = refs[15:]
    r, z, t = lax.axis_index("rep"), lax.axis_index("fs"), lax.axis_index("tp")
    right, left = lax.rem(z + 1, n_fs), lax.rem(z + n_fs - 1, n_fs)
    partner = {"rep": 1 - r}
    sources = (w_gate, w_up, w_down)
    targets = (full_gate, full_up, full_down)
    rows = w_gate.shape[0]
    hidden = w_down.shape[0]
    local = tokens.shape[1]

    def own_piece(m, half):
        size = (hidden if m == 2 else rows) // 2
        return sources[m].at[pl.ds(pl.multiple_of(half * size, size), size), :]

    def piece(m, owner, half):
        if m == 2:
            size = hidden // 2
            return targets[m].at[
                pl.ds(pl.multiple_of(half * size, size), size),
                pl.ds(pl.multiple_of(owner * rows, rows), rows),
            ]
        size = rows // 2
        return targets[m].at[
            pl.ds(pl.multiple_of(owner * rows + half * size, size), size), :
        ]

    peers = [{"fs": right}, {"fs": left}, partner]
    peers += [{"tp": lax.rem(t + j, n_tp)} for j in range(1, n_tp)]
    greet(peers)

    def owner_of(side, back):
        return lax.rem(z + (n_fs - back if side == 0 else back), n_fs)

    def hop(m, side, d):
        place = piece(m, owner_of(side, d - 1), r)
        return remote(
            own_piece(m, r) if d == 1 else place,
            place,
            ring_send.at[m, side, d - 1],
            ring_recv.at[m, side, d - 1],
            {"fs": right if side == 0 else left},
        )

    def arrival(m, side, d):
        place = piece(m, owner_of(side, d), r)
        return remote(
            place,
            place,
            ring_send.at[m, side, d - 1],
            ring_recv.at[m, side, d - 1],
            {"fs": right if side == 0 else left},
        )

    def across(m, side, d):
        place = piece(m, owner_of(side, d), r)
        return remote(
            place, place, rep_send.at[m, side, d - 1], rep_recv.at[m, side, d - 1], partner
        )

    for m in range(3):
        for side in range(2):

            @pl.when(line_sends(z, n_fs, side, 1))
            def _():
                hop(m, side, 1).start()

    ends = []
    for a, (source, target) in enumerate(((tokens, whole_x), (cot, whole_dy))):
        place = target.at[:, pl.ds(pl.multiple_of(t * local, local), local)]
        for j in range(1, n_tp):
            copy = remote(
                source,
                place,
                tp_send.at[a, j - 1],
                tp_recv.at[a, j - 1],
                {"tp": lax.rem(t + j, n_tp)},
            )
            copy.start()
            ends.append(copy)
    mine = pl.ds(pl.multiple_of(t * local, local), local)
    band = pl.ds(pl.multiple_of(z * rows, rows), rows)
    finish = keep_own(
        (tokens, cot, w_gate, w_up, w_down),
        holders,
        (
            whole_x.at[:, mine],
            whole_dy.at[:, mine],
            full_gate.at[band, :],
            full_up.at[band, :],
            full_down.at[:, band],
        ),
        own_sem,
    )
    finish()
    for d in range(1, n_fs):
        for m in range(3):
            for side in range(2):

                @pl.when(line_receives(z, n_fs, side, d))
                def _():
                    arrival(m, side, d).wait_recv()
                    if d < n_fs - 1:

                        @pl.when(line_sends(z, n_fs, side, d + 1))
                        def _():
                            hop(m, side, d + 1).start()

                    across(m, side, d).start()

    for d in range(1, n_fs):
        for m in range(3):
            for side in range(2):

                @pl.when(line_sends(z, n_fs, side, d))
                def _():
                    hop(m, side, d).wait_send()

                @pl.when(line_receives(z, n_fs, side, d))
                def _():
                    across(m, side, d).wait()

    for copy in ends:
        copy.wait()


def gather_weights(n_fs, n_tp, tokens, cot, w_gate, w_up, w_down):
    count, local = tokens.shape
    rows, hidden = w_gate.shape
    width = rows * n_fs
    dtype = tokens.dtype
    shapes = [
        (count, width),
        (count, width),
        (width, hidden),
        (width, hidden),
        (hidden, width),
    ]
    held = (tokens, cot, w_gate, w_up, w_down)
    moved = sum(2 * a * b for a, b in shapes)
    dma = pltpu.SemaphoreType.DMA
    return pl.pallas_call(
        functools.partial(weights_kernel, n_fs, n_tp),
        out_shape=[jax.ShapeDtypeStruct(s, dtype) for s in shapes],
        in_specs=[pl.BlockSpec(memory_space=pl.ANY)] * 5,
        out_specs=[pl.BlockSpec(memory_space=pl.ANY)] * 5,
        scratch_shapes=[pltpu.VMEM(a.shape, a.dtype) for a in held]
        + [
            dma((2, 5)),
            dma((3, 2, n_fs - 1)),
            dma((3, 2, n_fs - 1)),
            dma((3, 2, n_fs - 1)),
            dma((3, 2, n_fs - 1)),
            dma((2, n_tp - 1)),
            dma((2, n_tp - 1)),
        ],
        compiler_params=pltpu.CompilerParams(collective_id=0, has_side_effects=True),
        cost_estimate=pl.CostEstimate(flops=0, bytes_accessed=16 * moved, transcendentals=0),
        name="gather_weights",
    )(*held)


def tokens_kernel(n_fs, n_tp, n_act, n_swap, *refs):
    total = n_act + n_swap
    acts, swaps = refs[:n_act], refs[n_act:total]
    act_outs, swap_outs = refs[total : total + n_act], refs[total + n_act : 2 * total]
    holders = refs[2 * total : 3 * total]
    own_sem, ring_send, ring_recv = refs[3 * total : 3 * total + 3]
    swap_send, swap_recv, relay_send, relay_recv = refs[3 * total + 3 :]
    z, t = lax.axis_index("fs"), lax.axis_index("tp")
    right, left = lax.rem(z + 1, n_fs), lax.rem(z + n_fs - 1, n_fs)
    count = acts[0].shape[0]
    peers = [{"fs": lax.rem(z + j, n_fs)} for j in range(1, n_fs)]
    if n_swap:
        peers += [{"tp": lax.rem(t + j, n_tp)} for j in range(1, n_tp)]
    greet(peers)

    def rows_of(owner):
        return pl.ds(pl.multiple_of(owner * count, count), count)

    def owner_of(side, back):
        return lax.rem(z + (n_fs - back if side == 0 else back), n_fs)

    def hop(m, side, d):
        place = act_outs[m].at[rows_of(owner_of(side, d - 1)), :]
        return remote(
            acts[m] if d == 1 else place,
            place,
            ring_send.at[m, side, d - 1],
            ring_recv.at[m, side, d - 1],
            {"fs": right if side == 0 else left},
        )

    def arrival(m, side, d):
        place = act_outs[m].at[rows_of(owner_of(side, d)), :]
        return remote(
            place,
            place,
            ring_send.at[m, side, d - 1],
            ring_recv.at[m, side, d - 1],
            {"fs": right if side == 0 else left},
        )

    def swap(a, j):
        peer = lax.rem(z + j, n_fs)
        cut = swap_outs[a].shape[1]
        return remote(
            swaps[a].at[:, pl.ds(pl.multiple_of(peer * cut, cut), cut)],
            swap_outs[a].at[rows_of(z), :],
            swap_send.at[a, j - 1],
            swap_recv.at[a, j - 1],
            {"fs": peer},
        )

    def swapped(a, j):
        place = swap_outs[a].at[rows_of(owner_of(0, j)), :]
        return remote(
            place,
            place,
            swap_send.at[a, j - 1],
            swap_recv.at[a, j - 1],
            {"fs": lax.rem(z + j, n_fs)},
        )

    def relay(a, j, k):
        place = swap_outs[a].at[rows_of(owner_of(0, j)), :]
        return remote(
            place,
            place,
            relay_send.at[a, j - 1, k - 1],
            relay_recv.at[a, j - 1],
            {"tp": lax.rem(t + k, n_tp)},
        )

    hub = lax.rem(z, n_tp) == t

    def feeds(j):
        return lax.rem(lax.rem(z + j, n_fs), n_tp) == t

    for a in range(n_swap):
        for j in range(1, n_fs):

            @pl.when(feeds(j))
            def _():
                swap(a, j).start()

    for m in range(n_act):
        for side in range(2):

            @pl.when(line_sends(z, n_fs, side, 1))
            def _():
                hop(m, side, 1).start()

    sources = list(acts)
    for a in range(n_swap):
        cut = swap_outs[a].shape[1]
        sources.append(swaps[a].at[:, pl.ds(pl.multiple_of(z * cut, cut), cut)])
    finish = keep_own(
        sources, holders, [out.at[rows_of(z), :] for out in act_outs + swap_outs], own_sem
    )
    finish()
    if n_swap:

        @pl.when(hub)
        def _():
            for a in range(n_swap):
                for j in range(1, n_fs):
                    swapped(a, j).wait_recv()
                    for k in range(1, n_tp):
                        relay(a, j, k).start()

    for d in range(1, n_fs):
        for m in range(n_act):
            for side in range(2):

                @pl.when(line_receives(z, n_fs, side, d))
                def _():
                    arrival(m, side, d).wait_recv()
                    if d < n_fs - 1:

                        @pl.when(line_sends(z, n_fs, side, d + 1))
                        def _():
                            hop(m, side, d + 1).start()

    for d in range(1, n_fs):
        for m in range(n_act):
            for side in range(2):

                @pl.when(line_sends(z, n_fs, side, d))
                def _():
                    hop(m, side, d).wait_send()

    for a in range(n_swap):
        for j in range(1, n_fs):

            @pl.when(feeds(j))
            def _():
                swap(a, j).wait_send()

            @pl.when(hub)
            def _():
                for k in range(1, n_tp):
                    relay(a, j, k).wait_send()

            @pl.when(jnp.logical_not(hub))
            def _():
                relay(a, j, 1).wait_recv()


def gather_tokens(n_fs, n_tp, collective_id, acts, swaps):
    count = acts[0].shape[0]
    outs = [jax.ShapeDtypeStruct((n_fs * count, a.shape[1]), a.dtype) for a in acts]
    outs += [jax.ShapeDtypeStruct((n_fs * count, a.shape[1] // n_fs), a.dtype) for a in swaps]
    dma = pltpu.SemaphoreType.DMA
    total = len(outs)
    n_swap = max(len(swaps), 1)
    moved = sum(2 * o.shape[0] * o.shape[1] for o in outs)
    return pl.pallas_call(
        functools.partial(tokens_kernel, n_fs, n_tp, len(acts), len(swaps)),
        out_shape=outs,
        in_specs=[pl.BlockSpec(memory_space=pl.ANY)] * total,
        out_specs=[pl.BlockSpec(memory_space=pl.ANY)] * total,
        scratch_shapes=[pltpu.VMEM((count, o.shape[1]), o.dtype) for o in outs]
        + [
            dma((2, total)),
            dma((len(acts), 2, n_fs - 1)),
            dma((len(acts), 2, n_fs - 1)),
            dma((n_swap, n_fs - 1)),
            dma((n_swap, n_fs - 1)),
            dma((n_swap, n_fs - 1, n_tp - 1)),
            dma((n_swap, n_fs - 1)),
        ],
        compiler_params=pltpu.CompilerParams(
            collective_id=collective_id, has_side_effects=True
        ),
        cost_estimate=pl.CostEstimate(flops=0, bytes_accessed=16 * moved, transcendentals=0),
        name=f"gather_tokens_{collective_id}",
    )(*acts, *swaps)


def over_rep(part):
    part = part.astype(jnp.bfloat16)
    n_rep = lax.axis_size("rep")
    other = lax.ppermute(part, "rep", [(i, (i + 1) % n_rep) for i in range(n_rep)])
    return part, other


def added(pair):
    return pair[0].astype(jnp.float32) + pair[1].astype(jnp.float32)


def on_device(tokens, norm_gain, w_gate, w_up, w_down, cotangent):
    n_fs, n_tp = lax.axis_size("fs"), lax.axis_size("tp")
    whole_x, whole_dy, full_gate, full_up, full_down = gather_weights(
        n_fs, n_tp, tokens, cotangent, w_gate, w_up, w_down
    )
    width = whole_x.shape[1]
    wide_tokens = whole_x.astype(jnp.float32)
    gain_f = norm_gain.astype(jnp.float32)
    inverse = lax.rsqrt(jnp.mean(wide_tokens * wide_tokens, axis=-1, keepdims=True) + 1e-06)
    normed = (wide_tokens * inverse * gain_f).astype(jnp.bfloat16)
    gate = jnp.dot(normed, full_gate, preferred_element_type=jnp.float32)
    up_proj = jnp.dot(normed, full_up, preferred_element_type=jnp.float32)
    sigma = jax.nn.sigmoid(gate)
    active = gate * sigma
    hidden = (active * up_proj).astype(jnp.bfloat16)
    back = 0.5 * contract_last(whole_dy, full_down)
    d_up = (back * active).astype(jnp.bfloat16)
    d_gate = (back * up_proj * sigma * (1.0 + gate * (1.0 - sigma))).astype(jnp.bfloat16)

    all_hidden, rows_dy = gather_tokens(n_fs, n_tp, 1, [hidden], [whole_dy])
    down_pair = over_rep(0.5 * contract_first(all_hidden, rows_dy))

    partial_normed = contract_last(d_gate, full_gate) + contract_last(d_up, full_up)
    d_normed = lax.psum_scatter(
        partial_normed.astype(jnp.bfloat16), "tp", scatter_dimension=1, tiled=True
    ).astype(jnp.float32)

    all_gate, rows_normed = gather_tokens(n_fs, n_tp, 2, [d_gate], [normed])
    gate_pair = over_rep(contract_first(rows_normed, all_gate))
    (all_up,) = gather_tokens(n_fs, n_tp, 3, [d_up], [])
    up_pair = over_rep(contract_first(rows_normed, all_up))

    local_width = d_normed.shape[1]
    local_gain = lax.dynamic_slice_in_dim(
        gain_f, lax.axis_index("tp") * local_width, local_width, 0
    )
    local_tokens = tokens.astype(jnp.float32)
    scaled_grad = d_normed * local_gain
    rowdot = lax.psum(jnp.sum(scaled_grad * local_tokens, axis=-1), "tp")
    grad_tokens = (
        cotangent.astype(jnp.float32)
        + inverse * scaled_grad
        - local_tokens * inverse**3 * rowdot[:, None] / width
    ).astype(jnp.bfloat16)
    grad_gain = lax.psum(jnp.sum(d_normed * local_tokens * inverse, axis=0), ("rep", "fs"))

    grad_down = added(down_pair)
    down_sq = lax.psum(jnp.sum(grad_down * grad_down, axis=1), "fs")
    grad_gate = added(gate_pair)
    grad_up = added(up_pair)
    gate_up_sq = lax.psum(
        jnp.stack([jnp.sum(grad_gate * grad_gate, axis=1), jnp.sum(grad_up * grad_up, axis=1)]),
        "tp",
    )
    return (grad_tokens, grad_gain, grad_gate, grad_up, grad_down, gate_up_sq, down_sq)


CORES = 2


def line_next(z, n_fs, side):
    return z <= n_fs - 2 if side == 0 else z >= 1


def pull_kernel(n_fs, *refs):
    tokens, cot, w_gate, w_up, w_down = refs[:5]
    outs = refs[5:10]
    act_hold, weight_hold, down_hold = refs[10:13]
    (own_sem, az_own, az_fwd, az_recv, ay_own, ay_fwd, ay_recv, ap_send, ap_recv) = refs[13:22]
    (w_send, w_recv, wx_send, wx_recv, wp_send, wp_recv, wo_send, wo_recv) = refs[22:]
    r, z, t = lax.axis_index("rep"), lax.axis_index("fs"), lax.axis_index("tp")
    y, c = lax.div(t, CORES), lax.rem(t, CORES)
    acts, weights = (tokens, cot), (w_gate, w_up, w_down)
    half, local = tokens.shape[0] // CORES, tokens.shape[1]
    rows = w_gate.shape[0]
    kb = n_fs // CORES
    width = w_gate.shape[1] // kb
    partner = {"tp": y * CORES + 1 - c}
    across = {"rep": 1 - r}
    owner = lax.div(z, kb)

    peers = [partner, across]
    peers += [{"tp": (1 - y) * CORES + h} for h in range(CORES)]
    for j in range(1, n_fs):
        for h in range(CORES):
            peers.append({"fs": lax.rem(z + j, n_fs), "tp": y * CORES + h})
    greet(peers)

    def own_act(a, h):
        return acts[a].at[pl.ds(pl.multiple_of(h * half, half), half), :]

    def act_place(a, source, column):
        return outs[a].at[
            pl.ds(pl.multiple_of(source * half, half), half),
            pl.ds(pl.multiple_of(column * local, local), local),
        ]

    def source_of(side, d):
        return z - d if side == 0 else z + d

    def next_of(side):
        return z + 1 if side == 0 else z - 1

    def act_first(a, side, h):
        return remote(
            own_act(a, h),
            act_place(a, z, t),
            az_own.at[a, side, h],
            az_recv.at[a, side, 0, c],
            {"fs": next_of(side), "tp": y * CORES + h},
        )

    def act_arrival(a, side, d, core):
        place = act_place(a, source_of(side, d), y * CORES + core)
        return remote(
            place, place, az_fwd.at[a, side, d - 1, core], az_recv.at[a, side, d - 1, core], partner
        )

    def act_forward(a, side, d, core):
        place = act_place(a, source_of(side, d), y * CORES + core)
        return remote(
            place,
            place,
            az_fwd.at[a, side, d - 1, core],
            az_recv.at[a, side, d, core],
            {"fs": next_of(side)},
        )

    def act_over(a, side, d, core):
        source = source_of(side, d)
        place = act_place(a, source, y * CORES + core)
        return remote(
            place,
            place,
            ay_fwd.at[a, side, d - 1, core],
            ay_recv.at[a, source, core],
            {"tp": (1 - y) * CORES + c},
        )

    def act_over_own(a, h):
        return remote(
            own_act(a, h),
            act_place(a, z, t),
            ay_own.at[a, h],
            ay_recv.at[a, z, c],
            {"tp": (1 - y) * CORES + h},
        )

    def act_over_arrival(a, source, core):
        place = act_place(a, source, (1 - y) * CORES + core)
        return remote(place, place, ay_own.at[a, 0], ay_recv.at[a, source, core], partner)

    def act_partner(a):
        return remote(own_act(a, 1 - c), act_place(a, z, t), ap_send.at[a], ap_recv.at[a], partner)

    def act_partner_arrival(a):
        place = act_place(a, z, y * CORES + 1 - c)
        return remote(place, place, ap_send.at[a], ap_recv.at[a], partner)

    def block_of(m, k):
        if m == 2:
            return weights[m].at[pl.ds(pl.multiple_of(k * width, width), width), :]
        return weights[m].at[:, pl.ds(pl.multiple_of(k * width, width), width)]

    def band_of(m, source):
        band = pl.ds(pl.multiple_of(source * rows, rows), rows)
        return outs[2 + m].at[:, band] if m == 2 else outs[2 + m].at[band, :]

    def quarter(m, source, rep, core):
        if m == 2:
            size = width // (2 * CORES)
            return outs[4].at[
                pl.ds(pl.multiple_of((rep * CORES + core) * size, size), size),
                pl.ds(pl.multiple_of(source * rows, rows), rows),
            ]
        size = rows // (2 * CORES)
        start = source * rows + (rep * CORES + core) * size
        return outs[2 + m].at[pl.ds(pl.multiple_of(start, size), size), :]

    def own_quarter(m, k, core):
        if m == 2:
            size = width // (2 * CORES)
            start = k * width + (r * CORES + core) * size
            return weights[m].at[pl.ds(pl.multiple_of(start, size), size), :]
        size = rows // (2 * CORES)
        return weights[m].at[
            pl.ds(pl.multiple_of((r * CORES + core) * size, size), size),
            pl.ds(k * width, width),
        ]

    def weight_send(m, k, core):
        return remote(
            own_quarter(m, k, core),
            quarter(m, z, r, core),
            w_send.at[m, k, core],
            w_recv.at[m, z],
            {"fs": kb * c + k, "tp": y * CORES + core},
        )

    def weight_arrival(m, source):
        place = quarter(m, source, r, c)
        return remote(place, place, wx_send.at[m, source], w_recv.at[m, source], partner)

    def weight_across(m, source):
        place = quarter(m, source, r, c)
        return remote(place, place, wx_send.at[m, source], wx_recv.at[m, source], across)

    def weight_across_arrival(m, source):
        place = quarter(m, source, 1 - r, c)
        return remote(place, place, wx_send.at[m, source], wx_recv.at[m, source], across)

    def weight_beside(m, source, which):
        place = quarter(m, source, r if which == 0 else 1 - r, c)
        return remote(
            place, place, wp_send.at[m, source, which], wp_recv.at[m, source, which], partner
        )

    def weight_beside_arrival(m, source, which):
        place = quarter(m, source, r if which == 0 else 1 - r, 1 - c)
        return remote(
            place, place, wp_send.at[m, source, which], wp_recv.at[m, source, which], partner
        )

    def own_beside(m):
        return remote(
            block_of(m, z - kb * owner), band_of(m, z), wo_send.at[m], wo_recv.at[m], partner
        )

    def own_beside_arrival(m):
        return remote(band_of(m, z), band_of(m, z), wo_send.at[m], wo_recv.at[m], partner)

    for a in range(2):
        for h in range(CORES):
            for side in range(2):

                @pl.when(line_next(z, n_fs, side))
                def _():
                    act_first(a, side, h).start()

            act_over_own(a, h).start()
    for a in range(2):
        act_partner(a).start()

    @pl.when(c == owner)
    def _():
        for m in range(3):
            own_beside(m).start()

    holders = [act_hold.at[0], act_hold.at[1]]
    loads = [pltpu.make_async_copy(own_act(a, c), holders[a], own_sem.at[0, a]) for a in range(2)]
    stores = [
        pltpu.make_async_copy(holders[a], act_place(a, z, t), own_sem.at[1, a]) for a in range(2)
    ]
    for load in loads:
        load.start()
    for load, store in zip(loads, stores):
        load.wait()
        store.start()
    for store in stores:
        store.wait()

    @pl.when(c == owner)
    def _():
        places = [weight_hold.at[0], weight_hold.at[1], down_hold]
        loads = [
            pltpu.make_async_copy(block_of(m, z - kb * owner), places[m], own_sem.at[0, 2 + m])
            for m in range(3)
        ]
        stores = [
            pltpu.make_async_copy(places[m], band_of(m, z), own_sem.at[1, 2 + m])
            for m in range(3)
        ]
        for load in loads:
            load.start()
        for load, store in zip(loads, stores):
            load.wait()
            store.start()
        for store in stores:
            store.wait()

    def act_round(d):
        for a in range(2):
            for core in range(CORES):
                for side in range(2):

                    @pl.when(line_receives(z, n_fs, side, d))
                    def _():
                        act_arrival(a, side, d, core).wait_recv()
                        if d < n_fs - 1:

                            @pl.when(line_next(z, n_fs, side))
                            def _():
                                act_forward(a, side, d, core).start()

                        act_over(a, side, d, core).start()

    def weight_round(d):
        for m in range(3):
            for side in range(2):

                @pl.when(line_receives(z, n_fs, side, d))
                def _():
                    source = source_of(side, d)
                    weight_arrival(m, source).wait_recv()
                    weight_across(m, source).start()
                    weight_beside(m, source, 0).start()

    def across_round(d):
        for m in range(3):
            for side in range(2):

                @pl.when(line_receives(z, n_fs, side, d))
                def _():
                    source = source_of(side, d)
                    weight_across_arrival(m, source).wait_recv()
                    weight_beside(m, source, 1).start()

    act_round(1)
    for m in range(3):
        for k in range(kb):

            @pl.when(kb * c + k != z)
            def _():
                for core in range(CORES):
                    weight_send(m, k, core).start()

    for d in range(1, n_fs):
        if d + 1 < n_fs:
            act_round(d + 1)
        weight_round(d)
        if d > 1:
            across_round(d - 1)
    across_round(n_fs - 1)

    for d in range(1, n_fs):
        for side in range(2):

            @pl.when(line_receives(z, n_fs, side, d))
            def _():
                source = source_of(side, d)
                for a in range(2):
                    for core in range(CORES):
                        act_over_arrival(a, source, core).wait_recv()
                        act_over(a, side, d, core).wait_send()
                        if d < n_fs - 1:

                            @pl.when(line_next(z, n_fs, side))
                            def _():
                                act_forward(a, side, d, core).wait_send()

                for m in range(3):
                    weight_across(m, source).wait_send()
                    for which in range(2):
                        weight_beside_arrival(m, source, which).wait_recv()
                        weight_beside(m, source, which).wait_send()

    for a in range(2):
        act_partner_arrival(a).wait_recv()
        act_partner(a).wait_send()
        for h in range(CORES):
            act_over_arrival(a, z, h).wait_recv()
            act_over_own(a, h).wait_send()
            for side in range(2):

                @pl.when(line_next(z, n_fs, side))
                def _():
                    act_first(a, side, h).wait_send()

    for m in range(3):
        for k in range(kb):

            @pl.when(kb * c + k != z)
            def _():
                for core in range(CORES):
                    weight_send(m, k, core).wait_send()

    @pl.when(c == owner)
    def _():
        for m in range(3):
            own_beside(m).wait_send()

    @pl.when(c != owner)
    def _():
        for m in range(3):
            own_beside_arrival(m).wait_recv()


def pull(n_fs, n_tp, tokens, cot, w_gate, w_up, w_down):
    half, local = tokens.shape[0] // CORES, tokens.shape[1]
    rows, hidden = w_gate.shape
    width = hidden * CORES // n_fs
    model = rows * n_fs
    dtype = tokens.dtype
    shapes = [(half * n_fs, model)] * 2 + [(model, width)] * 2 + [(width, model)]
    dma = pltpu.SemaphoreType.DMA
    kb = n_fs // CORES
    line = (2, 2, n_fs - 1, CORES)
    return pl.pallas_call(
        functools.partial(pull_kernel, n_fs),
        out_shape=[jax.ShapeDtypeStruct(s, dtype) for s in shapes],
        in_specs=[pl.BlockSpec(memory_space=pl.ANY)] * 5,
        out_specs=[pl.BlockSpec(memory_space=pl.ANY)] * 5,
        scratch_shapes=[
            pltpu.VMEM((2, half, local), dtype),
            pltpu.VMEM((2, rows, width), dtype),
            pltpu.VMEM((width, rows), dtype),
            dma((2, 5)),
            dma((2, 2, CORES)),
            dma(line),
            dma(line),
            dma((2, CORES)),
            dma(line),
            dma((2, n_fs, CORES)),
            dma((2,)),
            dma((2,)),
            dma((3, kb, CORES)),
            dma((3, n_fs)),
            dma((3, n_fs)),
            dma((3, n_fs)),
            dma((3, n_fs, 2)),
            dma((3, n_fs, 2)),
            dma((3,)),
            dma((3,)),
        ],
        compiler_params=pltpu.CompilerParams(collective_id=4, has_side_effects=True),
        cost_estimate=pl.CostEstimate(
            flops=0, bytes_accessed=sum(2 * a * b for a, b in shapes), transcendentals=0
        ),
        name="pull",
    )(tokens, cot, w_gate, w_up, w_down)


def push_kernel(n_fs, *refs):
    partial, g_gate, g_up, g_down, inv = refs[:5]
    o_gate, o_up, o_down, o_normed, o_inv = refs[5:10]
    pair_wide, pair_tall, sum_wide, sum_tall, x_wide, x_tall, t_wide, t_tall = refs[10:18]
    y_buf, d_buf, z_buf, n_buf = refs[18:22]
    (p_send, p_recv, x_send, x_recv, z_send, z_recv, f_send, f_recv) = refs[22:30]
    (y_send, y_recv, d_send, d_recv, n_send, n_recv, own_sem) = refs[30:]
    r, z, t = lax.axis_index("rep"), lax.axis_index("fs"), lax.axis_index("tp")
    y, c = lax.div(t, CORES), lax.rem(t, CORES)
    kb = n_fs // CORES
    half = partial.shape[0] // n_fs
    reach = partial.shape[1] // 2
    local = reach // CORES
    width = g_gate.shape[1]
    rows = g_gate.shape[0] // n_fs
    strip = rows // 2
    partner = {"tp": y * CORES + 1 - c}
    across = {"rep": 1 - r}
    beside = {"tp": (1 - y) * CORES + c}
    owner = lax.div(z, kb)
    grads, outs = (g_gate, g_up, g_down), (o_gate, o_up, o_down)

    peers = [partner, across, beside]
    for j in range(1, n_fs):
        for h in range(CORES):
            peers.append({"fs": lax.rem(z + j, n_fs), "tp": y * CORES + h})
    greet(peers)

    def slot(wide, tall, m, *where):
        return tall.at[where] if m == 2 else wide.at[(m,) + where]

    def strip_of(band, rep):
        return pl.ds(pl.multiple_of(band * rows + rep * strip, strip), strip)

    def grad_piece(m, band, rep):
        if m == 2:
            return grads[m].at[:, strip_of(band, rep)]
        return grads[m].at[strip_of(band, rep), :]

    def rep_of(j):
        return 1 - r if j == 0 else r

    def pair(m, k, j):
        return remote(
            grad_piece(m, kb * (1 - c) + k, rep_of(j)),
            slot(pair_wide, pair_tall, m, k, j),
            p_send.at[m, k, j],
            p_recv.at[m, k, j],
            partner,
        )

    def swap(m, k):
        return remote(
            slot(sum_wide, sum_tall, m, k),
            slot(x_wide, x_tall, m, k),
            x_send.at[m, k],
            x_recv.at[m, k],
            across,
        )

    def place(m, block, rep):
        strips = pl.ds(pl.multiple_of(rep * strip, strip), strip)
        blocks = pl.ds(pl.multiple_of(block * width, width), width)
        return outs[m].at[blocks, strips] if m == 2 else outs[m].at[strips, blocks]

    def deliver(m, k):
        block = lax.rem(z, kb)
        return remote(
            slot(t_wide, t_tall, m, k),
            place(m, block, r),
            z_send.at[m, k],
            z_recv.at[m, block],
            {"fs": kb * c + k, "tp": y * CORES + owner},
        )

    def delivered(m, k):
        return remote(place(m, k, r), place(m, k, r), z_send.at[m, k], z_recv.at[m, k], partner)

    def keep(m, k):
        return pltpu.make_async_copy(slot(t_wide, t_tall, m, k), place(m, k, r), own_sem.at[m])

    def spread(m, k, source):
        return remote(source, place(m, k, r), f_send.at[m, k], f_recv.at[m, k], across)

    def spread_arrival(m, k):
        return remote(
            place(m, k, 1 - r), place(m, k, 1 - r), f_send.at[m, k], f_recv.at[m, k], across
        )

    def band_rows(band):
        return pl.ds(pl.multiple_of(band * half, half), half)

    def side_columns(which):
        return pl.ds(pl.multiple_of(which * reach, reach), reach)

    def over(j):
        band = lax.rem(z + j, n_fs)
        return remote(
            partial.at[band_rows(band), side_columns(1 - y)],
            y_buf.at[j],
            y_send.at[j],
            y_recv.at[j],
            beside,
        )

    def normed_send(j):
        return remote(
            d_buf.at[j], z_buf.at[z], d_send.at[j], d_recv.at[z], {"fs": lax.rem(z + j, n_fs)}
        )

    def normed_arrival(j):
        source = lax.rem(z + j, n_fs)
        return remote(z_buf.at[source], z_buf.at[source], d_send.at[j], d_recv.at[source], partner)

    def own_rows(core):
        return pl.ds(pl.multiple_of(core * half, half), half)

    def inv_send():
        return remote(inv, o_inv.at[own_rows(c), :], n_send.at[0], n_recv.at[0], partner)

    def inv_arrival():
        at = o_inv.at[own_rows(1 - c), :]
        return remote(at, at, n_send.at[0], n_recv.at[0], partner)

    def last_send():
        return remote(n_buf, o_normed.at[own_rows(c), :], n_send.at[1], n_recv.at[1], partner)

    def last_arrival():
        at = o_normed.at[own_rows(1 - c), :]
        return remote(at, at, n_send.at[1], n_recv.at[1], partner)

    items = [(m, k) for m in (2, 0, 1) for k in range(kb)]
    order = list(range(1, n_fs)) + [0]
    for m, k in items:
        pair(m, k, 0).start()
    for j in order:
        over(j).start()
    for m, k in items:
        pair(m, k, 1).start()
    inv_send().start()
    o_inv[own_rows(c), :] = inv[...]

    def added(m, k, j):
        own = grad_piece(m, kb * c + k, rep_of(j))[...].astype(jnp.float32)
        return own + slot(pair_wide, pair_tall, m, k, j)[...].astype(jnp.float32)

    def put(wide, tall, m, k, value):
        if m == 2:
            tall[k] = value
        else:
            wide[m, k] = value

    def first(m, k):
        pair(m, k, 0).wait_recv()
        put(sum_wide, sum_tall, m, k, added(m, k, 0).astype(jnp.bfloat16))
        swap(m, k).start()

    def second(m, k):
        pair(m, k, 1).wait_recv()
        swap(m, k).wait_recv()
        whole = added(m, k, 1) + slot(x_wide, x_tall, m, k)[...].astype(jnp.float32)
        put(t_wide, t_tall, m, k, whole.astype(jnp.bfloat16))
        mine = kb * c + k == z

        @pl.when(mine)
        def _():
            keep(m, k).start()
            spread(m, k, slot(t_wide, t_tall, m, k)).start()

        @pl.when(jnp.logical_not(mine))
        def _():
            deliver(m, k).start()

    def third(m, k):
        @pl.when(kb * c + k != z)
        def _():
            delivered(m, k).wait_recv()
            spread(m, k, place(m, k, r)).start()

    def normed_step(j):
        over(j).wait_recv()
        band = lax.rem(z + j, n_fs)
        own = partial[band_rows(band), side_columns(y)].astype(jnp.float32)
        d_buf[j] = (own + y_buf[j].astype(jnp.float32)).astype(jnp.bfloat16)
        if j:
            normed_send(j).start()

    for m, k in items:
        first(m, k)
    n_items = len(items)
    for i in range(n_items + 2):
        if i < n_items:
            second(*items[i])
        if i < n_fs:
            normed_step(order[i])
        if i >= 2:
            third(*items[i - 2])

    for j in range(1, n_fs):
        normed_arrival(j).wait_recv()
    total = d_buf[0].astype(jnp.float32)
    for j in range(1, n_fs):
        total = total + z_buf[lax.rem(z + j, n_fs)].astype(jnp.float32)
    total = total.astype(jnp.bfloat16)

    @pl.when(c == 0)
    def _():
        o_normed[pl.ds(0, half), :] = total[:, :local]
        n_buf[...] = total[:, local:]

    @pl.when(c == 1)
    def _():
        o_normed[pl.ds(half, half), :] = total[:, local:]
        n_buf[...] = total[:, :local]

    last_send().start()

    for m, k in items:
        for j in range(2):
            pair(m, k, j).wait_send()
        swap(m, k).wait_send()
        mine = kb * c + k == z

        @pl.when(mine)
        def _():
            keep(m, k).wait()

        @pl.when(jnp.logical_not(mine))
        def _():
            deliver(m, k).wait_send()

        spread(m, k, place(m, k, r)).wait_send()
        spread_arrival(m, k).wait_recv()
    for j in range(n_fs):
        over(j).wait_send()
        if j:
            normed_send(j).wait_send()
    inv_send().wait_send()
    inv_arrival().wait_recv()
    last_send().wait_send()
    last_arrival().wait_recv()


def push(n_fs, partial, g_gate, g_up, g_down, inv):
    kb = n_fs // CORES
    half, model = partial.shape[0] // n_fs, partial.shape[1]
    width, rows = g_gate.shape[1], g_gate.shape[0] // n_fs
    strip = rows // 2
    reach = model // 2
    local = reach // CORES
    dtype = partial.dtype
    dma = pltpu.SemaphoreType.DMA
    vmem = pl.BlockSpec(memory_space=pltpu.VMEM)
    hbm = pl.BlockSpec(memory_space=pl.ANY)
    wide, tall = (strip, width), (width, strip)
    shapes = [(rows, kb * width)] * 2 + [(kb * width, rows)]
    pairs = dma((3, kb, 2))
    singles = dma((3, kb))
    return pl.pallas_call(
        functools.partial(push_kernel, n_fs),
        out_shape=[jax.ShapeDtypeStruct(s, dtype) for s in shapes]
        + [
            jax.ShapeDtypeStruct((CORES * half, local), dtype),
            jax.ShapeDtypeStruct((CORES * half, inv.shape[1]), inv.dtype),
        ],
        in_specs=[vmem] * 5,
        out_specs=[hbm] * 3 + [vmem] * 2,
        scratch_shapes=[
            pltpu.VMEM((2, kb, 2) + wide, dtype),
            pltpu.VMEM((kb, 2) + tall, dtype),
            pltpu.VMEM((2, kb) + wide, dtype),
            pltpu.VMEM((kb,) + tall, dtype),
            pltpu.VMEM((2, kb) + wide, dtype),
            pltpu.VMEM((kb,) + tall, dtype),
            pltpu.VMEM((2, kb) + wide, dtype),
            pltpu.VMEM((kb,) + tall, dtype),
            pltpu.VMEM((n_fs, half, reach), dtype),
            pltpu.VMEM((n_fs, half, reach), dtype),
            pltpu.VMEM((n_fs, half, reach), dtype),
            pltpu.VMEM((half, local), dtype),
            pairs,
            pairs,
            singles,
            singles,
            singles,
            singles,
            singles,
            singles,
            dma((n_fs,)),
            dma((n_fs,)),
            dma((n_fs,)),
            dma((n_fs,)),
            dma((2,)),
            dma((2,)),
            dma((3,)),
        ],
        compiler_params=pltpu.CompilerParams(
            collective_id=5, has_side_effects=True, vmem_limit_bytes=56 * 1024 * 1024
        ),
        cost_estimate=pl.CostEstimate(
            flops=0, bytes_accessed=sum(2 * a * b for a, b in shapes), transcendentals=0
        ),
        name="push",
    )(partial, g_gate, g_up, g_down, inv)


def sums_kernel(n_fs, n_tp, n_rep, here, there, all_here, all_there, h_send, h_recv, o_send, o_recv):
    r, z, t = lax.axis_index("rep"), lax.axis_index("fs"), lax.axis_index("tp")
    groups = n_rep * n_fs
    spot = r * n_fs + z

    def group_of(j):
        at = lax.rem(spot + j, groups)
        return {"rep": lax.div(at, n_fs), "fs": lax.rem(at, n_fs)}

    def lane_of(j):
        return {"tp": lax.rem(t + j, n_tp)}

    greet([lane_of(j) for j in range(1, n_tp)] + [group_of(j) for j in range(1, groups)])
    sends = []
    for j in range(1, n_tp):
        sends.append(
            remote(here, all_here.at[t], h_send.at[j - 1], h_recv.at[n_tp - j - 1], lane_of(j))
        )
    for j in range(1, groups):
        sends.append(
            remote(there, all_there.at[spot], o_send.at[j - 1], o_recv.at[groups - j - 1], group_of(j))
        )
    for copy in sends:
        copy.start()
    all_here[t] = here[...]
    all_there[spot] = there[...]
    for j in range(1, n_tp):
        place = all_here.at[lax.rem(t + j, n_tp)]
        remote(place, place, h_send.at[j - 1], h_recv.at[j - 1], lane_of(j)).wait_recv()
    for j in range(1, groups):
        place = all_there.at[lax.rem(spot + j, groups)]
        remote(place, place, o_send.at[j - 1], o_recv.at[j - 1], group_of(j)).wait_recv()
    for copy in sends:
        copy.wait_send()


def exchange_sums(n_fs, n_tp, n_rep, here, there):
    dma = pltpu.SemaphoreType.DMA
    vmem = pl.BlockSpec(memory_space=pltpu.VMEM)
    groups = n_rep * n_fs
    return pl.pallas_call(
        functools.partial(sums_kernel, n_fs, n_tp, n_rep),
        out_shape=[
            jax.ShapeDtypeStruct((n_tp,) + here.shape, here.dtype),
            jax.ShapeDtypeStruct((groups,) + there.shape, there.dtype),
        ],
        in_specs=[vmem] * 2,
        out_specs=[vmem] * 2,
        scratch_shapes=[dma((n_tp - 1,)), dma((n_tp - 1,)), dma((groups - 1,)), dma((groups - 1,))],
        compiler_params=pltpu.CompilerParams(collective_id=6, has_side_effects=True),
        name="exchange_sums",
    )(here, there)


def packed(parts):
    flat = jnp.concatenate([p.reshape(-1) for p in parts])
    size = -(-flat.shape[0] // 1024) * 1024
    return jnp.pad(flat, (0, size - flat.shape[0])).reshape(-1, 128)


def by_chip(tokens, norm_gain, w_gate, w_up, w_down, cotangent):
    n_rep, n_fs, n_tp = lax.axis_size("rep"), lax.axis_size("fs"), lax.axis_size("tp")
    count, local = tokens.shape
    rows, wide = w_gate.shape
    half = count // CORES
    x, dy, f_gate, f_up, f_down = pull(n_fs, n_tp, tokens, cotangent, w_gate, w_up, w_down)
    model = x.shape[1]
    wide_tokens = x.astype(jnp.float32)
    gain_f = norm_gain.astype(jnp.float32)
    inverse = lax.rsqrt(jnp.mean(wide_tokens * wide_tokens, axis=-1, keepdims=True) + 1e-06)
    normed = (wide_tokens * inverse * gain_f).astype(jnp.bfloat16)
    gate = jnp.dot(normed, f_gate, preferred_element_type=jnp.float32)
    up_proj = jnp.dot(normed, f_up, preferred_element_type=jnp.float32)
    sigma = jax.nn.sigmoid(gate)
    active = gate * sigma
    hidden = (active * up_proj).astype(jnp.bfloat16)
    back = 0.5 * contract_last(dy, f_down)
    d_up = (back * active).astype(jnp.bfloat16)
    d_gate = (back * up_proj * sigma * (1.0 + gate * (1.0 - sigma))).astype(jnp.bfloat16)
    partial = (contract_last(d_gate, f_gate) + contract_last(d_up, f_up)).astype(jnp.bfloat16)
    g_down = (0.5 * contract_first(hidden, dy)).astype(jnp.bfloat16)
    g_gate = contract_first(normed, d_gate).astype(jnp.bfloat16)
    g_up = contract_first(normed, d_up).astype(jnp.bfloat16)
    own = lax.dynamic_slice_in_dim(inverse, lax.axis_index("fs") * half, half, 0)
    s_gate, s_up, s_down, d_normed, inv = push(
        n_fs, partial, g_gate, g_up, g_down, jnp.broadcast_to(own, (half, 128))
    )

    grad_gate, grad_up, grad_down = (s.astype(jnp.float32) for s in (s_gate, s_up, s_down))
    d_normed = d_normed.astype(jnp.float32)
    inv = inv[:, :1]
    gain_here = lax.dynamic_slice_in_dim(gain_f, lax.axis_index("tp") * local, local, 0)
    local_tokens = tokens.astype(jnp.float32)
    scaled = d_normed * gain_here
    here = packed(
        [
            jnp.sum(scaled * local_tokens, axis=-1),
            jnp.sum(grad_gate * grad_gate, axis=1),
            jnp.sum(grad_up * grad_up, axis=1),
        ]
    )
    there = packed(
        [
            jnp.sum(d_normed * local_tokens * inv, axis=0),
            jnp.sum(grad_down * grad_down, axis=1),
        ]
    )
    all_here, all_there = exchange_sums(n_fs, n_tp, n_rep, here, there)
    here = jnp.sum(all_here, axis=0).reshape(-1)
    rowdot = here[:count]
    gate_up_sq = here[count : count + 2 * rows].reshape(2, rows)
    flat = all_there.reshape(n_rep, n_fs, -1)
    grad_gain = jnp.sum(flat[:, :, :local], axis=(0, 1))
    down_sq = jnp.sum(flat[0, :, local : local + wide], axis=0)
    grad_tokens = (
        cotangent.astype(jnp.float32)
        + inv * scaled
        - local_tokens * inv**3 * rowdot[:, None] / model
    ).astype(jnp.bfloat16)
    return (grad_tokens, grad_gain, grad_gate, grad_up, grad_down, gate_up_sq, down_sq)


def fits_chips(mesh):
    n_rep, n_fs, n_tp = mesh.shape["rep"], mesh.shape["fs"], mesh.shape["tp"]
    return n_rep == 2 and n_tp == 2 * CORES and n_fs == 2 * CORES


def solution(mesh):
    placed = (
        P(("rep", "fs"), "tp"),
        P(),
        P("fs", "tp"),
        P("fs", "tp"),
        P("tp", "fs"),
        P(("rep", "fs"), "tp"),
    )
    return jax.shard_map(
        by_chip if fits_chips(mesh) else on_device,
        mesh=mesh,
        in_specs=placed,
        out_specs=(
            P(("rep", "fs"), "tp"),
            P("tp"),
            P("fs", "tp"),
            P("fs", "tp"),
            P("tp", "fs"),
            P(None, "fs"),
            P("tp"),
        ),
        check_vma=False,
    )
```

```python
import functools

import jax
import jax.numpy as jnp
from jax import lax
from jax.experimental import pallas as pl
from jax.experimental.pallas import tpu as pltpu
from jax.sharding import PartitionSpec as P

MESH = pl.DeviceIdType.MESH


def contract_last(left, right):
    return lax.dot_general(
        left, right, (((1,), (1,)), ((), ())), preferred_element_type=jnp.float32
    )


def contract_first(left, right):
    return lax.dot_general(
        left, right, (((0,), (0,)), ((), ())), preferred_element_type=jnp.float32
    )


def remote(source, target, send_sem, recv_sem, where):
    return pltpu.make_async_remote_copy(
        src_ref=source,
        dst_ref=target,
        send_sem=send_sem,
        recv_sem=recv_sem,
        device_id=where,
        device_id_type=MESH,
    )


def line_sends(z, n_fs, side, d):
    if side == 0:
        return jnp.logical_and(z >= d - 1, z <= n_fs - 2)
    return jnp.logical_and(z + d <= n_fs, z >= 1)


def line_receives(z, n_fs, side, d):
    return z >= d if side == 0 else z + d <= n_fs - 1


def greet(peers):
    barrier = pltpu.get_barrier_semaphore()
    for peer in peers:
        pl.semaphore_signal(barrier, inc=1, device_id=peer, device_id_type=MESH)
    pl.semaphore_wait(barrier, len(peers))


def keep_own(sources, holders, targets, sems):
    count = len(sources)
    loads = [
        pltpu.make_async_copy(sources[i], holders[i], sems.at[0, i]) for i in range(count)
    ]
    stores = [
        pltpu.make_async_copy(holders[i], targets[i], sems.at[1, i]) for i in range(count)
    ]
    for load in loads:
        load.start()

    def finish():
        for load, store in zip(loads, stores):
            load.wait()
            store.start()
        for store in stores:
            store.wait()

    return finish


def weights_kernel(n_fs, n_tp, *refs):
    tokens, cot, w_gate, w_up, w_down = refs[:5]
    whole_x, whole_dy, full_gate, full_up, full_down = refs[5:10]
    holders = refs[10:15]
    own_sem, ring_send, ring_recv, rep_send, rep_recv, tp_send, tp_recv = refs[15:]
    r, z, t = lax.axis_index("rep"), lax.axis_index("fs"), lax.axis_index("tp")
    right, left = lax.rem(z + 1, n_fs), lax.rem(z + n_fs - 1, n_fs)
    partner = {"rep": 1 - r}
    sources = (w_gate, w_up, w_down)
    targets = (full_gate, full_up, full_down)
    rows = w_gate.shape[0]
    hidden = w_down.shape[0]
    local = tokens.shape[1]

    def own_piece(m, half):
        size = (hidden if m == 2 else rows) // 2
        return sources[m].at[pl.ds(pl.multiple_of(half * size, size), size), :]

    def piece(m, owner, half):
        if m == 2:
            size = hidden // 2
            return targets[m].at[
                pl.ds(pl.multiple_of(half * size, size), size),
                pl.ds(pl.multiple_of(owner * rows, rows), rows),
            ]
        size = rows // 2
        return targets[m].at[
            pl.ds(pl.multiple_of(owner * rows + half * size, size), size), :
        ]

    peers = [{"fs": right}, {"fs": left}, partner]
    peers += [{"tp": lax.rem(t + j, n_tp)} for j in range(1, n_tp)]
    greet(peers)

    def owner_of(side, back):
        return lax.rem(z + (n_fs - back if side == 0 else back), n_fs)

    def hop(m, side, d):
        place = piece(m, owner_of(side, d - 1), r)
        return remote(
            own_piece(m, r) if d == 1 else place,
            place,
            ring_send.at[m, side, d - 1],
            ring_recv.at[m, side, d - 1],
            {"fs": right if side == 0 else left},
        )

    def arrival(m, side, d):
        place = piece(m, owner_of(side, d), r)
        return remote(
            place,
            place,
            ring_send.at[m, side, d - 1],
            ring_recv.at[m, side, d - 1],
            {"fs": right if side == 0 else left},
        )

    def across(m, side, d):
        place = piece(m, owner_of(side, d), r)
        return remote(
            place, place, rep_send.at[m, side, d - 1], rep_recv.at[m, side, d - 1], partner
        )

    for m in range(3):
        for side in range(2):

            @pl.when(line_sends(z, n_fs, side, 1))
            def _():
                hop(m, side, 1).start()

    ends = []
    for a, (source, target) in enumerate(((tokens, whole_x), (cot, whole_dy))):
        place = target.at[:, pl.ds(pl.multiple_of(t * local, local), local)]
        for j in range(1, n_tp):
            copy = remote(
                source,
                place,
                tp_send.at[a, j - 1],
                tp_recv.at[a, j - 1],
                {"tp": lax.rem(t + j, n_tp)},
            )
            copy.start()
            ends.append(copy)
    mine = pl.ds(pl.multiple_of(t * local, local), local)
    band = pl.ds(pl.multiple_of(z * rows, rows), rows)
    finish = keep_own(
        (tokens, cot, w_gate, w_up, w_down),
        holders,
        (
            whole_x.at[:, mine],
            whole_dy.at[:, mine],
            full_gate.at[band, :],
            full_up.at[band, :],
            full_down.at[:, band],
        ),
        own_sem,
    )
    finish()
    for d in range(1, n_fs):
        for m in range(3):
            for side in range(2):

                @pl.when(line_receives(z, n_fs, side, d))
                def _():
                    arrival(m, side, d).wait_recv()
                    if d < n_fs - 1:

                        @pl.when(line_sends(z, n_fs, side, d + 1))
                        def _():
                            hop(m, side, d + 1).start()

                    across(m, side, d).start()

    for d in range(1, n_fs):
        for m in range(3):
            for side in range(2):

                @pl.when(line_sends(z, n_fs, side, d))
                def _():
                    hop(m, side, d).wait_send()

                @pl.when(line_receives(z, n_fs, side, d))
                def _():
                    across(m, side, d).wait()

    for copy in ends:
        copy.wait()


def gather_weights(n_fs, n_tp, tokens, cot, w_gate, w_up, w_down):
    count, local = tokens.shape
    rows, hidden = w_gate.shape
    width = rows * n_fs
    dtype = tokens.dtype
    shapes = [
        (count, width),
        (count, width),
        (width, hidden),
        (width, hidden),
        (hidden, width),
    ]
    held = (tokens, cot, w_gate, w_up, w_down)
    moved = sum(2 * a * b for a, b in shapes)
    dma = pltpu.SemaphoreType.DMA
    return pl.pallas_call(
        functools.partial(weights_kernel, n_fs, n_tp),
        out_shape=[jax.ShapeDtypeStruct(s, dtype) for s in shapes],
        in_specs=[pl.BlockSpec(memory_space=pl.ANY)] * 5,
        out_specs=[pl.BlockSpec(memory_space=pl.ANY)] * 5,
        scratch_shapes=[pltpu.VMEM(a.shape, a.dtype) for a in held]
        + [
            dma((2, 5)),
            dma((3, 2, n_fs - 1)),
            dma((3, 2, n_fs - 1)),
            dma((3, 2, n_fs - 1)),
            dma((3, 2, n_fs - 1)),
            dma((2, n_tp - 1)),
            dma((2, n_tp - 1)),
        ],
        compiler_params=pltpu.CompilerParams(collective_id=0, has_side_effects=True),
        cost_estimate=pl.CostEstimate(flops=0, bytes_accessed=16 * moved, transcendentals=0),
        name="gather_weights",
    )(*held)


def tokens_kernel(n_fs, n_tp, n_act, n_swap, *refs):
    total = n_act + n_swap
    acts, swaps = refs[:n_act], refs[n_act:total]
    act_outs, swap_outs = refs[total : total + n_act], refs[total + n_act : 2 * total]
    holders = refs[2 * total : 3 * total]
    own_sem, ring_send, ring_recv = refs[3 * total : 3 * total + 3]
    swap_send, swap_recv, relay_send, relay_recv = refs[3 * total + 3 :]
    z, t = lax.axis_index("fs"), lax.axis_index("tp")
    right, left = lax.rem(z + 1, n_fs), lax.rem(z + n_fs - 1, n_fs)
    count = acts[0].shape[0]
    peers = [{"fs": lax.rem(z + j, n_fs)} for j in range(1, n_fs)]
    if n_swap:
        peers += [{"tp": lax.rem(t + j, n_tp)} for j in range(1, n_tp)]
    greet(peers)

    def rows_of(owner):
        return pl.ds(pl.multiple_of(owner * count, count), count)

    def owner_of(side, back):
        return lax.rem(z + (n_fs - back if side == 0 else back), n_fs)

    def hop(m, side, d):
        place = act_outs[m].at[rows_of(owner_of(side, d - 1)), :]
        return remote(
            acts[m] if d == 1 else place,
            place,
            ring_send.at[m, side, d - 1],
            ring_recv.at[m, side, d - 1],
            {"fs": right if side == 0 else left},
        )

    def arrival(m, side, d):
        place = act_outs[m].at[rows_of(owner_of(side, d)), :]
        return remote(
            place,
            place,
            ring_send.at[m, side, d - 1],
            ring_recv.at[m, side, d - 1],
            {"fs": right if side == 0 else left},
        )

    def swap(a, j):
        peer = lax.rem(z + j, n_fs)
        cut = swap_outs[a].shape[1]
        return remote(
            swaps[a].at[:, pl.ds(pl.multiple_of(peer * cut, cut), cut)],
            swap_outs[a].at[rows_of(z), :],
            swap_send.at[a, j - 1],
            swap_recv.at[a, j - 1],
            {"fs": peer},
        )

    def swapped(a, j):
        place = swap_outs[a].at[rows_of(owner_of(0, j)), :]
        return remote(
            place,
            place,
            swap_send.at[a, j - 1],
            swap_recv.at[a, j - 1],
            {"fs": lax.rem(z + j, n_fs)},
        )

    def relay(a, j, k):
        place = swap_outs[a].at[rows_of(owner_of(0, j)), :]
        return remote(
            place,
            place,
            relay_send.at[a, j - 1, k - 1],
            relay_recv.at[a, j - 1],
            {"tp": lax.rem(t + k, n_tp)},
        )

    hub = lax.rem(z, n_tp) == t

    def feeds(j):
        return lax.rem(lax.rem(z + j, n_fs), n_tp) == t

    for a in range(n_swap):
        for j in range(1, n_fs):

            @pl.when(feeds(j))
            def _():
                swap(a, j).start()

    for m in range(n_act):
        for side in range(2):

            @pl.when(line_sends(z, n_fs, side, 1))
            def _():
                hop(m, side, 1).start()

    sources = list(acts)
    for a in range(n_swap):
        cut = swap_outs[a].shape[1]
        sources.append(swaps[a].at[:, pl.ds(pl.multiple_of(z * cut, cut), cut)])
    finish = keep_own(
        sources, holders, [out.at[rows_of(z), :] for out in act_outs + swap_outs], own_sem
    )
    finish()
    if n_swap:

        @pl.when(hub)
        def _():
            for a in range(n_swap):
                for j in range(1, n_fs):
                    swapped(a, j).wait_recv()
                    for k in range(1, n_tp):
                        relay(a, j, k).start()

    for d in range(1, n_fs):
        for m in range(n_act):
            for side in range(2):

                @pl.when(line_receives(z, n_fs, side, d))
                def _():
                    arrival(m, side, d).wait_recv()
                    if d < n_fs - 1:

                        @pl.when(line_sends(z, n_fs, side, d + 1))
                        def _():
                            hop(m, side, d + 1).start()

    for d in range(1, n_fs):
        for m in range(n_act):
            for side in range(2):

                @pl.when(line_sends(z, n_fs, side, d))
                def _():
                    hop(m, side, d).wait_send()

    for a in range(n_swap):
        for j in range(1, n_fs):

            @pl.when(feeds(j))
            def _():
                swap(a, j).wait_send()

            @pl.when(hub)
            def _():
                for k in range(1, n_tp):
                    relay(a, j, k).wait_send()

            @pl.when(jnp.logical_not(hub))
            def _():
                relay(a, j, 1).wait_recv()


def gather_tokens(n_fs, n_tp, collective_id, acts, swaps):
    count = acts[0].shape[0]
    outs = [jax.ShapeDtypeStruct((n_fs * count, a.shape[1]), a.dtype) for a in acts]
    outs += [jax.ShapeDtypeStruct((n_fs * count, a.shape[1] // n_fs), a.dtype) for a in swaps]
    dma = pltpu.SemaphoreType.DMA
    total = len(outs)
    n_swap = max(len(swaps), 1)
    moved = sum(2 * o.shape[0] * o.shape[1] for o in outs)
    return pl.pallas_call(
        functools.partial(tokens_kernel, n_fs, n_tp, len(acts), len(swaps)),
        out_shape=outs,
        in_specs=[pl.BlockSpec(memory_space=pl.ANY)] * total,
        out_specs=[pl.BlockSpec(memory_space=pl.ANY)] * total,
        scratch_shapes=[pltpu.VMEM((count, o.shape[1]), o.dtype) for o in outs]
        + [
            dma((2, total)),
            dma((len(acts), 2, n_fs - 1)),
            dma((len(acts), 2, n_fs - 1)),
            dma((n_swap, n_fs - 1)),
            dma((n_swap, n_fs - 1)),
            dma((n_swap, n_fs - 1, n_tp - 1)),
            dma((n_swap, n_fs - 1)),
        ],
        compiler_params=pltpu.CompilerParams(
            collective_id=collective_id, has_side_effects=True
        ),
        cost_estimate=pl.CostEstimate(flops=0, bytes_accessed=16 * moved, transcendentals=0),
        name=f"gather_tokens_{collective_id}",
    )(*acts, *swaps)


def over_rep(part):
    part = part.astype(jnp.bfloat16)
    n_rep = lax.axis_size("rep")
    other = lax.ppermute(part, "rep", [(i, (i + 1) % n_rep) for i in range(n_rep)])
    return part, other


def added(pair):
    return pair[0].astype(jnp.float32) + pair[1].astype(jnp.float32)


def on_device(tokens, norm_gain, w_gate, w_up, w_down, cotangent):
    n_fs, n_tp = lax.axis_size("fs"), lax.axis_size("tp")
    whole_x, whole_dy, full_gate, full_up, full_down = gather_weights(
        n_fs, n_tp, tokens, cotangent, w_gate, w_up, w_down
    )
    width = whole_x.shape[1]
    wide_tokens = whole_x.astype(jnp.float32)
    gain_f = norm_gain.astype(jnp.float32)
    inverse = lax.rsqrt(jnp.mean(wide_tokens * wide_tokens, axis=-1, keepdims=True) + 1e-06)
    normed = (wide_tokens * inverse * gain_f).astype(jnp.bfloat16)
    gate = jnp.dot(normed, full_gate, preferred_element_type=jnp.float32)
    up_proj = jnp.dot(normed, full_up, preferred_element_type=jnp.float32)
    sigma = jax.nn.sigmoid(gate)
    active = gate * sigma
    hidden = (active * up_proj).astype(jnp.bfloat16)
    back = 0.5 * contract_last(whole_dy, full_down)
    d_up = (back * active).astype(jnp.bfloat16)
    d_gate = (back * up_proj * sigma * (1.0 + gate * (1.0 - sigma))).astype(jnp.bfloat16)

    all_hidden, rows_dy = gather_tokens(n_fs, n_tp, 1, [hidden], [whole_dy])
    down_pair = over_rep(0.5 * contract_first(all_hidden, rows_dy))

    partial_normed = contract_last(d_gate, full_gate) + contract_last(d_up, full_up)
    d_normed = lax.psum_scatter(
        partial_normed.astype(jnp.bfloat16), "tp", scatter_dimension=1, tiled=True
    ).astype(jnp.float32)

    all_gate, rows_normed = gather_tokens(n_fs, n_tp, 2, [d_gate], [normed])
    gate_pair = over_rep(contract_first(rows_normed, all_gate))
    (all_up,) = gather_tokens(n_fs, n_tp, 3, [d_up], [])
    up_pair = over_rep(contract_first(rows_normed, all_up))

    local_width = d_normed.shape[1]
    local_gain = lax.dynamic_slice_in_dim(
        gain_f, lax.axis_index("tp") * local_width, local_width, 0
    )
    local_tokens = tokens.astype(jnp.float32)
    scaled_grad = d_normed * local_gain
    rowdot = lax.psum(jnp.sum(scaled_grad * local_tokens, axis=-1), "tp")
    grad_tokens = (
        cotangent.astype(jnp.float32)
        + inverse * scaled_grad
        - local_tokens * inverse**3 * rowdot[:, None] / width
    ).astype(jnp.bfloat16)
    grad_gain = lax.psum(jnp.sum(d_normed * local_tokens * inverse, axis=0), ("rep", "fs"))

    grad_down = added(down_pair)
    down_sq = lax.psum(jnp.sum(grad_down * grad_down, axis=1), "fs")
    grad_gate = added(gate_pair)
    grad_up = added(up_pair)
    gate_up_sq = lax.psum(
        jnp.stack([jnp.sum(grad_gate * grad_gate, axis=1), jnp.sum(grad_up * grad_up, axis=1)]),
        "tp",
    )
    return (grad_tokens, grad_gain, grad_gate, grad_up, grad_down, gate_up_sq, down_sq)


CORES = 2
LANES = 128
TILE = 256


def line_next(z, n_fs, side):
    return z <= n_fs - 2 if side == 0 else z >= 1


def layer_kernel(n_fs, *refs):
    tokens, cot, w_gate, w_up, w_down, gain = refs[:6]
    o_gate, o_up, o_down, o_normed, o_inv = refs[6:11]
    full = refs[11:16]
    x_full, dy_full, f_gate, f_up, f_down = full
    normed, normed_t, hidden_t, act_f, slope_f, d_gate, d_up, inv_all = refs[16:24]
    g_gate, g_up, g_down = refs[24:27]
    pair_wide, pair_tall, sum_wide, sum_tall, x_wide, x_tall, t_wide, t_tall = refs[27:35]
    y_buf, d_buf, z_buf, n_buf = refs[35:39]
    (load_sem, az_own, az_fwd, az_recv, ay_own, ay_fwd, ay_recv, ap_send, ap_recv) = refs[39:48]
    (w_send, w_recv, wx_send, wx_recv, wp_send, wp_recv, wo_send, wo_recv) = refs[48:56]
    (p_send, p_recv, x_send, x_recv, z_send, z_recv, f_send, f_recv) = refs[56:64]
    (y_send, y_recv, d_send, d_recv, n_send, n_recv, own_sem) = refs[64:]
    r, z, t = lax.axis_index("rep"), lax.axis_index("fs"), lax.axis_index("tp")
    y, c = lax.div(t, CORES), lax.rem(t, CORES)
    acts, weights = (tokens, cot), (w_gate, w_up, w_down)
    grads, outs = (g_gate, g_up, g_down), (o_gate, o_up, o_down)
    half, local = tokens.shape[0] // CORES, tokens.shape[1]
    count, model = x_full.shape
    rows = w_gate.shape[0]
    kb = n_fs // CORES
    width = w_gate.shape[1] // kb
    strip = rows // 2
    reach = model // 2
    partner = {"tp": y * CORES + 1 - c}
    across = {"rep": 1 - r}
    beside = {"tp": (1 - y) * CORES + c}
    owner = lax.div(z, kb)

    peers = [partner, across]
    peers += [{"tp": (1 - y) * CORES + h} for h in range(CORES)]
    for j in range(1, n_fs):
        for h in range(CORES):
            peers.append({"fs": lax.rem(z + j, n_fs), "tp": y * CORES + h})
    greet(peers)

    def own_act(a, h):
        return acts[a].at[pl.ds(pl.multiple_of(h * half, half), half), :]

    def act_place(a, source, column):
        return full[a].at[
            pl.ds(pl.multiple_of(source * half, half), half),
            pl.ds(pl.multiple_of(column * local, local), local),
        ]

    def source_of(side, d):
        return z - d if side == 0 else z + d

    def next_of(side):
        return z + 1 if side == 0 else z - 1

    def act_first(a, side, h):
        return remote(
            own_act(a, h),
            act_place(a, z, t),
            az_own.at[a, side, h],
            az_recv.at[a, side, 0, c],
            {"fs": next_of(side), "tp": y * CORES + h},
        )

    def act_arrival(a, side, d, core):
        place = act_place(a, source_of(side, d), y * CORES + core)
        return remote(
            place, place, az_fwd.at[a, side, d - 1, core], az_recv.at[a, side, d - 1, core], partner
        )

    def act_forward(a, side, d, core):
        place = act_place(a, source_of(side, d), y * CORES + core)
        return remote(
            place,
            place,
            az_fwd.at[a, side, d - 1, core],
            az_recv.at[a, side, d, core],
            {"fs": next_of(side)},
        )

    def act_over(a, side, d, core):
        source = source_of(side, d)
        place = act_place(a, source, y * CORES + core)
        return remote(
            place,
            place,
            ay_fwd.at[a, side, d - 1, core],
            ay_recv.at[a, source, core],
            {"tp": (1 - y) * CORES + c},
        )

    def act_over_own(a, h):
        return remote(
            own_act(a, h),
            act_place(a, z, t),
            ay_own.at[a, h],
            ay_recv.at[a, z, c],
            {"tp": (1 - y) * CORES + h},
        )

    def act_over_arrival(a, source, core):
        place = act_place(a, source, (1 - y) * CORES + core)
        return remote(place, place, ay_own.at[a, 0], ay_recv.at[a, source, core], partner)

    def act_partner(a):
        return remote(own_act(a, 1 - c), act_place(a, z, t), ap_send.at[a], ap_recv.at[a], partner)

    def act_partner_arrival(a):
        place = act_place(a, z, y * CORES + 1 - c)
        return remote(place, place, ap_send.at[a], ap_recv.at[a], partner)

    def block_of(m, k):
        if m == 2:
            return weights[m].at[pl.ds(pl.multiple_of(k * width, width), width), :]
        return weights[m].at[:, pl.ds(pl.multiple_of(k * width, width), width)]

    def band_of(m, source):
        band = pl.ds(pl.multiple_of(source * rows, rows), rows)
        return full[2 + m].at[:, band] if m == 2 else full[2 + m].at[band, :]

    def quarter(m, source, rep, core):
        if m == 2:
            size = width // (2 * CORES)
            return full[4].at[
                pl.ds(pl.multiple_of((rep * CORES + core) * size, size), size),
                pl.ds(pl.multiple_of(source * rows, rows), rows),
            ]
        size = rows // (2 * CORES)
        start = source * rows + (rep * CORES + core) * size
        return full[2 + m].at[pl.ds(pl.multiple_of(start, size), size), :]

    def own_quarter(m, k, core):
        if m == 2:
            size = width // (2 * CORES)
            start = k * width + (r * CORES + core) * size
            return weights[m].at[pl.ds(pl.multiple_of(start, size), size), :]
        size = rows // (2 * CORES)
        return weights[m].at[
            pl.ds(pl.multiple_of((r * CORES + core) * size, size), size),
            pl.ds(k * width, width),
        ]

    def weight_send(m, k, core):
        return remote(
            own_quarter(m, k, core),
            quarter(m, z, r, core),
            w_send.at[m, k, core],
            w_recv.at[m, z],
            {"fs": kb * c + k, "tp": y * CORES + core},
        )

    def weight_arrival(m, source):
        place = quarter(m, source, r, c)
        return remote(place, place, wx_send.at[m, source], w_recv.at[m, source], partner)

    def weight_across(m, source):
        place = quarter(m, source, r, c)
        return remote(place, place, wx_send.at[m, source], wx_recv.at[m, source], across)

    def weight_across_arrival(m, source):
        place = quarter(m, source, 1 - r, c)
        return remote(place, place, wx_send.at[m, source], wx_recv.at[m, source], across)

    def weight_beside(m, source, which):
        place = quarter(m, source, r if which == 0 else 1 - r, c)
        return remote(
            place, place, wp_send.at[m, source, which], wp_recv.at[m, source, which], partner
        )

    def weight_beside_arrival(m, source, which):
        place = quarter(m, source, r if which == 0 else 1 - r, 1 - c)
        return remote(
            place, place, wp_send.at[m, source, which], wp_recv.at[m, source, which], partner
        )

    def own_beside(m):
        return remote(
            block_of(m, z - kb * owner), band_of(m, z), wo_send.at[m], wo_recv.at[m], partner
        )

    def own_beside_arrival(m):
        return remote(band_of(m, z), band_of(m, z), wo_send.at[m], wo_recv.at[m], partner)

    def slot(wide, tall, m, *where):
        return tall.at[where] if m == 2 else wide.at[(m,) + where]

    def strip_of(band, rep):
        return pl.ds(pl.multiple_of(band * rows + rep * strip, strip), strip)

    def grad_piece(m, band, rep):
        if m == 2:
            return grads[m].at[:, strip_of(band, rep)]
        return grads[m].at[strip_of(band, rep), :]

    def rep_of(j):
        return 1 - r if j == 0 else r

    def pair(m, k, j):
        return remote(
            grad_piece(m, kb * (1 - c) + k, rep_of(j)),
            slot(pair_wide, pair_tall, m, k, j),
            p_send.at[m, k, j],
            p_recv.at[m, k, j],
            partner,
        )

    def swap(m, k):
        return remote(
            slot(sum_wide, sum_tall, m, k),
            slot(x_wide, x_tall, m, k),
            x_send.at[m, k],
            x_recv.at[m, k],
            across,
        )

    def place(m, block, rep):
        strips = pl.ds(pl.multiple_of(rep * strip, strip), strip)
        blocks = pl.ds(pl.multiple_of(block * width, width), width)
        return outs[m].at[blocks, strips] if m == 2 else outs[m].at[strips, blocks]

    def deliver(m, k):
        block = lax.rem(z, kb)
        return remote(
            slot(t_wide, t_tall, m, k),
            place(m, block, r),
            z_send.at[m, k],
            z_recv.at[m, block],
            {"fs": kb * c + k, "tp": y * CORES + owner},
        )

    def delivered(m, k):
        return remote(place(m, k, r), place(m, k, r), z_send.at[m, k], z_recv.at[m, k], partner)

    def keep(m, k):
        return pltpu.make_async_copy(slot(t_wide, t_tall, m, k), place(m, k, r), own_sem.at[m])

    def spread(m, k, source):
        return remote(source, place(m, k, r), f_send.at[m, k], f_recv.at[m, k], across)

    def spread_arrival(m, k):
        return remote(
            place(m, k, 1 - r), place(m, k, 1 - r), f_send.at[m, k], f_recv.at[m, k], across
        )

    def band_rows(band):
        return pl.ds(pl.multiple_of(band * half, half), half)

    def side_columns(which):
        return pl.ds(pl.multiple_of(which * reach, reach), reach)

    def over(j):
        band = lax.rem(z + j, n_fs)
        return remote(
            x_full.at[band_rows(band), side_columns(1 - y)],
            y_buf.at[j],
            y_send.at[j],
            y_recv.at[j],
            beside,
        )

    def normed_send(j):
        return remote(
            d_buf.at[j], z_buf.at[z], d_send.at[j], d_recv.at[z], {"fs": lax.rem(z + j, n_fs)}
        )

    def normed_arrival(j):
        source = lax.rem(z + j, n_fs)
        return remote(z_buf.at[source], z_buf.at[source], d_send.at[j], d_recv.at[source], partner)

    def own_rows(core):
        return pl.ds(pl.multiple_of(core * half, half), half)

    def inv_send():
        return remote(inv_all.at[band_rows(z), :], o_inv.at[own_rows(c), :], n_send.at[0], n_recv.at[0], partner)

    def inv_arrival():
        at = o_inv.at[own_rows(1 - c), :]
        return remote(at, at, n_send.at[0], n_recv.at[0], partner)

    def last_send():
        return remote(n_buf, o_normed.at[own_rows(c), :], n_send.at[1], n_recv.at[1], partner)

    def last_arrival():
        at = o_normed.at[own_rows(1 - c), :]
        return remote(at, at, n_send.at[1], n_recv.at[1], partner)

    def loaded(a):
        return pltpu.make_async_copy(own_act(a, c), act_place(a, z, t), load_sem.at[a])

    def block_loaded(m):
        return pltpu.make_async_copy(
            block_of(m, z - kb * owner), band_of(m, z), load_sem.at[2 + m]
        )

    def act_start(a):
        for h in range(CORES):
            for side in range(2):

                @pl.when(line_next(z, n_fs, side))
                def _():
                    act_first(a, side, h).start()

            act_over_own(a, h).start()
        act_partner(a).start()

    def own_start(m):
        @pl.when(c == owner)
        def _():
            own_beside(m).start()

    def act_round(a, d):
        for core in range(CORES):
            for side in range(2):

                @pl.when(line_receives(z, n_fs, side, d))
                def _():
                    act_arrival(a, side, d, core).wait_recv()
                    if d < n_fs - 1:

                        @pl.when(line_next(z, n_fs, side))
                        def _():
                            act_forward(a, side, d, core).start()

                    act_over(a, side, d, core).start()

    def weight_start(m):
        for k in range(kb):

            @pl.when(kb * c + k != z)
            def _():
                for core in range(CORES):
                    weight_send(m, k, core).start()

    def weight_round(ms, d):
        for m in ms:
            for side in range(2):

                @pl.when(line_receives(z, n_fs, side, d))
                def _():
                    source = source_of(side, d)
                    weight_arrival(m, source).wait_recv()
                    weight_across(m, source).start()
                    weight_beside(m, source, 0).start()

    def across_round(ms, d):
        for m in ms:
            for side in range(2):

                @pl.when(line_receives(z, n_fs, side, d))
                def _():
                    source = source_of(side, d)
                    weight_across_arrival(m, source).wait_recv()
                    weight_beside(m, source, 1).start()

    def act_ready(a):
        for d in range(1, n_fs):
            for side in range(2):

                @pl.when(line_receives(z, n_fs, side, d))
                def _():
                    for core in range(CORES):
                        act_over_arrival(a, source_of(side, d), core).wait_recv()

        act_partner_arrival(a).wait_recv()
        for h in range(CORES):
            act_over_arrival(a, z, h).wait_recv()
        loaded(a).wait()

    def act_sent(a):
        for d in range(1, n_fs):
            for side in range(2):

                @pl.when(line_receives(z, n_fs, side, d))
                def _():
                    for core in range(CORES):
                        act_over(a, side, d, core).wait_send()
                        if d < n_fs - 1:

                            @pl.when(line_next(z, n_fs, side))
                            def _():
                                act_forward(a, side, d, core).wait_send()

        act_partner(a).wait_send()
        for h in range(CORES):
            act_over_own(a, h).wait_send()
            for side in range(2):

                @pl.when(line_next(z, n_fs, side))
                def _():
                    act_first(a, side, h).wait_send()

    def weight_ready(ms):
        for m in ms:
            for d in range(1, n_fs):
                for side in range(2):

                    @pl.when(line_receives(z, n_fs, side, d))
                    def _():
                        for which in range(2):
                            weight_beside_arrival(m, source_of(side, d), which).wait_recv()

            @pl.when(c == owner)
            def _():
                block_loaded(m).wait()

            @pl.when(c != owner)
            def _():
                own_beside_arrival(m).wait_recv()

    def weight_sent(m):
        for d in range(1, n_fs):
            for side in range(2):

                @pl.when(line_receives(z, n_fs, side, d))
                def _():
                    source = source_of(side, d)
                    weight_across(m, source).wait_send()
                    for which in range(2):
                        weight_beside(m, source, which).wait_send()

        for k in range(kb):

            @pl.when(kb * c + k != z)
            def _():
                for core in range(CORES):
                    weight_send(m, k, core).wait_send()

        @pl.when(c == owner)
        def _():
            own_beside(m).wait_send()

    def tile(i, size):
        return pl.ds(pl.multiple_of(i * size, size), size)

    def normalize(i):
        at = tile(i, LANES)
        wide = x_full[at, :].astype(jnp.float32)
        inv = lax.rsqrt(jnp.mean(wide * wide, axis=-1, keepdims=True) + 1e-06)
        value = wide * inv * gain[...]
        normed[at, :] = value.astype(jnp.bfloat16)
        normed_t[:, at] = value.T.astype(jnp.bfloat16)
        inv_all[at, :] = jnp.broadcast_to(inv, (LANES, LANES))

    def forward(i):
        at = tile(i, TILE)
        gate = jnp.dot(normed[at, :], f_gate[...], preferred_element_type=jnp.float32)
        up = jnp.dot(normed[at, :], f_up[...], preferred_element_type=jnp.float32)
        sigma = jax.nn.sigmoid(gate)
        active = gate * sigma
        act_f[at, :] = active
        slope_f[at, :] = up * sigma * (1.0 + gate * (1.0 - sigma))
        hidden_t[:, at] = (active * up).T.astype(jnp.bfloat16)

    def backward(i):
        at = tile(i, TILE)
        back = 0.5 * contract_last(dy_full[at, :], f_down[...])
        d_up[at, :] = (back * act_f[at, :]).astype(jnp.bfloat16)
        d_gate[at, :] = (back * slope_f[at, :]).astype(jnp.bfloat16)

    def gradient(m, own, j, k):
        band = kb * (c if own else 1 - c) + k
        at = strip_of(band, 1 - r if j == 0 else r)
        if m == 2:
            value = 0.5 * jnp.dot(
                hidden_t[...], dy_full[:, at], preferred_element_type=jnp.float32
            )
            g_down[:, at] = value.astype(jnp.bfloat16)
        else:
            right = d_gate if m == 0 else d_up
            value = jnp.dot(normed_t[at, :], right[...], preferred_element_type=jnp.float32)
            grads[m][at, :] = value.astype(jnp.bfloat16)

    def gradients(m, j):
        @pl.loop(0, kb)
        def _(k):
            gradient(m, False, j, k)
            pair(m, k, j).start()

        @pl.loop(0, kb)
        def _(k):
            gradient(m, True, j, k)

    def pull_back(band, which):
        at, columns = band_rows(band), side_columns(which)
        value = contract_last(d_gate[at, :], f_gate[columns, :])
        value = value + contract_last(d_up[at, :], f_up[columns, :])
        x_full[at, columns] = value.astype(jnp.bfloat16)

    def added(m, k, j):
        own = grad_piece(m, kb * c + k, rep_of(j))[...].astype(jnp.float32)
        return own + slot(pair_wide, pair_tall, m, k, j)[...].astype(jnp.float32)

    def put(wide, tall, m, k, value):
        if m == 2:
            tall[k] = value
        else:
            wide[m, k] = value

    def first(m, k):
        pair(m, k, 0).wait_recv()
        put(sum_wide, sum_tall, m, k, added(m, k, 0).astype(jnp.bfloat16))
        swap(m, k).start()

    def second(m, k):
        pair(m, k, 1).wait_recv()
        swap(m, k).wait_recv()
        whole = added(m, k, 1) + slot(x_wide, x_tall, m, k)[...].astype(jnp.float32)
        put(t_wide, t_tall, m, k, whole.astype(jnp.bfloat16))
        mine = kb * c + k == z

        @pl.when(mine)
        def _():
            keep(m, k).start()
            spread(m, k, slot(t_wide, t_tall, m, k)).start()

        @pl.when(jnp.logical_not(mine))
        def _():
            deliver(m, k).start()

    def third(m, k):
        @pl.when(kb * c + k != z)
        def _():
            delivered(m, k).wait_recv()
            spread(m, k, place(m, k, r)).start()

    def normed_step(j):
        over(j).wait_recv()
        band = lax.rem(z + j, n_fs)
        own = x_full[band_rows(band), side_columns(y)].astype(jnp.float32)
        d_buf[j] = (own + y_buf[j].astype(jnp.float32)).astype(jnp.bfloat16)
        if j:
            normed_send(j).start()


    for a in range(2):
        loaded(a).start()

    @pl.when(c == owner)
    def _():
        for m in range(3):
            block_loaded(m).start()

    act_start(0)
    own_start(0)
    own_start(1)
    act_round(0, 1)
    weight_start(0)
    weight_start(1)
    act_round(0, 2)
    act_start(1)
    own_start(2)
    for d in range(3, n_fs):
        act_round(0, d)
    weight_round((0, 1), 1)
    weight_round((0, 1), 2)
    across_round((0, 1), 1)
    act_round(1, 1)
    weight_start(2)
    for d in range(3, n_fs):
        weight_round((0, 1), d)
        across_round((0, 1), d - 1)
    act_round(1, 2)
    across_round((0, 1), n_fs - 1)
    act_ready(0)
    pl.loop(0, count // LANES)(normalize)
    weight_round((2,), 1)
    weight_ready((0, 1))
    pl.loop(0, count // TILE)(forward)
    for d in range(3, n_fs):
        act_round(1, d)
    weight_round((2,), 2)
    across_round((2,), 1)
    for d in range(3, n_fs):
        weight_round((2,), d)
        across_round((2,), d - 1)
    act_ready(1)
    gradients(2, 0)
    across_round((2,), n_fs - 1)
    for k in range(kb):
        first(2, k)
    gradients(2, 1)
    weight_ready((2,))
    pl.loop(0, count // TILE)(backward)
    gradients(0, 0)
    for k in range(kb):
        first(0, k)
    for k in range(kb):
        second(2, k)
    gradients(1, 0)
    for k in range(kb):
        first(1, k)
    gradients(0, 1)
    act_sent(0)

    @pl.loop(0, n_fs)
    def _(i):
        j = lax.rem(i + 1, n_fs)
        pull_back(lax.rem(z + j, n_fs), 1 - y)
        over(j).start()

    gradients(1, 1)
    for k in range(kb):
        third(2, k)

    @pl.loop(0, n_fs)
    def _(i):
        pull_back(i, y)

    inv_send().start()
    o_inv[own_rows(c), :] = inv_all[band_rows(z), :]
    order = list(range(1, n_fs)) + [0]
    items = [(m, k) for m in range(2) for k in range(kb)]
    n_items = len(items)
    for i in range(n_items + 2):
        if i < n_items:
            second(*items[i])
        if i < n_fs:
            normed_step(order[i])
        if i >= 2:
            third(*items[i - 2])
    items += [(2, k) for k in range(kb)]

    for j in range(1, n_fs):
        normed_arrival(j).wait_recv()
    total = d_buf[0].astype(jnp.float32)
    for j in range(1, n_fs):
        total = total + z_buf[lax.rem(z + j, n_fs)].astype(jnp.float32)
    total = total.astype(jnp.bfloat16)

    @pl.when(c == 0)
    def _():
        o_normed[pl.ds(0, half), :] = total[:, :local]
        n_buf[...] = total[:, local:]

    @pl.when(c == 1)
    def _():
        o_normed[pl.ds(half, half), :] = total[:, local:]
        n_buf[...] = total[:, :local]

    last_send().start()

    for m, k in items:
        for j in range(2):
            pair(m, k, j).wait_send()
        swap(m, k).wait_send()
        mine = kb * c + k == z

        @pl.when(mine)
        def _():
            keep(m, k).wait()

        @pl.when(jnp.logical_not(mine))
        def _():
            deliver(m, k).wait_send()

        spread(m, k, place(m, k, r)).wait_send()
        spread_arrival(m, k).wait_recv()
    for j in range(n_fs):
        over(j).wait_send()
        if j:
            normed_send(j).wait_send()
    inv_send().wait_send()
    inv_arrival().wait_recv()
    last_send().wait_send()
    last_arrival().wait_recv()


    act_sent(1)
    for m in range(3):
        weight_sent(m)


def layer(n_fs, tokens, cot, w_gate, w_up, w_down, gain):
    half, local = tokens.shape[0] // CORES, tokens.shape[1]
    rows, hidden = w_gate.shape
    width = hidden * CORES // n_fs
    model = rows * n_fs
    count = half * n_fs
    dtype = tokens.dtype
    kb = n_fs // CORES
    strip = rows // 2
    reach = model // 2
    wide, tall = (strip, width), (width, strip)
    dma = pltpu.SemaphoreType.DMA
    vmem = pl.BlockSpec(memory_space=pltpu.VMEM)
    hbm = pl.BlockSpec(memory_space=pl.ANY)
    line = dma((2, 2, n_fs - 1, CORES))
    pairs, singles = dma((3, kb, 2)), dma((3, kb))

    def bf(*shape):
        return pltpu.VMEM(shape, dtype)

    def f32(*shape):
        return pltpu.VMEM(shape, jnp.float32)

    shapes = [(rows, kb * width)] * 2 + [(kb * width, rows)]
    return pl.pallas_call(
        functools.partial(layer_kernel, n_fs),
        out_shape=[jax.ShapeDtypeStruct(s, dtype) for s in shapes]
        + [
            jax.ShapeDtypeStruct((CORES * half, local), dtype),
            jax.ShapeDtypeStruct((CORES * half, LANES), jnp.float32),
        ],
        in_specs=[hbm] * 5 + [vmem],
        out_specs=[hbm] * 3 + [vmem] * 2,
        scratch_shapes=[
            bf(count, model),
            bf(count, model),
            bf(model, width),
            bf(model, width),
            bf(width, model),
            bf(count, model),
            bf(model, count),
            bf(width, count),
            f32(count, width),
            f32(count, width),
            bf(count, width),
            bf(count, width),
            f32(count, LANES),
            bf(model, width),
            bf(model, width),
            bf(width, model),
            bf(2, kb, 2, *wide),
            bf(kb, 2, *tall),
            bf(2, kb, *wide),
            bf(kb, *tall),
            bf(2, kb, *wide),
            bf(kb, *tall),
            bf(2, kb, *wide),
            bf(kb, *tall),
            bf(n_fs, half, reach),
            bf(n_fs, half, reach),
            bf(n_fs, half, reach),
            bf(half, local),
            dma((5,)),
            dma((2, 2, CORES)),
            line,
            line,
            dma((2, CORES)),
            line,
            dma((2, n_fs, CORES)),
            dma((2,)),
            dma((2,)),
            dma((3, kb, CORES)),
            dma((3, n_fs)),
            dma((3, n_fs)),
            dma((3, n_fs)),
            dma((3, n_fs, 2)),
            dma((3, n_fs, 2)),
            dma((3,)),
            dma((3,)),
            pairs,
            pairs,
            singles,
            singles,
            singles,
            singles,
            singles,
            singles,
            dma((n_fs,)),
            dma((n_fs,)),
            dma((n_fs,)),
            dma((n_fs,)),
            dma((2,)),
            dma((2,)),
            dma((3,)),
        ],
        compiler_params=pltpu.CompilerParams(
            collective_id=4, has_side_effects=True, vmem_limit_bytes=67043328
        ),
        name="layer",
    )(tokens, cot, w_gate, w_up, w_down, gain)


def sums_kernel(n_fs, n_tp, n_rep, here, there, all_here, all_there, h_send, h_recv, o_send, o_recv):
    r, z, t = lax.axis_index("rep"), lax.axis_index("fs"), lax.axis_index("tp")
    groups = n_rep * n_fs
    spot = r * n_fs + z

    def group_of(j):
        at = lax.rem(spot + j, groups)
        return {"rep": lax.div(at, n_fs), "fs": lax.rem(at, n_fs)}

    def lane_of(j):
        return {"tp": lax.rem(t + j, n_tp)}

    greet([lane_of(j) for j in range(1, n_tp)] + [group_of(j) for j in range(1, groups)])
    sends = []
    for j in range(1, n_tp):
        sends.append(
            remote(here, all_here.at[t], h_send.at[j - 1], h_recv.at[n_tp - j - 1], lane_of(j))
        )
    for j in range(1, groups):
        sends.append(
            remote(there, all_there.at[spot], o_send.at[j - 1], o_recv.at[groups - j - 1], group_of(j))
        )
    for copy in sends:
        copy.start()
    all_here[t] = here[...]
    all_there[spot] = there[...]
    for j in range(1, n_tp):
        place = all_here.at[lax.rem(t + j, n_tp)]
        remote(place, place, h_send.at[j - 1], h_recv.at[j - 1], lane_of(j)).wait_recv()
    for j in range(1, groups):
        place = all_there.at[lax.rem(spot + j, groups)]
        remote(place, place, o_send.at[j - 1], o_recv.at[j - 1], group_of(j)).wait_recv()
    for copy in sends:
        copy.wait_send()


def exchange_sums(n_fs, n_tp, n_rep, here, there):
    dma = pltpu.SemaphoreType.DMA
    vmem = pl.BlockSpec(memory_space=pltpu.VMEM)
    groups = n_rep * n_fs
    return pl.pallas_call(
        functools.partial(sums_kernel, n_fs, n_tp, n_rep),
        out_shape=[
            jax.ShapeDtypeStruct((n_tp,) + here.shape, here.dtype),
            jax.ShapeDtypeStruct((groups,) + there.shape, there.dtype),
        ],
        in_specs=[vmem] * 2,
        out_specs=[vmem] * 2,
        scratch_shapes=[dma((n_tp - 1,)), dma((n_tp - 1,)), dma((groups - 1,)), dma((groups - 1,))],
        compiler_params=pltpu.CompilerParams(collective_id=6, has_side_effects=True),
        name="exchange_sums",
    )(here, there)


def packed(parts):
    flat = jnp.concatenate([p.reshape(-1) for p in parts])
    size = -(-flat.shape[0] // 1024) * 1024
    return jnp.pad(flat, (0, size - flat.shape[0])).reshape(-1, 128)


def by_chip(tokens, norm_gain, w_gate, w_up, w_down, cotangent):
    n_rep, n_fs, n_tp = lax.axis_size("rep"), lax.axis_size("fs"), lax.axis_size("tp")
    count, local = tokens.shape
    rows, wide = w_gate.shape
    model = rows * n_fs
    gain_f = norm_gain.astype(jnp.float32)
    s_gate, s_up, s_down, d_normed, inv = layer(
        n_fs, tokens, cotangent, w_gate, w_up, w_down, gain_f[None, :]
    )

    grad_gate, grad_up, grad_down = (s.astype(jnp.float32) for s in (s_gate, s_up, s_down))
    d_normed = d_normed.astype(jnp.float32)
    inv = inv[:, :1]
    gain_here = lax.dynamic_slice_in_dim(gain_f, lax.axis_index("tp") * local, local, 0)
    local_tokens = tokens.astype(jnp.float32)
    scaled = d_normed * gain_here
    here = packed(
        [
            jnp.sum(scaled * local_tokens, axis=-1),
            jnp.sum(grad_gate * grad_gate, axis=1),
            jnp.sum(grad_up * grad_up, axis=1),
        ]
    )
    there = packed(
        [
            jnp.sum(d_normed * local_tokens * inv, axis=0),
            jnp.sum(grad_down * grad_down, axis=1),
        ]
    )
    all_here, all_there = exchange_sums(n_fs, n_tp, n_rep, here, there)
    here = jnp.sum(all_here, axis=0).reshape(-1)
    rowdot = here[:count]
    gate_up_sq = here[count : count + 2 * rows].reshape(2, rows)
    flat = all_there.reshape(n_rep, n_fs, -1)
    grad_gain = jnp.sum(flat[:, :, :local], axis=(0, 1))
    down_sq = jnp.sum(flat[0, :, local : local + wide], axis=0)
    grad_tokens = (
        cotangent.astype(jnp.float32)
        + inv * scaled
        - local_tokens * inv**3 * rowdot[:, None] / model
    ).astype(jnp.bfloat16)
    return (grad_tokens, grad_gain, grad_gate, grad_up, grad_down, gate_up_sq, down_sq)


def fits_chips(mesh):
    n_rep, n_fs, n_tp = mesh.shape["rep"], mesh.shape["fs"], mesh.shape["tp"]
    return n_rep == 2 and n_tp == 2 * CORES and n_fs == 2 * CORES


def solution(mesh):
    placed = (
        P(("rep", "fs"), "tp"),
        P(),
        P("fs", "tp"),
        P("fs", "tp"),
        P("tp", "fs"),
        P(("rep", "fs"), "tp"),
    )
    return jax.shard_map(
        by_chip if fits_chips(mesh) else on_device,
        mesh=mesh,
        in_specs=placed,
        out_specs=(
            P(("rep", "fs"), "tp"),
            P("tp"),
            P("fs", "tp"),
            P("fs", "tp"),
            P("tp", "fs"),
            P(None, "fs"),
            P("tp"),
        ),
        check_vma=False,
    )
```

```python
import functools

import jax
import jax.numpy as jnp
from jax import lax
from jax.experimental import pallas as pl
from jax.experimental.pallas import tpu as pltpu
from jax.sharding import PartitionSpec as P

MESH = pl.DeviceIdType.MESH


def contract_last(left, right):
    return lax.dot_general(
        left, right, (((1,), (1,)), ((), ())), preferred_element_type=jnp.float32
    )


def contract_first(left, right):
    return lax.dot_general(
        left, right, (((0,), (0,)), ((), ())), preferred_element_type=jnp.float32
    )


def remote(source, target, send_sem, recv_sem, where):
    return pltpu.make_async_remote_copy(
        src_ref=source,
        dst_ref=target,
        send_sem=send_sem,
        recv_sem=recv_sem,
        device_id=where,
        device_id_type=MESH,
    )


def line_sends(z, n_fs, side, d):
    if side == 0:
        return jnp.logical_and(z >= d - 1, z <= n_fs - 2)
    return jnp.logical_and(z + d <= n_fs, z >= 1)


def line_receives(z, n_fs, side, d):
    return z >= d if side == 0 else z + d <= n_fs - 1


def greet(peers):
    barrier = pltpu.get_barrier_semaphore()
    for peer in peers:
        pl.semaphore_signal(barrier, inc=1, device_id=peer, device_id_type=MESH)
    pl.semaphore_wait(barrier, len(peers))


def keep_own(sources, holders, targets, sems):
    count = len(sources)
    loads = [
        pltpu.make_async_copy(sources[i], holders[i], sems.at[0, i]) for i in range(count)
    ]
    stores = [
        pltpu.make_async_copy(holders[i], targets[i], sems.at[1, i]) for i in range(count)
    ]
    for load in loads:
        load.start()

    def finish():
        for load, store in zip(loads, stores):
            load.wait()
            store.start()
        for store in stores:
            store.wait()

    return finish


def weights_kernel(n_fs, n_tp, *refs):
    tokens, cot, w_gate, w_up, w_down = refs[:5]
    whole_x, whole_dy, full_gate, full_up, full_down = refs[5:10]
    holders = refs[10:15]
    own_sem, ring_send, ring_recv, rep_send, rep_recv, tp_send, tp_recv = refs[15:]
    r, z, t = lax.axis_index("rep"), lax.axis_index("fs"), lax.axis_index("tp")
    right, left = lax.rem(z + 1, n_fs), lax.rem(z + n_fs - 1, n_fs)
    partner = {"rep": 1 - r}
    sources = (w_gate, w_up, w_down)
    targets = (full_gate, full_up, full_down)
    rows = w_gate.shape[0]
    hidden = w_down.shape[0]
    local = tokens.shape[1]

    def own_piece(m, half):
        size = (hidden if m == 2 else rows) // 2
        return sources[m].at[pl.ds(pl.multiple_of(half * size, size), size), :]

    def piece(m, owner, half):
        if m == 2:
            size = hidden // 2
            return targets[m].at[
                pl.ds(pl.multiple_of(half * size, size), size),
                pl.ds(pl.multiple_of(owner * rows, rows), rows),
            ]
        size = rows // 2
        return targets[m].at[
            pl.ds(pl.multiple_of(owner * rows + half * size, size), size), :
        ]

    peers = [{"fs": right}, {"fs": left}, partner]
    peers += [{"tp": lax.rem(t + j, n_tp)} for j in range(1, n_tp)]
    greet(peers)

    def owner_of(side, back):
        return lax.rem(z + (n_fs - back if side == 0 else back), n_fs)

    def hop(m, side, d):
        place = piece(m, owner_of(side, d - 1), r)
        return remote(
            own_piece(m, r) if d == 1 else place,
            place,
            ring_send.at[m, side, d - 1],
            ring_recv.at[m, side, d - 1],
            {"fs": right if side == 0 else left},
        )

    def arrival(m, side, d):
        place = piece(m, owner_of(side, d), r)
        return remote(
            place,
            place,
            ring_send.at[m, side, d - 1],
            ring_recv.at[m, side, d - 1],
            {"fs": right if side == 0 else left},
        )

    def across(m, side, d):
        place = piece(m, owner_of(side, d), r)
        return remote(
            place, place, rep_send.at[m, side, d - 1], rep_recv.at[m, side, d - 1], partner
        )

    for m in range(3):
        for side in range(2):

            @pl.when(line_sends(z, n_fs, side, 1))
            def _():
                hop(m, side, 1).start()

    ends = []
    for a, (source, target) in enumerate(((tokens, whole_x), (cot, whole_dy))):
        place = target.at[:, pl.ds(pl.multiple_of(t * local, local), local)]
        for j in range(1, n_tp):
            copy = remote(
                source,
                place,
                tp_send.at[a, j - 1],
                tp_recv.at[a, j - 1],
                {"tp": lax.rem(t + j, n_tp)},
            )
            copy.start()
            ends.append(copy)
    mine = pl.ds(pl.multiple_of(t * local, local), local)
    band = pl.ds(pl.multiple_of(z * rows, rows), rows)
    finish = keep_own(
        (tokens, cot, w_gate, w_up, w_down),
        holders,
        (
            whole_x.at[:, mine],
            whole_dy.at[:, mine],
            full_gate.at[band, :],
            full_up.at[band, :],
            full_down.at[:, band],
        ),
        own_sem,
    )
    finish()
    for d in range(1, n_fs):
        for m in range(3):
            for side in range(2):

                @pl.when(line_receives(z, n_fs, side, d))
                def _():
                    arrival(m, side, d).wait_recv()
                    if d < n_fs - 1:

                        @pl.when(line_sends(z, n_fs, side, d + 1))
                        def _():
                            hop(m, side, d + 1).start()

                    across(m, side, d).start()

    for d in range(1, n_fs):
        for m in range(3):
            for side in range(2):

                @pl.when(line_sends(z, n_fs, side, d))
                def _():
                    hop(m, side, d).wait_send()

                @pl.when(line_receives(z, n_fs, side, d))
                def _():
                    across(m, side, d).wait()

    for copy in ends:
        copy.wait()


def gather_weights(n_fs, n_tp, tokens, cot, w_gate, w_up, w_down):
    count, local = tokens.shape
    rows, hidden = w_gate.shape
    width = rows * n_fs
    dtype = tokens.dtype
    shapes = [
        (count, width),
        (count, width),
        (width, hidden),
        (width, hidden),
        (hidden, width),
    ]
    held = (tokens, cot, w_gate, w_up, w_down)
    moved = sum(2 * a * b for a, b in shapes)
    dma = pltpu.SemaphoreType.DMA
    return pl.pallas_call(
        functools.partial(weights_kernel, n_fs, n_tp),
        out_shape=[jax.ShapeDtypeStruct(s, dtype) for s in shapes],
        in_specs=[pl.BlockSpec(memory_space=pl.ANY)] * 5,
        out_specs=[pl.BlockSpec(memory_space=pl.ANY)] * 5,
        scratch_shapes=[pltpu.VMEM(a.shape, a.dtype) for a in held]
        + [
            dma((2, 5)),
            dma((3, 2, n_fs - 1)),
            dma((3, 2, n_fs - 1)),
            dma((3, 2, n_fs - 1)),
            dma((3, 2, n_fs - 1)),
            dma((2, n_tp - 1)),
            dma((2, n_tp - 1)),
        ],
        compiler_params=pltpu.CompilerParams(collective_id=0, has_side_effects=True),
        cost_estimate=pl.CostEstimate(flops=0, bytes_accessed=16 * moved, transcendentals=0),
        name="gather_weights",
    )(*held)


def tokens_kernel(n_fs, n_tp, n_act, n_swap, *refs):
    total = n_act + n_swap
    acts, swaps = refs[:n_act], refs[n_act:total]
    act_outs, swap_outs = refs[total : total + n_act], refs[total + n_act : 2 * total]
    holders = refs[2 * total : 3 * total]
    own_sem, ring_send, ring_recv = refs[3 * total : 3 * total + 3]
    swap_send, swap_recv, relay_send, relay_recv = refs[3 * total + 3 :]
    z, t = lax.axis_index("fs"), lax.axis_index("tp")
    right, left = lax.rem(z + 1, n_fs), lax.rem(z + n_fs - 1, n_fs)
    count = acts[0].shape[0]
    peers = [{"fs": lax.rem(z + j, n_fs)} for j in range(1, n_fs)]
    if n_swap:
        peers += [{"tp": lax.rem(t + j, n_tp)} for j in range(1, n_tp)]
    greet(peers)

    def rows_of(owner):
        return pl.ds(pl.multiple_of(owner * count, count), count)

    def owner_of(side, back):
        return lax.rem(z + (n_fs - back if side == 0 else back), n_fs)

    def hop(m, side, d):
        place = act_outs[m].at[rows_of(owner_of(side, d - 1)), :]
        return remote(
            acts[m] if d == 1 else place,
            place,
            ring_send.at[m, side, d - 1],
            ring_recv.at[m, side, d - 1],
            {"fs": right if side == 0 else left},
        )

    def arrival(m, side, d):
        place = act_outs[m].at[rows_of(owner_of(side, d)), :]
        return remote(
            place,
            place,
            ring_send.at[m, side, d - 1],
            ring_recv.at[m, side, d - 1],
            {"fs": right if side == 0 else left},
        )

    def swap(a, j):
        peer = lax.rem(z + j, n_fs)
        cut = swap_outs[a].shape[1]
        return remote(
            swaps[a].at[:, pl.ds(pl.multiple_of(peer * cut, cut), cut)],
            swap_outs[a].at[rows_of(z), :],
            swap_send.at[a, j - 1],
            swap_recv.at[a, j - 1],
            {"fs": peer},
        )

    def swapped(a, j):
        place = swap_outs[a].at[rows_of(owner_of(0, j)), :]
        return remote(
            place,
            place,
            swap_send.at[a, j - 1],
            swap_recv.at[a, j - 1],
            {"fs": lax.rem(z + j, n_fs)},
        )

    def relay(a, j, k):
        place = swap_outs[a].at[rows_of(owner_of(0, j)), :]
        return remote(
            place,
            place,
            relay_send.at[a, j - 1, k - 1],
            relay_recv.at[a, j - 1],
            {"tp": lax.rem(t + k, n_tp)},
        )

    hub = lax.rem(z, n_tp) == t

    def feeds(j):
        return lax.rem(lax.rem(z + j, n_fs), n_tp) == t

    for a in range(n_swap):
        for j in range(1, n_fs):

            @pl.when(feeds(j))
            def _():
                swap(a, j).start()

    for m in range(n_act):
        for side in range(2):

            @pl.when(line_sends(z, n_fs, side, 1))
            def _():
                hop(m, side, 1).start()

    sources = list(acts)
    for a in range(n_swap):
        cut = swap_outs[a].shape[1]
        sources.append(swaps[a].at[:, pl.ds(pl.multiple_of(z * cut, cut), cut)])
    finish = keep_own(
        sources, holders, [out.at[rows_of(z), :] for out in act_outs + swap_outs], own_sem
    )
    finish()
    if n_swap:

        @pl.when(hub)
        def _():
            for a in range(n_swap):
                for j in range(1, n_fs):
                    swapped(a, j).wait_recv()
                    for k in range(1, n_tp):
                        relay(a, j, k).start()

    for d in range(1, n_fs):
        for m in range(n_act):
            for side in range(2):

                @pl.when(line_receives(z, n_fs, side, d))
                def _():
                    arrival(m, side, d).wait_recv()
                    if d < n_fs - 1:

                        @pl.when(line_sends(z, n_fs, side, d + 1))
                        def _():
                            hop(m, side, d + 1).start()

    for d in range(1, n_fs):
        for m in range(n_act):
            for side in range(2):

                @pl.when(line_sends(z, n_fs, side, d))
                def _():
                    hop(m, side, d).wait_send()

    for a in range(n_swap):
        for j in range(1, n_fs):

            @pl.when(feeds(j))
            def _():
                swap(a, j).wait_send()

            @pl.when(hub)
            def _():
                for k in range(1, n_tp):
                    relay(a, j, k).wait_send()

            @pl.when(jnp.logical_not(hub))
            def _():
                relay(a, j, 1).wait_recv()


def gather_tokens(n_fs, n_tp, collective_id, acts, swaps):
    count = acts[0].shape[0]
    outs = [jax.ShapeDtypeStruct((n_fs * count, a.shape[1]), a.dtype) for a in acts]
    outs += [jax.ShapeDtypeStruct((n_fs * count, a.shape[1] // n_fs), a.dtype) for a in swaps]
    dma = pltpu.SemaphoreType.DMA
    total = len(outs)
    n_swap = max(len(swaps), 1)
    moved = sum(2 * o.shape[0] * o.shape[1] for o in outs)
    return pl.pallas_call(
        functools.partial(tokens_kernel, n_fs, n_tp, len(acts), len(swaps)),
        out_shape=outs,
        in_specs=[pl.BlockSpec(memory_space=pl.ANY)] * total,
        out_specs=[pl.BlockSpec(memory_space=pl.ANY)] * total,
        scratch_shapes=[pltpu.VMEM((count, o.shape[1]), o.dtype) for o in outs]
        + [
            dma((2, total)),
            dma((len(acts), 2, n_fs - 1)),
            dma((len(acts), 2, n_fs - 1)),
            dma((n_swap, n_fs - 1)),
            dma((n_swap, n_fs - 1)),
            dma((n_swap, n_fs - 1, n_tp - 1)),
            dma((n_swap, n_fs - 1)),
        ],
        compiler_params=pltpu.CompilerParams(
            collective_id=collective_id, has_side_effects=True
        ),
        cost_estimate=pl.CostEstimate(flops=0, bytes_accessed=16 * moved, transcendentals=0),
        name=f"gather_tokens_{collective_id}",
    )(*acts, *swaps)


def over_rep(part):
    part = part.astype(jnp.bfloat16)
    n_rep = lax.axis_size("rep")
    other = lax.ppermute(part, "rep", [(i, (i + 1) % n_rep) for i in range(n_rep)])
    return part, other


def added(pair):
    return pair[0].astype(jnp.float32) + pair[1].astype(jnp.float32)


def on_device(tokens, norm_gain, w_gate, w_up, w_down, cotangent):
    n_fs, n_tp = lax.axis_size("fs"), lax.axis_size("tp")
    whole_x, whole_dy, full_gate, full_up, full_down = gather_weights(
        n_fs, n_tp, tokens, cotangent, w_gate, w_up, w_down
    )
    width = whole_x.shape[1]
    wide_tokens = whole_x.astype(jnp.float32)
    gain_f = norm_gain.astype(jnp.float32)
    inverse = lax.rsqrt(jnp.mean(wide_tokens * wide_tokens, axis=-1, keepdims=True) + 1e-06)
    normed = (wide_tokens * inverse * gain_f).astype(jnp.bfloat16)
    gate = jnp.dot(normed, full_gate, preferred_element_type=jnp.float32)
    up_proj = jnp.dot(normed, full_up, preferred_element_type=jnp.float32)
    sigma = jax.nn.sigmoid(gate)
    active = gate * sigma
    hidden = (active * up_proj).astype(jnp.bfloat16)
    back = 0.5 * contract_last(whole_dy, full_down)
    d_up = (back * active).astype(jnp.bfloat16)
    d_gate = (back * up_proj * sigma * (1.0 + gate * (1.0 - sigma))).astype(jnp.bfloat16)

    all_hidden, rows_dy = gather_tokens(n_fs, n_tp, 1, [hidden], [whole_dy])
    down_pair = over_rep(0.5 * contract_first(all_hidden, rows_dy))

    partial_normed = contract_last(d_gate, full_gate) + contract_last(d_up, full_up)
    d_normed = lax.psum_scatter(
        partial_normed.astype(jnp.bfloat16), "tp", scatter_dimension=1, tiled=True
    ).astype(jnp.float32)

    all_gate, rows_normed = gather_tokens(n_fs, n_tp, 2, [d_gate], [normed])
    gate_pair = over_rep(contract_first(rows_normed, all_gate))
    (all_up,) = gather_tokens(n_fs, n_tp, 3, [d_up], [])
    up_pair = over_rep(contract_first(rows_normed, all_up))

    local_width = d_normed.shape[1]
    local_gain = lax.dynamic_slice_in_dim(
        gain_f, lax.axis_index("tp") * local_width, local_width, 0
    )
    local_tokens = tokens.astype(jnp.float32)
    scaled_grad = d_normed * local_gain
    rowdot = lax.psum(jnp.sum(scaled_grad * local_tokens, axis=-1), "tp")
    grad_tokens = (
        cotangent.astype(jnp.float32)
        + inverse * scaled_grad
        - local_tokens * inverse**3 * rowdot[:, None] / width
    ).astype(jnp.bfloat16)
    grad_gain = lax.psum(jnp.sum(d_normed * local_tokens * inverse, axis=0), ("rep", "fs"))

    grad_down = added(down_pair)
    down_sq = lax.psum(jnp.sum(grad_down * grad_down, axis=1), "fs")
    grad_gate = added(gate_pair)
    grad_up = added(up_pair)
    gate_up_sq = lax.psum(
        jnp.stack([jnp.sum(grad_gate * grad_gate, axis=1), jnp.sum(grad_up * grad_up, axis=1)]),
        "tp",
    )
    return (grad_tokens, grad_gain, grad_gate, grad_up, grad_down, gate_up_sq, down_sq)


CORES = 2
LANES = 128
TILE = 256


def line_next(z, n_fs, side):
    return z <= n_fs - 2 if side == 0 else z >= 1


def layer_kernel(n_fs, n_tp, *refs):
    tokens, cot, w_gate, w_up, w_down, gain = refs[:6]
    o_gate, o_up, o_down, o_tokens, o_gain, o_wide_sq, o_tall_sq = refs[6:13]
    full = refs[13:18]
    x_full, dy_full, f_gate, f_up, f_down = full
    normed, normed_t, hidden_t, act_f, slope_f, d_gate, d_up, inv_all = refs[18:26]
    g_gate, g_up, g_down = refs[26:29]
    pair_wide, pair_tall, sum_wide, sum_tall, x_wide, x_tall, t_wide, t_tall = refs[29:37]
    y_buf, d_buf, z_buf, n_buf = refs[37:41]
    v_gate, v_up, v_down, v_tokens, v_cot, v_normed, v_inv, v_out = refs[41:49]
    lane_sq, row_all, gain_all, wide_all, tall_all = refs[49:54]
    (load_sem, az_own, az_fwd, az_recv, ay_own, ay_fwd, ay_recv, ap_send, ap_recv) = refs[54:63]
    (w_send, w_recv, wx_send, wx_recv, wp_send, wp_recv, wo_send, wo_recv) = refs[63:71]
    (p_send, p_recv, x_send, x_recv, z_send, z_recv, f_send, f_recv) = refs[71:79]
    (y_send, y_recv, d_send, d_recv, n_send, n_recv, own_sem) = refs[79:86]
    (row_send, row_recv, gain_send, gain_recv) = refs[86:90]
    (wide_send, wide_recv, tall_send, tall_recv, out_sem, total, gain_sum) = refs[90:]
    r, z, t = lax.axis_index("rep"), lax.axis_index("fs"), lax.axis_index("tp")
    y, c = lax.div(t, CORES), lax.rem(t, CORES)
    acts, weights = (tokens, cot), (w_gate, w_up, w_down)
    grads, outs = (g_gate, g_up, g_down), (v_gate, v_up, v_down)
    half, local = tokens.shape[0] // CORES, tokens.shape[1]
    count, model = x_full.shape
    rows = w_gate.shape[0]
    kb = n_fs // CORES
    width = w_gate.shape[1] // kb
    strip = rows // 2
    reach = model // 2
    partner = {"tp": y * CORES + 1 - c}
    across = {"rep": 1 - r}
    beside = {"tp": (1 - y) * CORES + c}
    owner = lax.div(z, kb)

    peers = [partner, across]
    peers += [{"tp": (1 - y) * CORES + h} for h in range(CORES)]
    for j in range(1, n_fs):
        for h in range(CORES):
            peers.append({"fs": lax.rem(z + j, n_fs), "tp": y * CORES + h})
        peers.append({"rep": 1 - r, "fs": lax.rem(z + j, n_fs)})
    greet(peers)

    def own_act(a, h):
        return acts[a].at[pl.ds(pl.multiple_of(h * half, half), half), :]

    def act_place(a, source, column):
        return full[a].at[
            pl.ds(pl.multiple_of(source * half, half), half),
            pl.ds(pl.multiple_of(column * local, local), local),
        ]

    def source_of(side, d):
        return z - d if side == 0 else z + d

    def next_of(side):
        return z + 1 if side == 0 else z - 1

    def act_first(a, side, h):
        return remote(
            own_act(a, h),
            act_place(a, z, t),
            az_own.at[a, side, h],
            az_recv.at[a, side, 0, c],
            {"fs": next_of(side), "tp": y * CORES + h},
        )

    def act_arrival(a, side, d, core):
        place = act_place(a, source_of(side, d), y * CORES + core)
        return remote(
            place, place, az_fwd.at[a, side, d - 1, core], az_recv.at[a, side, d - 1, core], partner
        )

    def act_forward(a, side, d, core):
        place = act_place(a, source_of(side, d), y * CORES + core)
        return remote(
            place,
            place,
            az_fwd.at[a, side, d - 1, core],
            az_recv.at[a, side, d, core],
            {"fs": next_of(side)},
        )

    def act_over(a, side, d, core):
        source = source_of(side, d)
        place = act_place(a, source, y * CORES + core)
        return remote(
            place,
            place,
            ay_fwd.at[a, side, d - 1, core],
            ay_recv.at[a, source, core],
            {"tp": (1 - y) * CORES + c},
        )

    def act_over_own(a, h):
        return remote(
            own_act(a, h),
            act_place(a, z, t),
            ay_own.at[a, h],
            ay_recv.at[a, z, c],
            {"tp": (1 - y) * CORES + h},
        )

    def act_over_arrival(a, source, core):
        place = act_place(a, source, (1 - y) * CORES + core)
        return remote(place, place, ay_own.at[a, 0], ay_recv.at[a, source, core], partner)

    def act_partner(a):
        return remote(own_act(a, 1 - c), act_place(a, z, t), ap_send.at[a], ap_recv.at[a], partner)

    def act_partner_arrival(a):
        place = act_place(a, z, y * CORES + 1 - c)
        return remote(place, place, ap_send.at[a], ap_recv.at[a], partner)

    def block_of(m, k):
        if m == 2:
            return weights[m].at[pl.ds(pl.multiple_of(k * width, width), width), :]
        return weights[m].at[:, pl.ds(pl.multiple_of(k * width, width), width)]

    def band_of(m, source):
        band = pl.ds(pl.multiple_of(source * rows, rows), rows)
        return full[2 + m].at[:, band] if m == 2 else full[2 + m].at[band, :]

    def quarter(m, source, rep, core):
        if m == 2:
            size = width // (2 * CORES)
            return full[4].at[
                pl.ds(pl.multiple_of((rep * CORES + core) * size, size), size),
                pl.ds(pl.multiple_of(source * rows, rows), rows),
            ]
        size = rows // (2 * CORES)
        start = source * rows + (rep * CORES + core) * size
        return full[2 + m].at[pl.ds(pl.multiple_of(start, size), size), :]

    def own_quarter(m, k, core):
        if m == 2:
            size = width // (2 * CORES)
            start = k * width + (r * CORES + core) * size
            return weights[m].at[pl.ds(pl.multiple_of(start, size), size), :]
        size = rows // (2 * CORES)
        return weights[m].at[
            pl.ds(pl.multiple_of((r * CORES + core) * size, size), size),
            pl.ds(k * width, width),
        ]

    def weight_send(m, k, core):
        return remote(
            own_quarter(m, k, core),
            quarter(m, z, r, core),
            w_send.at[m, k, core],
            w_recv.at[m, z],
            {"fs": kb * c + k, "tp": y * CORES + core},
        )

    def weight_arrival(m, source):
        place = quarter(m, source, r, c)
        return remote(place, place, wx_send.at[m, source], w_recv.at[m, source], partner)

    def weight_across(m, source):
        place = quarter(m, source, r, c)
        return remote(place, place, wx_send.at[m, source], wx_recv.at[m, source], across)

    def weight_across_arrival(m, source):
        place = quarter(m, source, 1 - r, c)
        return remote(place, place, wx_send.at[m, source], wx_recv.at[m, source], across)

    def weight_beside(m, source, which):
        place = quarter(m, source, r if which == 0 else 1 - r, c)
        return remote(
            place, place, wp_send.at[m, source, which], wp_recv.at[m, source, which], partner
        )

    def weight_beside_arrival(m, source, which):
        place = quarter(m, source, r if which == 0 else 1 - r, 1 - c)
        return remote(
            place, place, wp_send.at[m, source, which], wp_recv.at[m, source, which], partner
        )

    def own_beside(m):
        return remote(
            block_of(m, z - kb * owner), band_of(m, z), wo_send.at[m], wo_recv.at[m], partner
        )

    def own_beside_arrival(m):
        return remote(band_of(m, z), band_of(m, z), wo_send.at[m], wo_recv.at[m], partner)

    def slot(wide, tall, m, *where):
        return tall.at[where] if m == 2 else wide.at[(m,) + where]

    def strip_of(band, rep):
        return pl.ds(pl.multiple_of(band * rows + rep * strip, strip), strip)

    def grad_piece(m, band, rep):
        if m == 2:
            return grads[m].at[:, strip_of(band, rep)]
        return grads[m].at[strip_of(band, rep), :]

    def rep_of(j):
        return 1 - r if j == 0 else r

    def pair(m, k, j):
        return remote(
            grad_piece(m, kb * (1 - c) + k, rep_of(j)),
            slot(pair_wide, pair_tall, m, k, j),
            p_send.at[m, k, j],
            p_recv.at[m, k, j],
            partner,
        )

    def swap(m, k):
        return remote(
            slot(sum_wide, sum_tall, m, k),
            slot(x_wide, x_tall, m, k),
            x_send.at[m, k],
            x_recv.at[m, k],
            across,
        )

    def place(m, block, rep):
        strips = pl.ds(pl.multiple_of(rep * strip, strip), strip)
        blocks = pl.ds(pl.multiple_of(block * width, width), width)
        return outs[m].at[blocks, strips] if m == 2 else outs[m].at[strips, blocks]

    def deliver(m, k):
        block = lax.rem(z, kb)
        return remote(
            slot(t_wide, t_tall, m, k),
            place(m, block, r),
            z_send.at[m, k],
            z_recv.at[m, block],
            {"fs": kb * c + k, "tp": y * CORES + owner},
        )

    def delivered(m, k):
        return remote(place(m, k, r), place(m, k, r), z_send.at[m, k], z_recv.at[m, k], partner)

    def keep(m, k):
        return pltpu.make_async_copy(slot(t_wide, t_tall, m, k), place(m, k, r), own_sem.at[m, k])

    def spread(m, k, source):
        return remote(source, place(m, k, r), f_send.at[m, k], f_recv.at[m, k], across)

    def spread_arrival(m, k):
        return remote(
            place(m, k, 1 - r), place(m, k, 1 - r), f_send.at[m, k], f_recv.at[m, k], across
        )

    def band_rows(band):
        return pl.ds(pl.multiple_of(band * half, half), half)

    def side_columns(which):
        return pl.ds(pl.multiple_of(which * reach, reach), reach)

    def over(band):
        return remote(
            x_full.at[band_rows(band), side_columns(1 - y)],
            y_buf.at[band],
            y_send.at[band],
            y_recv.at[band],
            beside,
        )

    low = z < n_fs // 2
    inner = jnp.logical_and(z > 0, z < n_fs - 1)
    line_slot = jnp.where(low, 0, 1)

    def line_band(i):
        return jnp.where(low, n_fs - 1 - i, i)

    def y_turn(i):
        return jnp.where(jnp.logical_and(inner, i >= 2), n_fs + 1 - i, i)

    def line_send(i, target):
        band = line_band(i)
        return remote(
            d_buf.at[i],
            z_buf.at[line_slot, band],
            d_send.at[i],
            d_recv.at[line_slot, band],
            {"fs": target},
        )

    def line_arrival(which, band):
        place = z_buf.at[which, band]
        return remote(place, place, d_send.at[0], d_recv.at[which, band], partner)

    def own_rows(core):
        return pl.ds(pl.multiple_of(core * half, half), half)

    def inv_send():
        return remote(inv_all.at[band_rows(z), :], v_inv.at[own_rows(c), :], n_send.at[0], n_recv.at[0], partner)

    def inv_arrival():
        at = v_inv.at[own_rows(1 - c), :]
        return remote(at, at, n_send.at[0], n_recv.at[0], partner)

    def last_send():
        return remote(n_buf, v_normed.at[own_rows(c), :], n_send.at[1], n_recv.at[1], partner)

    def last_arrival():
        at = v_normed.at[own_rows(1 - c), :]
        return remote(at, at, n_send.at[1], n_recv.at[1], partner)

    def loaded(a):
        return pltpu.make_async_copy(own_act(a, c), act_place(a, z, t), load_sem.at[a])

    def block_loaded(m):
        return pltpu.make_async_copy(
            block_of(m, z - kb * owner), band_of(m, z), load_sem.at[2 + m]
        )

    def act_start(a):
        for h in range(CORES):
            for side in range(2):

                @pl.when(line_next(z, n_fs, side))
                def _():
                    act_first(a, side, h).start()

            act_over_own(a, h).start()
        act_partner(a).start()

    def own_start(m):
        @pl.when(c == owner)
        def _():
            own_beside(m).start()

    def act_round(a, d):
        for core in range(CORES):
            for side in range(2):

                @pl.when(line_receives(z, n_fs, side, d))
                def _():
                    act_arrival(a, side, d, core).wait_recv()
                    if d < n_fs - 1:

                        @pl.when(line_next(z, n_fs, side))
                        def _():
                            act_forward(a, side, d, core).start()

                    act_over(a, side, d, core).start()

    def weight_start(m):
        for k in range(kb):

            @pl.when(kb * c + k != z)
            def _():
                for core in range(CORES):
                    weight_send(m, k, core).start()

    def weight_round(ms, d):
        for m in ms:
            for side in range(2):

                @pl.when(line_receives(z, n_fs, side, d))
                def _():
                    source = source_of(side, d)
                    weight_arrival(m, source).wait_recv()
                    weight_across(m, source).start()
                    weight_beside(m, source, 0).start()

    def across_round(ms, d):
        for m in ms:
            for side in range(2):

                @pl.when(line_receives(z, n_fs, side, d))
                def _():
                    source = source_of(side, d)
                    weight_across_arrival(m, source).wait_recv()
                    weight_beside(m, source, 1).start()

    def weight_all(m):
        for d in range(1, n_fs):
            weight_round((m,), d)

    def across_all(m):
        for d in range(1, n_fs):
            across_round((m,), d)

    def act_ready(a):
        for d in range(1, n_fs):
            for side in range(2):

                @pl.when(line_receives(z, n_fs, side, d))
                def _():
                    for core in range(CORES):
                        act_over_arrival(a, source_of(side, d), core).wait_recv()

        act_partner_arrival(a).wait_recv()
        for h in range(CORES):
            act_over_arrival(a, z, h).wait_recv()
        loaded(a).wait()

    def act_sent(a):
        for d in range(1, n_fs):
            for side in range(2):

                @pl.when(line_receives(z, n_fs, side, d))
                def _():
                    for core in range(CORES):
                        act_over(a, side, d, core).wait_send()
                        if d < n_fs - 1:

                            @pl.when(line_next(z, n_fs, side))
                            def _():
                                act_forward(a, side, d, core).wait_send()

        act_partner(a).wait_send()
        for h in range(CORES):
            act_over_own(a, h).wait_send()
            for side in range(2):

                @pl.when(line_next(z, n_fs, side))
                def _():
                    act_first(a, side, h).wait_send()

    def weight_ready(ms):
        for m in ms:
            for d in range(1, n_fs):
                for side in range(2):

                    @pl.when(line_receives(z, n_fs, side, d))
                    def _():
                        for which in range(2):
                            weight_beside_arrival(m, source_of(side, d), which).wait_recv()

            @pl.when(c == owner)
            def _():
                block_loaded(m).wait()

            @pl.when(c != owner)
            def _():
                own_beside_arrival(m).wait_recv()

    def weight_sent(m):
        for d in range(1, n_fs):
            for side in range(2):

                @pl.when(line_receives(z, n_fs, side, d))
                def _():
                    source = source_of(side, d)
                    weight_across(m, source).wait_send()
                    for which in range(2):
                        weight_beside(m, source, which).wait_send()

        for k in range(kb):

            @pl.when(kb * c + k != z)
            def _():
                for core in range(CORES):
                    weight_send(m, k, core).wait_send()

        @pl.when(c == owner)
        def _():
            own_beside(m).wait_send()

    def tile(i, size):
        return pl.ds(pl.multiple_of(i * size, size), size)

    def normalize(i):
        at = tile(i, LANES)
        wide = x_full[at, :].astype(jnp.float32)
        inv = lax.rsqrt(jnp.mean(wide * wide, axis=-1, keepdims=True) + 1e-06)
        value = wide * inv * gain[...].astype(jnp.float32)
        normed[at, :] = value.astype(jnp.bfloat16)
        normed_t[:, at] = value.T.astype(jnp.bfloat16)
        inv_all[at, :] = jnp.broadcast_to(inv, (LANES, LANES))

    def forward(i):
        at = tile(i, TILE)
        gate = jnp.dot(normed[at, :], f_gate[...], preferred_element_type=jnp.float32)
        up = jnp.dot(normed[at, :], f_up[...], preferred_element_type=jnp.float32)
        sigma = jax.nn.sigmoid(gate)
        active = gate * sigma
        act_f[at, :] = active
        slope_f[at, :] = up * sigma * (1.0 + gate * (1.0 - sigma))
        hidden_t[:, at] = (active * up).T.astype(jnp.bfloat16)

    def backward(i):
        at = tile(i, TILE)
        back = 0.5 * contract_last(dy_full[at, :], f_down[...])
        d_up[at, :] = (back * act_f[at, :]).astype(jnp.bfloat16)
        d_gate[at, :] = (back * slope_f[at, :]).astype(jnp.bfloat16)

    def gradient(m, own, j, k):
        band = kb * (c if own else 1 - c) + k
        at = strip_of(band, 1 - r if j == 0 else r)
        if m == 2:
            value = 0.5 * jnp.dot(
                hidden_t[...], dy_full[:, at], preferred_element_type=jnp.float32
            )
            g_down[:, at] = value.astype(jnp.bfloat16)
        else:
            right = d_gate if m == 0 else d_up
            value = jnp.dot(normed_t[at, :], right[...], preferred_element_type=jnp.float32)
            grads[m][at, :] = value.astype(jnp.bfloat16)

    def gradients(m, j):
        @pl.loop(0, kb)
        def _(k):
            gradient(m, False, j, k)
            pair(m, k, j).start()

        @pl.loop(0, kb)
        def _(k):
            gradient(m, True, j, k)

    def pull_back(band, which):
        at, columns = band_rows(band), side_columns(which)
        value = contract_last(d_gate[at, :], f_gate[columns, :])
        value = value + contract_last(d_up[at, :], f_up[columns, :])
        x_full[at, columns] = value.astype(jnp.bfloat16)

    def added(m, k, j):
        own = grad_piece(m, kb * c + k, rep_of(j))[...].astype(jnp.float32)
        return own + slot(pair_wide, pair_tall, m, k, j)[...].astype(jnp.float32)

    def put(wide, tall, m, k, value):
        if m == 2:
            tall[k] = value
        else:
            wide[m, k] = value

    def first(m, k):
        pair(m, k, 0).wait_recv()
        put(sum_wide, sum_tall, m, k, added(m, k, 0).astype(jnp.bfloat16))
        swap(m, k).start()

    def second(m, k):
        pair(m, k, 1).wait_recv()
        swap(m, k).wait_recv()
        whole = added(m, k, 1) + slot(x_wide, x_tall, m, k)[...].astype(jnp.float32)
        put(t_wide, t_tall, m, k, whole.astype(jnp.bfloat16))
        mine = kb * c + k == z

        @pl.when(mine)
        def _():
            keep(m, k).start()
            spread(m, k, slot(t_wide, t_tall, m, k)).start()

        @pl.when(jnp.logical_not(mine))
        def _():
            deliver(m, k).start()

    def third(m, k):
        @pl.when(kb * c + k != z)
        def _():
            delivered(m, k).wait_recv()
            spread(m, k, place(m, k, r)).start()

    def own_share(band):
        over(band).wait_recv()
        own = x_full[band_rows(band), side_columns(y)].astype(jnp.float32)
        return own + y_buf[band].astype(jnp.float32)

    def line_target(i):
        if i == n_fs - 1:
            return jnp.where(low, z - 1, z + 1)
        return line_band(i)

    def normed_outer(i):
        @pl.when(jnp.logical_not(inner))
        def _():
            d_buf[i] = own_share(line_band(i)).astype(jnp.bfloat16)
            line_send(i, jnp.where(low, z + 1, z - 1)).start()

    def normed_inner(i):
        @pl.when(inner)
        def _():
            band = line_band(i)
            value = own_share(band)
            if i < n_fs - 1:
                line_arrival(line_slot, band).wait_recv()
                value = value + z_buf[line_slot, band].astype(jnp.float32)
            d_buf[i] = value.astype(jnp.bfloat16)
            line_send(i, line_target(i)).start()

    def normed_sent():
        for i in range(n_fs):
            if i < n_fs - 1:

                @pl.when(jnp.logical_not(inner))
                def _():
                    line_send(i, jnp.where(low, z + 1, z - 1)).wait_send()

            if i != n_fs - 2:

                @pl.when(inner)
                def _():
                    line_send(i, line_target(i)).wait_send()

    def normed_last():
        value = own_share(z)
        for which in range(2):
            line_arrival(which, z).wait_recv()
            value = value + z_buf[which, z].astype(jnp.float32)
        total[...] = value

        for core in range(CORES):

            @pl.when(c == core)
            def _():
                mine = slice(core * local, (core + 1) * local)
                theirs = slice((1 - core) * local, (2 - core) * local)
                v_normed[core * half : (core + 1) * half, :] = total[:, mine].astype(jnp.bfloat16)
                n_buf[...] = total[:, theirs].astype(jnp.bfloat16)

        last_send().start()

    def fold(value):
        out = value[:, :LANES]
        for i in range(1, value.shape[1] // LANES):
            out = out + value[:, i * LANES : (i + 1) * LANES]
        return out

    def row_of(value):
        return jnp.sum(value.T, axis=0, keepdims=True)

    def lane_peer(j):
        return {"tp": lax.rem(t + j, n_tp)}

    def group_peer(j):
        at = lax.rem(r * n_fs + z + j, 2 * n_fs)
        return {"rep": lax.div(at, n_fs), "fs": lax.rem(at, n_fs)}

    def fan(buffer, count_of, mine, send, recv, peer):
        def sent(j):
            return remote(
                buffer.at[mine], buffer.at[mine], send.at[j - 1], recv.at[count_of - j - 1], peer(j)
            )

        def received(j):
            place = buffer.at[lax.rem(mine + j, count_of)]
            return remote(place, place, send.at[j - 1], recv.at[j - 1], peer(j))

        return sent, received

    row_fan = fan(row_all, n_tp, t, row_send, row_recv, lane_peer)
    wide_fan = fan(wide_all, n_tp, t, wide_send, wide_recv, lane_peer)
    gain_fan = fan(gain_all, 2 * n_fs, r * n_fs + z, gain_send, gain_recv, group_peer)
    tall_fan = fan(
        tall_all, n_fs, z, tall_send, tall_recv, lambda j: {"fs": lax.rem(z + j, n_fs)}
    )

    def fan_start(pair_of, count_of):
        for j in range(1, count_of):
            pair_of[0](j).start()

    def fan_ready(pair_of, count_of):
        for j in range(1, count_of):
            pair_of[1](j).wait_recv()

    def fan_sent(pair_of, count_of):
        for j in range(1, count_of):
            pair_of[0](j).wait_send()

    def gain_here():
        return gain[:, pl.ds(pl.multiple_of(t * local, local), local)].astype(jnp.float32)

    def token_sums():
        last_arrival().wait_recv()
        inv_arrival().wait_recv()
        for i in range(2):
            own_loaded(i).wait()
        gain_l = gain_here()
        gain_sum[...] = jnp.zeros_like(gain_sum)

        @pl.loop(0, CORES * half // LANES)
        def _(i):
            at = tile(i, LANES)
            d_tokens = v_normed[at, :].astype(jnp.float32) * v_tokens[at, :].astype(jnp.float32)
            row_all[t, :, at] = row_of(fold(d_tokens * gain_l))
            inv = v_inv[at, :1]
            gain_sum[...] += jnp.sum(d_tokens * inv, axis=0, keepdims=True)

        gain_all[r * n_fs + z] = gain_sum[...]
        fan_start(row_fan, n_tp)
        fan_start(gain_fan, 2 * n_fs)

    def token_grads():
        fan_ready(row_fan, n_tp)
        gain_l = gain_here()

        @pl.loop(0, CORES * half // LANES)
        def _(i):
            at = tile(i, LANES)
            dots = row_all[0, :, at]
            for j in range(1, n_tp):
                dots = dots + row_all[j, :, at]
            rowdot = jnp.broadcast_to(dots, (LANES, LANES)).T[:, :1]
            inv = v_inv[at, :1]
            value = v_cot[at, :].astype(jnp.float32)
            value = value + inv * (v_normed[at, :].astype(jnp.float32) * gain_l)
            scale = inv**3 * rowdot / model
            value = value - v_tokens[at, :].astype(jnp.float32) * scale
            v_out[at, :] = value.astype(jnp.bfloat16)

        pltpu.make_async_copy(v_out, o_tokens, out_sem.at[3, 0]).start()

    def own_loaded(i):
        source, target = ((tokens, v_tokens), (cot, v_cot))[i]
        return pltpu.make_async_copy(source, target, load_sem.at[5 + i])

    def block_out(m, k):
        at = pl.ds(k * width, width)
        if m == 2:
            return pltpu.make_async_copy(v_down.at[at, :], o_down.at[at, :], out_sem.at[m, k])
        return pltpu.make_async_copy(
            outs[m].at[:, at], (o_gate, o_up)[m].at[:, at], out_sem.at[m, k]
        )

    def squares(m, k):
        spread_arrival(m, k).wait_recv()
        mine = kb * c + k == z

        @pl.when(mine)
        def _():
            keep(m, k).wait()

        block_out(m, k).start()
        if m == 2:

            @pl.loop(0, width // LANES)
            def _(i):
                at = pl.ds(pl.multiple_of(k * width + i * LANES, LANES), LANES)
                value = v_down[at, :].astype(jnp.float32)
                tall_all[z, :, at] = row_of(fold(value * value))
        else:

            @pl.loop(0, rows // LANES)
            def _(i):
                at = tile(i, LANES)
                value = outs[m][at, k * width : (k + 1) * width].astype(jnp.float32)
                part = fold(value * value)
                if k > 0:
                    part = part + lane_sq[m, at, :]
                if k < kb - 1:
                    lane_sq[m, at, :] = part
                else:
                    wide_all[t, m : m + 1, at] = row_of(part)

    for a in range(2):
        loaded(a).start()

    @pl.when(c == owner)
    def _():
        for m in range(3):
            block_loaded(m).start()

    act_start(0)
    own_start(0)
    own_start(1)
    for i in range(2):
        own_loaded(i).start()
    act_round(0, 1)
    act_round(0, 2)
    weight_start(0)
    weight_start(1)
    act_start(1)
    own_start(2)
    for d in range(3, n_fs):
        act_round(0, d)
    weight_all(0)
    act_round(1, 1)
    weight_all(1)
    across_all(0)
    act_ready(0)
    pl.loop(0, count // LANES)(normalize)
    inv_send().start()
    v_inv[own_rows(c), :] = inv_all[band_rows(z), :]
    weight_start(2)
    across_all(1)
    act_round(1, 2)
    weight_ready((0, 1))
    pl.loop(0, count // TILE)(forward)
    weight_all(2)
    for d in range(3, n_fs):
        act_round(1, d)
    across_all(2)
    act_ready(1)
    gradients(2, 0)
    for k in range(kb):
        first(2, k)
    gradients(2, 1)
    weight_ready((2,))
    pl.loop(0, count // TILE)(backward)
    act_sent(0)

    @pl.loop(0, n_fs)
    def _(i):
        band = line_band(y_turn(i))
        pull_back(band, 1 - y)
        over(band).start()

    gradients(0, 0)
    for k in range(kb):
        first(0, k)
    gradients(1, 0)
    for k in range(kb):
        first(1, k)
    gradients(0, 1)
    for k in range(kb):
        second(2, k)

    @pl.loop(0, n_fs)
    def _(i):
        pull_back(i, y)

    gradients(1, 1)
    second(0, 0)
    normed_outer(0)
    second(0, 1)
    third(2, 0)
    third(2, 1)
    normed_outer(1)
    second(1, 0)
    normed_inner(n_fs - 1)
    normed_inner(0)
    second(1, 1)
    normed_outer(2)
    third(0, 0)
    third(0, 1)
    normed_inner(1)
    third(1, 0)
    third(1, 1)
    normed_last()
    squares(2, 0)
    squares(2, 1)
    fan_start(tall_fan, n_fs)
    token_sums()
    squares(0, 0)
    squares(0, 1)
    token_grads()
    squares(1, 0)
    squares(1, 1)
    fan_start(wide_fan, n_tp)
    fan_ready(gain_fan, 2 * n_fs)
    gain_total = gain_all[0]
    for j in range(1, 2 * n_fs):
        gain_total = gain_total + gain_all[j]
    o_gain[...] = gain_total
    fan_ready(tall_fan, n_fs)
    tall_total = tall_all[0]
    for j in range(1, n_fs):
        tall_total = tall_total + tall_all[j]
    o_tall_sq[...] = tall_total

    for m in range(3):
        for k in range(kb):
            for j in range(2):
                pair(m, k, j).wait_send()
            swap(m, k).wait_send()

            @pl.when(kb * c + k != z)
            def _():
                deliver(m, k).wait_send()

            spread(m, k, place(m, k, r)).wait_send()
            block_out(m, k).wait()
    pltpu.make_async_copy(v_out, o_tokens, out_sem.at[3, 0]).wait()
    for b in range(n_fs):
        over(b).wait_send()
    normed_sent()
    inv_send().wait_send()
    last_send().wait_send()
    act_sent(1)
    for m in range(3):
        weight_sent(m)
    fan_sent(row_fan, n_tp)
    fan_sent(gain_fan, 2 * n_fs)
    fan_sent(tall_fan, n_fs)
    fan_ready(wide_fan, n_tp)
    wide_total = wide_all[0]
    for j in range(1, n_tp):
        wide_total = wide_total + wide_all[j]
    o_wide_sq[...] = wide_total
    fan_sent(wide_fan, n_tp)


def layer(n_fs, n_tp, tokens, cot, w_gate, w_up, w_down, gain):
    half, local = tokens.shape[0] // CORES, tokens.shape[1]
    rows, hidden = w_gate.shape
    width = hidden * CORES // n_fs
    model = rows * n_fs
    count = half * n_fs
    dtype = tokens.dtype
    kb = n_fs // CORES
    strip = rows // 2
    reach = model // 2
    wide, tall = (strip, width), (width, strip)
    dma = pltpu.SemaphoreType.DMA
    vmem = pl.BlockSpec(memory_space=pltpu.VMEM)
    hbm = pl.BlockSpec(memory_space=pl.ANY)
    line = dma((2, 2, n_fs - 1, CORES))
    pairs, singles = dma((3, kb, 2)), dma((3, kb))

    def bf(*shape):
        return pltpu.VMEM(shape, dtype)

    def f32(*shape):
        return pltpu.VMEM(shape, jnp.float32)

    hidden = kb * width
    shapes = [(rows, hidden)] * 2 + [(hidden, rows)]
    return pl.pallas_call(
        functools.partial(layer_kernel, n_fs, n_tp),
        out_shape=[jax.ShapeDtypeStruct(s, dtype) for s in shapes]
        + [jax.ShapeDtypeStruct((CORES * half, local), dtype)]
        + [jax.ShapeDtypeStruct(s, jnp.float32) for s in ((1, local), (2, rows), (1, hidden))],
        in_specs=[hbm] * 5 + [vmem],
        out_specs=[hbm] * 4 + [vmem] * 3,
        scratch_shapes=[
            bf(count, model),
            bf(count, model),
            bf(model, width),
            bf(model, width),
            bf(width, model),
            bf(count, model),
            bf(model, count),
            bf(width, count),
            f32(count, width),
            f32(count, width),
            bf(count, width),
            bf(count, width),
            f32(count, LANES),
            bf(model, width),
            bf(model, width),
            bf(width, model),
            bf(2, kb, 2, *wide),
            bf(kb, 2, *tall),
            bf(2, kb, *wide),
            bf(kb, *tall),
            bf(2, kb, *wide),
            bf(kb, *tall),
            bf(2, kb, *wide),
            bf(kb, *tall),
            bf(n_fs, half, reach),
            bf(n_fs, half, reach),
            bf(2, n_fs, half, reach),
            bf(half, local),
            bf(rows, hidden),
            bf(rows, hidden),
            bf(hidden, rows),
            bf(CORES * half, local),
            bf(CORES * half, local),
            bf(CORES * half, local),
            f32(CORES * half, LANES),
            bf(CORES * half, local),
            f32(2, rows, LANES),
            f32(n_tp, 1, CORES * half),
            f32(2 * n_fs, 1, local),
            f32(n_tp, 2, rows),
            f32(n_fs, 1, hidden),
            dma((7,)),
            dma((2, 2, CORES)),
            line,
            line,
            dma((2, CORES)),
            line,
            dma((2, n_fs, CORES)),
            dma((2,)),
            dma((2,)),
            dma((3, kb, CORES)),
            dma((3, n_fs)),
            dma((3, n_fs)),
            dma((3, n_fs)),
            dma((3, n_fs, 2)),
            dma((3, n_fs, 2)),
            dma((3,)),
            dma((3,)),
            pairs,
            pairs,
            singles,
            singles,
            singles,
            singles,
            singles,
            singles,
            dma((n_fs,)),
            dma((n_fs,)),
            dma((n_fs,)),
            dma((2, n_fs)),
            dma((2,)),
            dma((2,)),
            dma((3, kb)),
            dma((n_tp - 1,)),
            dma((n_tp - 1,)),
            dma((2 * n_fs - 1,)),
            dma((2 * n_fs - 1,)),
            dma((n_tp - 1,)),
            dma((n_tp - 1,)),
            dma((n_fs - 1,)),
            dma((n_fs - 1,)),
            dma((4, kb)),
            f32(half, reach),
            f32(1, local),
        ],
        compiler_params=pltpu.CompilerParams(
            collective_id=4, has_side_effects=True, vmem_limit_bytes=67043328
        ),
        name="layer",
    )(tokens, cot, w_gate, w_up, w_down, gain)


def by_chip(tokens, norm_gain, w_gate, w_up, w_down, cotangent):
    s_gate, s_up, s_down, grad_tokens, grad_gain, gate_up_sq, down_sq = layer(
        lax.axis_size("fs"),
        lax.axis_size("tp"),
        tokens,
        cotangent,
        w_gate,
        w_up,
        w_down,
        norm_gain[None, :],
    )
    grad_gate, grad_up, grad_down = (s.astype(jnp.float32) for s in (s_gate, s_up, s_down))
    return (grad_tokens, grad_gain[0], grad_gate, grad_up, grad_down, gate_up_sq, down_sq[0])


def fits_chips(mesh):
    n_rep, n_fs, n_tp = mesh.shape["rep"], mesh.shape["fs"], mesh.shape["tp"]
    return n_rep == 2 and n_tp == 2 * CORES and n_fs == 2 * CORES


def solution(mesh):
    placed = (
        P(("rep", "fs"), "tp"),
        P(),
        P("fs", "tp"),
        P("fs", "tp"),
        P("tp", "fs"),
        P(("rep", "fs"), "tp"),
    )
    return jax.shard_map(
        by_chip if fits_chips(mesh) else on_device,
        mesh=mesh,
        in_specs=placed,
        out_specs=(
            P(("rep", "fs"), "tp"),
            P("tp"),
            P("fs", "tp"),
            P("fs", "tp"),
            P("tp", "fs"),
            P(None, "fs"),
            P("tp"),
        ),
        check_vma=False,
    )
```

```python
import functools

import jax
import jax.numpy as jnp
from jax import lax
from jax.experimental import pallas as pl
from jax.experimental.pallas import tpu as pltpu
from jax.sharding import PartitionSpec as P

MESH = pl.DeviceIdType.MESH


def contract_last(left, right):
    return lax.dot_general(
        left, right, (((1,), (1,)), ((), ())), preferred_element_type=jnp.float32
    )


def contract_first(left, right):
    return lax.dot_general(
        left, right, (((0,), (0,)), ((), ())), preferred_element_type=jnp.float32
    )


def remote(source, target, send_sem, recv_sem, where):
    return pltpu.make_async_remote_copy(
        src_ref=source,
        dst_ref=target,
        send_sem=send_sem,
        recv_sem=recv_sem,
        device_id=where,
        device_id_type=MESH,
    )


def line_sends(z, n_fs, side, d):
    if side == 0:
        return jnp.logical_and(z >= d - 1, z <= n_fs - 2)
    return jnp.logical_and(z + d <= n_fs, z >= 1)


def line_receives(z, n_fs, side, d):
    return z >= d if side == 0 else z + d <= n_fs - 1


def greet(peers):
    barrier = pltpu.get_barrier_semaphore()
    for peer in peers:
        pl.semaphore_signal(barrier, inc=1, device_id=peer, device_id_type=MESH)
    pl.semaphore_wait(barrier, len(peers))


def keep_own(sources, holders, targets, sems):
    count = len(sources)
    loads = [
        pltpu.make_async_copy(sources[i], holders[i], sems.at[0, i]) for i in range(count)
    ]
    stores = [
        pltpu.make_async_copy(holders[i], targets[i], sems.at[1, i]) for i in range(count)
    ]
    for load in loads:
        load.start()

    def finish():
        for load, store in zip(loads, stores):
            load.wait()
            store.start()
        for store in stores:
            store.wait()

    return finish


def weights_kernel(n_fs, n_tp, *refs):
    tokens, cot, w_gate, w_up, w_down = refs[:5]
    whole_x, whole_dy, full_gate, full_up, full_down = refs[5:10]
    holders = refs[10:15]
    own_sem, ring_send, ring_recv, rep_send, rep_recv, tp_send, tp_recv = refs[15:]
    r, z, t = lax.axis_index("rep"), lax.axis_index("fs"), lax.axis_index("tp")
    right, left = lax.rem(z + 1, n_fs), lax.rem(z + n_fs - 1, n_fs)
    partner = {"rep": 1 - r}
    sources = (w_gate, w_up, w_down)
    targets = (full_gate, full_up, full_down)
    rows = w_gate.shape[0]
    hidden = w_down.shape[0]
    local = tokens.shape[1]

    def own_piece(m, half):
        size = (hidden if m == 2 else rows) // 2
        return sources[m].at[pl.ds(pl.multiple_of(half * size, size), size), :]

    def piece(m, owner, half):
        if m == 2:
            size = hidden // 2
            return targets[m].at[
                pl.ds(pl.multiple_of(half * size, size), size),
                pl.ds(pl.multiple_of(owner * rows, rows), rows),
            ]
        size = rows // 2
        return targets[m].at[
            pl.ds(pl.multiple_of(owner * rows + half * size, size), size), :
        ]

    peers = [{"fs": right}, {"fs": left}, partner]
    peers += [{"tp": lax.rem(t + j, n_tp)} for j in range(1, n_tp)]
    greet(peers)

    def owner_of(side, back):
        return lax.rem(z + (n_fs - back if side == 0 else back), n_fs)

    def hop(m, side, d):
        place = piece(m, owner_of(side, d - 1), r)
        return remote(
            own_piece(m, r) if d == 1 else place,
            place,
            ring_send.at[m, side, d - 1],
            ring_recv.at[m, side, d - 1],
            {"fs": right if side == 0 else left},
        )

    def arrival(m, side, d):
        place = piece(m, owner_of(side, d), r)
        return remote(
            place,
            place,
            ring_send.at[m, side, d - 1],
            ring_recv.at[m, side, d - 1],
            {"fs": right if side == 0 else left},
        )

    def across(m, side, d):
        place = piece(m, owner_of(side, d), r)
        return remote(
            place, place, rep_send.at[m, side, d - 1], rep_recv.at[m, side, d - 1], partner
        )

    for m in range(3):
        for side in range(2):

            @pl.when(line_sends(z, n_fs, side, 1))
            def _():
                hop(m, side, 1).start()

    ends = []
    for a, (source, target) in enumerate(((tokens, whole_x), (cot, whole_dy))):
        place = target.at[:, pl.ds(pl.multiple_of(t * local, local), local)]
        for j in range(1, n_tp):
            copy = remote(
                source,
                place,
                tp_send.at[a, j - 1],
                tp_recv.at[a, j - 1],
                {"tp": lax.rem(t + j, n_tp)},
            )
            copy.start()
            ends.append(copy)
    mine = pl.ds(pl.multiple_of(t * local, local), local)
    band = pl.ds(pl.multiple_of(z * rows, rows), rows)
    finish = keep_own(
        (tokens, cot, w_gate, w_up, w_down),
        holders,
        (
            whole_x.at[:, mine],
            whole_dy.at[:, mine],
            full_gate.at[band, :],
            full_up.at[band, :],
            full_down.at[:, band],
        ),
        own_sem,
    )
    finish()
    for d in range(1, n_fs):
        for m in range(3):
            for side in range(2):

                @pl.when(line_receives(z, n_fs, side, d))
                def _():
                    arrival(m, side, d).wait_recv()
                    if d < n_fs - 1:

                        @pl.when(line_sends(z, n_fs, side, d + 1))
                        def _():
                            hop(m, side, d + 1).start()

                    across(m, side, d).start()

    for d in range(1, n_fs):
        for m in range(3):
            for side in range(2):

                @pl.when(line_sends(z, n_fs, side, d))
                def _():
                    hop(m, side, d).wait_send()

                @pl.when(line_receives(z, n_fs, side, d))
                def _():
                    across(m, side, d).wait()

    for copy in ends:
        copy.wait()


def gather_weights(n_fs, n_tp, tokens, cot, w_gate, w_up, w_down):
    count, local = tokens.shape
    rows, hidden = w_gate.shape
    width = rows * n_fs
    dtype = tokens.dtype
    shapes = [
        (count, width),
        (count, width),
        (width, hidden),
        (width, hidden),
        (hidden, width),
    ]
    held = (tokens, cot, w_gate, w_up, w_down)
    moved = sum(2 * a * b for a, b in shapes)
    dma = pltpu.SemaphoreType.DMA
    return pl.pallas_call(
        functools.partial(weights_kernel, n_fs, n_tp),
        out_shape=[jax.ShapeDtypeStruct(s, dtype) for s in shapes],
        in_specs=[pl.BlockSpec(memory_space=pl.ANY)] * 5,
        out_specs=[pl.BlockSpec(memory_space=pl.ANY)] * 5,
        scratch_shapes=[pltpu.VMEM(a.shape, a.dtype) for a in held]
        + [
            dma((2, 5)),
            dma((3, 2, n_fs - 1)),
            dma((3, 2, n_fs - 1)),
            dma((3, 2, n_fs - 1)),
            dma((3, 2, n_fs - 1)),
            dma((2, n_tp - 1)),
            dma((2, n_tp - 1)),
        ],
        compiler_params=pltpu.CompilerParams(collective_id=0, has_side_effects=True),
        cost_estimate=pl.CostEstimate(flops=0, bytes_accessed=16 * moved, transcendentals=0),
        name="gather_weights",
    )(*held)


def tokens_kernel(n_fs, n_tp, n_act, n_swap, *refs):
    total = n_act + n_swap
    acts, swaps = refs[:n_act], refs[n_act:total]
    act_outs, swap_outs = refs[total : total + n_act], refs[total + n_act : 2 * total]
    holders = refs[2 * total : 3 * total]
    own_sem, ring_send, ring_recv = refs[3 * total : 3 * total + 3]
    swap_send, swap_recv, relay_send, relay_recv = refs[3 * total + 3 :]
    z, t = lax.axis_index("fs"), lax.axis_index("tp")
    right, left = lax.rem(z + 1, n_fs), lax.rem(z + n_fs - 1, n_fs)
    count = acts[0].shape[0]
    peers = [{"fs": lax.rem(z + j, n_fs)} for j in range(1, n_fs)]
    if n_swap:
        peers += [{"tp": lax.rem(t + j, n_tp)} for j in range(1, n_tp)]
    greet(peers)

    def rows_of(owner):
        return pl.ds(pl.multiple_of(owner * count, count), count)

    def owner_of(side, back):
        return lax.rem(z + (n_fs - back if side == 0 else back), n_fs)

    def hop(m, side, d):
        place = act_outs[m].at[rows_of(owner_of(side, d - 1)), :]
        return remote(
            acts[m] if d == 1 else place,
            place,
            ring_send.at[m, side, d - 1],
            ring_recv.at[m, side, d - 1],
            {"fs": right if side == 0 else left},
        )

    def arrival(m, side, d):
        place = act_outs[m].at[rows_of(owner_of(side, d)), :]
        return remote(
            place,
            place,
            ring_send.at[m, side, d - 1],
            ring_recv.at[m, side, d - 1],
            {"fs": right if side == 0 else left},
        )

    def swap(a, j):
        peer = lax.rem(z + j, n_fs)
        cut = swap_outs[a].shape[1]
        return remote(
            swaps[a].at[:, pl.ds(pl.multiple_of(peer * cut, cut), cut)],
            swap_outs[a].at[rows_of(z), :],
            swap_send.at[a, j - 1],
            swap_recv.at[a, j - 1],
            {"fs": peer},
        )

    def swapped(a, j):
        place = swap_outs[a].at[rows_of(owner_of(0, j)), :]
        return remote(
            place,
            place,
            swap_send.at[a, j - 1],
            swap_recv.at[a, j - 1],
            {"fs": lax.rem(z + j, n_fs)},
        )

    def relay(a, j, k):
        place = swap_outs[a].at[rows_of(owner_of(0, j)), :]
        return remote(
            place,
            place,
            relay_send.at[a, j - 1, k - 1],
            relay_recv.at[a, j - 1],
            {"tp": lax.rem(t + k, n_tp)},
        )

    hub = lax.rem(z, n_tp) == t

    def feeds(j):
        return lax.rem(lax.rem(z + j, n_fs), n_tp) == t

    for a in range(n_swap):
        for j in range(1, n_fs):

            @pl.when(feeds(j))
            def _():
                swap(a, j).start()

    for m in range(n_act):
        for side in range(2):

            @pl.when(line_sends(z, n_fs, side, 1))
            def _():
                hop(m, side, 1).start()

    sources = list(acts)
    for a in range(n_swap):
        cut = swap_outs[a].shape[1]
        sources.append(swaps[a].at[:, pl.ds(pl.multiple_of(z * cut, cut), cut)])
    finish = keep_own(
        sources, holders, [out.at[rows_of(z), :] for out in act_outs + swap_outs], own_sem
    )
    finish()
    if n_swap:

        @pl.when(hub)
        def _():
            for a in range(n_swap):
                for j in range(1, n_fs):
                    swapped(a, j).wait_recv()
                    for k in range(1, n_tp):
                        relay(a, j, k).start()

    for d in range(1, n_fs):
        for m in range(n_act):
            for side in range(2):

                @pl.when(line_receives(z, n_fs, side, d))
                def _():
                    arrival(m, side, d).wait_recv()
                    if d < n_fs - 1:

                        @pl.when(line_sends(z, n_fs, side, d + 1))
                        def _():
                            hop(m, side, d + 1).start()

    for d in range(1, n_fs):
        for m in range(n_act):
            for side in range(2):

                @pl.when(line_sends(z, n_fs, side, d))
                def _():
                    hop(m, side, d).wait_send()

    for a in range(n_swap):
        for j in range(1, n_fs):

            @pl.when(feeds(j))
            def _():
                swap(a, j).wait_send()

            @pl.when(hub)
            def _():
                for k in range(1, n_tp):
                    relay(a, j, k).wait_send()

            @pl.when(jnp.logical_not(hub))
            def _():
                relay(a, j, 1).wait_recv()


def gather_tokens(n_fs, n_tp, collective_id, acts, swaps):
    count = acts[0].shape[0]
    outs = [jax.ShapeDtypeStruct((n_fs * count, a.shape[1]), a.dtype) for a in acts]
    outs += [jax.ShapeDtypeStruct((n_fs * count, a.shape[1] // n_fs), a.dtype) for a in swaps]
    dma = pltpu.SemaphoreType.DMA
    total = len(outs)
    n_swap = max(len(swaps), 1)
    moved = sum(2 * o.shape[0] * o.shape[1] for o in outs)
    return pl.pallas_call(
        functools.partial(tokens_kernel, n_fs, n_tp, len(acts), len(swaps)),
        out_shape=outs,
        in_specs=[pl.BlockSpec(memory_space=pl.ANY)] * total,
        out_specs=[pl.BlockSpec(memory_space=pl.ANY)] * total,
        scratch_shapes=[pltpu.VMEM((count, o.shape[1]), o.dtype) for o in outs]
        + [
            dma((2, total)),
            dma((len(acts), 2, n_fs - 1)),
            dma((len(acts), 2, n_fs - 1)),
            dma((n_swap, n_fs - 1)),
            dma((n_swap, n_fs - 1)),
            dma((n_swap, n_fs - 1, n_tp - 1)),
            dma((n_swap, n_fs - 1)),
        ],
        compiler_params=pltpu.CompilerParams(
            collective_id=collective_id, has_side_effects=True
        ),
        cost_estimate=pl.CostEstimate(flops=0, bytes_accessed=16 * moved, transcendentals=0),
        name=f"gather_tokens_{collective_id}",
    )(*acts, *swaps)


def over_rep(part):
    part = part.astype(jnp.bfloat16)
    n_rep = lax.axis_size("rep")
    other = lax.ppermute(part, "rep", [(i, (i + 1) % n_rep) for i in range(n_rep)])
    return part, other


def added(pair):
    return pair[0].astype(jnp.float32) + pair[1].astype(jnp.float32)


def on_device(tokens, norm_gain, w_gate, w_up, w_down, cotangent):
    n_fs, n_tp = lax.axis_size("fs"), lax.axis_size("tp")
    whole_x, whole_dy, full_gate, full_up, full_down = gather_weights(
        n_fs, n_tp, tokens, cotangent, w_gate, w_up, w_down
    )
    width = whole_x.shape[1]
    wide_tokens = whole_x.astype(jnp.float32)
    gain_f = norm_gain.astype(jnp.float32)
    inverse = lax.rsqrt(jnp.mean(wide_tokens * wide_tokens, axis=-1, keepdims=True) + 1e-06)
    normed = (wide_tokens * inverse * gain_f).astype(jnp.bfloat16)
    gate = jnp.dot(normed, full_gate, preferred_element_type=jnp.float32)
    up_proj = jnp.dot(normed, full_up, preferred_element_type=jnp.float32)
    sigma = jax.nn.sigmoid(gate)
    active = gate * sigma
    hidden = (active * up_proj).astype(jnp.bfloat16)
    back = 0.5 * contract_last(whole_dy, full_down)
    d_up = (back * active).astype(jnp.bfloat16)
    d_gate = (back * up_proj * sigma * (1.0 + gate * (1.0 - sigma))).astype(jnp.bfloat16)

    all_hidden, rows_dy = gather_tokens(n_fs, n_tp, 1, [hidden], [whole_dy])
    down_pair = over_rep(0.5 * contract_first(all_hidden, rows_dy))

    partial_normed = contract_last(d_gate, full_gate) + contract_last(d_up, full_up)
    d_normed = lax.psum_scatter(
        partial_normed.astype(jnp.bfloat16), "tp", scatter_dimension=1, tiled=True
    ).astype(jnp.float32)

    all_gate, rows_normed = gather_tokens(n_fs, n_tp, 2, [d_gate], [normed])
    gate_pair = over_rep(contract_first(rows_normed, all_gate))
    (all_up,) = gather_tokens(n_fs, n_tp, 3, [d_up], [])
    up_pair = over_rep(contract_first(rows_normed, all_up))

    local_width = d_normed.shape[1]
    local_gain = lax.dynamic_slice_in_dim(
        gain_f, lax.axis_index("tp") * local_width, local_width, 0
    )
    local_tokens = tokens.astype(jnp.float32)
    scaled_grad = d_normed * local_gain
    rowdot = lax.psum(jnp.sum(scaled_grad * local_tokens, axis=-1), "tp")
    grad_tokens = (
        cotangent.astype(jnp.float32)
        + inverse * scaled_grad
        - local_tokens * inverse**3 * rowdot[:, None] / width
    ).astype(jnp.bfloat16)
    grad_gain = lax.psum(jnp.sum(d_normed * local_tokens * inverse, axis=0), ("rep", "fs"))

    grad_down = added(down_pair)
    down_sq = lax.psum(jnp.sum(grad_down * grad_down, axis=1), "fs")
    grad_gate = added(gate_pair)
    grad_up = added(up_pair)
    gate_up_sq = lax.psum(
        jnp.stack([jnp.sum(grad_gate * grad_gate, axis=1), jnp.sum(grad_up * grad_up, axis=1)]),
        "tp",
    )
    return (grad_tokens, grad_gain, grad_gate, grad_up, grad_down, gate_up_sq, down_sq)


CORES = 2
LANES = 128
TILE = 256
PARTS = 2


def line_next(z, n_fs, side):
    return z <= n_fs - 2 if side == 0 else z >= 1


def layer_kernel(n_fs, n_tp, *refs):
    tokens, cot, w_gate, w_up, w_down, gain_in = refs[:6]
    o_gate, o_up, o_down, o_tokens, o_gain, o_wide_sq, o_tall_sq = refs[6:13]
    full = refs[13:18]
    x_full, dy_full, f_gate, f_up, f_down = full
    normed, normed_t, hidden_t, act_f, slope_f, d_gate, d_up, inv_all = refs[18:26]
    g_gate, g_up, g_down = refs[26:29]
    pair_wide, pair_tall, sum_wide, sum_tall, x_wide, x_tall, t_wide, t_tall = refs[29:37]
    y_buf, d_buf, z_buf, n_buf = refs[37:41]
    v_gate, v_up, v_down, v_tokens, v_cot, v_normed, v_inv, v_out = refs[41:49]
    lane_sq, row_all, gain_all, wide_all, tall_all = refs[49:54]
    (load_sem, az_own, az_fwd, az_recv, ay_own, ay_fwd, ay_recv, ap_send, ap_recv) = refs[54:63]
    (w_send, w_recv, wx_send, wx_recv, wp_send, wp_recv, wo_send, wo_recv) = refs[63:71]
    (p_send, p_recv, x_send, x_recv, z_send, z_recv, f_send, f_recv) = refs[71:79]
    (y_send, y_recv, d_send, d_recv, n_send, n_recv, own_sem) = refs[79:86]
    (row_send, row_recv, gain_send, gain_recv) = refs[86:90]
    (wide_send, wide_recv, tall_send, tall_recv, out_sem, total, gain_sum) = refs[90:97]
    gain_load, gain, v_wide, v_tall, v_half = refs[97:]
    r, z, t = lax.axis_index("rep"), lax.axis_index("fs"), lax.axis_index("tp")
    y, c = lax.div(t, CORES), lax.rem(t, CORES)
    acts, weights = (tokens, cot), (w_gate, w_up, w_down)
    grads, outs = (g_gate, g_up, g_down), (v_gate, v_up, v_down)
    half, local = tokens.shape[0] // CORES, tokens.shape[1]
    count, model = x_full.shape
    rows = w_gate.shape[0]
    kb = n_fs // CORES
    width = w_gate.shape[1] // kb
    strip = rows // 2
    reach = model // 2
    partner = {"tp": y * CORES + 1 - c}
    across = {"rep": 1 - r}
    beside = {"tp": (1 - y) * CORES + c}
    owner = lax.div(z, kb)

    peers = [partner, across]
    peers += [{"tp": (1 - y) * CORES + h} for h in range(CORES)]
    for j in range(1, n_fs):
        for h in range(CORES):
            peers.append({"fs": lax.rem(z + j, n_fs), "tp": y * CORES + h})
        peers.append({"rep": 1 - r, "fs": lax.rem(z + j, n_fs)})
    greet(peers)

    def own_act(a, h):
        return acts[a].at[pl.ds(pl.multiple_of(h * half, half), half), :]

    def act_place(a, source, column):
        return full[a].at[
            pl.ds(pl.multiple_of(source * half, half), half),
            pl.ds(pl.multiple_of(column * local, local), local),
        ]

    sub = half // PARTS

    def own_part(a, h, q):
        start = h * half + q * sub
        return acts[a].at[pl.ds(start, sub), :]

    def act_part(a, source, column, q):
        return full[a].at[
            pl.ds(pl.multiple_of(source * half + q * sub, sub), sub),
            pl.ds(pl.multiple_of(column * local, local), local),
        ]

    def source_of(side, d):
        return z - d if side == 0 else z + d

    def next_of(side):
        return z + 1 if side == 0 else z - 1

    def line_turn(source, at):
        return lax.rem(source - at + n_fs, n_fs) - 1

    def act_first(a, side, h, q):
        return remote(
            own_part(a, h, q),
            act_part(a, z, t, q),
            az_own.at[a, side],
            az_recv.at[a, line_turn(z, next_of(side)), c, q],
            {"fs": next_of(side), "tp": y * CORES + h},
        )

    def act_arrival(a, side, d, core, q):
        place = act_part(a, source_of(side, d), y * CORES + core, q)
        return remote(
            place,
            place,
            az_fwd.at[a],
            az_recv.at[a, line_turn(source_of(side, d), z), core, q],
            partner,
        )

    def act_forward(a, side, d, core, q):
        place = act_part(a, source_of(side, d), y * CORES + core, q)
        return remote(
            place,
            place,
            az_fwd.at[a],
            az_recv.at[a, line_turn(source_of(side, d), next_of(side)), core, q],
            {"fs": next_of(side)},
        )

    def act_over(a, side, d, core, q):
        source = source_of(side, d)
        place = act_part(a, source, y * CORES + core, q)
        return remote(
            place,
            place,
            ay_fwd.at[a],
            ay_recv.at[a, source, core, q],
            {"tp": (1 - y) * CORES + c},
        )

    def act_over_arrival(a, source, core, q):
        place = act_part(a, source, (1 - y) * CORES + core, q)
        return remote(place, place, ay_own.at[a], ay_recv.at[a, source, core, q], partner)

    def act_over_own(a, h):
        return remote(
            own_act(a, h),
            act_place(a, z, t),
            ay_own.at[a],
            ay_recv.at[a, z, c, 0],
            {"tp": (1 - y) * CORES + h},
        )

    def act_over_own_arrival(a, core):
        place = act_place(a, z, (1 - y) * CORES + core)
        return remote(place, place, ay_own.at[a], ay_recv.at[a, z, core, 0], partner)

    def act_partner(a):
        return remote(own_act(a, 1 - c), act_place(a, z, t), ap_send.at[a], ap_recv.at[a], partner)

    def act_partner_arrival(a):
        place = act_place(a, z, y * CORES + 1 - c)
        return remote(place, place, ap_send.at[a], ap_recv.at[a], partner)

    def block_of(m, k):
        if m == 2:
            return weights[m].at[pl.ds(pl.multiple_of(k * width, width), width), :]
        return weights[m].at[:, pl.ds(pl.multiple_of(k * width, width), width)]

    def band_of(m, source):
        band = pl.ds(pl.multiple_of(source * rows, rows), rows)
        return full[2 + m].at[:, band] if m == 2 else full[2 + m].at[band, :]

    def quarter(m, source, rep, core):
        if m == 2:
            size = width // (2 * CORES)
            return full[4].at[
                pl.ds(pl.multiple_of((rep * CORES + core) * size, size), size),
                pl.ds(pl.multiple_of(source * rows, rows), rows),
            ]
        size = rows // (2 * CORES)
        start = source * rows + (rep * CORES + core) * size
        return full[2 + m].at[pl.ds(pl.multiple_of(start, size), size), :]

    def own_quarter(m, k, core):
        if m == 2:
            size = width // (2 * CORES)
            start = k * width + (r * CORES + core) * size
            return weights[m].at[pl.ds(pl.multiple_of(start, size), size), :]
        size = rows // (2 * CORES)
        return weights[m].at[
            pl.ds(pl.multiple_of((r * CORES + core) * size, size), size),
            pl.ds(k * width, width),
        ]

    def weight_send(m, k, core):
        return remote(
            own_quarter(m, k, core),
            quarter(m, z, r, core),
            w_send.at[m, k],
            w_recv.at[m, z],
            {"fs": kb * c + k, "tp": y * CORES + core},
        )

    def weight_arrival(m, source):
        place = quarter(m, source, r, c)
        return remote(place, place, wx_send.at[m], w_recv.at[m, source], partner)

    def weight_across(m, source):
        place = quarter(m, source, r, c)
        return remote(place, place, wx_send.at[m], wx_recv.at[m, source], across)

    def weight_across_arrival(m, source):
        place = quarter(m, source, 1 - r, c)
        return remote(place, place, wx_send.at[m], wx_recv.at[m, source], across)

    def weight_beside(m, source, which):
        place = quarter(m, source, r if which == 0 else 1 - r, c)
        return remote(
            place, place, wp_send.at[m], wp_recv.at[m, source, which], partner
        )

    def weight_beside_arrival(m, source, which):
        place = quarter(m, source, r if which == 0 else 1 - r, 1 - c)
        return remote(
            place, place, wp_send.at[m], wp_recv.at[m, source, which], partner
        )

    def own_beside(m):
        return remote(
            block_of(m, z - kb * owner), band_of(m, z), wo_send.at[m], wo_recv.at[m], partner
        )

    def own_beside_arrival(m):
        return remote(band_of(m, z), band_of(m, z), wo_send.at[m], wo_recv.at[m], partner)

    def slot(wide, tall, m, *where):
        return tall.at[where] if m == 2 else wide.at[(m,) + where]

    def strip_of(band, rep):
        return pl.ds(pl.multiple_of(band * rows + rep * strip, strip), strip)

    def grad_piece(m, band, rep):
        if m == 2:
            return grads[m].at[:, strip_of(band, rep)]
        return grads[m].at[strip_of(band, rep), :]

    def rep_of(j):
        return 1 - r if j == 0 else r

    def pair(m, k, j):
        return remote(
            grad_piece(m, kb * (1 - c) + k, rep_of(j)),
            slot(pair_wide, pair_tall, m, k, j),
            p_send.at[m],
            p_recv.at[m, k, j],
            partner,
        )

    def swap(m, k):
        return remote(
            slot(sum_wide, sum_tall, m, k),
            slot(x_wide, x_tall, m, k),
            x_send.at[m],
            x_recv.at[m, k],
            across,
        )

    def place(m, block, rep):
        strips = pl.ds(pl.multiple_of(rep * strip, strip), strip)
        blocks = pl.ds(pl.multiple_of(block * width, width), width)
        return outs[m].at[blocks, strips] if m == 2 else outs[m].at[strips, blocks]

    def deliver(m, k):
        block = lax.rem(z, kb)
        return remote(
            slot(t_wide, t_tall, m, k),
            place(m, block, r),
            z_send.at[m, k],
            z_recv.at[m, block],
            {"fs": kb * c + k, "tp": y * CORES + owner},
        )

    def delivered(m, k):
        return remote(place(m, k, r), place(m, k, r), z_send.at[m, k], z_recv.at[m, k], partner)

    def keep(m, k):
        return pltpu.make_async_copy(slot(t_wide, t_tall, m, k), place(m, k, r), own_sem.at[m, k])

    def spread(m, k, source):
        return remote(source, place(m, k, r), f_send.at[m], f_recv.at[m, k], across)

    def spread_arrival(m, k):
        return remote(
            place(m, k, 1 - r), place(m, k, 1 - r), f_send.at[m], f_recv.at[m, k], across
        )

    def band_rows(band):
        return pl.ds(pl.multiple_of(band * half, half), half)

    def side_columns(which):
        return pl.ds(pl.multiple_of(which * reach, reach), reach)

    def over(band):
        return remote(
            x_full.at[band_rows(band), side_columns(1 - y)],
            y_buf.at[band],
            y_send.at[0],
            y_recv.at[band],
            beside,
        )

    low = z < n_fs // 2
    inner = jnp.logical_and(z > 0, z < n_fs - 1)
    line_slot = jnp.where(low, 0, 1)

    def line_band(i):
        return jnp.where(low, n_fs - 1 - i, i)

    def y_turn(i):
        return jnp.where(jnp.logical_and(inner, i >= 2), n_fs + 1 - i, i)

    def line_send(i, target):
        band = line_band(i)
        return remote(
            d_buf.at[i],
            z_buf.at[line_slot, band],
            d_send.at[i],
            d_recv.at[line_slot, band],
            {"fs": target},
        )

    def line_arrival(which, band):
        place = z_buf.at[which, band]
        return remote(place, place, d_send.at[0], d_recv.at[which, band], partner)

    def own_rows(core):
        return pl.ds(pl.multiple_of(core * half, half), half)

    def inv_send():
        return remote(inv_all.at[band_rows(z), :], v_inv.at[own_rows(c), :], n_send.at[0], n_recv.at[0], partner)

    def inv_arrival():
        at = v_inv.at[own_rows(1 - c), :]
        return remote(at, at, n_send.at[0], n_recv.at[0], partner)

    def last_send():
        return remote(n_buf, v_normed.at[own_rows(c), :], n_send.at[1], n_recv.at[1], partner)

    def last_arrival():
        at = v_normed.at[own_rows(1 - c), :]
        return remote(at, at, n_send.at[1], n_recv.at[1], partner)

    def loaded(a):
        return pltpu.make_async_copy(own_act(a, c), act_place(a, z, t), load_sem.at[a])

    def block_loaded(m):
        return pltpu.make_async_copy(
            block_of(m, z - kb * owner), band_of(m, z), load_sem.at[2 + m]
        )

    def act_start(a):
        for h in range(CORES):
            for side in range(2):

                @pl.when(line_next(z, n_fs, side))
                def _():
                    for q in range(PARTS):
                        act_first(a, side, h, q).start()

            act_over_own(a, h).start()
        act_partner(a).start()

    def own_start(m):
        @pl.when(c == owner)
        def _():
            own_beside(m).start()

    def act_round(a, d):
        for core in range(CORES):
            for q in range(PARTS):
                for side in range(2):

                    @pl.when(line_receives(z, n_fs, side, d))
                    def _():
                        act_arrival(a, side, d, core, q).wait_recv()
                        if d < n_fs - 1:

                            @pl.when(line_next(z, n_fs, side))
                            def _():
                                act_forward(a, side, d, core, q).start()

                        act_over(a, side, d, core, q).start()

    def weight_start(m):
        for k in range(kb):

            @pl.when(kb * c + k != z)
            def _():
                for core in range(CORES):
                    weight_send(m, k, core).start()

    def weight_round(ms, d):
        for m in ms:
            for side in range(2):

                @pl.when(line_receives(z, n_fs, side, d))
                def _():
                    source = source_of(side, d)
                    weight_arrival(m, source).wait_recv()
                    weight_across(m, source).start()
                    weight_beside(m, source, 0).start()

    def across_round(ms, d):
        for m in ms:
            for side in range(2):

                @pl.when(line_receives(z, n_fs, side, d))
                def _():
                    source = source_of(side, d)
                    weight_across_arrival(m, source).wait_recv()
                    weight_beside(m, source, 1).start()

    def weight_all(m):
        for d in range(1, n_fs):
            weight_round((m,), d)

    def across_all(m):
        for d in range(1, n_fs):
            across_round((m,), d)

    def act_ready(a):
        for d in range(1, n_fs):
            for side in range(2):

                @pl.when(line_receives(z, n_fs, side, d))
                def _():
                    for core in range(CORES):
                        for q in range(PARTS):
                            act_over_arrival(a, source_of(side, d), core, q).wait_recv()

        act_partner_arrival(a).wait_recv()
        for h in range(CORES):
            act_over_own_arrival(a, h).wait_recv()
        loaded(a).wait()

    def sent(ref, sem):
        remote(ref, ref, sem, sem, partner).wait_send()

    def act_sent(a, landed):
        others = full[a].at[pl.ds(0, count - half), pl.ds(0, CORES * local)]
        if landed:
            sent(others, ay_fwd.at[a])

            @pl.when(inner)
            def _():
                sent(others, az_fwd.at[a])

        if a == 1 or not landed:
            act_partner(a).wait_send()
            sent(acts[a], ay_own.at[a])
            for side in range(2):

                @pl.when(line_next(z, n_fs, side))
                def _():
                    sent(acts[a], az_own.at[a, side])

    def weight_ready(ms):
        for m in ms:
            for d in range(1, n_fs):
                for side in range(2):

                    @pl.when(line_receives(z, n_fs, side, d))
                    def _():
                        for which in range(2):
                            weight_beside_arrival(m, source_of(side, d), which).wait_recv()

            @pl.when(c == owner)
            def _():
                block_loaded(m).wait()

            @pl.when(c != owner)
            def _():
                own_beside_arrival(m).wait_recv()

    def weight_sent(m):
        size = full[2 + m].shape[0 if m < 2 else 1] - rows
        part = (rows if m < 2 else width) // (2 * CORES)
        if m < 2:
            sent(full[2 + m].at[pl.ds(0, (n_fs - 1) * part), :], wx_send.at[m])
            sent(full[2 + m].at[pl.ds(0, 2 * (n_fs - 1) * part), :], wp_send.at[m])
            half_block = weights[m].at[pl.ds(0, CORES * part), pl.ds(0, width)]
        else:
            sent(full[4].at[pl.ds(0, part), pl.ds(0, size)], wx_send.at[m])
            sent(full[4].at[pl.ds(0, 2 * part), pl.ds(0, size)], wp_send.at[m])
            half_block = weights[m].at[pl.ds(0, CORES * part), :]
        for k in range(kb):

            @pl.when(kb * c + k != z)
            def _():
                sent(half_block, w_send.at[m, k])

        @pl.when(c == owner)
        def _():
            own_beside(m).wait_send()

    def pairs_sent(m):
        span = pl.ds(0, kb * rows)
        sent(g_down.at[:, span] if m == 2 else grads[m].at[span, :], p_send.at[m])

    def swaps_sent(m):
        sent(sum_tall if m == 2 else sum_wide.at[m], x_send.at[m])

    def spreads_sent(m):
        sent(sum_tall if m == 2 else sum_wide.at[m], f_send.at[m])

    def over_sent():
        sent(x_full.at[:, side_columns(1 - y)], y_send.at[0])

    def tile(i, size):
        return pl.ds(pl.multiple_of(i * size, size), size)

    def normalize(i):
        at = tile(i, LANES)
        wide = x_full[at, :].astype(jnp.float32)
        inv = lax.rsqrt(jnp.mean(wide * wide, axis=-1, keepdims=True) + 1e-06)
        value = wide * inv * gain[...]
        normed[at, :] = value.astype(jnp.bfloat16)
        normed_t[:, at] = value.T.astype(jnp.bfloat16)
        inv_all[at, :] = jnp.broadcast_to(inv, (LANES, LANES))

    def forward(i):
        at = tile(i, TILE)
        gate = jnp.dot(normed[at, :], f_gate[...], preferred_element_type=jnp.float32)
        up = jnp.dot(normed[at, :], f_up[...], preferred_element_type=jnp.float32)
        sigma = jax.nn.sigmoid(gate)
        active = gate * sigma
        act_f[at, :] = active
        slope_f[at, :] = up * sigma * (1.0 + gate * (1.0 - sigma))
        hidden_t[:, at] = (active * up).T.astype(jnp.bfloat16)

    def backward(i):
        at = tile(i, TILE)
        back = 0.5 * contract_last(dy_full[at, :], f_down[...])
        d_up[at, :] = (back * act_f[at, :]).astype(jnp.bfloat16)
        d_gate[at, :] = (back * slope_f[at, :]).astype(jnp.bfloat16)

    def gradient(m, own, j, k):
        band = kb * (c if own else 1 - c) + k
        at = strip_of(band, 1 - r if j == 0 else r)
        if m == 2:
            value = 0.5 * jnp.dot(
                hidden_t[...], dy_full[:, at], preferred_element_type=jnp.float32
            )
            g_down[:, at] = value.astype(jnp.bfloat16)
        else:
            right = d_gate if m == 0 else d_up
            value = jnp.dot(normed_t[at, :], right[...], preferred_element_type=jnp.float32)
            grads[m][at, :] = value.astype(jnp.bfloat16)

    def gradients(m, j):
        @pl.loop(0, kb)
        def _(k):
            gradient(m, False, j, k)
            pair(m, k, j).start()

        @pl.loop(0, kb)
        def _(k):
            gradient(m, True, j, k)

    def pull_back(band, which):
        at, columns = band_rows(band), side_columns(which)
        value = contract_last(d_gate[at, :], f_gate[columns, :])
        value = value + contract_last(d_up[at, :], f_up[columns, :])
        x_full[at, columns] = value.astype(jnp.bfloat16)

    def added(m, k, j):
        own = grad_piece(m, kb * c + k, rep_of(j))[...].astype(jnp.float32)
        return own + slot(pair_wide, pair_tall, m, k, j)[...].astype(jnp.float32)

    def put(wide, tall, m, k, value):
        if m == 2:
            tall[k] = value
        else:
            wide[m, k] = value

    def first(m, k):
        pair(m, k, 0).wait_recv()
        put(sum_wide, sum_tall, m, k, added(m, k, 0).astype(jnp.bfloat16))
        swap(m, k).start()

    def second(m, k):
        pair(m, k, 1).wait_recv()
        swap(m, k).wait_recv()
        whole = added(m, k, 1) + slot(x_wide, x_tall, m, k)[...].astype(jnp.float32)
        put(t_wide, t_tall, m, k, whole.astype(jnp.bfloat16))
        mine = kb * c + k == z

        @pl.when(mine)
        def _():
            keep(m, k).start()
            spread(m, k, slot(t_wide, t_tall, m, k)).start()

        @pl.when(jnp.logical_not(mine))
        def _():
            deliver(m, k).start()

    def third(m, k):
        @pl.when(kb * c + k != z)
        def _():
            delivered(m, k).wait_recv()
            spread(m, k, place(m, k, r)).start()

    def own_share(band):
        over(band).wait_recv()
        own = x_full[band_rows(band), side_columns(y)].astype(jnp.float32)
        return own + y_buf[band].astype(jnp.float32)

    def line_target(i):
        if i == n_fs - 1:
            return jnp.where(low, z - 1, z + 1)
        return line_band(i)

    def normed_outer(i):
        @pl.when(jnp.logical_not(inner))
        def _():
            d_buf[i] = own_share(line_band(i)).astype(jnp.bfloat16)
            line_send(i, jnp.where(low, z + 1, z - 1)).start()

    def normed_inner(i):
        @pl.when(inner)
        def _():
            band = line_band(i)
            value = own_share(band)
            if i < n_fs - 1:
                line_arrival(line_slot, band).wait_recv()
                value = value + z_buf[line_slot, band].astype(jnp.float32)
            d_buf[i] = value.astype(jnp.bfloat16)
            line_send(i, line_target(i)).start()

    def normed_sent():
        for i in range(n_fs):
            if i < n_fs - 1:

                @pl.when(jnp.logical_not(inner))
                def _():
                    line_send(i, jnp.where(low, z + 1, z - 1)).wait_send()

            if i != n_fs - 2:

                @pl.when(inner)
                def _():
                    line_send(i, line_target(i)).wait_send()

    def normed_last():
        value = own_share(z)
        for which in range(2):
            line_arrival(which, z).wait_recv()
            value = value + z_buf[which, z].astype(jnp.float32)
        total[...] = value

        for core in range(CORES):

            @pl.when(c == core)
            def _():
                mine = slice(core * local, (core + 1) * local)
                theirs = slice((1 - core) * local, (2 - core) * local)
                v_normed[core * half : (core + 1) * half, :] = total[:, mine].astype(jnp.bfloat16)
                n_buf[...] = total[:, theirs].astype(jnp.bfloat16)

        last_send().start()

    def fold(value):
        out = value[:, :LANES]
        for i in range(1, value.shape[1] // LANES):
            out = out + value[:, i * LANES : (i + 1) * LANES]
        return out

    def row_of(value):
        return jnp.sum(value.T, axis=0, keepdims=True)

    def lane_peer(j):
        return {"tp": lax.rem(t + j, n_tp)}

    def group_peer(j):
        at = lax.rem(r * n_fs + z + j, 2 * n_fs)
        return {"rep": lax.div(at, n_fs), "fs": lax.rem(at, n_fs)}

    def fan(buffer, count_of, mine, send, recv, peer):
        def sent(j):
            return remote(
                buffer.at[mine], buffer.at[mine], send.at[j - 1], recv.at[count_of - j - 1], peer(j)
            )

        def received(j):
            place = buffer.at[lax.rem(mine + j, count_of)]
            return remote(place, place, send.at[j - 1], recv.at[j - 1], peer(j))

        return sent, received

    row_fan = fan(row_all, n_tp, t, row_send, row_recv, lane_peer)
    wide_fan = fan(wide_all, n_tp, t, wide_send, wide_recv, lane_peer)
    gain_fan = fan(gain_all, 2 * n_fs, r * n_fs + z, gain_send, gain_recv, group_peer)
    tall_fan = fan(tall_all, 2 * n_fs, r * n_fs + z, tall_send, tall_recv, group_peer)

    def fan_start(pair_of, count_of):
        for j in range(1, count_of):
            pair_of[0](j).start()

    def fan_ready(pair_of, count_of):
        for j in range(1, count_of):
            pair_of[1](j).wait_recv()

    def fan_sent(pair_of, count_of):
        for j in range(1, count_of):
            pair_of[0](j).wait_send()

    def gain_here():
        return gain[:, pl.ds(pl.multiple_of(t * local, local), local)]

    def token_sums():
        last_arrival().wait_recv()
        inv_arrival().wait_recv()
        for i in range(2):
            own_loaded(i).wait()
        gain_l = gain_here()
        gain_sum[...] = jnp.zeros_like(gain_sum)

        @pl.loop(0, CORES * half // LANES)
        def _(i):
            at = tile(i, LANES)
            d_tokens = v_normed[at, :].astype(jnp.float32) * v_tokens[at, :].astype(jnp.float32)
            row_all[t, :, at] = row_of(fold(d_tokens * gain_l))
            inv = v_inv[at, :1]
            gain_sum[...] += jnp.sum(d_tokens * inv, axis=0, keepdims=True)

        gain_all[r * n_fs + z] = gain_sum[...]
        fan_start(row_fan, n_tp)
        fan_start(gain_fan, 2 * n_fs)

    def token_grads():
        fan_ready(row_fan, n_tp)
        gain_l = gain_here()

        @pl.loop(0, CORES * half // LANES)
        def _(i):
            at = tile(i, LANES)
            dots = row_all[0, :, at]
            for j in range(1, n_tp):
                dots = dots + row_all[j, :, at]
            rowdot = jnp.broadcast_to(dots, (LANES, LANES)).T[:, :1]
            inv = v_inv[at, :1]
            value = v_cot[at, :].astype(jnp.float32)
            value = value + inv * (v_normed[at, :].astype(jnp.float32) * gain_l)
            scale = inv**3 * rowdot / model
            value = value - v_tokens[at, :].astype(jnp.float32) * scale
            v_out[at, :] = value.astype(jnp.bfloat16)

        pltpu.make_async_copy(v_out, o_tokens, out_sem.at[3, 0]).start()

    def own_loaded(i):
        source, target = ((tokens, v_tokens), (cot, v_cot))[i]
        return pltpu.make_async_copy(source, target, load_sem.at[5 + i])

    def block_out(m, k):
        at = pl.ds(k * width, width)
        if m == 2:
            return pltpu.make_async_copy(v_down.at[at, :], o_down.at[at, :], out_sem.at[m, k])
        return pltpu.make_async_copy(
            outs[m].at[:, at], (o_gate, o_up)[m].at[:, at], out_sem.at[m, k]
        )

    def strip_squares(m, k):
        @pl.when(kb * c + k == z)
        def _():
            keep(m, k).wait()

        if m == 2:
            columns = pl.ds(pl.multiple_of(r * strip, strip), strip)

            @pl.loop(0, width // LANES)
            def _(i):
                at = pl.ds(pl.multiple_of(k * width + i * LANES, LANES), LANES)
                value = v_down[at, columns].astype(jnp.float32)
                tall_all[r * n_fs + z, :, at] = row_of(fold(value * value))
        else:

            @pl.loop(0, strip // LANES)
            def _(i):
                at = tile(i, LANES)
                from_row = pl.ds(pl.multiple_of(r * strip + i * LANES, LANES), LANES)
                value = outs[m][from_row, k * width : (k + 1) * width].astype(jnp.float32)
                part = fold(value * value)
                if k > 0:
                    part = part + lane_sq[m, at, :]
                if k < kb - 1:
                    lane_sq[m, at, :] = part
                else:
                    wide_all[t, m : m + 1, at] = row_of(part)

    def wide_cross():
        strips = pl.ds(pl.multiple_of(r * strip, strip), strip)
        return remote(v_half, v_wide.at[:, strips], n_send.at[2], n_recv.at[2], across)

    def wide_cross_arrival():
        place = v_wide.at[:, pl.ds(pl.multiple_of((1 - r) * strip, strip), strip)]
        return remote(place, place, n_send.at[2], n_recv.at[2], across)

    def summed(buffer, count_of):
        value = buffer[0]
        for j in range(1, count_of):
            value = value + buffer[j]
        return value

    def whole_block(m, k):
        spread_arrival(m, k).wait_recv()
        block_out(m, k).start()

    gain_copy = pltpu.make_async_copy(gain_in, gain_load, out_sem.at[3, 1])
    gain_copy.start()
    for a in range(2):
        loaded(a).start()

    @pl.when(c == owner)
    def _():
        for m in range(3):
            block_loaded(m).start()

    act_start(0)
    own_start(0)
    own_start(1)
    for i in range(2):
        own_loaded(i).start()
    act_round(0, 1)
    act_round(0, 2)
    weight_start(0)
    weight_start(1)
    act_start(1)
    own_start(2)
    for d in range(3, n_fs):
        act_round(0, d)
    weight_all(0)
    act_round(1, 1)
    weight_all(1)
    across_all(0)
    gain_copy.wait()
    for i in range(model // LANES):
        gain[:, i * LANES : (i + 1) * LANES] = gain_load[i : i + 1, :].astype(jnp.float32)
    act_ready(0)
    pl.loop(0, count // LANES)(normalize)
    inv_send().start()
    v_inv[own_rows(c), :] = inv_all[band_rows(z), :]
    weight_start(2)
    across_all(1)
    act_round(1, 2)
    weight_ready((0, 1))
    pl.loop(0, count // TILE)(forward)
    weight_all(2)
    for d in range(3, n_fs):
        act_round(1, d)
    across_all(2)
    act_ready(1)
    gradients(2, 0)
    for k in range(kb):
        first(2, k)
    gradients(2, 1)
    weight_ready((2,))
    pl.loop(0, count // TILE)(backward)
    act_sent(0, True)

    @pl.loop(0, n_fs)
    def _(i):
        band = line_band(y_turn(i))
        pull_back(band, 1 - y)
        over(band).start()

    gradients(0, 0)
    for k in range(kb):
        first(0, k)
    gradients(1, 0)
    for k in range(kb):
        first(1, k)
    gradients(0, 1)
    for k in range(kb):
        second(2, k)

    @pl.loop(0, n_fs)
    def _(i):
        pull_back(i, y)

    gradients(1, 1)
    second(0, 0)
    normed_outer(0)
    second(0, 1)
    third(2, 0)
    third(2, 1)
    normed_outer(1)
    second(1, 0)
    normed_inner(n_fs - 1)
    normed_inner(0)
    second(1, 1)
    normed_outer(2)
    third(0, 0)
    third(0, 1)
    normed_inner(1)
    for k in range(kb):
        strip_squares(2, k)
    fan_start(tall_fan, 2 * n_fs)
    for k in range(kb):
        strip_squares(0, k)
    third(1, 0)
    strip_squares(1, 0)
    third(1, 1)
    strip_squares(1, 1)
    fan_start(wide_fan, n_tp)
    normed_last()
    whole_block(2, 0)
    whole_block(2, 1)
    token_sums()
    fan_ready(wide_fan, n_tp)
    v_half[...] = summed(wide_all, n_tp)
    wide_cross().start()
    v_wide[:, pl.ds(pl.multiple_of(r * strip, strip), strip)] = v_half[...]
    fan_ready(tall_fan, 2 * n_fs)
    v_tall[...] = summed(tall_all, 2 * n_fs)
    tall_out = pltpu.make_async_copy(v_tall, o_tall_sq, out_sem.at[4, 1])
    tall_out.start()
    token_grads()
    whole_block(0, 0)
    whole_block(0, 1)
    act_sent(0, False)
    act_sent(1, True)
    for m in range(3):
        weight_sent(m)
    over_sent()
    normed_sent()
    inv_send().wait_send()
    last_send().wait_send()
    fan_sent(row_fan, n_tp)
    fan_sent(wide_fan, n_tp)
    for m in range(3):
        pairs_sent(m)
        swaps_sent(m)
        for k in range(kb):

            @pl.when(kb * c + k != z)
            def _():
                deliver(m, k).wait_send()

    whole_block(1, 0)
    fan_ready(gain_fan, 2 * n_fs)
    gain_sum[...] = summed(gain_all, 2 * n_fs)
    gain_out = pltpu.make_async_copy(gain_sum, o_gain, out_sem.at[4, 0])
    gain_out.start()
    wide_cross_arrival().wait_recv()
    wide_out = pltpu.make_async_copy(v_wide, o_wide_sq, out_sem.at[4, 2])
    wide_out.start()
    whole_block(1, 1)
    wide_cross().wait_send()
    fan_sent(gain_fan, 2 * n_fs)
    fan_sent(tall_fan, 2 * n_fs)
    gain_out.wait()
    tall_out.wait()
    wide_out.wait()
    pltpu.make_async_copy(v_out, o_tokens, out_sem.at[3, 0]).wait()
    for m in range(3):
        spreads_sent(m)
        for k in range(kb):
            block_out(m, k).wait()


def layer(n_fs, n_tp, tokens, cot, w_gate, w_up, w_down, gain):
    half, local = tokens.shape[0] // CORES, tokens.shape[1]
    rows, hidden = w_gate.shape
    width = hidden * CORES // n_fs
    model = rows * n_fs
    count = half * n_fs
    dtype = tokens.dtype
    kb = n_fs // CORES
    strip = rows // 2
    reach = model // 2
    wide, tall = (strip, width), (width, strip)
    dma = pltpu.SemaphoreType.DMA
    hbm = pl.BlockSpec(memory_space=pl.ANY)
    pairs, singles = dma((3, kb, 2)), dma((3, kb))

    def bf(*shape):
        return pltpu.VMEM(shape, dtype)

    def f32(*shape):
        return pltpu.VMEM(shape, jnp.float32)

    hidden = kb * width
    shapes = [(rows, hidden)] * 2 + [(hidden, rows)]
    return pl.pallas_call(
        functools.partial(layer_kernel, n_fs, n_tp),
        out_shape=[jax.ShapeDtypeStruct(s, dtype) for s in shapes]
        + [jax.ShapeDtypeStruct((CORES * half, local), dtype)]
        + [jax.ShapeDtypeStruct(s, jnp.float32) for s in ((1, local), (2, rows), (1, hidden))],
        in_specs=[hbm] * 6,
        out_specs=[hbm] * 7,
        scratch_shapes=[
            bf(count, model),
            bf(count, model),
            bf(model, width),
            bf(model, width),
            bf(width, model),
            bf(count, model),
            bf(model, count),
            bf(width, count),
            f32(count, width),
            f32(count, width),
            bf(count, width),
            bf(count, width),
            f32(count, LANES),
            bf(model, width),
            bf(model, width),
            bf(width, model),
            bf(2, kb, 2, *wide),
            bf(kb, 2, *tall),
            bf(2, kb, *wide),
            bf(kb, *tall),
            bf(2, kb, *wide),
            bf(kb, *tall),
            bf(2, kb, *wide),
            bf(kb, *tall),
            bf(n_fs, half, reach),
            bf(n_fs, half, reach),
            bf(2, n_fs, half, reach),
            bf(half, local),
            bf(rows, hidden),
            bf(rows, hidden),
            bf(hidden, rows),
            bf(CORES * half, local),
            bf(CORES * half, local),
            bf(CORES * half, local),
            f32(CORES * half, LANES),
            bf(CORES * half, local),
            f32(2, strip, LANES),
            f32(n_tp, 1, CORES * half),
            f32(2 * n_fs, 1, local),
            f32(n_tp, 2, strip),
            f32(2 * n_fs, 1, hidden),
            dma((7,)),
            dma((2, 2)),
            dma((2,)),
            dma((2, n_fs - 1, CORES, PARTS)),
            dma((2,)),
            dma((2,)),
            dma((2, n_fs, CORES, PARTS)),
            dma((2,)),
            dma((2,)),
            dma((3, kb)),
            dma((3, n_fs)),
            dma((3,)),
            dma((3, n_fs)),
            dma((3,)),
            dma((3, n_fs, 2)),
            dma((3,)),
            dma((3,)),
            dma((3,)),
            pairs,
            dma((3,)),
            singles,
            singles,
            singles,
            dma((3,)),
            singles,
            dma((1,)),
            dma((n_fs,)),
            dma((n_fs,)),
            dma((2, n_fs)),
            dma((3,)),
            dma((3,)),
            dma((3, kb)),
            dma((n_tp - 1,)),
            dma((n_tp - 1,)),
            dma((2 * n_fs - 1,)),
            dma((2 * n_fs - 1,)),
            dma((n_tp - 1,)),
            dma((n_tp - 1,)),
            dma((2 * n_fs - 1,)),
            dma((2 * n_fs - 1,)),
            dma((5, max(kb, 3))),
            f32(half, reach),
            f32(1, local),
            bf(model // LANES, LANES),
            f32(1, model),
            f32(2, rows),
            f32(1, hidden),
            f32(2, strip),
        ],
        compiler_params=pltpu.CompilerParams(
            collective_id=4, has_side_effects=True, vmem_limit_bytes=67043328
        ),
        name="layer",
    )(tokens, cot, w_gate, w_up, w_down, gain)


def by_chip(tokens, norm_gain, w_gate, w_up, w_down, cotangent):
    s_gate, s_up, s_down, grad_tokens, grad_gain, gate_up_sq, down_sq = layer(
        lax.axis_size("fs"),
        lax.axis_size("tp"),
        tokens,
        cotangent,
        w_gate,
        w_up,
        w_down,
        norm_gain.reshape(-1, LANES),
    )
    grad_gate, grad_up, grad_down = (s.astype(jnp.float32) for s in (s_gate, s_up, s_down))
    return (grad_tokens, grad_gain[0], grad_gate, grad_up, grad_down, gate_up_sq, down_sq[0])


def fits_chips(mesh):
    n_rep, n_fs, n_tp = mesh.shape["rep"], mesh.shape["fs"], mesh.shape["tp"]
    return n_rep == 2 and n_tp == 2 * CORES and n_fs == 2 * CORES


def solution(mesh):
    placed = (
        P(("rep", "fs"), "tp"),
        P(),
        P("fs", "tp"),
        P("fs", "tp"),
        P("tp", "fs"),
        P(("rep", "fs"), "tp"),
    )
    return jax.shard_map(
        by_chip if fits_chips(mesh) else on_device,
        mesh=mesh,
        in_specs=placed,
        out_specs=(
            P(("rep", "fs"), "tp"),
            P("tp"),
            P("fs", "tp"),
            P("fs", "tp"),
            P("tp", "fs"),
            P(None, "fs"),
            P("tp"),
        ),
        check_vma=False,
    )
```

```python
import functools

import jax
import jax.numpy as jnp
from jax import lax
from jax.experimental import pallas as pl
from jax.experimental.pallas import tpu as pltpu
from jax.sharding import PartitionSpec as P

MESH = pl.DeviceIdType.MESH


def contract_last(left, right):
    return lax.dot_general(
        left, right, (((1,), (1,)), ((), ())), preferred_element_type=jnp.float32
    )


def contract_first(left, right):
    return lax.dot_general(
        left, right, (((0,), (0,)), ((), ())), preferred_element_type=jnp.float32
    )


def remote(source, target, send_sem, recv_sem, where):
    return pltpu.make_async_remote_copy(
        src_ref=source,
        dst_ref=target,
        send_sem=send_sem,
        recv_sem=recv_sem,
        device_id=where,
        device_id_type=MESH,
    )


def line_sends(z, n_fs, side, d):
    if side == 0:
        return jnp.logical_and(z >= d - 1, z <= n_fs - 2)
    return jnp.logical_and(z + d <= n_fs, z >= 1)


def line_receives(z, n_fs, side, d):
    return z >= d if side == 0 else z + d <= n_fs - 1


def greet(peers):
    barrier = pltpu.get_barrier_semaphore()
    for peer in peers:
        pl.semaphore_signal(barrier, inc=1, device_id=peer, device_id_type=MESH)
    pl.semaphore_wait(barrier, len(peers))


def keep_own(sources, holders, targets, sems):
    count = len(sources)
    loads = [
        pltpu.make_async_copy(sources[i], holders[i], sems.at[0, i]) for i in range(count)
    ]
    stores = [
        pltpu.make_async_copy(holders[i], targets[i], sems.at[1, i]) for i in range(count)
    ]
    for load in loads:
        load.start()

    def finish():
        for load, store in zip(loads, stores):
            load.wait()
            store.start()
        for store in stores:
            store.wait()

    return finish


def weights_kernel(n_fs, n_tp, *refs):
    tokens, cot, w_gate, w_up, w_down = refs[:5]
    whole_x, whole_dy, full_gate, full_up, full_down = refs[5:10]
    holders = refs[10:15]
    own_sem, ring_send, ring_recv, rep_send, rep_recv, tp_send, tp_recv = refs[15:]
    r, z, t = lax.axis_index("rep"), lax.axis_index("fs"), lax.axis_index("tp")
    right, left = lax.rem(z + 1, n_fs), lax.rem(z + n_fs - 1, n_fs)
    partner = {"rep": 1 - r}
    sources = (w_gate, w_up, w_down)
    targets = (full_gate, full_up, full_down)
    rows = w_gate.shape[0]
    hidden = w_down.shape[0]
    local = tokens.shape[1]

    def own_piece(m, half):
        size = (hidden if m == 2 else rows) // 2
        return sources[m].at[pl.ds(pl.multiple_of(half * size, size), size), :]

    def piece(m, owner, half):
        if m == 2:
            size = hidden // 2
            return targets[m].at[
                pl.ds(pl.multiple_of(half * size, size), size),
                pl.ds(pl.multiple_of(owner * rows, rows), rows),
            ]
        size = rows // 2
        return targets[m].at[
            pl.ds(pl.multiple_of(owner * rows + half * size, size), size), :
        ]

    peers = [{"fs": right}, {"fs": left}, partner]
    peers += [{"tp": lax.rem(t + j, n_tp)} for j in range(1, n_tp)]
    greet(peers)

    def owner_of(side, back):
        return lax.rem(z + (n_fs - back if side == 0 else back), n_fs)

    def hop(m, side, d):
        place = piece(m, owner_of(side, d - 1), r)
        return remote(
            own_piece(m, r) if d == 1 else place,
            place,
            ring_send.at[m, side, d - 1],
            ring_recv.at[m, side, d - 1],
            {"fs": right if side == 0 else left},
        )

    def arrival(m, side, d):
        place = piece(m, owner_of(side, d), r)
        return remote(
            place,
            place,
            ring_send.at[m, side, d - 1],
            ring_recv.at[m, side, d - 1],
            {"fs": right if side == 0 else left},
        )

    def across(m, side, d):
        place = piece(m, owner_of(side, d), r)
        return remote(
            place, place, rep_send.at[m, side, d - 1], rep_recv.at[m, side, d - 1], partner
        )

    for m in range(3):
        for side in range(2):

            @pl.when(line_sends(z, n_fs, side, 1))
            def _():
                hop(m, side, 1).start()

    ends = []
    for a, (source, target) in enumerate(((tokens, whole_x), (cot, whole_dy))):
        place = target.at[:, pl.ds(pl.multiple_of(t * local, local), local)]
        for j in range(1, n_tp):
            copy = remote(
                source,
                place,
                tp_send.at[a, j - 1],
                tp_recv.at[a, j - 1],
                {"tp": lax.rem(t + j, n_tp)},
            )
            copy.start()
            ends.append(copy)
    mine = pl.ds(pl.multiple_of(t * local, local), local)
    band = pl.ds(pl.multiple_of(z * rows, rows), rows)
    finish = keep_own(
        (tokens, cot, w_gate, w_up, w_down),
        holders,
        (
            whole_x.at[:, mine],
            whole_dy.at[:, mine],
            full_gate.at[band, :],
            full_up.at[band, :],
            full_down.at[:, band],
        ),
        own_sem,
    )
    finish()
    for d in range(1, n_fs):
        for m in range(3):
            for side in range(2):

                @pl.when(line_receives(z, n_fs, side, d))
                def _():
                    arrival(m, side, d).wait_recv()
                    if d < n_fs - 1:

                        @pl.when(line_sends(z, n_fs, side, d + 1))
                        def _():
                            hop(m, side, d + 1).start()

                    across(m, side, d).start()

    for d in range(1, n_fs):
        for m in range(3):
            for side in range(2):

                @pl.when(line_sends(z, n_fs, side, d))
                def _():
                    hop(m, side, d).wait_send()

                @pl.when(line_receives(z, n_fs, side, d))
                def _():
                    across(m, side, d).wait()

    for copy in ends:
        copy.wait()


def gather_weights(n_fs, n_tp, tokens, cot, w_gate, w_up, w_down):
    count, local = tokens.shape
    rows, hidden = w_gate.shape
    width = rows * n_fs
    dtype = tokens.dtype
    shapes = [
        (count, width),
        (count, width),
        (width, hidden),
        (width, hidden),
        (hidden, width),
    ]
    held = (tokens, cot, w_gate, w_up, w_down)
    moved = sum(2 * a * b for a, b in shapes)
    dma = pltpu.SemaphoreType.DMA
    return pl.pallas_call(
        functools.partial(weights_kernel, n_fs, n_tp),
        out_shape=[jax.ShapeDtypeStruct(s, dtype) for s in shapes],
        in_specs=[pl.BlockSpec(memory_space=pl.ANY)] * 5,
        out_specs=[pl.BlockSpec(memory_space=pl.ANY)] * 5,
        scratch_shapes=[pltpu.VMEM(a.shape, a.dtype) for a in held]
        + [
            dma((2, 5)),
            dma((3, 2, n_fs - 1)),
            dma((3, 2, n_fs - 1)),
            dma((3, 2, n_fs - 1)),
            dma((3, 2, n_fs - 1)),
            dma((2, n_tp - 1)),
            dma((2, n_tp - 1)),
        ],
        compiler_params=pltpu.CompilerParams(collective_id=0, has_side_effects=True),
        cost_estimate=pl.CostEstimate(flops=0, bytes_accessed=16 * moved, transcendentals=0),
        name="gather_weights",
    )(*held)


def tokens_kernel(n_fs, n_tp, n_act, n_swap, *refs):
    total = n_act + n_swap
    acts, swaps = refs[:n_act], refs[n_act:total]
    act_outs, swap_outs = refs[total : total + n_act], refs[total + n_act : 2 * total]
    holders = refs[2 * total : 3 * total]
    own_sem, ring_send, ring_recv = refs[3 * total : 3 * total + 3]
    swap_send, swap_recv, relay_send, relay_recv = refs[3 * total + 3 :]
    z, t = lax.axis_index("fs"), lax.axis_index("tp")
    right, left = lax.rem(z + 1, n_fs), lax.rem(z + n_fs - 1, n_fs)
    count = acts[0].shape[0]
    peers = [{"fs": lax.rem(z + j, n_fs)} for j in range(1, n_fs)]
    if n_swap:
        peers += [{"tp": lax.rem(t + j, n_tp)} for j in range(1, n_tp)]
    greet(peers)

    def rows_of(owner):
        return pl.ds(pl.multiple_of(owner * count, count), count)

    def owner_of(side, back):
        return lax.rem(z + (n_fs - back if side == 0 else back), n_fs)

    def hop(m, side, d):
        place = act_outs[m].at[rows_of(owner_of(side, d - 1)), :]
        return remote(
            acts[m] if d == 1 else place,
            place,
            ring_send.at[m, side, d - 1],
            ring_recv.at[m, side, d - 1],
            {"fs": right if side == 0 else left},
        )

    def arrival(m, side, d):
        place = act_outs[m].at[rows_of(owner_of(side, d)), :]
        return remote(
            place,
            place,
            ring_send.at[m, side, d - 1],
            ring_recv.at[m, side, d - 1],
            {"fs": right if side == 0 else left},
        )

    def swap(a, j):
        peer = lax.rem(z + j, n_fs)
        cut = swap_outs[a].shape[1]
        return remote(
            swaps[a].at[:, pl.ds(pl.multiple_of(peer * cut, cut), cut)],
            swap_outs[a].at[rows_of(z), :],
            swap_send.at[a, j - 1],
            swap_recv.at[a, j - 1],
            {"fs": peer},
        )

    def swapped(a, j):
        place = swap_outs[a].at[rows_of(owner_of(0, j)), :]
        return remote(
            place,
            place,
            swap_send.at[a, j - 1],
            swap_recv.at[a, j - 1],
            {"fs": lax.rem(z + j, n_fs)},
        )

    def relay(a, j, k):
        place = swap_outs[a].at[rows_of(owner_of(0, j)), :]
        return remote(
            place,
            place,
            relay_send.at[a, j - 1, k - 1],
            relay_recv.at[a, j - 1],
            {"tp": lax.rem(t + k, n_tp)},
        )

    hub = lax.rem(z, n_tp) == t

    def feeds(j):
        return lax.rem(lax.rem(z + j, n_fs), n_tp) == t

    for a in range(n_swap):
        for j in range(1, n_fs):

            @pl.when(feeds(j))
            def _():
                swap(a, j).start()

    for m in range(n_act):
        for side in range(2):

            @pl.when(line_sends(z, n_fs, side, 1))
            def _():
                hop(m, side, 1).start()

    sources = list(acts)
    for a in range(n_swap):
        cut = swap_outs[a].shape[1]
        sources.append(swaps[a].at[:, pl.ds(pl.multiple_of(z * cut, cut), cut)])
    finish = keep_own(
        sources, holders, [out.at[rows_of(z), :] for out in act_outs + swap_outs], own_sem
    )
    finish()
    if n_swap:

        @pl.when(hub)
        def _():
            for a in range(n_swap):
                for j in range(1, n_fs):
                    swapped(a, j).wait_recv()
                    for k in range(1, n_tp):
                        relay(a, j, k).start()

    for d in range(1, n_fs):
        for m in range(n_act):
            for side in range(2):

                @pl.when(line_receives(z, n_fs, side, d))
                def _():
                    arrival(m, side, d).wait_recv()
                    if d < n_fs - 1:

                        @pl.when(line_sends(z, n_fs, side, d + 1))
                        def _():
                            hop(m, side, d + 1).start()

    for d in range(1, n_fs):
        for m in range(n_act):
            for side in range(2):

                @pl.when(line_sends(z, n_fs, side, d))
                def _():
                    hop(m, side, d).wait_send()

    for a in range(n_swap):
        for j in range(1, n_fs):

            @pl.when(feeds(j))
            def _():
                swap(a, j).wait_send()

            @pl.when(hub)
            def _():
                for k in range(1, n_tp):
                    relay(a, j, k).wait_send()

            @pl.when(jnp.logical_not(hub))
            def _():
                relay(a, j, 1).wait_recv()


def gather_tokens(n_fs, n_tp, collective_id, acts, swaps):
    count = acts[0].shape[0]
    outs = [jax.ShapeDtypeStruct((n_fs * count, a.shape[1]), a.dtype) for a in acts]
    outs += [jax.ShapeDtypeStruct((n_fs * count, a.shape[1] // n_fs), a.dtype) for a in swaps]
    dma = pltpu.SemaphoreType.DMA
    total = len(outs)
    n_swap = max(len(swaps), 1)
    moved = sum(2 * o.shape[0] * o.shape[1] for o in outs)
    return pl.pallas_call(
        functools.partial(tokens_kernel, n_fs, n_tp, len(acts), len(swaps)),
        out_shape=outs,
        in_specs=[pl.BlockSpec(memory_space=pl.ANY)] * total,
        out_specs=[pl.BlockSpec(memory_space=pl.ANY)] * total,
        scratch_shapes=[pltpu.VMEM((count, o.shape[1]), o.dtype) for o in outs]
        + [
            dma((2, total)),
            dma((len(acts), 2, n_fs - 1)),
            dma((len(acts), 2, n_fs - 1)),
            dma((n_swap, n_fs - 1)),
            dma((n_swap, n_fs - 1)),
            dma((n_swap, n_fs - 1, n_tp - 1)),
            dma((n_swap, n_fs - 1)),
        ],
        compiler_params=pltpu.CompilerParams(
            collective_id=collective_id, has_side_effects=True
        ),
        cost_estimate=pl.CostEstimate(flops=0, bytes_accessed=16 * moved, transcendentals=0),
        name=f"gather_tokens_{collective_id}",
    )(*acts, *swaps)


def over_rep(part):
    part = part.astype(jnp.bfloat16)
    n_rep = lax.axis_size("rep")
    other = lax.ppermute(part, "rep", [(i, (i + 1) % n_rep) for i in range(n_rep)])
    return part, other


def added(pair):
    return pair[0].astype(jnp.float32) + pair[1].astype(jnp.float32)


def on_device(tokens, norm_gain, w_gate, w_up, w_down, cotangent):
    n_fs, n_tp = lax.axis_size("fs"), lax.axis_size("tp")
    whole_x, whole_dy, full_gate, full_up, full_down = gather_weights(
        n_fs, n_tp, tokens, cotangent, w_gate, w_up, w_down
    )
    width = whole_x.shape[1]
    wide_tokens = whole_x.astype(jnp.float32)
    gain_f = norm_gain.astype(jnp.float32)
    inverse = lax.rsqrt(jnp.mean(wide_tokens * wide_tokens, axis=-1, keepdims=True) + 1e-06)
    normed = (wide_tokens * inverse * gain_f).astype(jnp.bfloat16)
    gate = jnp.dot(normed, full_gate, preferred_element_type=jnp.float32)
    up_proj = jnp.dot(normed, full_up, preferred_element_type=jnp.float32)
    sigma = jax.nn.sigmoid(gate)
    active = gate * sigma
    hidden = (active * up_proj).astype(jnp.bfloat16)
    back = 0.5 * contract_last(whole_dy, full_down)
    d_up = (back * active).astype(jnp.bfloat16)
    d_gate = (back * up_proj * sigma * (1.0 + gate * (1.0 - sigma))).astype(jnp.bfloat16)

    all_hidden, rows_dy = gather_tokens(n_fs, n_tp, 1, [hidden], [whole_dy])
    down_pair = over_rep(0.5 * contract_first(all_hidden, rows_dy))

    partial_normed = contract_last(d_gate, full_gate) + contract_last(d_up, full_up)
    d_normed = lax.psum_scatter(
        partial_normed.astype(jnp.bfloat16), "tp", scatter_dimension=1, tiled=True
    ).astype(jnp.float32)

    all_gate, rows_normed = gather_tokens(n_fs, n_tp, 2, [d_gate], [normed])
    gate_pair = over_rep(contract_first(rows_normed, all_gate))
    (all_up,) = gather_tokens(n_fs, n_tp, 3, [d_up], [])
    up_pair = over_rep(contract_first(rows_normed, all_up))

    local_width = d_normed.shape[1]
    local_gain = lax.dynamic_slice_in_dim(
        gain_f, lax.axis_index("tp") * local_width, local_width, 0
    )
    local_tokens = tokens.astype(jnp.float32)
    scaled_grad = d_normed * local_gain
    rowdot = lax.psum(jnp.sum(scaled_grad * local_tokens, axis=-1), "tp")
    grad_tokens = (
        cotangent.astype(jnp.float32)
        + inverse * scaled_grad
        - local_tokens * inverse**3 * rowdot[:, None] / width
    ).astype(jnp.bfloat16)
    grad_gain = lax.psum(jnp.sum(d_normed * local_tokens * inverse, axis=0), ("rep", "fs"))

    grad_down = added(down_pair)
    down_sq = lax.psum(jnp.sum(grad_down * grad_down, axis=1), "fs")
    grad_gate = added(gate_pair)
    grad_up = added(up_pair)
    gate_up_sq = lax.psum(
        jnp.stack([jnp.sum(grad_gate * grad_gate, axis=1), jnp.sum(grad_up * grad_up, axis=1)]),
        "tp",
    )
    return (grad_tokens, grad_gain, grad_gate, grad_up, grad_down, gate_up_sq, down_sq)


CORES = 2
LANES = 128
TILE = 256
PARTS = 2
STEPS = 2


def line_next(z, n_fs, side):
    return z <= n_fs - 2 if side == 0 else z >= 1


def layer_kernel(n_fs, n_tp, *refs):
    tokens, cot, w_gate, w_up, w_down, gain_in = refs[:6]
    o_gate, o_up, o_down, o_tokens, o_gain, o_wide_sq, o_tall_sq = refs[6:13]
    full = refs[13:18]
    x_full, dy_full, f_gate, f_up, f_down = full
    normed, normed_t, hidden_t, act_f, slope_f, d_gate, d_up, inv_all = refs[18:26]
    g_gate, g_up, g_down = refs[26:29]
    pair_wide, pair_tall, sum_wide, sum_tall, x_wide, x_tall, t_wide, t_tall = refs[29:37]
    y_buf, d_buf, z_buf, n_buf = refs[37:41]
    v_gate, v_up, v_down, v_tokens, v_cot, v_normed, v_inv, v_out = refs[41:49]
    lane_sq, row_all, gain_all, wide_all, tall_all = refs[49:54]
    (load_sem, az_own, az_fwd, az_recv, ay_own, ay_fwd, ay_recv, ap_send, ap_recv) = refs[54:63]
    (w_send, w_recv, wx_send, wx_recv, wp_send, wp_recv, wo_send, wo_recv) = refs[63:71]
    (p_send, p_recv, x_send, x_recv, z_send, z_recv, f_send, f_recv) = refs[71:79]
    (y_send, y_recv, d_send, d_recv, n_send, n_recv, own_sem) = refs[79:86]
    (row_send, row_recv, gain_send, gain_recv) = refs[86:90]
    (wide_send, wide_recv, tall_send, tall_recv, out_sem, total, gain_sum) = refs[90:97]
    gain_load, gain, v_wide, v_tall, v_half = refs[97:]
    r, z, t = lax.axis_index("rep"), lax.axis_index("fs"), lax.axis_index("tp")
    y, c = lax.div(t, CORES), lax.rem(t, CORES)
    acts, weights = (tokens, cot), (w_gate, w_up, w_down)
    grads, outs = (g_gate, g_up, g_down), (v_gate, v_up, v_down)
    half, local = tokens.shape[0] // CORES, tokens.shape[1]
    count, model = x_full.shape
    rows = w_gate.shape[0]
    kb = n_fs // CORES
    width = w_gate.shape[1] // kb
    strip = rows // 2
    reach = model // 2
    partner = {"tp": y * CORES + 1 - c}
    across = {"rep": 1 - r}
    beside = {"tp": (1 - y) * CORES + c}
    owner = lax.div(z, kb)

    peers = [partner, across]
    peers += [{"tp": (1 - y) * CORES + h} for h in range(CORES)]
    for j in range(1, n_fs):
        for h in range(CORES):
            peers.append({"fs": lax.rem(z + j, n_fs), "tp": y * CORES + h})
        peers.append({"rep": 1 - r, "fs": lax.rem(z + j, n_fs)})
    greet(peers)

    def own_act(a, h):
        return acts[a].at[pl.ds(pl.multiple_of(h * half, half), half), :]

    def act_place(a, source, column):
        return full[a].at[
            pl.ds(pl.multiple_of(source * half, half), half),
            pl.ds(pl.multiple_of(column * local, local), local),
        ]

    sub = half // PARTS

    def own_part(a, h, q):
        start = h * half + q * sub
        return acts[a].at[pl.ds(start, sub), :]

    def act_part(a, source, column, q):
        return full[a].at[
            pl.ds(pl.multiple_of(source * half + q * sub, sub), sub),
            pl.ds(pl.multiple_of(column * local, local), local),
        ]

    def source_of(side, d):
        return z - d if side == 0 else z + d

    def next_of(side):
        return z + 1 if side == 0 else z - 1

    def line_turn(source, at):
        return lax.rem(source - at + n_fs, n_fs) - 1

    def act_first(a, side, h, q):
        return remote(
            own_part(a, h, q),
            act_part(a, z, t, q),
            az_own.at[a, side],
            az_recv.at[a, line_turn(z, next_of(side)), c, q],
            {"fs": next_of(side), "tp": y * CORES + h},
        )

    def act_arrival(a, side, d, core, q):
        place = act_part(a, source_of(side, d), y * CORES + core, q)
        return remote(
            place,
            place,
            az_fwd.at[a],
            az_recv.at[a, line_turn(source_of(side, d), z), core, q],
            partner,
        )

    def act_forward(a, side, d, core, q):
        place = act_part(a, source_of(side, d), y * CORES + core, q)
        return remote(
            place,
            place,
            az_fwd.at[a],
            az_recv.at[a, line_turn(source_of(side, d), next_of(side)), core, q],
            {"fs": next_of(side)},
        )

    def act_over(a, side, d, core, q):
        source = source_of(side, d)
        place = act_part(a, source, y * CORES + core, q)
        return remote(
            place,
            place,
            ay_fwd.at[a],
            ay_recv.at[a],
            {"tp": (1 - y) * CORES + c},
        )

    def act_over_own(a, h):
        return remote(
            own_act(a, h),
            act_place(a, z, t),
            ay_own.at[a],
            ay_recv.at[a],
            {"tp": (1 - y) * CORES + h},
        )

    def act_over_arrivals(a):
        place = full[a].at[:, side_columns(1 - y)]
        return remote(place, place, ay_own.at[a], ay_recv.at[a], partner)

    def act_partner(a):
        return remote(own_act(a, 1 - c), act_place(a, z, t), ap_send.at[a], ap_recv.at[a], partner)

    def act_partner_arrival(a):
        place = act_place(a, z, y * CORES + 1 - c)
        return remote(place, place, ap_send.at[a], ap_recv.at[a], partner)

    def block_of(m, k):
        if m == 2:
            return weights[m].at[pl.ds(pl.multiple_of(k * width, width), width), :]
        return weights[m].at[:, pl.ds(pl.multiple_of(k * width, width), width)]

    def band_of(m, source):
        band = pl.ds(pl.multiple_of(source * rows, rows), rows)
        return full[2 + m].at[:, band] if m == 2 else full[2 + m].at[band, :]

    def quarter(m, source, rep, core):
        if m == 2:
            size = width // (2 * CORES)
            return full[4].at[
                pl.ds(pl.multiple_of((rep * CORES + core) * size, size), size),
                pl.ds(pl.multiple_of(source * rows, rows), rows),
            ]
        size = rows // (2 * CORES)
        start = source * rows + (rep * CORES + core) * size
        return full[2 + m].at[pl.ds(pl.multiple_of(start, size), size), :]

    def own_quarter(m, k, core):
        if m == 2:
            size = width // (2 * CORES)
            start = k * width + (r * CORES + core) * size
            return weights[m].at[pl.ds(pl.multiple_of(start, size), size), :]
        size = rows // (2 * CORES)
        return weights[m].at[
            pl.ds(pl.multiple_of((r * CORES + core) * size, size), size),
            pl.ds(k * width, width),
        ]

    def weight_send(m, k, core):
        return remote(
            own_quarter(m, k, core),
            quarter(m, z, r, core),
            w_send.at[m, k],
            w_recv.at[m, z],
            {"fs": kb * c + k, "tp": y * CORES + core},
        )

    def weight_arrival(m, source):
        place = quarter(m, source, r, c)
        return remote(place, place, wx_send.at[m], w_recv.at[m, source], partner)

    def weight_across(m, source):
        place = quarter(m, source, r, c)
        return remote(place, place, wx_send.at[m], wx_recv.at[m, source], across)

    def weight_across_arrival(m, source):
        place = quarter(m, source, 1 - r, c)
        return remote(place, place, wx_send.at[m], wx_recv.at[m, source], across)

    def weight_beside(m, source, which):
        place = quarter(m, source, r if which == 0 else 1 - r, c)
        return remote(
            place, place, wp_send.at[m], wp_recv.at[m], partner
        )

    def weight_beside_arrivals(m):
        part = (width if m == 2 else rows) // (2 * CORES)
        if m == 2:
            place = full[4].at[pl.ds(0, 2 * part), pl.ds(0, model - rows)]
        else:
            place = full[2 + m].at[pl.ds(0, 2 * (n_fs - 1) * part), :]
        return remote(place, place, wp_send.at[m], wp_recv.at[m], partner)

    def own_beside(m):
        return remote(
            block_of(m, z - kb * owner), band_of(m, z), wo_send.at[m], wo_recv.at[m], partner
        )

    def own_beside_arrival(m):
        return remote(band_of(m, z), band_of(m, z), wo_send.at[m], wo_recv.at[m], partner)

    def slot(wide, tall, m, *where):
        return tall.at[where] if m == 2 else wide.at[(m,) + where]

    def strip_of(band, rep):
        return pl.ds(pl.multiple_of(band * rows + rep * strip, strip), strip)

    def grad_piece(m, band, rep):
        if m == 2:
            return grads[m].at[:, strip_of(band, rep)]
        return grads[m].at[strip_of(band, rep), :]

    def rep_of(j):
        return 1 - r if j == 0 else r

    def pair(m, k, j):
        return remote(
            grad_piece(m, kb * (1 - c) + k, rep_of(j)),
            slot(pair_wide, pair_tall, m, k, j),
            p_send.at[m],
            p_recv.at[m, k, j],
            partner,
        )

    def swap(m, k):
        return remote(
            slot(sum_wide, sum_tall, m, k),
            slot(x_wide, x_tall, m, k),
            x_send.at[m],
            x_recv.at[m, k],
            across,
        )

    def place(m, block, rep):
        strips = pl.ds(pl.multiple_of(rep * strip, strip), strip)
        blocks = pl.ds(pl.multiple_of(block * width, width), width)
        return outs[m].at[blocks, strips] if m == 2 else outs[m].at[strips, blocks]

    def deliver(m, k):
        block = lax.rem(z, kb)
        return remote(
            slot(t_wide, t_tall, m, k),
            place(m, block, r),
            z_send.at[m, k],
            z_recv.at[m, block],
            {"fs": kb * c + k, "tp": y * CORES + owner},
        )

    def delivered(m, k):
        return remote(place(m, k, r), place(m, k, r), z_send.at[m, k], z_recv.at[m, k], partner)

    def keep(m, k):
        return pltpu.make_async_copy(slot(t_wide, t_tall, m, k), place(m, k, r), own_sem.at[m, k])

    def spread(m, k, source):
        return remote(source, place(m, k, r), f_send.at[m], f_recv.at[m, k], across)

    def spread_arrival(m, k):
        return remote(
            place(m, k, 1 - r), place(m, k, 1 - r), f_send.at[m], f_recv.at[m, k], across
        )

    def band_rows(band):
        return pl.ds(pl.multiple_of(band * half, half), half)

    def side_columns(which):
        return pl.ds(pl.multiple_of(which * reach, reach), reach)

    def over(band):
        return remote(
            x_full.at[band_rows(band), side_columns(1 - y)],
            y_buf.at[band],
            y_send.at[0],
            y_recv.at[band],
            beside,
        )

    low = z < n_fs // 2
    inner = jnp.logical_and(z > 0, z < n_fs - 1)
    line_slot = jnp.where(low, 0, 1)

    def line_band(i):
        return jnp.where(low, n_fs - 1 - i, i)

    def y_turn(i):
        return jnp.where(jnp.logical_and(inner, i >= 2), n_fs + 1 - i, i)

    def line_send(i, target):
        band = line_band(i)
        return remote(
            d_buf.at[i],
            z_buf.at[line_slot, band],
            d_send.at[i],
            d_recv.at[line_slot, band],
            {"fs": target},
        )

    def line_arrival(which, band):
        place = z_buf.at[which, band]
        return remote(place, place, d_send.at[0], d_recv.at[which, band], partner)

    def own_rows(core):
        return pl.ds(pl.multiple_of(core * half, half), half)

    def inv_send():
        return remote(inv_all.at[band_rows(z), :], v_inv.at[own_rows(c), :], n_send.at[0], n_recv.at[0], partner)

    def inv_arrival():
        at = v_inv.at[own_rows(1 - c), :]
        return remote(at, at, n_send.at[0], n_recv.at[0], partner)

    def last_send():
        return remote(n_buf, v_normed.at[own_rows(c), :], n_send.at[1], n_recv.at[1], partner)

    def last_arrival():
        at = v_normed.at[own_rows(1 - c), :]
        return remote(at, at, n_send.at[1], n_recv.at[1], partner)

    def loaded(a):
        return pltpu.make_async_copy(own_act(a, c), act_place(a, z, t), load_sem.at[a])

    def block_loaded(m):
        return pltpu.make_async_copy(
            block_of(m, z - kb * owner), band_of(m, z), load_sem.at[2 + m]
        )

    def act_start(a):
        for h in range(CORES):
            for side in range(2):

                @pl.when(line_next(z, n_fs, side))
                def _():
                    for q in range(PARTS):
                        act_first(a, side, h, q).start()

            act_over_own(a, h).start()
        act_partner(a).start()

    def own_start(m):
        @pl.when(c == owner)
        def _():
            own_beside(m).start()

    def act_round(a, d):
        for core in range(CORES):
            for q in range(PARTS):
                for side in range(2):

                    @pl.when(line_receives(z, n_fs, side, d))
                    def _():
                        act_arrival(a, side, d, core, q).wait_recv()
                        if d < n_fs - 1:

                            @pl.when(line_next(z, n_fs, side))
                            def _():
                                act_forward(a, side, d, core, q).start()

                        act_over(a, side, d, core, q).start()

    def weight_start(m):
        for k in range(kb):

            @pl.when(kb * c + k != z)
            def _():
                for core in range(CORES):
                    weight_send(m, k, core).start()

    def weight_round(ms, d):
        for m in ms:
            for side in range(2):

                @pl.when(line_receives(z, n_fs, side, d))
                def _():
                    source = source_of(side, d)
                    weight_arrival(m, source).wait_recv()
                    weight_across(m, source).start()
                    weight_beside(m, source, 0).start()

    def across_round(ms, d):
        for m in ms:
            for side in range(2):

                @pl.when(line_receives(z, n_fs, side, d))
                def _():
                    source = source_of(side, d)
                    weight_across_arrival(m, source).wait_recv()
                    weight_beside(m, source, 1).start()

    def weight_all(m):
        for d in range(1, n_fs):
            weight_round((m,), d)

    def across_all(m):
        for d in range(1, n_fs):
            across_round((m,), d)

    def act_ready(a):
        act_over_arrivals(a).wait_recv()
        act_partner_arrival(a).wait_recv()
        loaded(a).wait()

    def sent(ref, sem):
        remote(ref, ref, sem, sem, partner).wait_send()

    def act_sent(a, landed):
        others = full[a].at[pl.ds(0, count - half), pl.ds(0, CORES * local)]
        if landed:
            sent(others, ay_fwd.at[a])

            @pl.when(inner)
            def _():
                sent(others, az_fwd.at[a])

        if a == 1 or not landed:
            act_partner(a).wait_send()
            sent(acts[a], ay_own.at[a])
            for side in range(2):

                @pl.when(line_next(z, n_fs, side))
                def _():
                    sent(acts[a], az_own.at[a, side])

    def weight_ready(ms):
        for m in ms:
            weight_beside_arrivals(m).wait_recv()

            @pl.when(c == owner)
            def _():
                block_loaded(m).wait()

            @pl.when(c != owner)
            def _():
                own_beside_arrival(m).wait_recv()

    def weight_sent(m):
        size = full[2 + m].shape[0 if m < 2 else 1] - rows
        part = (rows if m < 2 else width) // (2 * CORES)
        if m < 2:
            sent(full[2 + m].at[pl.ds(0, (n_fs - 1) * part), :], wx_send.at[m])
            sent(full[2 + m].at[pl.ds(0, 2 * (n_fs - 1) * part), :], wp_send.at[m])
            half_block = weights[m].at[pl.ds(0, CORES * part), pl.ds(0, width)]
        else:
            sent(full[4].at[pl.ds(0, part), pl.ds(0, size)], wx_send.at[m])
            sent(full[4].at[pl.ds(0, 2 * part), pl.ds(0, size)], wp_send.at[m])
            half_block = weights[m].at[pl.ds(0, CORES * part), :]
        for k in range(kb):

            @pl.when(kb * c + k != z)
            def _():
                sent(half_block, w_send.at[m, k])

        @pl.when(c == owner)
        def _():
            own_beside(m).wait_send()

    def pairs_sent(m):
        span = pl.ds(0, kb * rows)
        sent(g_down.at[:, span] if m == 2 else grads[m].at[span, :], p_send.at[m])

    def swaps_sent(m):
        sent(sum_tall if m == 2 else sum_wide.at[m], x_send.at[m])

    def spreads_sent(m):
        sent(sum_tall if m == 2 else sum_wide.at[m], f_send.at[m])

    def over_sent():
        sent(x_full.at[:, side_columns(1 - y)], y_send.at[0])

    def tile(i, size):
        return pl.ds(pl.multiple_of(i * size, size), size)

    def normalize(i):
        at = tile(i, LANES)
        wide = x_full[at, :].astype(jnp.float32)
        inv = lax.rsqrt(jnp.mean(wide * wide, axis=-1, keepdims=True) + 1e-06)
        value = wide * inv * gain[...]
        normed[at, :] = value.astype(jnp.bfloat16)
        normed_t[:, at] = value.T.astype(jnp.bfloat16)
        inv_all[at, :] = jnp.broadcast_to(inv, (LANES, LANES))

    def forward(i):
        at = tile(i, TILE)
        gate = jnp.dot(normed[at, :], f_gate[...], preferred_element_type=jnp.float32)
        up = jnp.dot(normed[at, :], f_up[...], preferred_element_type=jnp.float32)
        sigma = jax.nn.sigmoid(gate)
        active = gate * sigma
        act_f[at, :] = active
        slope_f[at, :] = up * sigma * (1.0 + gate * (1.0 - sigma))
        hidden_t[:, at] = (active * up).T.astype(jnp.bfloat16)

    def backward(i):
        at = tile(i, TILE)
        back = 0.5 * contract_last(dy_full[at, :], f_down[...])
        d_up[at, :] = (back * act_f[at, :]).astype(jnp.bfloat16)
        d_gate[at, :] = (back * slope_f[at, :]).astype(jnp.bfloat16)

    def gradient(m, own, j, k):
        band = kb * (c if own else 1 - c) + k
        at = strip_of(band, 1 - r if j == 0 else r)
        if m == 2:
            value = 0.5 * jnp.dot(
                hidden_t[...], dy_full[:, at], preferred_element_type=jnp.float32
            )
            g_down[:, at] = value.astype(jnp.bfloat16)
        else:
            right = d_gate if m == 0 else d_up
            value = jnp.dot(normed_t[at, :], right[...], preferred_element_type=jnp.float32)
            grads[m][at, :] = value.astype(jnp.bfloat16)

    def gradients(m, j):
        @pl.loop(0, kb)
        def _(k):
            gradient(m, False, j, k)
            pair(m, k, j).start()

        @pl.loop(0, kb)
        def _(k):
            gradient(m, True, j, k)

    def pull_back(band, which):
        at, columns = band_rows(band), side_columns(which)
        value = contract_last(d_gate[at, :], f_gate[columns, :])
        value = value + contract_last(d_up[at, :], f_up[columns, :])
        x_full[at, columns] = value.astype(jnp.bfloat16)

    def added(m, k, j):
        own = grad_piece(m, kb * c + k, rep_of(j))[...].astype(jnp.float32)
        return own + slot(pair_wide, pair_tall, m, k, j)[...].astype(jnp.float32)

    def put(wide, tall, m, k, value):
        if m == 2:
            tall[k] = value
        else:
            wide[m, k] = value

    def first(m, k):
        pair(m, k, 0).wait_recv()
        put(sum_wide, sum_tall, m, k, added(m, k, 0).astype(jnp.bfloat16))
        swap(m, k).start()

    def second(m, k):
        pair(m, k, 1).wait_recv()
        swap(m, k).wait_recv()
        whole = added(m, k, 1) + slot(x_wide, x_tall, m, k)[...].astype(jnp.float32)
        put(t_wide, t_tall, m, k, whole.astype(jnp.bfloat16))
        mine = kb * c + k == z

        @pl.when(mine)
        def _():
            keep(m, k).start()
            spread(m, k, slot(t_wide, t_tall, m, k)).start()

        @pl.when(jnp.logical_not(mine))
        def _():
            deliver(m, k).start()

    def third(m, k):
        @pl.when(kb * c + k != z)
        def _():
            delivered(m, k).wait_recv()
            spread(m, k, place(m, k, r)).start()

    def own_share(band):
        over(band).wait_recv()
        own = x_full[band_rows(band), side_columns(y)].astype(jnp.float32)
        return own + y_buf[band].astype(jnp.float32)

    def line_target(i):
        if i == n_fs - 1:
            return jnp.where(low, z - 1, z + 1)
        return line_band(i)

    def normed_outer(i):
        @pl.when(jnp.logical_not(inner))
        def _():
            d_buf[i] = own_share(line_band(i)).astype(jnp.bfloat16)
            line_send(i, jnp.where(low, z + 1, z - 1)).start()

    def normed_inner(i):
        @pl.when(inner)
        def _():
            band = line_band(i)
            value = own_share(band)
            if i < n_fs - 1:
                line_arrival(line_slot, band).wait_recv()
                value = value + z_buf[line_slot, band].astype(jnp.float32)
            d_buf[i] = value.astype(jnp.bfloat16)
            line_send(i, line_target(i)).start()

    def normed_sent():
        for i in range(n_fs):
            if i < n_fs - 1:

                @pl.when(jnp.logical_not(inner))
                def _():
                    line_send(i, jnp.where(low, z + 1, z - 1)).wait_send()

            if i != n_fs - 2:

                @pl.when(inner)
                def _():
                    line_send(i, line_target(i)).wait_send()

    def normed_last():
        value = own_share(z)
        for which in range(2):
            line_arrival(which, z).wait_recv()
            value = value + z_buf[which, z].astype(jnp.float32)
        total[...] = value

        for core in range(CORES):

            @pl.when(c == core)
            def _():
                mine = slice(core * local, (core + 1) * local)
                theirs = slice((1 - core) * local, (2 - core) * local)
                v_normed[core * half : (core + 1) * half, :] = total[:, mine].astype(jnp.bfloat16)
                n_buf[...] = total[:, theirs].astype(jnp.bfloat16)

        last_send().start()

    def fold(value):
        out = value[:, :LANES]
        for i in range(1, value.shape[1] // LANES):
            out = out + value[:, i * LANES : (i + 1) * LANES]
        return out

    def row_of(value):
        return jnp.sum(value.T, axis=0, keepdims=True)

    def lane_peer(j):
        return {"tp": lax.rem(t + j, n_tp)}

    def group_peer(j):
        at = lax.rem(r * n_fs + z + j, 2 * n_fs)
        return {"rep": lax.div(at, n_fs), "fs": lax.rem(at, n_fs)}

    def fan(buffer, count_of, mine, send, recv, peer):
        def start():
            for j in range(1, count_of):
                place = buffer.at[mine]
                remote(place, place, send.at[0], recv.at[0], peer(j)).start()

        def others():
            place = buffer.at[pl.ds(0, count_of - 1)]
            return remote(place, place, send.at[0], recv.at[0], partner)

        return start, others

    row_fan = fan(row_all, n_tp, t, row_send, row_recv, lane_peer)
    wide_fan = fan(wide_all, n_tp, t, wide_send, wide_recv, lane_peer)
    gain_fan = fan(gain_all, 2 * n_fs, r * n_fs + z, gain_send, gain_recv, group_peer)
    tall_fan = fan(tall_all, 2 * n_fs, r * n_fs + z, tall_send, tall_recv, group_peer)

    def gain_here():
        return gain[:, pl.ds(pl.multiple_of(t * local, local), local)]

    def token_sums():
        last_arrival().wait_recv()
        inv_arrival().wait_recv()
        for i in range(2):
            own_loaded(i).wait()
        gain_l = gain_here()
        gain_sum[...] = jnp.zeros_like(gain_sum)

        @pl.loop(0, CORES * half // LANES)
        def _(i):
            at = tile(i, LANES)
            d_tokens = v_normed[at, :].astype(jnp.float32) * v_tokens[at, :].astype(jnp.float32)
            row_all[t, :, at] = row_of(fold(d_tokens * gain_l))
            inv = v_inv[at, :1]
            gain_sum[...] += jnp.sum(d_tokens * inv, axis=0, keepdims=True)

        gain_all[r * n_fs + z] = gain_sum[...]
        row_fan[0]()
        gain_fan[0]()

    def token_grads():
        row_fan[1]().wait_recv()
        gain_l = gain_here()

        @pl.loop(0, CORES * half // LANES)
        def _(i):
            at = tile(i, LANES)
            dots = row_all[0, :, at]
            for j in range(1, n_tp):
                dots = dots + row_all[j, :, at]
            rowdot = jnp.broadcast_to(dots, (LANES, LANES)).T[:, :1]
            inv = v_inv[at, :1]
            value = v_cot[at, :].astype(jnp.float32)
            value = value + inv * (v_normed[at, :].astype(jnp.float32) * gain_l)
            scale = inv**3 * rowdot / model
            value = value - v_tokens[at, :].astype(jnp.float32) * scale
            v_out[at, :] = value.astype(jnp.bfloat16)

        pltpu.make_async_copy(v_out, o_tokens, out_sem.at[3]).start()

    def own_loaded(i):
        source, target = ((tokens, v_tokens), (cot, v_cot))[i]
        return pltpu.make_async_copy(source, target, load_sem.at[5 + i])

    def block_out(m, k):
        at = pl.ds(k * width, width)
        if m == 2:
            return pltpu.make_async_copy(v_down.at[at, :], o_down.at[at, :], out_sem.at[m])
        return pltpu.make_async_copy(
            outs[m].at[:, at], (o_gate, o_up)[m].at[:, at], out_sem.at[m]
        )

    def strip_squares(m, k):
        @pl.when(kb * c + k == z)
        def _():
            keep(m, k).wait()

        if m == 2:
            columns = pl.ds(pl.multiple_of(r * strip, strip), strip)

            @pl.loop(0, width // LANES)
            def _(i):
                at = pl.ds(pl.multiple_of(k * width + i * LANES, LANES), LANES)
                value = v_down[at, columns].astype(jnp.float32)
                tall_all[r * n_fs + z, :, at] = row_of(fold(value * value))
        else:

            @pl.loop(0, strip // LANES)
            def _(i):
                at = tile(i, LANES)
                from_row = pl.ds(pl.multiple_of(r * strip + i * LANES, LANES), LANES)
                value = outs[m][from_row, k * width : (k + 1) * width].astype(jnp.float32)
                part = fold(value * value)
                if k > 0:
                    part = part + lane_sq[m, at, :]
                if k < kb - 1:
                    lane_sq[m, at, :] = part
                else:
                    wide_all[t, m : m + 1, at] = row_of(part)

    def wide_cross():
        strips = pl.ds(pl.multiple_of(r * strip, strip), strip)
        return remote(v_half, v_wide.at[:, strips], n_send.at[2], n_recv.at[2], across)

    def wide_cross_arrival():
        place = v_wide.at[:, pl.ds(pl.multiple_of((1 - r) * strip, strip), strip)]
        return remote(place, place, n_send.at[2], n_recv.at[2], across)

    def summed(buffer, count_of):
        value = buffer[0]
        for j in range(1, count_of):
            value = value + buffer[j]
        return value

    def whole_block(m, k):
        spread_arrival(m, k).wait_recv()
        block_out(m, k).start()

    gain_copy = pltpu.make_async_copy(gain_in, gain_load, out_sem.at[4])
    gain_copy.start()
    for a in range(2):
        loaded(a).start()

    @pl.when(c == owner)
    def _():
        for m in range(3):
            block_loaded(m).start()

    act_start(0)
    own_start(0)
    own_start(1)
    for i in range(2):
        own_loaded(i).start()
    act_round(0, 1)
    act_round(0, 2)
    weight_start(0)
    weight_start(1)
    act_start(1)
    own_start(2)
    for d in range(3, n_fs):
        act_round(0, d)
    weight_all(0)
    act_round(1, 1)
    weight_all(1)
    across_all(0)
    gain_copy.wait()
    for i in range(model // LANES):
        gain[:, i * LANES : (i + 1) * LANES] = gain_load[i : i + 1, :].astype(jnp.float32)
    act_ready(0)
    pl.loop(0, count // LANES)(normalize)
    inv_send().start()
    v_inv[own_rows(c), :] = inv_all[band_rows(z), :]
    weight_start(2)
    across_all(1)
    act_round(1, 2)
    weight_ready((0, 1))
    pl.loop(0, count // TILE)(forward)
    weight_all(2)
    for d in range(3, n_fs):
        act_round(1, d)
    across_all(2)
    act_ready(1)
    gradients(2, 0)
    for k in range(kb):
        first(2, k)
    gradients(2, 1)
    weight_ready((2,))
    pl.loop(0, count // TILE)(backward)
    act_sent(0, True)

    @pl.loop(0, n_fs)
    def _(i):
        band = line_band(y_turn(i))
        pull_back(band, 1 - y)
        over(band).start()

    gradients(0, 0)
    for k in range(kb):
        first(0, k)
    gradients(1, 0)
    for k in range(kb):
        first(1, k)
    gradients(0, 1)
    for k in range(kb):
        second(2, k)

    @pl.loop(0, n_fs)
    def _(i):
        pull_back(i, y)

    gradients(1, 1)
    second(0, 0)
    normed_outer(0)
    second(0, 1)
    third(2, 0)
    third(2, 1)
    normed_outer(1)
    second(1, 0)
    normed_inner(n_fs - 1)
    normed_inner(0)
    second(1, 1)
    normed_outer(2)
    third(0, 0)
    third(0, 1)
    normed_inner(1)
    for k in range(kb):
        strip_squares(2, k)
    tall_fan[0]()
    for k in range(kb):
        strip_squares(0, k)
    third(1, 0)
    strip_squares(1, 0)
    third(1, 1)
    strip_squares(1, 1)
    wide_fan[0]()
    normed_last()
    whole_block(2, 0)
    whole_block(2, 1)
    token_sums()
    wide_fan[1]().wait_recv()
    v_half[...] = summed(wide_all, n_tp)
    wide_cross().start()
    v_wide[:, pl.ds(pl.multiple_of(r * strip, strip), strip)] = v_half[...]
    tall_fan[1]().wait_recv()
    v_tall[...] = summed(tall_all, 2 * n_fs)
    tall_out = pltpu.make_async_copy(v_tall, o_tall_sq, out_sem.at[6])
    tall_out.start()
    token_grads()
    whole_block(0, 0)
    whole_block(0, 1)
    act_sent(0, False)
    act_sent(1, True)
    for m in range(3):
        weight_sent(m)
    over_sent()
    normed_sent()
    inv_send().wait_send()
    last_send().wait_send()
    row_fan[1]().wait_send()
    wide_fan[1]().wait_send()
    for m in range(3):
        pairs_sent(m)
        swaps_sent(m)
        for k in range(kb):

            @pl.when(kb * c + k != z)
            def _():
                deliver(m, k).wait_send()

    whole_block(1, 0)
    gain_fan[1]().wait_recv()
    gain_sum[...] = summed(gain_all, 2 * n_fs)
    gain_out = pltpu.make_async_copy(gain_sum, o_gain, out_sem.at[5])
    gain_out.start()
    wide_cross_arrival().wait_recv()
    wide_out = pltpu.make_async_copy(v_wide, o_wide_sq, out_sem.at[7])
    wide_out.start()
    whole_block(1, 1)
    wide_cross().wait_send()
    gain_fan[1]().wait_send()
    tall_fan[1]().wait_send()
    gain_out.wait()
    tall_out.wait()
    wide_out.wait()
    pltpu.make_async_copy(v_out, o_tokens, out_sem.at[3]).wait()
    for m in range(3):
        spreads_sent(m)
        pltpu.make_async_copy(outs[m], (o_gate, o_up, o_down)[m], out_sem.at[m]).wait()


def layer(n_fs, n_tp, tokens, cot, w_gate, w_up, w_down, gain):
    half, local = tokens.shape[0] // CORES, tokens.shape[1]
    rows, hidden = w_gate.shape
    width = hidden * CORES // n_fs
    model = rows * n_fs
    count = half * n_fs
    dtype = tokens.dtype
    kb = n_fs // CORES
    strip = rows // 2
    reach = model // 2
    wide, tall = (strip, width), (width, strip)
    dma = pltpu.SemaphoreType.DMA
    hbm = pl.BlockSpec(memory_space=pl.ANY)
    pairs, singles = dma((3, kb, 2)), dma((3, kb))

    def bf(*shape):
        return pltpu.VMEM(shape, dtype)

    def f32(*shape):
        return pltpu.VMEM(shape, jnp.float32)

    hidden = kb * width
    shapes = [(rows, hidden)] * 2 + [(hidden, rows)]
    return pl.pallas_call(
        functools.partial(layer_kernel, n_fs, n_tp),
        out_shape=[jax.ShapeDtypeStruct(s, dtype) for s in shapes]
        + [jax.ShapeDtypeStruct((CORES * half, local), dtype)]
        + [jax.ShapeDtypeStruct(s, jnp.float32) for s in ((1, local), (2, rows), (1, hidden))],
        in_specs=[hbm] * 6,
        out_specs=[hbm] * 7,
        scratch_shapes=[
            bf(count, model),
            bf(count, model),
            bf(model, width),
            bf(model, width),
            bf(width, model),
            bf(count, model),
            bf(model, count),
            bf(width, count),
            f32(count, width),
            f32(count, width),
            bf(count, width),
            bf(count, width),
            f32(count, LANES),
            bf(model, width),
            bf(model, width),
            bf(width, model),
            bf(2, kb, 2, *wide),
            bf(kb, 2, *tall),
            bf(2, kb, *wide),
            bf(kb, *tall),
            bf(2, kb, *wide),
            bf(kb, *tall),
            bf(2, kb, *wide),
            bf(kb, *tall),
            bf(n_fs, half, reach),
            bf(n_fs, half, reach),
            bf(2, n_fs, half, reach),
            bf(half, local),
            bf(rows, hidden),
            bf(rows, hidden),
            bf(hidden, rows),
            bf(CORES * half, local),
            bf(CORES * half, local),
            bf(CORES * half, local),
            f32(CORES * half, LANES),
            bf(CORES * half, local),
            f32(2, strip, LANES),
            f32(n_tp, 1, CORES * half),
            f32(2 * n_fs, 1, local),
            f32(n_tp, 2, strip),
            f32(2 * n_fs, 1, hidden),
            dma((7,)),
            dma((2, 2)),
            dma((2,)),
            dma((2, n_fs - 1, CORES, PARTS)),
            dma((2,)),
            dma((2,)),
            dma((2,)),
            dma((2,)),
            dma((2,)),
            dma((3, kb)),
            dma((3, n_fs)),
            dma((3,)),
            dma((3, n_fs)),
            dma((3,)),
            dma((3,)),
            dma((3,)),
            dma((3,)),
            dma((3,)),
            pairs,
            dma((3,)),
            singles,
            singles,
            singles,
            dma((3,)),
            singles,
            dma((1,)),
            dma((n_fs,)),
            dma((n_fs,)),
            dma((2, n_fs)),
            dma((3,)),
            dma((3,)),
            dma((3, kb)),
            dma((1,)),
            dma((1,)),
            dma((1,)),
            dma((1,)),
            dma((1,)),
            dma((1,)),
            dma((1,)),
            dma((1,)),
            dma((8,)),
            f32(half, reach),
            f32(1, local),
            bf(model // LANES, LANES),
            f32(1, model),
            f32(2, rows),
            f32(1, hidden),
            f32(2, strip),
        ],
        compiler_params=pltpu.CompilerParams(
            collective_id=4, has_side_effects=True, vmem_limit_bytes=67043328
        ),
        name="layer",
    )(tokens, cot, w_gate, w_up, w_down, gain)


def widen_kernel(*refs):
    g_gate, g_up, g_down, tokens, gain, wide_sq, tall_sq = refs[:7]
    o_gate, o_up, o_down, o_tokens, o_gain, o_wide_sq, o_tall_sq = refs[7:]
    o_gate[...] = g_gate[...].astype(jnp.float32)
    o_up[...] = g_up[...].astype(jnp.float32)
    o_down[...] = g_down[...].astype(jnp.float32)
    o_tokens[...] = tokens[...]
    o_gain[...] = gain[0, :]
    o_wide_sq[...] = wide_sq[...]
    o_tall_sq[...] = tall_sq[0, :]


def widen(*arrays):
    shapes = [a.shape for a in arrays]

    def split(shape):
        return pl.BlockSpec((shape[0] // STEPS, shape[1]), lambda i: (i, 0))

    def whole(shape):
        return pl.BlockSpec(shape, lambda i: (0,) * len(shape))

    outs = shapes[:4] + [shapes[4][1:], shapes[5], shapes[6][1:]]
    kinds = [jnp.float32] * 3 + [arrays[3].dtype] + [jnp.float32] * 3
    return pl.pallas_call(
        widen_kernel,
        grid=(STEPS,),
        out_shape=[jax.ShapeDtypeStruct(s, k) for s, k in zip(outs, kinds)],
        in_specs=[split(s) for s in shapes[:4]] + [whole(s) for s in shapes[4:]],
        out_specs=[split(s) for s in outs[:4]] + [whole(s) for s in outs[4:]],
        compiler_params=pltpu.CompilerParams(dimension_semantics=("arbitrary",)),
        name="widen",
    )(*arrays)


def by_chip(tokens, norm_gain, w_gate, w_up, w_down, cotangent):
    found = layer(
        lax.axis_size("fs"),
        lax.axis_size("tp"),
        tokens,
        cotangent,
        w_gate,
        w_up,
        w_down,
        norm_gain.reshape(-1, LANES),
    )
    grad_gate, grad_up, grad_down, grad_tokens, grad_gain, gate_up_sq, down_sq = widen(*found)
    return (grad_tokens, grad_gain, grad_gate, grad_up, grad_down, gate_up_sq, down_sq)


def fits_chips(mesh):
    n_rep, n_fs, n_tp = mesh.shape["rep"], mesh.shape["fs"], mesh.shape["tp"]
    return n_rep == 2 and n_tp == 2 * CORES and n_fs == 2 * CORES


def solution(mesh):
    placed = (
        P(("rep", "fs"), "tp"),
        P(),
        P("fs", "tp"),
        P("fs", "tp"),
        P("tp", "fs"),
        P(("rep", "fs"), "tp"),
    )
    return jax.shard_map(
        by_chip if fits_chips(mesh) else on_device,
        mesh=mesh,
        in_specs=placed,
        out_specs=(
            P(("rep", "fs"), "tp"),
            P("tp"),
            P("fs", "tp"),
            P("fs", "tp"),
            P("tp", "fs"),
            P(None, "fs"),
            P("tp"),
        ),
        check_vma=False,
    )
```

```python
import functools

import jax
import jax.numpy as jnp
from jax import lax
from jax.experimental import pallas as pl
from jax.experimental.pallas import tpu as pltpu
from jax.sharding import PartitionSpec as P

MESH = pl.DeviceIdType.MESH


def contract_last(left, right):
    return lax.dot_general(
        left, right, (((1,), (1,)), ((), ())), preferred_element_type=jnp.float32
    )


def contract_first(left, right):
    return lax.dot_general(
        left, right, (((0,), (0,)), ((), ())), preferred_element_type=jnp.float32
    )


def remote(source, target, send_sem, recv_sem, where):
    return pltpu.make_async_remote_copy(
        src_ref=source,
        dst_ref=target,
        send_sem=send_sem,
        recv_sem=recv_sem,
        device_id=where,
        device_id_type=MESH,
    )


def line_sends(z, n_fs, side, d):
    if side == 0:
        return jnp.logical_and(z >= d - 1, z <= n_fs - 2)
    return jnp.logical_and(z + d <= n_fs, z >= 1)


def line_receives(z, n_fs, side, d):
    return z >= d if side == 0 else z + d <= n_fs - 1


def greet(peers):
    barrier = pltpu.get_barrier_semaphore()
    for peer in peers:
        pl.semaphore_signal(barrier, inc=1, device_id=peer, device_id_type=MESH)
    pl.semaphore_wait(barrier, len(peers))


def keep_own(sources, holders, targets, sems):
    count = len(sources)
    loads = [
        pltpu.make_async_copy(sources[i], holders[i], sems.at[0, i]) for i in range(count)
    ]
    stores = [
        pltpu.make_async_copy(holders[i], targets[i], sems.at[1, i]) for i in range(count)
    ]
    for load in loads:
        load.start()

    def finish():
        for load, store in zip(loads, stores):
            load.wait()
            store.start()
        for store in stores:
            store.wait()

    return finish


def weights_kernel(n_fs, n_tp, *refs):
    tokens, cot, w_gate, w_up, w_down = refs[:5]
    whole_x, whole_dy, full_gate, full_up, full_down = refs[5:10]
    holders = refs[10:15]
    own_sem, ring_send, ring_recv, rep_send, rep_recv, tp_send, tp_recv = refs[15:]
    r, z, t = lax.axis_index("rep"), lax.axis_index("fs"), lax.axis_index("tp")
    right, left = lax.rem(z + 1, n_fs), lax.rem(z + n_fs - 1, n_fs)
    partner = {"rep": 1 - r}
    sources = (w_gate, w_up, w_down)
    targets = (full_gate, full_up, full_down)
    rows = w_gate.shape[0]
    hidden = w_down.shape[0]
    local = tokens.shape[1]

    def own_piece(m, half):
        size = (hidden if m == 2 else rows) // 2
        return sources[m].at[pl.ds(pl.multiple_of(half * size, size), size), :]

    def piece(m, owner, half):
        if m == 2:
            size = hidden // 2
            return targets[m].at[
                pl.ds(pl.multiple_of(half * size, size), size),
                pl.ds(pl.multiple_of(owner * rows, rows), rows),
            ]
        size = rows // 2
        return targets[m].at[
            pl.ds(pl.multiple_of(owner * rows + half * size, size), size), :
        ]

    peers = [{"fs": right}, {"fs": left}, partner]
    peers += [{"tp": lax.rem(t + j, n_tp)} for j in range(1, n_tp)]
    greet(peers)

    def owner_of(side, back):
        return lax.rem(z + (n_fs - back if side == 0 else back), n_fs)

    def hop(m, side, d):
        place = piece(m, owner_of(side, d - 1), r)
        return remote(
            own_piece(m, r) if d == 1 else place,
            place,
            ring_send.at[m, side, d - 1],
            ring_recv.at[m, side, d - 1],
            {"fs": right if side == 0 else left},
        )

    def arrival(m, side, d):
        place = piece(m, owner_of(side, d), r)
        return remote(
            place,
            place,
            ring_send.at[m, side, d - 1],
            ring_recv.at[m, side, d - 1],
            {"fs": right if side == 0 else left},
        )

    def across(m, side, d):
        place = piece(m, owner_of(side, d), r)
        return remote(
            place, place, rep_send.at[m, side, d - 1], rep_recv.at[m, side, d - 1], partner
        )

    for m in range(3):
        for side in range(2):

            @pl.when(line_sends(z, n_fs, side, 1))
            def _():
                hop(m, side, 1).start()

    ends = []
    for a, (source, target) in enumerate(((tokens, whole_x), (cot, whole_dy))):
        place = target.at[:, pl.ds(pl.multiple_of(t * local, local), local)]
        for j in range(1, n_tp):
            copy = remote(
                source,
                place,
                tp_send.at[a, j - 1],
                tp_recv.at[a, j - 1],
                {"tp": lax.rem(t + j, n_tp)},
            )
            copy.start()
            ends.append(copy)
    mine = pl.ds(pl.multiple_of(t * local, local), local)
    band = pl.ds(pl.multiple_of(z * rows, rows), rows)
    finish = keep_own(
        (tokens, cot, w_gate, w_up, w_down),
        holders,
        (
            whole_x.at[:, mine],
            whole_dy.at[:, mine],
            full_gate.at[band, :],
            full_up.at[band, :],
            full_down.at[:, band],
        ),
        own_sem,
    )
    finish()
    for d in range(1, n_fs):
        for m in range(3):
            for side in range(2):

                @pl.when(line_receives(z, n_fs, side, d))
                def _():
                    arrival(m, side, d).wait_recv()
                    if d < n_fs - 1:

                        @pl.when(line_sends(z, n_fs, side, d + 1))
                        def _():
                            hop(m, side, d + 1).start()

                    across(m, side, d).start()

    for d in range(1, n_fs):
        for m in range(3):
            for side in range(2):

                @pl.when(line_sends(z, n_fs, side, d))
                def _():
                    hop(m, side, d).wait_send()

                @pl.when(line_receives(z, n_fs, side, d))
                def _():
                    across(m, side, d).wait()

    for copy in ends:
        copy.wait()


def gather_weights(n_fs, n_tp, tokens, cot, w_gate, w_up, w_down):
    count, local = tokens.shape
    rows, hidden = w_gate.shape
    width = rows * n_fs
    dtype = tokens.dtype
    shapes = [
        (count, width),
        (count, width),
        (width, hidden),
        (width, hidden),
        (hidden, width),
    ]
    held = (tokens, cot, w_gate, w_up, w_down)
    moved = sum(2 * a * b for a, b in shapes)
    dma = pltpu.SemaphoreType.DMA
    return pl.pallas_call(
        functools.partial(weights_kernel, n_fs, n_tp),
        out_shape=[jax.ShapeDtypeStruct(s, dtype) for s in shapes],
        in_specs=[pl.BlockSpec(memory_space=pl.ANY)] * 5,
        out_specs=[pl.BlockSpec(memory_space=pl.ANY)] * 5,
        scratch_shapes=[pltpu.VMEM(a.shape, a.dtype) for a in held]
        + [
            dma((2, 5)),
            dma((3, 2, n_fs - 1)),
            dma((3, 2, n_fs - 1)),
            dma((3, 2, n_fs - 1)),
            dma((3, 2, n_fs - 1)),
            dma((2, n_tp - 1)),
            dma((2, n_tp - 1)),
        ],
        compiler_params=pltpu.CompilerParams(collective_id=0, has_side_effects=True),
        cost_estimate=pl.CostEstimate(flops=0, bytes_accessed=16 * moved, transcendentals=0),
        name="gather_weights",
    )(*held)


def tokens_kernel(n_fs, n_tp, n_act, n_swap, *refs):
    total = n_act + n_swap
    acts, swaps = refs[:n_act], refs[n_act:total]
    act_outs, swap_outs = refs[total : total + n_act], refs[total + n_act : 2 * total]
    holders = refs[2 * total : 3 * total]
    own_sem, ring_send, ring_recv = refs[3 * total : 3 * total + 3]
    swap_send, swap_recv, relay_send, relay_recv = refs[3 * total + 3 :]
    z, t = lax.axis_index("fs"), lax.axis_index("tp")
    right, left = lax.rem(z + 1, n_fs), lax.rem(z + n_fs - 1, n_fs)
    count = acts[0].shape[0]
    peers = [{"fs": lax.rem(z + j, n_fs)} for j in range(1, n_fs)]
    if n_swap:
        peers += [{"tp": lax.rem(t + j, n_tp)} for j in range(1, n_tp)]
    greet(peers)

    def rows_of(owner):
        return pl.ds(pl.multiple_of(owner * count, count), count)

    def owner_of(side, back):
        return lax.rem(z + (n_fs - back if side == 0 else back), n_fs)

    def hop(m, side, d):
        place = act_outs[m].at[rows_of(owner_of(side, d - 1)), :]
        return remote(
            acts[m] if d == 1 else place,
            place,
            ring_send.at[m, side, d - 1],
            ring_recv.at[m, side, d - 1],
            {"fs": right if side == 0 else left},
        )

    def arrival(m, side, d):
        place = act_outs[m].at[rows_of(owner_of(side, d)), :]
        return remote(
            place,
            place,
            ring_send.at[m, side, d - 1],
            ring_recv.at[m, side, d - 1],
            {"fs": right if side == 0 else left},
        )

    def swap(a, j):
        peer = lax.rem(z + j, n_fs)
        cut = swap_outs[a].shape[1]
        return remote(
            swaps[a].at[:, pl.ds(pl.multiple_of(peer * cut, cut), cut)],
            swap_outs[a].at[rows_of(z), :],
            swap_send.at[a, j - 1],
            swap_recv.at[a, j - 1],
            {"fs": peer},
        )

    def swapped(a, j):
        place = swap_outs[a].at[rows_of(owner_of(0, j)), :]
        return remote(
            place,
            place,
            swap_send.at[a, j - 1],
            swap_recv.at[a, j - 1],
            {"fs": lax.rem(z + j, n_fs)},
        )

    def relay(a, j, k):
        place = swap_outs[a].at[rows_of(owner_of(0, j)), :]
        return remote(
            place,
            place,
            relay_send.at[a, j - 1, k - 1],
            relay_recv.at[a, j - 1],
            {"tp": lax.rem(t + k, n_tp)},
        )

    hub = lax.rem(z, n_tp) == t

    def feeds(j):
        return lax.rem(lax.rem(z + j, n_fs), n_tp) == t

    for a in range(n_swap):
        for j in range(1, n_fs):

            @pl.when(feeds(j))
            def _():
                swap(a, j).start()

    for m in range(n_act):
        for side in range(2):

            @pl.when(line_sends(z, n_fs, side, 1))
            def _():
                hop(m, side, 1).start()

    sources = list(acts)
    for a in range(n_swap):
        cut = swap_outs[a].shape[1]
        sources.append(swaps[a].at[:, pl.ds(pl.multiple_of(z * cut, cut), cut)])
    finish = keep_own(
        sources, holders, [out.at[rows_of(z), :] for out in act_outs + swap_outs], own_sem
    )
    finish()
    if n_swap:

        @pl.when(hub)
        def _():
            for a in range(n_swap):
                for j in range(1, n_fs):
                    swapped(a, j).wait_recv()
                    for k in range(1, n_tp):
                        relay(a, j, k).start()

    for d in range(1, n_fs):
        for m in range(n_act):
            for side in range(2):

                @pl.when(line_receives(z, n_fs, side, d))
                def _():
                    arrival(m, side, d).wait_recv()
                    if d < n_fs - 1:

                        @pl.when(line_sends(z, n_fs, side, d + 1))
                        def _():
                            hop(m, side, d + 1).start()

    for d in range(1, n_fs):
        for m in range(n_act):
            for side in range(2):

                @pl.when(line_sends(z, n_fs, side, d))
                def _():
                    hop(m, side, d).wait_send()

    for a in range(n_swap):
        for j in range(1, n_fs):

            @pl.when(feeds(j))
            def _():
                swap(a, j).wait_send()

            @pl.when(hub)
            def _():
                for k in range(1, n_tp):
                    relay(a, j, k).wait_send()

            @pl.when(jnp.logical_not(hub))
            def _():
                relay(a, j, 1).wait_recv()


def gather_tokens(n_fs, n_tp, collective_id, acts, swaps):
    count = acts[0].shape[0]
    outs = [jax.ShapeDtypeStruct((n_fs * count, a.shape[1]), a.dtype) for a in acts]
    outs += [jax.ShapeDtypeStruct((n_fs * count, a.shape[1] // n_fs), a.dtype) for a in swaps]
    dma = pltpu.SemaphoreType.DMA
    total = len(outs)
    n_swap = max(len(swaps), 1)
    moved = sum(2 * o.shape[0] * o.shape[1] for o in outs)
    return pl.pallas_call(
        functools.partial(tokens_kernel, n_fs, n_tp, len(acts), len(swaps)),
        out_shape=outs,
        in_specs=[pl.BlockSpec(memory_space=pl.ANY)] * total,
        out_specs=[pl.BlockSpec(memory_space=pl.ANY)] * total,
        scratch_shapes=[pltpu.VMEM((count, o.shape[1]), o.dtype) for o in outs]
        + [
            dma((2, total)),
            dma((len(acts), 2, n_fs - 1)),
            dma((len(acts), 2, n_fs - 1)),
            dma((n_swap, n_fs - 1)),
            dma((n_swap, n_fs - 1)),
            dma((n_swap, n_fs - 1, n_tp - 1)),
            dma((n_swap, n_fs - 1)),
        ],
        compiler_params=pltpu.CompilerParams(
            collective_id=collective_id, has_side_effects=True
        ),
        cost_estimate=pl.CostEstimate(flops=0, bytes_accessed=16 * moved, transcendentals=0),
        name=f"gather_tokens_{collective_id}",
    )(*acts, *swaps)


def over_rep(part):
    part = part.astype(jnp.bfloat16)
    n_rep = lax.axis_size("rep")
    other = lax.ppermute(part, "rep", [(i, (i + 1) % n_rep) for i in range(n_rep)])
    return part, other


def added(pair):
    return pair[0].astype(jnp.float32) + pair[1].astype(jnp.float32)


def on_device(tokens, norm_gain, w_gate, w_up, w_down, cotangent):
    n_fs, n_tp = lax.axis_size("fs"), lax.axis_size("tp")
    whole_x, whole_dy, full_gate, full_up, full_down = gather_weights(
        n_fs, n_tp, tokens, cotangent, w_gate, w_up, w_down
    )
    width = whole_x.shape[1]
    wide_tokens = whole_x.astype(jnp.float32)
    gain_f = norm_gain.astype(jnp.float32)
    inverse = lax.rsqrt(jnp.mean(wide_tokens * wide_tokens, axis=-1, keepdims=True) + 1e-06)
    normed = (wide_tokens * inverse * gain_f).astype(jnp.bfloat16)
    gate = jnp.dot(normed, full_gate, preferred_element_type=jnp.float32)
    up_proj = jnp.dot(normed, full_up, preferred_element_type=jnp.float32)
    sigma = jax.nn.sigmoid(gate)
    active = gate * sigma
    hidden = (active * up_proj).astype(jnp.bfloat16)
    back = 0.5 * contract_last(whole_dy, full_down)
    d_up = (back * active).astype(jnp.bfloat16)
    d_gate = (back * up_proj * sigma * (1.0 + gate * (1.0 - sigma))).astype(jnp.bfloat16)

    all_hidden, rows_dy = gather_tokens(n_fs, n_tp, 1, [hidden], [whole_dy])
    down_pair = over_rep(0.5 * contract_first(all_hidden, rows_dy))

    partial_normed = contract_last(d_gate, full_gate) + contract_last(d_up, full_up)
    d_normed = lax.psum_scatter(
        partial_normed.astype(jnp.bfloat16), "tp", scatter_dimension=1, tiled=True
    ).astype(jnp.float32)

    all_gate, rows_normed = gather_tokens(n_fs, n_tp, 2, [d_gate], [normed])
    gate_pair = over_rep(contract_first(rows_normed, all_gate))
    (all_up,) = gather_tokens(n_fs, n_tp, 3, [d_up], [])
    up_pair = over_rep(contract_first(rows_normed, all_up))

    local_width = d_normed.shape[1]
    local_gain = lax.dynamic_slice_in_dim(
        gain_f, lax.axis_index("tp") * local_width, local_width, 0
    )
    local_tokens = tokens.astype(jnp.float32)
    scaled_grad = d_normed * local_gain
    rowdot = lax.psum(jnp.sum(scaled_grad * local_tokens, axis=-1), "tp")
    grad_tokens = (
        cotangent.astype(jnp.float32)
        + inverse * scaled_grad
        - local_tokens * inverse**3 * rowdot[:, None] / width
    ).astype(jnp.bfloat16)
    grad_gain = lax.psum(jnp.sum(d_normed * local_tokens * inverse, axis=0), ("rep", "fs"))

    grad_down = added(down_pair)
    down_sq = lax.psum(jnp.sum(grad_down * grad_down, axis=1), "fs")
    grad_gate = added(gate_pair)
    grad_up = added(up_pair)
    gate_up_sq = lax.psum(
        jnp.stack([jnp.sum(grad_gate * grad_gate, axis=1), jnp.sum(grad_up * grad_up, axis=1)]),
        "tp",
    )
    return (grad_tokens, grad_gain, grad_gate, grad_up, grad_down, gate_up_sq, down_sq)


CORES = 2
LANES = 128
TILE = 256
PARTS = 4
STEPS = 4


def line_next(z, n_fs, side):
    return z <= n_fs - 2 if side == 0 else z >= 1


def layer_kernel(n_fs, n_tp, *refs):
    tokens, cot, w_gate, w_up, w_down, gain_in = refs[:6]
    o_gate, o_up, o_down, o_tokens, o_gain, o_wide_sq, o_tall_sq = refs[6:13]
    full = refs[13:18]
    x_full, dy_full, f_gate, f_up, f_down = full
    normed, normed_t, hidden_t, act_f, slope_f, d_gate, d_up, inv_all = refs[18:26]
    g_gate, g_up, g_down = refs[26:29]
    pair_wide, pair_tall, sum_wide, sum_tall, x_wide, x_tall, t_wide, t_tall = refs[29:37]
    y_buf, d_buf, z_buf, n_buf = refs[37:41]
    v_gate, v_up, v_down, v_tokens, v_cot, v_normed, v_inv, v_out = refs[41:49]
    lane_sq, row_all, gain_all, wide_all, tall_all = refs[49:54]
    (load_sem, az_own, az_fwd, az_recv, ay_own, ay_fwd, ay_recv, ap_send, ap_recv) = refs[54:63]
    (w_send, w_recv, wx_send, wx_recv, wp_send, wp_recv, wo_send, wo_recv) = refs[63:71]
    (p_send, p_recv, x_send, x_recv, z_send, z_recv, f_send, f_recv) = refs[71:79]
    (y_send, y_recv, d_send, d_recv, n_send, n_recv, own_sem) = refs[79:86]
    (row_send, row_recv, gain_send, gain_recv) = refs[86:90]
    (wide_send, wide_recv, tall_send, tall_recv, out_sem, total, gain_sum) = refs[90:97]
    gain_load, gain, v_wide, v_tall, v_half = refs[97:]
    r, z, t = lax.axis_index("rep"), lax.axis_index("fs"), lax.axis_index("tp")
    y, c = lax.div(t, CORES), lax.rem(t, CORES)
    acts, weights = (tokens, cot), (w_gate, w_up, w_down)
    grads, outs = (g_gate, g_up, g_down), (v_gate, v_up, v_down)
    half, local = tokens.shape[0] // CORES, tokens.shape[1]
    count, model = x_full.shape
    rows = w_gate.shape[0]
    kb = n_fs // CORES
    width = w_gate.shape[1] // kb
    strip = rows // 2
    reach = model // 2
    partner = {"tp": y * CORES + 1 - c}
    across = {"rep": 1 - r}
    beside = {"tp": (1 - y) * CORES + c}
    owner = lax.div(z, kb)

    peers = [partner, across]
    peers += [{"tp": (1 - y) * CORES + h} for h in range(CORES)]
    for j in range(1, n_fs):
        for h in range(CORES):
            peers.append({"fs": lax.rem(z + j, n_fs), "tp": y * CORES + h})
        peers.append({"rep": 1 - r, "fs": lax.rem(z + j, n_fs)})
    greet(peers)

    def own_act(a, h):
        return acts[a].at[pl.ds(pl.multiple_of(h * half, half), half), :]

    def act_place(a, source, column):
        return full[a].at[
            pl.ds(pl.multiple_of(source * half, half), half),
            pl.ds(pl.multiple_of(column * local, local), local),
        ]

    sub = half // PARTS

    def own_part(a, h, q):
        start = h * half + q * sub
        return acts[a].at[pl.ds(start, sub), :]

    def act_part(a, source, column, q):
        return full[a].at[
            pl.ds(pl.multiple_of(source * half + q * sub, sub), sub),
            pl.ds(pl.multiple_of(column * local, local), local),
        ]

    def source_of(side, d):
        return z - d if side == 0 else z + d

    def next_of(side):
        return z + 1 if side == 0 else z - 1

    def line_turn(source, at):
        return lax.rem(source - at + n_fs, n_fs) - 1

    def act_first(a, side, h, q):
        return remote(
            own_part(a, h, q),
            act_part(a, z, t, q),
            az_own.at[a, side],
            az_recv.at[a, line_turn(z, next_of(side)), c, q],
            {"fs": next_of(side), "tp": y * CORES + h},
        )

    def act_arrival(a, side, d, core, q):
        place = act_part(a, source_of(side, d), y * CORES + core, q)
        return remote(
            place,
            place,
            az_fwd.at[a],
            az_recv.at[a, line_turn(source_of(side, d), z), core, q],
            partner,
        )

    def act_forward(a, side, d, core, q):
        place = act_part(a, source_of(side, d), y * CORES + core, q)
        return remote(
            place,
            place,
            az_fwd.at[a],
            az_recv.at[a, line_turn(source_of(side, d), next_of(side)), core, q],
            {"fs": next_of(side)},
        )

    def act_over(a, side, d, core, q):
        source = source_of(side, d)
        place = act_part(a, source, y * CORES + core, q)
        return remote(
            place,
            place,
            ay_fwd.at[a],
            ay_recv.at[a],
            {"tp": (1 - y) * CORES + c},
        )

    def act_over_own(a, h):
        return remote(
            own_act(a, h),
            act_place(a, z, t),
            ay_own.at[a],
            ay_recv.at[a],
            {"tp": (1 - y) * CORES + h},
        )

    def act_over_arrivals(a):
        place = full[a].at[:, side_columns(1 - y)]
        return remote(place, place, ay_own.at[a], ay_recv.at[a], partner)

    def act_partner(a):
        return remote(own_act(a, 1 - c), act_place(a, z, t), ap_send.at[a], ap_recv.at[a], partner)

    def act_partner_arrival(a):
        place = act_place(a, z, y * CORES + 1 - c)
        return remote(place, place, ap_send.at[a], ap_recv.at[a], partner)

    def block_of(m, k):
        if m == 2:
            return weights[m].at[pl.ds(pl.multiple_of(k * width, width), width), :]
        return weights[m].at[:, pl.ds(pl.multiple_of(k * width, width), width)]

    def band_of(m, source):
        band = pl.ds(pl.multiple_of(source * rows, rows), rows)
        return full[2 + m].at[:, band] if m == 2 else full[2 + m].at[band, :]

    def quarter(m, source, rep, core):
        if m == 2:
            size = width // (2 * CORES)
            return full[4].at[
                pl.ds(pl.multiple_of((rep * CORES + core) * size, size), size),
                pl.ds(pl.multiple_of(source * rows, rows), rows),
            ]
        size = rows // (2 * CORES)
        start = source * rows + (rep * CORES + core) * size
        return full[2 + m].at[pl.ds(pl.multiple_of(start, size), size), :]

    def own_quarter(m, k, core):
        if m == 2:
            size = width // (2 * CORES)
            start = k * width + (r * CORES + core) * size
            return weights[m].at[pl.ds(pl.multiple_of(start, size), size), :]
        size = rows // (2 * CORES)
        return weights[m].at[
            pl.ds(pl.multiple_of((r * CORES + core) * size, size), size),
            pl.ds(k * width, width),
        ]

    def weight_send(m, k, core):
        return remote(
            own_quarter(m, k, core),
            quarter(m, z, r, core),
            w_send.at[m, k],
            w_recv.at[m, z],
            {"fs": kb * c + k, "tp": y * CORES + core},
        )

    def weight_arrival(m, source):
        place = quarter(m, source, r, c)
        return remote(place, place, wx_send.at[m], w_recv.at[m, source], partner)

    def weight_across(m, source):
        place = quarter(m, source, r, c)
        return remote(place, place, wx_send.at[m], wx_recv.at[m, source], across)

    def weight_across_arrival(m, source):
        place = quarter(m, source, 1 - r, c)
        return remote(place, place, wx_send.at[m], wx_recv.at[m, source], across)

    def weight_beside(m, source, which):
        place = quarter(m, source, r if which == 0 else 1 - r, c)
        return remote(
            place, place, wp_send.at[m], wp_recv.at[m], partner
        )

    def weight_beside_arrivals(m):
        part = (width if m == 2 else rows) // (2 * CORES)
        if m == 2:
            place = full[4].at[pl.ds(0, 2 * part), pl.ds(0, model - rows)]
        else:
            place = full[2 + m].at[pl.ds(0, 2 * (n_fs - 1) * part), :]
        return remote(place, place, wp_send.at[m], wp_recv.at[m], partner)

    def own_beside(m):
        return remote(
            block_of(m, z - kb * owner), band_of(m, z), wo_send.at[m], wo_recv.at[m], partner
        )

    def own_beside_arrival(m):
        return remote(band_of(m, z), band_of(m, z), wo_send.at[m], wo_recv.at[m], partner)

    def slot(wide, tall, m, *where):
        return tall.at[where] if m == 2 else wide.at[(m,) + where]

    def strip_of(band, rep):
        return pl.ds(pl.multiple_of(band * rows + rep * strip, strip), strip)

    def grad_piece(m, band, rep):
        if m == 2:
            return grads[m].at[:, strip_of(band, rep)]
        return grads[m].at[strip_of(band, rep), :]

    def rep_of(j):
        return 1 - r if j == 0 else r

    def pair(m, k, j):
        return remote(
            grad_piece(m, kb * (1 - c) + k, rep_of(j)),
            slot(pair_wide, pair_tall, m, k, j),
            p_send.at[m],
            p_recv.at[m, k, j],
            partner,
        )

    def swap(m, k):
        return remote(
            slot(sum_wide, sum_tall, m, k),
            slot(x_wide, x_tall, m, k),
            x_send.at[m],
            x_recv.at[m, k],
            across,
        )

    def place(m, block, rep):
        strips = pl.ds(pl.multiple_of(rep * strip, strip), strip)
        blocks = pl.ds(pl.multiple_of(block * width, width), width)
        return outs[m].at[blocks, strips] if m == 2 else outs[m].at[strips, blocks]

    def deliver(m, k):
        block = lax.rem(z, kb)
        return remote(
            slot(t_wide, t_tall, m, k),
            place(m, block, r),
            z_send.at[m, k],
            z_recv.at[m, block],
            {"fs": kb * c + k, "tp": y * CORES + owner},
        )

    def delivered(m, k):
        return remote(place(m, k, r), place(m, k, r), z_send.at[m, k], z_recv.at[m, k], partner)

    def keep(m, k):
        return pltpu.make_async_copy(slot(t_wide, t_tall, m, k), place(m, k, r), own_sem.at[m, k])

    def spread(m, k, source):
        return remote(source, place(m, k, r), f_send.at[m], f_recv.at[m, k], across)

    def spread_arrival(m, k):
        return remote(
            place(m, k, 1 - r), place(m, k, 1 - r), f_send.at[m], f_recv.at[m, k], across
        )

    def band_rows(band):
        return pl.ds(pl.multiple_of(band * half, half), half)

    def side_columns(which):
        return pl.ds(pl.multiple_of(which * reach, reach), reach)

    def over(band):
        return remote(
            x_full.at[band_rows(band), side_columns(1 - y)],
            y_buf.at[band],
            y_send.at[0],
            y_recv.at[band],
            beside,
        )

    low = z < n_fs // 2
    inner = jnp.logical_and(z > 0, z < n_fs - 1)
    line_slot = jnp.where(low, 0, 1)

    def line_band(i):
        return jnp.where(low, n_fs - 1 - i, i)

    def y_turn(i):
        return jnp.where(jnp.logical_and(inner, i >= 2), n_fs + 1 - i, i)

    def line_send(i, target):
        band = line_band(i)
        return remote(
            d_buf.at[i],
            z_buf.at[line_slot, band],
            d_send.at[i],
            d_recv.at[line_slot, band],
            {"fs": target},
        )

    def line_arrival(which, band):
        place = z_buf.at[which, band]
        return remote(place, place, d_send.at[0], d_recv.at[which, band], partner)

    def own_rows(core):
        return pl.ds(pl.multiple_of(core * half, half), half)

    def inv_send():
        return remote(inv_all.at[band_rows(z), :], v_inv.at[own_rows(c), :], n_send.at[0], n_recv.at[0], partner)

    def inv_arrival():
        at = v_inv.at[own_rows(1 - c), :]
        return remote(at, at, n_send.at[0], n_recv.at[0], partner)

    def last_send():
        return remote(n_buf, v_normed.at[own_rows(c), :], n_send.at[1], n_recv.at[1], partner)

    def last_arrival():
        at = v_normed.at[own_rows(1 - c), :]
        return remote(at, at, n_send.at[1], n_recv.at[1], partner)

    def loaded(a):
        return pltpu.make_async_copy(own_act(a, c), act_place(a, z, t), load_sem.at[a])

    def block_loaded(m):
        return pltpu.make_async_copy(
            block_of(m, z - kb * owner), band_of(m, z), load_sem.at[2 + m]
        )

    def act_start(a):
        for h in range(CORES):
            for side in range(2):

                @pl.when(line_next(z, n_fs, side))
                def _():
                    for q in range(PARTS):
                        act_first(a, side, h, q).start()

            act_over_own(a, h).start()
        act_partner(a).start()

    def own_start(m):
        @pl.when(c == owner)
        def _():
            own_beside(m).start()

    def act_round(a, d):
        for core in range(CORES):
            for q in range(PARTS):
                for side in range(2):

                    @pl.when(line_receives(z, n_fs, side, d))
                    def _():
                        act_arrival(a, side, d, core, q).wait_recv()
                        if d < n_fs - 1:

                            @pl.when(line_next(z, n_fs, side))
                            def _():
                                act_forward(a, side, d, core, q).start()

                        act_over(a, side, d, core, q).start()

    def weight_start(m):
        for k in range(kb):

            @pl.when(kb * c + k != z)
            def _():
                for core in range(CORES):
                    weight_send(m, k, core).start()

    def weight_round(ms, d):
        for m in ms:
            for side in range(2):

                @pl.when(line_receives(z, n_fs, side, d))
                def _():
                    source = source_of(side, d)
                    weight_arrival(m, source).wait_recv()
                    weight_across(m, source).start()
                    weight_beside(m, source, 0).start()

    def across_round(ms, d):
        for m in ms:
            for side in range(2):

                @pl.when(line_receives(z, n_fs, side, d))
                def _():
                    source = source_of(side, d)
                    weight_across_arrival(m, source).wait_recv()
                    weight_beside(m, source, 1).start()

    def weight_all(m):
        for d in range(1, n_fs):
            weight_round((m,), d)

    def across_all(m):
        for d in range(1, n_fs):
            across_round((m,), d)

    def act_ready(a):
        act_over_arrivals(a).wait_recv()
        act_partner_arrival(a).wait_recv()
        loaded(a).wait()

    def sent(ref, sem):
        remote(ref, ref, sem, sem, partner).wait_send()

    def act_sent(a, landed):
        others = full[a].at[pl.ds(0, count - half), pl.ds(0, CORES * local)]
        if landed:
            sent(others, ay_fwd.at[a])

            @pl.when(inner)
            def _():
                sent(others, az_fwd.at[a])

        if a == 1 or not landed:
            act_partner(a).wait_send()
            sent(acts[a], ay_own.at[a])
            for side in range(2):

                @pl.when(line_next(z, n_fs, side))
                def _():
                    sent(acts[a], az_own.at[a, side])

    def weight_ready(ms):
        for m in ms:
            weight_beside_arrivals(m).wait_recv()

            @pl.when(c == owner)
            def _():
                block_loaded(m).wait()

            @pl.when(c != owner)
            def _():
                own_beside_arrival(m).wait_recv()

    def weight_sent(m):
        size = full[2 + m].shape[0 if m < 2 else 1] - rows
        part = (rows if m < 2 else width) // (2 * CORES)
        if m < 2:
            sent(full[2 + m].at[pl.ds(0, (n_fs - 1) * part), :], wx_send.at[m])
            sent(full[2 + m].at[pl.ds(0, 2 * (n_fs - 1) * part), :], wp_send.at[m])
            half_block = weights[m].at[pl.ds(0, CORES * part), pl.ds(0, width)]
        else:
            sent(full[4].at[pl.ds(0, part), pl.ds(0, size)], wx_send.at[m])
            sent(full[4].at[pl.ds(0, 2 * part), pl.ds(0, size)], wp_send.at[m])
            half_block = weights[m].at[pl.ds(0, CORES * part), :]
        for k in range(kb):

            @pl.when(kb * c + k != z)
            def _():
                sent(half_block, w_send.at[m, k])

        @pl.when(c == owner)
        def _():
            own_beside(m).wait_send()

    def pairs_sent(m):
        span = pl.ds(0, kb * rows)
        sent(g_down.at[:, span] if m == 2 else grads[m].at[span, :], p_send.at[m])

    def swaps_sent(m):
        sent(sum_tall if m == 2 else sum_wide.at[m], x_send.at[m])

    def spreads_sent(m):
        sent(sum_tall if m == 2 else sum_wide.at[m], f_send.at[m])

    def over_sent():
        sent(x_full.at[:, side_columns(1 - y)], y_send.at[0])

    def tile(i, size):
        return pl.ds(pl.multiple_of(i * size, size), size)

    def normalize(i):
        at = tile(i, LANES)
        wide = x_full[at, :].astype(jnp.float32)
        inv = lax.rsqrt(jnp.mean(wide * wide, axis=-1, keepdims=True) + 1e-06)
        value = wide * inv * gain[...]
        normed[at, :] = value.astype(jnp.bfloat16)
        normed_t[:, at] = value.T.astype(jnp.bfloat16)
        inv_all[at, :] = jnp.broadcast_to(inv, (LANES, LANES))

    def forward(i):
        at = tile(i, TILE)
        gate = jnp.dot(normed[at, :], f_gate[...], preferred_element_type=jnp.float32)
        up = jnp.dot(normed[at, :], f_up[...], preferred_element_type=jnp.float32)
        sigma = jax.nn.sigmoid(gate)
        active = gate * sigma
        act_f[at, :] = active
        slope_f[at, :] = up * sigma * (1.0 + gate * (1.0 - sigma))
        hidden_t[:, at] = (active * up).T.astype(jnp.bfloat16)

    def backward(i):
        at = tile(i, TILE)
        back = 0.5 * contract_last(dy_full[at, :], f_down[...])
        d_up[at, :] = (back * act_f[at, :]).astype(jnp.bfloat16)
        d_gate[at, :] = (back * slope_f[at, :]).astype(jnp.bfloat16)

    def gradient(m, own, j, k):
        band = kb * (c if own else 1 - c) + k
        at = strip_of(band, 1 - r if j == 0 else r)
        if m == 2:
            value = 0.5 * jnp.dot(
                hidden_t[...], dy_full[:, at], preferred_element_type=jnp.float32
            )
            g_down[:, at] = value.astype(jnp.bfloat16)
        else:
            right = d_gate if m == 0 else d_up
            value = jnp.dot(normed_t[at, :], right[...], preferred_element_type=jnp.float32)
            grads[m][at, :] = value.astype(jnp.bfloat16)

    def gradients(m, j):
        @pl.loop(0, kb)
        def _(k):
            gradient(m, False, j, k)
            pair(m, k, j).start()

        @pl.loop(0, kb)
        def _(k):
            gradient(m, True, j, k)

    def pull_back(band, which):
        at, columns = band_rows(band), side_columns(which)
        value = contract_last(d_gate[at, :], f_gate[columns, :])
        value = value + contract_last(d_up[at, :], f_up[columns, :])
        x_full[at, columns] = value.astype(jnp.bfloat16)

    def added(m, k, j):
        own = grad_piece(m, kb * c + k, rep_of(j))[...].astype(jnp.float32)
        return own + slot(pair_wide, pair_tall, m, k, j)[...].astype(jnp.float32)

    def put(wide, tall, m, k, value):
        if m == 2:
            tall[k] = value
        else:
            wide[m, k] = value

    def first(m, k):
        pair(m, k, 0).wait_recv()
        put(sum_wide, sum_tall, m, k, added(m, k, 0).astype(jnp.bfloat16))
        swap(m, k).start()

    def second(m, k):
        pair(m, k, 1).wait_recv()
        swap(m, k).wait_recv()
        whole = added(m, k, 1) + slot(x_wide, x_tall, m, k)[...].astype(jnp.float32)
        put(t_wide, t_tall, m, k, whole.astype(jnp.bfloat16))
        mine = kb * c + k == z

        @pl.when(mine)
        def _():
            keep(m, k).start()
            spread(m, k, slot(t_wide, t_tall, m, k)).start()

        @pl.when(jnp.logical_not(mine))
        def _():
            deliver(m, k).start()

    def third(m, k):
        @pl.when(kb * c + k != z)
        def _():
            delivered(m, k).wait_recv()
            spread(m, k, place(m, k, r)).start()

    def own_share(band):
        over(band).wait_recv()
        own = x_full[band_rows(band), side_columns(y)].astype(jnp.float32)
        return own + y_buf[band].astype(jnp.float32)

    def line_target(i):
        if i == n_fs - 1:
            return jnp.where(low, z - 1, z + 1)
        return line_band(i)

    def normed_outer(i):
        @pl.when(jnp.logical_not(inner))
        def _():
            d_buf[i] = own_share(line_band(i)).astype(jnp.bfloat16)
            line_send(i, jnp.where(low, z + 1, z - 1)).start()

    def normed_inner(i):
        @pl.when(inner)
        def _():
            band = line_band(i)
            value = own_share(band)
            if i < n_fs - 1:
                line_arrival(line_slot, band).wait_recv()
                value = value + z_buf[line_slot, band].astype(jnp.float32)
            d_buf[i] = value.astype(jnp.bfloat16)
            line_send(i, line_target(i)).start()

    def normed_sent():
        for i in range(n_fs):
            if i < n_fs - 1:

                @pl.when(jnp.logical_not(inner))
                def _():
                    line_send(i, jnp.where(low, z + 1, z - 1)).wait_send()

            if i != n_fs - 2:

                @pl.when(inner)
                def _():
                    line_send(i, line_target(i)).wait_send()

    def normed_last():
        value = own_share(z)
        for which in range(2):
            line_arrival(which, z).wait_recv()
            value = value + z_buf[which, z].astype(jnp.float32)
        total[...] = value

        for core in range(CORES):

            @pl.when(c == core)
            def _():
                mine = slice(core * local, (core + 1) * local)
                theirs = slice((1 - core) * local, (2 - core) * local)
                v_normed[core * half : (core + 1) * half, :] = total[:, mine].astype(jnp.bfloat16)
                n_buf[...] = total[:, theirs].astype(jnp.bfloat16)

        last_send().start()

    def fold(value):
        out = value[:, :LANES]
        for i in range(1, value.shape[1] // LANES):
            out = out + value[:, i * LANES : (i + 1) * LANES]
        return out

    def row_of(value):
        return jnp.sum(value.T, axis=0, keepdims=True)

    def lane_peer(j):
        return {"tp": lax.rem(t + j, n_tp)}

    def group_peer(j):
        at = lax.rem(r * n_fs + z + j, 2 * n_fs)
        return {"rep": lax.div(at, n_fs), "fs": lax.rem(at, n_fs)}

    def fan(buffer, count_of, mine, send, recv, peer):
        def start():
            for j in range(1, count_of):
                place = buffer.at[mine]
                remote(place, place, send.at[0], recv.at[0], peer(j)).start()

        def others():
            place = buffer.at[pl.ds(0, count_of - 1)]
            return remote(place, place, send.at[0], recv.at[0], partner)

        return start, others

    row_fan = fan(row_all, n_tp, t, row_send, row_recv, lane_peer)
    wide_fan = fan(wide_all, n_tp, t, wide_send, wide_recv, lane_peer)
    gain_fan = fan(gain_all, 2 * n_fs, r * n_fs + z, gain_send, gain_recv, group_peer)
    tall_fan = fan(tall_all, 2 * n_fs, r * n_fs + z, tall_send, tall_recv, group_peer)

    def gain_here():
        return gain[:, pl.ds(pl.multiple_of(t * local, local), local)]

    def token_sums():
        last_arrival().wait_recv()
        inv_arrival().wait_recv()
        for i in range(2):
            own_loaded(i).wait()
        gain_l = gain_here()
        gain_sum[...] = jnp.zeros_like(gain_sum)

        @pl.loop(0, CORES * half // LANES)
        def _(i):
            at = tile(i, LANES)
            d_tokens = v_normed[at, :].astype(jnp.float32) * v_tokens[at, :].astype(jnp.float32)
            row_all[t, :, at] = row_of(fold(d_tokens * gain_l))
            inv = v_inv[at, :1]
            gain_sum[...] += jnp.sum(d_tokens * inv, axis=0, keepdims=True)

        gain_all[r * n_fs + z] = gain_sum[...]
        row_fan[0]()
        gain_fan[0]()

    def token_grads():
        row_fan[1]().wait_recv()
        gain_l = gain_here()

        @pl.loop(0, CORES * half // LANES)
        def _(i):
            at = tile(i, LANES)
            dots = row_all[0, :, at]
            for j in range(1, n_tp):
                dots = dots + row_all[j, :, at]
            rowdot = jnp.broadcast_to(dots, (LANES, LANES)).T[:, :1]
            inv = v_inv[at, :1]
            value = v_cot[at, :].astype(jnp.float32)
            value = value + inv * (v_normed[at, :].astype(jnp.float32) * gain_l)
            scale = inv**3 * rowdot / model
            value = value - v_tokens[at, :].astype(jnp.float32) * scale
            v_out[at, :] = value.astype(jnp.bfloat16)

        pltpu.make_async_copy(v_out, o_tokens, out_sem.at[3]).start()

    def own_loaded(i):
        source, target = ((tokens, v_tokens), (cot, v_cot))[i]
        return pltpu.make_async_copy(source, target, load_sem.at[5 + i])

    def block_out(m, k):
        at = pl.ds(k * width, width)
        if m == 2:
            return pltpu.make_async_copy(v_down.at[at, :], o_down.at[at, :], out_sem.at[m])
        return pltpu.make_async_copy(
            outs[m].at[:, at], (o_gate, o_up)[m].at[:, at], out_sem.at[m]
        )

    def strip_squares(m, k):
        @pl.when(kb * c + k == z)
        def _():
            keep(m, k).wait()

        if m == 2:
            columns = pl.ds(pl.multiple_of(r * strip, strip), strip)

            @pl.loop(0, width // LANES)
            def _(i):
                at = pl.ds(pl.multiple_of(k * width + i * LANES, LANES), LANES)
                value = v_down[at, columns].astype(jnp.float32)
                tall_all[r * n_fs + z, :, at] = row_of(fold(value * value))
        else:

            @pl.loop(0, strip // LANES)
            def _(i):
                at = tile(i, LANES)
                from_row = pl.ds(pl.multiple_of(r * strip + i * LANES, LANES), LANES)
                value = outs[m][from_row, k * width : (k + 1) * width].astype(jnp.float32)
                part = fold(value * value)
                if k > 0:
                    part = part + lane_sq[m, at, :]
                if k < kb - 1:
                    lane_sq[m, at, :] = part
                else:
                    wide_all[t, m : m + 1, at] = row_of(part)

    def wide_cross():
        strips = pl.ds(pl.multiple_of(r * strip, strip), strip)
        return remote(v_half, v_wide.at[:, strips], n_send.at[2], n_recv.at[2], across)

    def wide_cross_arrival():
        place = v_wide.at[:, pl.ds(pl.multiple_of((1 - r) * strip, strip), strip)]
        return remote(place, place, n_send.at[2], n_recv.at[2], across)

    def summed(buffer, count_of):
        value = buffer[0]
        for j in range(1, count_of):
            value = value + buffer[j]
        return value

    def whole_block(m, k):
        spread_arrival(m, k).wait_recv()
        block_out(m, k).start()

    gain_copy = pltpu.make_async_copy(gain_in, gain_load, out_sem.at[4])
    gain_copy.start()
    for a in range(2):
        loaded(a).start()

    @pl.when(c == owner)
    def _():
        for m in range(3):
            block_loaded(m).start()

    act_start(0)
    own_start(0)
    own_start(1)
    for i in range(2):
        own_loaded(i).start()
    act_round(0, 1)
    act_round(0, 2)
    weight_start(0)
    weight_start(1)
    act_start(1)
    own_start(2)
    for d in range(3, n_fs):
        act_round(0, d)
    weight_all(0)
    act_round(1, 1)
    weight_all(1)
    across_all(0)
    gain_copy.wait()
    for i in range(model // LANES):
        gain[:, i * LANES : (i + 1) * LANES] = gain_load[i : i + 1, :].astype(jnp.float32)
    act_ready(0)
    pl.loop(0, count // LANES)(normalize)
    inv_send().start()
    v_inv[own_rows(c), :] = inv_all[band_rows(z), :]
    weight_start(2)
    across_all(1)
    act_round(1, 2)
    weight_ready((0, 1))
    pl.loop(0, count // TILE)(forward)
    weight_all(2)
    for d in range(3, n_fs):
        act_round(1, d)
    across_all(2)
    act_ready(1)
    for k in range(kb):
        gradient(2, False, 0, k)
        pair(2, k, 0).start()
        if k:
            first(2, k - 1)
        gradient(2, True, 0, k)
    first(2, kb - 1)
    gradients(2, 1)
    weight_ready((2,))
    pl.loop(0, count // TILE)(backward)
    act_sent(0, True)

    gradients(0, 0)
    for k in range(kb):
        first(0, k)

    @pl.loop(0, n_fs)
    def _(i):
        band = line_band(y_turn(i))
        pull_back(band, 1 - y)
        over(band).start()

    gradients(1, 0)
    for k in range(kb):
        first(1, k)
    gradients(0, 1)
    for k in range(kb):
        second(2, k)

    @pl.loop(0, n_fs)
    def _(i):
        pull_back(i, y)

    gradients(1, 1)
    second(0, 0)
    normed_outer(0)
    second(0, 1)
    third(2, 0)
    third(2, 1)
    normed_outer(1)
    second(1, 0)
    normed_inner(n_fs - 1)
    normed_inner(0)
    second(1, 1)
    normed_outer(2)
    third(0, 0)
    third(0, 1)
    normed_inner(1)
    for k in range(kb):
        strip_squares(2, k)
    tall_fan[0]()
    for k in range(kb):
        strip_squares(0, k)
    third(1, 0)
    strip_squares(1, 0)
    third(1, 1)
    strip_squares(1, 1)
    wide_fan[0]()
    normed_last()
    whole_block(2, 0)
    whole_block(2, 1)
    token_sums()
    wide_fan[1]().wait_recv()
    v_half[...] = summed(wide_all, n_tp)
    wide_cross().start()
    v_wide[:, pl.ds(pl.multiple_of(r * strip, strip), strip)] = v_half[...]
    tall_fan[1]().wait_recv()
    v_tall[...] = summed(tall_all, 2 * n_fs)
    tall_out = pltpu.make_async_copy(v_tall, o_tall_sq, out_sem.at[6])
    tall_out.start()
    token_grads()
    whole_block(0, 0)
    whole_block(0, 1)
    act_sent(0, False)
    act_sent(1, True)
    for m in range(3):
        weight_sent(m)
    over_sent()
    normed_sent()
    inv_send().wait_send()
    last_send().wait_send()
    row_fan[1]().wait_send()
    wide_fan[1]().wait_send()
    for m in range(3):
        pairs_sent(m)
        swaps_sent(m)
        for k in range(kb):

            @pl.when(kb * c + k != z)
            def _():
                deliver(m, k).wait_send()

    whole_block(1, 0)
    gain_fan[1]().wait_recv()
    gain_sum[...] = summed(gain_all, 2 * n_fs)
    gain_out = pltpu.make_async_copy(gain_sum, o_gain, out_sem.at[5])
    gain_out.start()
    wide_cross_arrival().wait_recv()
    wide_out = pltpu.make_async_copy(v_wide, o_wide_sq, out_sem.at[7])
    wide_out.start()
    whole_block(1, 1)
    wide_cross().wait_send()
    gain_fan[1]().wait_send()
    tall_fan[1]().wait_send()
    gain_out.wait()
    tall_out.wait()
    wide_out.wait()
    pltpu.make_async_copy(v_out, o_tokens, out_sem.at[3]).wait()
    for m in range(3):
        spreads_sent(m)
        pltpu.make_async_copy(outs[m], (o_gate, o_up, o_down)[m], out_sem.at[m]).wait()


def layer(n_fs, n_tp, tokens, cot, w_gate, w_up, w_down, gain):
    half, local = tokens.shape[0] // CORES, tokens.shape[1]
    rows, hidden = w_gate.shape
    width = hidden * CORES // n_fs
    model = rows * n_fs
    count = half * n_fs
    dtype = tokens.dtype
    kb = n_fs // CORES
    strip = rows // 2
    reach = model // 2
    wide, tall = (strip, width), (width, strip)
    dma = pltpu.SemaphoreType.DMA
    hbm = pl.BlockSpec(memory_space=pl.ANY)
    pairs, singles = dma((3, kb, 2)), dma((3, kb))

    def bf(*shape):
        return pltpu.VMEM(shape, dtype)

    def f32(*shape):
        return pltpu.VMEM(shape, jnp.float32)

    hidden = kb * width
    shapes = [(rows, hidden)] * 2 + [(hidden, rows)]
    return pl.pallas_call(
        functools.partial(layer_kernel, n_fs, n_tp),
        out_shape=[jax.ShapeDtypeStruct(s, dtype) for s in shapes]
        + [jax.ShapeDtypeStruct((CORES * half, local), dtype)]
        + [jax.ShapeDtypeStruct(s, jnp.float32) for s in ((1, local), (2, rows), (1, hidden))],
        in_specs=[hbm] * 6,
        out_specs=[hbm] * 7,
        scratch_shapes=[
            bf(count, model),
            bf(count, model),
            bf(model, width),
            bf(model, width),
            bf(width, model),
            bf(count, model),
            bf(model, count),
            bf(width, count),
            f32(count, width),
            f32(count, width),
            bf(count, width),
            bf(count, width),
            f32(count, LANES),
            bf(model, width),
            bf(model, width),
            bf(width, model),
            bf(2, kb, 2, *wide),
            bf(kb, 2, *tall),
            bf(2, kb, *wide),
            bf(kb, *tall),
            bf(2, kb, *wide),
            bf(kb, *tall),
            bf(2, kb, *wide),
            bf(kb, *tall),
            bf(n_fs, half, reach),
            bf(n_fs, half, reach),
            bf(2, n_fs, half, reach),
            bf(half, local),
            bf(rows, hidden),
            bf(rows, hidden),
            bf(hidden, rows),
            bf(CORES * half, local),
            bf(CORES * half, local),
            bf(CORES * half, local),
            f32(CORES * half, LANES),
            bf(CORES * half, local),
            f32(2, strip, LANES),
            f32(n_tp, 1, CORES * half),
            f32(2 * n_fs, 1, local),
            f32(n_tp, 2, strip),
            f32(2 * n_fs, 1, hidden),
            dma((7,)),
            dma((2, 2)),
            dma((2,)),
            dma((2, n_fs - 1, CORES, PARTS)),
            dma((2,)),
            dma((2,)),
            dma((2,)),
            dma((2,)),
            dma((2,)),
            dma((3, kb)),
            dma((3, n_fs)),
            dma((3,)),
            dma((3, n_fs)),
            dma((3,)),
            dma((3,)),
            dma((3,)),
            dma((3,)),
            dma((3,)),
            pairs,
            dma((3,)),
            singles,
            singles,
            singles,
            dma((3,)),
            singles,
            dma((1,)),
            dma((n_fs,)),
            dma((n_fs,)),
            dma((2, n_fs)),
            dma((3,)),
            dma((3,)),
            dma((3, kb)),
            dma((1,)),
            dma((1,)),
            dma((1,)),
            dma((1,)),
            dma((1,)),
            dma((1,)),
            dma((1,)),
            dma((1,)),
            dma((8,)),
            f32(half, reach),
            f32(1, local),
            bf(model // LANES, LANES),
            f32(1, model),
            f32(2, rows),
            f32(1, hidden),
            f32(2, strip),
        ],
        compiler_params=pltpu.CompilerParams(
            collective_id=4, has_side_effects=True, vmem_limit_bytes=67043328
        ),
        name="layer",
    )(tokens, cot, w_gate, w_up, w_down, gain)


def widen_kernel(n, *refs):
    sources, targets = refs[:n], refs[n : 2 * n]
    narrow, wide = refs[2 * n : 3 * n], refs[3 * n : 3 * n + 3]
    flat, load_sem, store_sem = refs[3 * n + 3 : -2], *refs[-2:]

    def rows_of(i, step):
        size = sources[i].shape[0] // STEPS
        return pl.ds(step * size, size)

    def load(i, step):
        at = rows_of(i, step)
        return pltpu.make_async_copy(sources[i].at[at], narrow[i].at[at], load_sem.at[i, step])

    def store(i, step):
        at = rows_of(i, step)
        return pltpu.make_async_copy(wide[i].at[at], targets[i].at[at], store_sem.at[i, step])

    def load_whole(i):
        return pltpu.make_async_copy(sources[i], narrow[i], load_sem.at[i, 0])

    def store_whole(i):
        source = {4: flat[0], 6: flat[1]}.get(i, narrow[i])
        return pltpu.make_async_copy(source, targets[i], store_sem.at[i, 0])

    for i in range(3, n):
        load_whole(i).start()
    for step in range(STEPS):
        for i in range(3):
            load(i, step).start()
    for i in range(3, n):
        load_whole(i).wait()
        if i in (4, 6):
            flat[(i - 4) // 2][...] = narrow[i][0, :]
        store_whole(i).start()
    for step in range(STEPS):
        for i in range(3):
            load(i, step).wait()
            at = rows_of(i, step)
            wide[i][at] = narrow[i][at].astype(jnp.float32)
            store(i, step).start()
    for step in range(STEPS):
        for i in range(3):
            store(i, step).wait()
    for i in range(3, n):
        store_whole(i).wait()


def widen(*arrays):
    n = len(arrays)
    hbm = pl.BlockSpec(memory_space=pl.ANY)
    shapes = [a.shape[1:] if a.shape[0] == 1 else a.shape for a in arrays]
    kinds = [jnp.float32] * 3 + [a.dtype for a in arrays[3:]]
    dma = pltpu.SemaphoreType.DMA
    return pl.pallas_call(
        functools.partial(widen_kernel, n),
        out_shape=[jax.ShapeDtypeStruct(s, k) for s, k in zip(shapes, kinds)],
        in_specs=[hbm] * n,
        out_specs=[hbm] * n,
        scratch_shapes=[pltpu.VMEM(a.shape, a.dtype) for a in arrays]
        + [pltpu.VMEM(a.shape, jnp.float32) for a in arrays[:3]]
        + [pltpu.VMEM(s, jnp.float32) for s in (shapes[4], shapes[6])]
        + [dma((n, STEPS)), dma((n, STEPS))],
        name="widen",
    )(*arrays)


def by_chip(tokens, norm_gain, w_gate, w_up, w_down, cotangent):
    found = layer(
        lax.axis_size("fs"),
        lax.axis_size("tp"),
        tokens,
        cotangent,
        w_gate,
        w_up,
        w_down,
        norm_gain.reshape(-1, LANES),
    )
    grad_gate, grad_up, grad_down, grad_tokens, grad_gain, gate_up_sq, down_sq = widen(*found)
    return (grad_tokens, grad_gain, grad_gate, grad_up, grad_down, gate_up_sq, down_sq)


def fits_chips(mesh):
    n_rep, n_fs, n_tp = mesh.shape["rep"], mesh.shape["fs"], mesh.shape["tp"]
    return n_rep == 2 and n_tp == 2 * CORES and n_fs == 2 * CORES


def solution(mesh):
    placed = (
        P(("rep", "fs"), "tp"),
        P(),
        P("fs", "tp"),
        P("fs", "tp"),
        P("tp", "fs"),
        P(("rep", "fs"), "tp"),
    )
    return jax.shard_map(
        by_chip if fits_chips(mesh) else on_device,
        mesh=mesh,
        in_specs=placed,
        out_specs=(
            P(("rep", "fs"), "tp"),
            P("tp"),
            P("fs", "tp"),
            P("fs", "tp"),
            P("tp", "fs"),
            P(None, "fs"),
            P("tp"),
        ),
        check_vma=False,
    )
```

```python
import functools

import jax
import jax.numpy as jnp
from jax import lax
from jax.experimental import pallas as pl
from jax.experimental.pallas import tpu as pltpu
from jax.sharding import PartitionSpec as P

MESH = pl.DeviceIdType.MESH


def contract_last(left, right):
    return lax.dot_general(
        left, right, (((1,), (1,)), ((), ())), preferred_element_type=jnp.float32
    )


def contract_first(left, right):
    return lax.dot_general(
        left, right, (((0,), (0,)), ((), ())), preferred_element_type=jnp.float32
    )


def remote(source, target, send_sem, recv_sem, where):
    return pltpu.make_async_remote_copy(
        src_ref=source,
        dst_ref=target,
        send_sem=send_sem,
        recv_sem=recv_sem,
        device_id=where,
        device_id_type=MESH,
    )


def line_sends(z, n_fs, side, d):
    if side == 0:
        return jnp.logical_and(z >= d - 1, z <= n_fs - 2)
    return jnp.logical_and(z + d <= n_fs, z >= 1)


def line_receives(z, n_fs, side, d):
    return z >= d if side == 0 else z + d <= n_fs - 1


def greet(peers):
    barrier = pltpu.get_barrier_semaphore()
    for peer in peers:
        pl.semaphore_signal(barrier, inc=1, device_id=peer, device_id_type=MESH)
    pl.semaphore_wait(barrier, len(peers))


def keep_own(sources, holders, targets, sems):
    count = len(sources)
    loads = [
        pltpu.make_async_copy(sources[i], holders[i], sems.at[0, i]) for i in range(count)
    ]
    stores = [
        pltpu.make_async_copy(holders[i], targets[i], sems.at[1, i]) for i in range(count)
    ]
    for load in loads:
        load.start()

    def finish():
        for load, store in zip(loads, stores):
            load.wait()
            store.start()
        for store in stores:
            store.wait()

    return finish


def weights_kernel(n_fs, n_tp, *refs):
    tokens, cot, w_gate, w_up, w_down = refs[:5]
    whole_x, whole_dy, full_gate, full_up, full_down = refs[5:10]
    holders = refs[10:15]
    own_sem, ring_send, ring_recv, rep_send, rep_recv, tp_send, tp_recv = refs[15:]
    r, z, t = lax.axis_index("rep"), lax.axis_index("fs"), lax.axis_index("tp")
    right, left = lax.rem(z + 1, n_fs), lax.rem(z + n_fs - 1, n_fs)
    partner = {"rep": 1 - r}
    sources = (w_gate, w_up, w_down)
    targets = (full_gate, full_up, full_down)
    rows = w_gate.shape[0]
    hidden = w_down.shape[0]
    local = tokens.shape[1]

    def own_piece(m, half):
        size = (hidden if m == 2 else rows) // 2
        return sources[m].at[pl.ds(pl.multiple_of(half * size, size), size), :]

    def piece(m, owner, half):
        if m == 2:
            size = hidden // 2
            return targets[m].at[
                pl.ds(pl.multiple_of(half * size, size), size),
                pl.ds(pl.multiple_of(owner * rows, rows), rows),
            ]
        size = rows // 2
        return targets[m].at[
            pl.ds(pl.multiple_of(owner * rows + half * size, size), size), :
        ]

    peers = [{"fs": right}, {"fs": left}, partner]
    peers += [{"tp": lax.rem(t + j, n_tp)} for j in range(1, n_tp)]
    greet(peers)

    def owner_of(side, back):
        return lax.rem(z + (n_fs - back if side == 0 else back), n_fs)

    def hop(m, side, d):
        place = piece(m, owner_of(side, d - 1), r)
        return remote(
            own_piece(m, r) if d == 1 else place,
            place,
            ring_send.at[m, side, d - 1],
            ring_recv.at[m, side, d - 1],
            {"fs": right if side == 0 else left},
        )

    def arrival(m, side, d):
        place = piece(m, owner_of(side, d), r)
        return remote(
            place,
            place,
            ring_send.at[m, side, d - 1],
            ring_recv.at[m, side, d - 1],
            {"fs": right if side == 0 else left},
        )

    def across(m, side, d):
        place = piece(m, owner_of(side, d), r)
        return remote(
            place, place, rep_send.at[m, side, d - 1], rep_recv.at[m, side, d - 1], partner
        )

    for m in range(3):
        for side in range(2):

            @pl.when(line_sends(z, n_fs, side, 1))
            def _():
                hop(m, side, 1).start()

    ends = []
    for a, (source, target) in enumerate(((tokens, whole_x), (cot, whole_dy))):
        place = target.at[:, pl.ds(pl.multiple_of(t * local, local), local)]
        for j in range(1, n_tp):
            copy = remote(
                source,
                place,
                tp_send.at[a, j - 1],
                tp_recv.at[a, j - 1],
                {"tp": lax.rem(t + j, n_tp)},
            )
            copy.start()
            ends.append(copy)
    mine = pl.ds(pl.multiple_of(t * local, local), local)
    band = pl.ds(pl.multiple_of(z * rows, rows), rows)
    finish = keep_own(
        (tokens, cot, w_gate, w_up, w_down),
        holders,
        (
            whole_x.at[:, mine],
            whole_dy.at[:, mine],
            full_gate.at[band, :],
            full_up.at[band, :],
            full_down.at[:, band],
        ),
        own_sem,
    )
    finish()
    for d in range(1, n_fs):
        for m in range(3):
            for side in range(2):

                @pl.when(line_receives(z, n_fs, side, d))
                def _():
                    arrival(m, side, d).wait_recv()
                    if d < n_fs - 1:

                        @pl.when(line_sends(z, n_fs, side, d + 1))
                        def _():
                            hop(m, side, d + 1).start()

                    across(m, side, d).start()

    for d in range(1, n_fs):
        for m in range(3):
            for side in range(2):

                @pl.when(line_sends(z, n_fs, side, d))
                def _():
                    hop(m, side, d).wait_send()

                @pl.when(line_receives(z, n_fs, side, d))
                def _():
                    across(m, side, d).wait()

    for copy in ends:
        copy.wait()


def gather_weights(n_fs, n_tp, tokens, cot, w_gate, w_up, w_down):
    count, local = tokens.shape
    rows, hidden = w_gate.shape
    width = rows * n_fs
    dtype = tokens.dtype
    shapes = [
        (count, width),
        (count, width),
        (width, hidden),
        (width, hidden),
        (hidden, width),
    ]
    held = (tokens, cot, w_gate, w_up, w_down)
    moved = sum(2 * a * b for a, b in shapes)
    dma = pltpu.SemaphoreType.DMA
    return pl.pallas_call(
        functools.partial(weights_kernel, n_fs, n_tp),
        out_shape=[jax.ShapeDtypeStruct(s, dtype) for s in shapes],
        in_specs=[pl.BlockSpec(memory_space=pl.ANY)] * 5,
        out_specs=[pl.BlockSpec(memory_space=pl.ANY)] * 5,
        scratch_shapes=[pltpu.VMEM(a.shape, a.dtype) for a in held]
        + [
            dma((2, 5)),
            dma((3, 2, n_fs - 1)),
            dma((3, 2, n_fs - 1)),
            dma((3, 2, n_fs - 1)),
            dma((3, 2, n_fs - 1)),
            dma((2, n_tp - 1)),
            dma((2, n_tp - 1)),
        ],
        compiler_params=pltpu.CompilerParams(collective_id=0, has_side_effects=True),
        cost_estimate=pl.CostEstimate(flops=0, bytes_accessed=16 * moved, transcendentals=0),
        name="gather_weights",
    )(*held)


def tokens_kernel(n_fs, n_tp, n_act, n_swap, *refs):
    total = n_act + n_swap
    acts, swaps = refs[:n_act], refs[n_act:total]
    act_outs, swap_outs = refs[total : total + n_act], refs[total + n_act : 2 * total]
    holders = refs[2 * total : 3 * total]
    own_sem, ring_send, ring_recv = refs[3 * total : 3 * total + 3]
    swap_send, swap_recv, relay_send, relay_recv = refs[3 * total + 3 :]
    z, t = lax.axis_index("fs"), lax.axis_index("tp")
    right, left = lax.rem(z + 1, n_fs), lax.rem(z + n_fs - 1, n_fs)
    count = acts[0].shape[0]
    peers = [{"fs": lax.rem(z + j, n_fs)} for j in range(1, n_fs)]
    if n_swap:
        peers += [{"tp": lax.rem(t + j, n_tp)} for j in range(1, n_tp)]
    greet(peers)

    def rows_of(owner):
        return pl.ds(pl.multiple_of(owner * count, count), count)

    def owner_of(side, back):
        return lax.rem(z + (n_fs - back if side == 0 else back), n_fs)

    def hop(m, side, d):
        place = act_outs[m].at[rows_of(owner_of(side, d - 1)), :]
        return remote(
            acts[m] if d == 1 else place,
            place,
            ring_send.at[m, side, d - 1],
            ring_recv.at[m, side, d - 1],
            {"fs": right if side == 0 else left},
        )

    def arrival(m, side, d):
        place = act_outs[m].at[rows_of(owner_of(side, d)), :]
        return remote(
            place,
            place,
            ring_send.at[m, side, d - 1],
            ring_recv.at[m, side, d - 1],
            {"fs": right if side == 0 else left},
        )

    def swap(a, j):
        peer = lax.rem(z + j, n_fs)
        cut = swap_outs[a].shape[1]
        return remote(
            swaps[a].at[:, pl.ds(pl.multiple_of(peer * cut, cut), cut)],
            swap_outs[a].at[rows_of(z), :],
            swap_send.at[a, j - 1],
            swap_recv.at[a, j - 1],
            {"fs": peer},
        )

    def swapped(a, j):
        place = swap_outs[a].at[rows_of(owner_of(0, j)), :]
        return remote(
            place,
            place,
            swap_send.at[a, j - 1],
            swap_recv.at[a, j - 1],
            {"fs": lax.rem(z + j, n_fs)},
        )

    def relay(a, j, k):
        place = swap_outs[a].at[rows_of(owner_of(0, j)), :]
        return remote(
            place,
            place,
            relay_send.at[a, j - 1, k - 1],
            relay_recv.at[a, j - 1],
            {"tp": lax.rem(t + k, n_tp)},
        )

    hub = lax.rem(z, n_tp) == t

    def feeds(j):
        return lax.rem(lax.rem(z + j, n_fs), n_tp) == t

    for a in range(n_swap):
        for j in range(1, n_fs):

            @pl.when(feeds(j))
            def _():
                swap(a, j).start()

    for m in range(n_act):
        for side in range(2):

            @pl.when(line_sends(z, n_fs, side, 1))
            def _():
                hop(m, side, 1).start()

    sources = list(acts)
    for a in range(n_swap):
        cut = swap_outs[a].shape[1]
        sources.append(swaps[a].at[:, pl.ds(pl.multiple_of(z * cut, cut), cut)])
    finish = keep_own(
        sources, holders, [out.at[rows_of(z), :] for out in act_outs + swap_outs], own_sem
    )
    finish()
    if n_swap:

        @pl.when(hub)
        def _():
            for a in range(n_swap):
                for j in range(1, n_fs):
                    swapped(a, j).wait_recv()
                    for k in range(1, n_tp):
                        relay(a, j, k).start()

    for d in range(1, n_fs):
        for m in range(n_act):
            for side in range(2):

                @pl.when(line_receives(z, n_fs, side, d))
                def _():
                    arrival(m, side, d).wait_recv()
                    if d < n_fs - 1:

                        @pl.when(line_sends(z, n_fs, side, d + 1))
                        def _():
                            hop(m, side, d + 1).start()

    for d in range(1, n_fs):
        for m in range(n_act):
            for side in range(2):

                @pl.when(line_sends(z, n_fs, side, d))
                def _():
                    hop(m, side, d).wait_send()

    for a in range(n_swap):
        for j in range(1, n_fs):

            @pl.when(feeds(j))
            def _():
                swap(a, j).wait_send()

            @pl.when(hub)
            def _():
                for k in range(1, n_tp):
                    relay(a, j, k).wait_send()

            @pl.when(jnp.logical_not(hub))
            def _():
                relay(a, j, 1).wait_recv()


def gather_tokens(n_fs, n_tp, collective_id, acts, swaps):
    count = acts[0].shape[0]
    outs = [jax.ShapeDtypeStruct((n_fs * count, a.shape[1]), a.dtype) for a in acts]
    outs += [jax.ShapeDtypeStruct((n_fs * count, a.shape[1] // n_fs), a.dtype) for a in swaps]
    dma = pltpu.SemaphoreType.DMA
    total = len(outs)
    n_swap = max(len(swaps), 1)
    moved = sum(2 * o.shape[0] * o.shape[1] for o in outs)
    return pl.pallas_call(
        functools.partial(tokens_kernel, n_fs, n_tp, len(acts), len(swaps)),
        out_shape=outs,
        in_specs=[pl.BlockSpec(memory_space=pl.ANY)] * total,
        out_specs=[pl.BlockSpec(memory_space=pl.ANY)] * total,
        scratch_shapes=[pltpu.VMEM((count, o.shape[1]), o.dtype) for o in outs]
        + [
            dma((2, total)),
            dma((len(acts), 2, n_fs - 1)),
            dma((len(acts), 2, n_fs - 1)),
            dma((n_swap, n_fs - 1)),
            dma((n_swap, n_fs - 1)),
            dma((n_swap, n_fs - 1, n_tp - 1)),
            dma((n_swap, n_fs - 1)),
        ],
        compiler_params=pltpu.CompilerParams(
            collective_id=collective_id, has_side_effects=True
        ),
        cost_estimate=pl.CostEstimate(flops=0, bytes_accessed=16 * moved, transcendentals=0),
        name=f"gather_tokens_{collective_id}",
    )(*acts, *swaps)


def over_rep(part):
    part = part.astype(jnp.bfloat16)
    n_rep = lax.axis_size("rep")
    other = lax.ppermute(part, "rep", [(i, (i + 1) % n_rep) for i in range(n_rep)])
    return part, other


def added(pair):
    return pair[0].astype(jnp.float32) + pair[1].astype(jnp.float32)


def on_device(tokens, norm_gain, w_gate, w_up, w_down, cotangent):
    n_fs, n_tp = lax.axis_size("fs"), lax.axis_size("tp")
    whole_x, whole_dy, full_gate, full_up, full_down = gather_weights(
        n_fs, n_tp, tokens, cotangent, w_gate, w_up, w_down
    )
    width = whole_x.shape[1]
    wide_tokens = whole_x.astype(jnp.float32)
    gain_f = norm_gain.astype(jnp.float32)
    inverse = lax.rsqrt(jnp.mean(wide_tokens * wide_tokens, axis=-1, keepdims=True) + 1e-06)
    normed = (wide_tokens * inverse * gain_f).astype(jnp.bfloat16)
    gate = jnp.dot(normed, full_gate, preferred_element_type=jnp.float32)
    up_proj = jnp.dot(normed, full_up, preferred_element_type=jnp.float32)
    sigma = jax.nn.sigmoid(gate)
    active = gate * sigma
    hidden = (active * up_proj).astype(jnp.bfloat16)
    back = 0.5 * contract_last(whole_dy, full_down)
    d_up = (back * active).astype(jnp.bfloat16)
    d_gate = (back * up_proj * sigma * (1.0 + gate * (1.0 - sigma))).astype(jnp.bfloat16)

    all_hidden, rows_dy = gather_tokens(n_fs, n_tp, 1, [hidden], [whole_dy])
    down_pair = over_rep(0.5 * contract_first(all_hidden, rows_dy))

    partial_normed = contract_last(d_gate, full_gate) + contract_last(d_up, full_up)
    d_normed = lax.psum_scatter(
        partial_normed.astype(jnp.bfloat16), "tp", scatter_dimension=1, tiled=True
    ).astype(jnp.float32)

    all_gate, rows_normed = gather_tokens(n_fs, n_tp, 2, [d_gate], [normed])
    gate_pair = over_rep(contract_first(rows_normed, all_gate))
    (all_up,) = gather_tokens(n_fs, n_tp, 3, [d_up], [])
    up_pair = over_rep(contract_first(rows_normed, all_up))

    local_width = d_normed.shape[1]
    local_gain = lax.dynamic_slice_in_dim(
        gain_f, lax.axis_index("tp") * local_width, local_width, 0
    )
    local_tokens = tokens.astype(jnp.float32)
    scaled_grad = d_normed * local_gain
    rowdot = lax.psum(jnp.sum(scaled_grad * local_tokens, axis=-1), "tp")
    grad_tokens = (
        cotangent.astype(jnp.float32)
        + inverse * scaled_grad
        - local_tokens * inverse**3 * rowdot[:, None] / width
    ).astype(jnp.bfloat16)
    grad_gain = lax.psum(jnp.sum(d_normed * local_tokens * inverse, axis=0), ("rep", "fs"))

    grad_down = added(down_pair)
    down_sq = lax.psum(jnp.sum(grad_down * grad_down, axis=1), "fs")
    grad_gate = added(gate_pair)
    grad_up = added(up_pair)
    gate_up_sq = lax.psum(
        jnp.stack([jnp.sum(grad_gate * grad_gate, axis=1), jnp.sum(grad_up * grad_up, axis=1)]),
        "tp",
    )
    return (grad_tokens, grad_gain, grad_gate, grad_up, grad_down, gate_up_sq, down_sq)


CORES = 2
LANES = 128
TILE = 256
PARTS = 4
STEPS = 4


def line_next(z, n_fs, side):
    return z <= n_fs - 2 if side == 0 else z >= 1


def layer_kernel(n_fs, n_tp, *refs):
    tokens, cot, w_gate, w_up, w_down, gain_in = refs[:6]
    o_gate, o_up, o_down, o_tokens, o_gain, o_wide_sq, o_tall_sq = refs[6:13]
    full = refs[13:18]
    x_full, dy_full, f_gate, f_up, f_down = full
    normed, normed_t, hidden_t, act_f, slope_f, d_gate, d_up, inv_all = refs[18:26]
    g_gate, g_up, g_down = refs[26:29]
    pair_wide, pair_tall, sum_wide, sum_tall, x_wide, x_tall, t_wide, t_tall = refs[29:37]
    y_buf, d_buf, z_buf, n_buf = refs[37:41]
    v_gate, v_up, v_down, v_tokens, v_cot, v_normed, v_inv, v_out = refs[41:49]
    lane_sq, row_all, gain_all, wide_all, tall_all = refs[49:54]
    (load_sem, az_own, az_fwd, az_recv, ay_own, ay_fwd, ay_recv, ap_send, ap_recv) = refs[54:63]
    (w_send, w_recv, wx_send, wx_recv, wp_send, wp_recv, wo_send, wo_recv) = refs[63:71]
    (p_send, p_recv, x_send, x_recv, z_send, z_recv, f_send, f_recv) = refs[71:79]
    (y_send, y_recv, d_send, d_recv, n_send, n_recv, own_sem) = refs[79:86]
    (row_send, row_recv, gain_send, gain_recv) = refs[86:90]
    (wide_send, wide_recv, tall_send, tall_recv, out_sem, total, gain_sum) = refs[90:97]
    gain_load, gain, v_wide, v_tall, v_half, relay_sem = refs[97:]
    r, z, t = lax.axis_index("rep"), lax.axis_index("fs"), lax.axis_index("tp")
    y, c = lax.div(t, CORES), lax.rem(t, CORES)
    acts, weights = (tokens, cot), (w_gate, w_up, w_down)
    grads, outs = (g_gate, g_up, g_down), (v_gate, v_up, v_down)
    half, local = tokens.shape[0] // CORES, tokens.shape[1]
    count, model = x_full.shape
    rows = w_gate.shape[0]
    kb = n_fs // CORES
    width = w_gate.shape[1] // kb
    strip = rows // 2
    reach = model // 2
    partner = {"tp": y * CORES + 1 - c}
    across = {"rep": 1 - r}
    beside = {"tp": (1 - y) * CORES + c}
    owner = lax.div(z, kb)

    ends = jnp.logical_or(z == 0, z == n_fs - 1)

    def beyond(side):
        return {"fs": z + 1 if side == 0 else z - 1}

    barrier = pltpu.get_barrier_semaphore()
    close = [partner, across] + [{"tp": (1 - y) * CORES + h} for h in range(CORES)]
    for peer in close:
        pl.semaphore_signal(barrier, inc=1, device_id=peer, device_id_type=MESH)
    for side in range(2):

        @pl.when(line_next(z, n_fs, side))
        def _():
            for h in range(CORES):
                peer = {**beyond(side), "tp": y * CORES + h}
                pl.semaphore_signal(barrier, inc=1, device_id=peer, device_id_type=MESH)

    pl.semaphore_wait(barrier, jnp.where(ends, len(close) + CORES, len(close) + 2 * CORES))

    def tell(side):
        pl.semaphore_signal(
            relay_sem.at[side], inc=1, device_id=beyond(side), device_id_type=MESH
        )

    for side in range(2):

        @pl.when(z == 0 if side == 0 else z == n_fs - 1)
        def _():
            tell(side)

    def greet_far():
        for side in range(2):

            @pl.when(line_next(z, n_fs, 1 - side))
            def _():
                pl.semaphore_wait(relay_sem.at[side], 1)

                @pl.when(line_next(z, n_fs, side))
                def _():
                    tell(side)

    def own_act(a, h):
        return acts[a].at[pl.ds(pl.multiple_of(h * half, half), half), :]

    def act_place(a, source, column):
        return full[a].at[
            pl.ds(pl.multiple_of(source * half, half), half),
            pl.ds(pl.multiple_of(column * local, local), local),
        ]

    sub = half // PARTS

    def own_part(a, h, q):
        start = h * half + q * sub
        return acts[a].at[pl.ds(start, sub), :]

    def act_part(a, source, column, q):
        return full[a].at[
            pl.ds(pl.multiple_of(source * half + q * sub, sub), sub),
            pl.ds(pl.multiple_of(column * local, local), local),
        ]

    def source_of(side, d):
        return z - d if side == 0 else z + d

    def next_of(side):
        return z + 1 if side == 0 else z - 1

    def line_turn(source, at):
        return lax.rem(source - at + n_fs, n_fs) - 1

    def act_first(a, side, h, q):
        return remote(
            own_part(a, h, q),
            act_part(a, z, t, q),
            az_own.at[a, side],
            az_recv.at[a, line_turn(z, next_of(side)), c, q],
            {"fs": next_of(side), "tp": y * CORES + h},
        )

    def act_arrival(a, side, d, core, q):
        place = act_part(a, source_of(side, d), y * CORES + core, q)
        return remote(
            place,
            place,
            az_fwd.at[a],
            az_recv.at[a, line_turn(source_of(side, d), z), core, q],
            partner,
        )

    def act_forward(a, side, d, core, q):
        place = act_part(a, source_of(side, d), y * CORES + core, q)
        return remote(
            place,
            place,
            az_fwd.at[a],
            az_recv.at[a, line_turn(source_of(side, d), next_of(side)), core, q],
            {"fs": next_of(side)},
        )

    def act_over(a, side, d, core, q):
        source = source_of(side, d)
        place = act_part(a, source, y * CORES + core, q)
        return remote(
            place,
            place,
            ay_fwd.at[a],
            ay_recv.at[a],
            {"tp": (1 - y) * CORES + c},
        )

    def act_over_own(a, h):
        return remote(
            own_act(a, h),
            act_place(a, z, t),
            ay_own.at[a],
            ay_recv.at[a],
            {"tp": (1 - y) * CORES + h},
        )

    def act_over_arrivals(a):
        place = full[a].at[:, side_columns(1 - y)]
        return remote(place, place, ay_own.at[a], ay_recv.at[a], partner)

    def act_partner(a):
        return remote(own_act(a, 1 - c), act_place(a, z, t), ap_send.at[a], ap_recv.at[a], partner)

    def act_partner_arrival(a):
        place = act_place(a, z, y * CORES + 1 - c)
        return remote(place, place, ap_send.at[a], ap_recv.at[a], partner)

    def block_of(m, k):
        if m == 2:
            return weights[m].at[pl.ds(pl.multiple_of(k * width, width), width), :]
        return weights[m].at[:, pl.ds(pl.multiple_of(k * width, width), width)]

    def band_of(m, source):
        band = pl.ds(pl.multiple_of(source * rows, rows), rows)
        return full[2 + m].at[:, band] if m == 2 else full[2 + m].at[band, :]

    def quarter(m, source, rep, core):
        if m == 2:
            size = width // (2 * CORES)
            return full[4].at[
                pl.ds(pl.multiple_of((rep * CORES + core) * size, size), size),
                pl.ds(pl.multiple_of(source * rows, rows), rows),
            ]
        size = rows // (2 * CORES)
        start = source * rows + (rep * CORES + core) * size
        return full[2 + m].at[pl.ds(pl.multiple_of(start, size), size), :]

    def own_quarter(m, k, core):
        if m == 2:
            size = width // (2 * CORES)
            start = k * width + (r * CORES + core) * size
            return weights[m].at[pl.ds(pl.multiple_of(start, size), size), :]
        size = rows // (2 * CORES)
        return weights[m].at[
            pl.ds(pl.multiple_of((r * CORES + core) * size, size), size),
            pl.ds(k * width, width),
        ]

    def weight_send(m, k, core):
        return remote(
            own_quarter(m, k, core),
            quarter(m, z, r, core),
            w_send.at[m, k],
            w_recv.at[m, z],
            {"fs": kb * c + k, "tp": y * CORES + core},
        )

    def weight_arrival(m, source):
        place = quarter(m, source, r, c)
        return remote(place, place, wx_send.at[m], w_recv.at[m, source], partner)

    def weight_across(m, source):
        place = quarter(m, source, r, c)
        return remote(place, place, wx_send.at[m], wx_recv.at[m, source], across)

    def weight_across_arrival(m, source):
        place = quarter(m, source, 1 - r, c)
        return remote(place, place, wx_send.at[m], wx_recv.at[m, source], across)

    def weight_beside(m, source, which):
        place = quarter(m, source, r if which == 0 else 1 - r, c)
        return remote(
            place, place, wp_send.at[m], wp_recv.at[m], partner
        )

    def weight_beside_arrivals(m):
        part = (width if m == 2 else rows) // (2 * CORES)
        if m == 2:
            place = full[4].at[pl.ds(0, 2 * part), pl.ds(0, model - rows)]
        else:
            place = full[2 + m].at[pl.ds(0, 2 * (n_fs - 1) * part), :]
        return remote(place, place, wp_send.at[m], wp_recv.at[m], partner)

    def own_beside(m):
        return remote(
            block_of(m, z - kb * owner), band_of(m, z), wo_send.at[m], wo_recv.at[m], partner
        )

    def own_beside_arrival(m):
        return remote(band_of(m, z), band_of(m, z), wo_send.at[m], wo_recv.at[m], partner)

    def slot(wide, tall, m, *where):
        return tall.at[where] if m == 2 else wide.at[(m,) + where]

    def strip_of(band, rep):
        return pl.ds(pl.multiple_of(band * rows + rep * strip, strip), strip)

    def grad_piece(m, band, rep):
        if m == 2:
            return grads[m].at[:, strip_of(band, rep)]
        return grads[m].at[strip_of(band, rep), :]

    def rep_of(j):
        return 1 - r if j == 0 else r

    def pair(m, k, j):
        return remote(
            grad_piece(m, kb * (1 - c) + k, rep_of(j)),
            slot(pair_wide, pair_tall, m, k, j),
            p_send.at[m],
            p_recv.at[m, k, j],
            partner,
        )

    def swap(m, k):
        return remote(
            slot(sum_wide, sum_tall, m, k),
            slot(x_wide, x_tall, m, k),
            x_send.at[m],
            x_recv.at[m, k],
            across,
        )

    def place(m, block, rep):
        strips = pl.ds(pl.multiple_of(rep * strip, strip), strip)
        blocks = pl.ds(pl.multiple_of(block * width, width), width)
        return outs[m].at[blocks, strips] if m == 2 else outs[m].at[strips, blocks]

    def deliver(m, k):
        block = lax.rem(z, kb)
        return remote(
            slot(t_wide, t_tall, m, k),
            place(m, block, r),
            z_send.at[m, k],
            z_recv.at[m, block],
            {"fs": kb * c + k, "tp": y * CORES + owner},
        )

    def delivered(m, k):
        return remote(place(m, k, r), place(m, k, r), z_send.at[m, k], z_recv.at[m, k], partner)

    def keep(m, k):
        return pltpu.make_async_copy(slot(t_wide, t_tall, m, k), place(m, k, r), own_sem.at[m, k])

    def spread(m, k, source):
        return remote(source, place(m, k, r), f_send.at[m], f_recv.at[m, k], across)

    def spread_arrival(m, k):
        return remote(
            place(m, k, 1 - r), place(m, k, 1 - r), f_send.at[m], f_recv.at[m, k], across
        )

    def band_rows(band):
        return pl.ds(pl.multiple_of(band * half, half), half)

    def side_columns(which):
        return pl.ds(pl.multiple_of(which * reach, reach), reach)

    def over(band):
        return remote(
            x_full.at[band_rows(band), side_columns(1 - y)],
            y_buf.at[band],
            y_send.at[0],
            y_recv.at[band],
            beside,
        )

    low = z < n_fs // 2
    inner = jnp.logical_and(z > 0, z < n_fs - 1)
    line_slot = jnp.where(low, 0, 1)

    def line_band(i):
        return jnp.where(low, n_fs - 1 - i, i)

    def y_turn(i):
        return jnp.where(jnp.logical_and(inner, i >= 2), n_fs + 1 - i, i)

    def line_send(i, target):
        band = line_band(i)
        return remote(
            d_buf.at[i],
            z_buf.at[line_slot, band],
            d_send.at[i],
            d_recv.at[line_slot, band],
            {"fs": target},
        )

    def line_arrival(which, band):
        place = z_buf.at[which, band]
        return remote(place, place, d_send.at[0], d_recv.at[which, band], partner)

    def own_rows(core):
        return pl.ds(pl.multiple_of(core * half, half), half)

    def inv_send():
        return remote(inv_all.at[band_rows(z), :], v_inv.at[own_rows(c), :], n_send.at[0], n_recv.at[0], partner)

    def inv_arrival():
        at = v_inv.at[own_rows(1 - c), :]
        return remote(at, at, n_send.at[0], n_recv.at[0], partner)

    def last_send():
        return remote(n_buf, v_normed.at[own_rows(c), :], n_send.at[1], n_recv.at[1], partner)

    def last_arrival():
        at = v_normed.at[own_rows(1 - c), :]
        return remote(at, at, n_send.at[1], n_recv.at[1], partner)

    def loaded(a):
        return pltpu.make_async_copy(own_act(a, c), act_place(a, z, t), load_sem.at[a])

    def block_loaded(m):
        return pltpu.make_async_copy(
            block_of(m, z - kb * owner), band_of(m, z), load_sem.at[2 + m]
        )

    def act_start(a):
        for h in range(CORES):
            for side in range(2):

                @pl.when(line_next(z, n_fs, side))
                def _():
                    for q in range(PARTS):
                        act_first(a, side, h, q).start()

            act_over_own(a, h).start()
        act_partner(a).start()

    def own_start(m):
        @pl.when(c == owner)
        def _():
            own_beside(m).start()

    def act_round(a, d):
        for core in range(CORES):
            for q in range(PARTS):
                for side in range(2):

                    @pl.when(line_receives(z, n_fs, side, d))
                    def _():
                        act_arrival(a, side, d, core, q).wait_recv()
                        if d < n_fs - 1:

                            @pl.when(line_next(z, n_fs, side))
                            def _():
                                act_forward(a, side, d, core, q).start()

                        act_over(a, side, d, core, q).start()

    def weight_start(m):
        for k in range(kb):

            @pl.when(kb * c + k != z)
            def _():
                for core in range(CORES):
                    weight_send(m, k, core).start()

    def weight_round(ms, d):
        for m in ms:
            for side in range(2):

                @pl.when(line_receives(z, n_fs, side, d))
                def _():
                    source = source_of(side, d)
                    weight_arrival(m, source).wait_recv()
                    weight_across(m, source).start()
                    weight_beside(m, source, 0).start()

    def across_round(ms, d):
        for m in ms:
            for side in range(2):

                @pl.when(line_receives(z, n_fs, side, d))
                def _():
                    source = source_of(side, d)
                    weight_across_arrival(m, source).wait_recv()
                    weight_beside(m, source, 1).start()

    def weight_all(m):
        for d in range(1, n_fs):
            weight_round((m,), d)

    def across_all(m):
        for d in range(1, n_fs):
            across_round((m,), d)

    def act_ready(a):
        act_over_arrivals(a).wait_recv()
        act_partner_arrival(a).wait_recv()
        loaded(a).wait()

    def sent(ref, sem):
        remote(ref, ref, sem, sem, partner).wait_send()

    def act_sent(a, landed):
        others = full[a].at[pl.ds(0, count - half), pl.ds(0, CORES * local)]
        if landed:
            sent(others, ay_fwd.at[a])

            @pl.when(inner)
            def _():
                sent(others, az_fwd.at[a])

        if a == 1 or not landed:
            act_partner(a).wait_send()
            sent(acts[a], ay_own.at[a])
            for side in range(2):

                @pl.when(line_next(z, n_fs, side))
                def _():
                    sent(acts[a], az_own.at[a, side])

    def weight_ready(ms):
        for m in ms:
            weight_beside_arrivals(m).wait_recv()

            @pl.when(c == owner)
            def _():
                block_loaded(m).wait()

            @pl.when(c != owner)
            def _():
                own_beside_arrival(m).wait_recv()

    def weight_sent(m):
        size = full[2 + m].shape[0 if m < 2 else 1] - rows
        part = (rows if m < 2 else width) // (2 * CORES)
        if m < 2:
            sent(full[2 + m].at[pl.ds(0, (n_fs - 1) * part), :], wx_send.at[m])
            sent(full[2 + m].at[pl.ds(0, 2 * (n_fs - 1) * part), :], wp_send.at[m])
            half_block = weights[m].at[pl.ds(0, CORES * part), pl.ds(0, width)]
        else:
            sent(full[4].at[pl.ds(0, part), pl.ds(0, size)], wx_send.at[m])
            sent(full[4].at[pl.ds(0, 2 * part), pl.ds(0, size)], wp_send.at[m])
            half_block = weights[m].at[pl.ds(0, CORES * part), :]
        for k in range(kb):

            @pl.when(kb * c + k != z)
            def _():
                sent(half_block, w_send.at[m, k])

        @pl.when(c == owner)
        def _():
            own_beside(m).wait_send()

    def pairs_sent(m):
        span = pl.ds(0, kb * rows)
        sent(g_down.at[:, span] if m == 2 else grads[m].at[span, :], p_send.at[m])

    def swaps_sent(m):
        sent(sum_tall if m == 2 else sum_wide.at[m], x_send.at[m])

    def spreads_sent(m):
        sent(sum_tall if m == 2 else sum_wide.at[m], f_send.at[m])

    def over_sent():
        sent(x_full.at[:, side_columns(1 - y)], y_send.at[0])

    def tile(i, size):
        return pl.ds(pl.multiple_of(i * size, size), size)

    def normalize(i):
        at = tile(i, LANES)
        wide = x_full[at, :].astype(jnp.float32)
        inv = lax.rsqrt(jnp.mean(wide * wide, axis=-1, keepdims=True) + 1e-06)
        value = wide * inv * gain[...]
        normed[at, :] = value.astype(jnp.bfloat16)
        normed_t[:, at] = value.T.astype(jnp.bfloat16)
        inv_all[at, :] = jnp.broadcast_to(inv, (LANES, LANES))

    def forward(i):
        at = tile(i, TILE)
        gate = jnp.dot(normed[at, :], f_gate[...], preferred_element_type=jnp.float32)
        up = jnp.dot(normed[at, :], f_up[...], preferred_element_type=jnp.float32)
        sigma = jax.nn.sigmoid(gate)
        active = gate * sigma
        act_f[at, :] = active
        slope_f[at, :] = up * sigma * (1.0 + gate * (1.0 - sigma))
        hidden_t[:, at] = (active * up).T.astype(jnp.bfloat16)

    def backward(i):
        at = tile(i, TILE)
        back = 0.5 * contract_last(dy_full[at, :], f_down[...])
        d_up[at, :] = (back * act_f[at, :]).astype(jnp.bfloat16)
        d_gate[at, :] = (back * slope_f[at, :]).astype(jnp.bfloat16)

    def gradient(m, own, j, k):
        band = kb * (c if own else 1 - c) + k
        at = strip_of(band, 1 - r if j == 0 else r)
        if m == 2:
            value = 0.5 * jnp.dot(
                hidden_t[...], dy_full[:, at], preferred_element_type=jnp.float32
            )
            g_down[:, at] = value.astype(jnp.bfloat16)
        else:
            right = d_gate if m == 0 else d_up
            value = jnp.dot(normed_t[at, :], right[...], preferred_element_type=jnp.float32)
            grads[m][at, :] = value.astype(jnp.bfloat16)

    def gradients(m, j):
        @pl.loop(0, kb)
        def _(k):
            gradient(m, False, j, k)
            pair(m, k, j).start()

        @pl.loop(0, kb)
        def _(k):
            gradient(m, True, j, k)

    def pull_back(band, which):
        at, columns = band_rows(band), side_columns(which)
        value = contract_last(d_gate[at, :], f_gate[columns, :])
        value = value + contract_last(d_up[at, :], f_up[columns, :])
        x_full[at, columns] = value.astype(jnp.bfloat16)

    def added(m, k, j):
        own = grad_piece(m, kb * c + k, rep_of(j))[...].astype(jnp.float32)
        return own + slot(pair_wide, pair_tall, m, k, j)[...].astype(jnp.float32)

    def put(wide, tall, m, k, value):
        if m == 2:
            tall[k] = value
        else:
            wide[m, k] = value

    def first(m, k):
        pair(m, k, 0).wait_recv()
        put(sum_wide, sum_tall, m, k, added(m, k, 0).astype(jnp.bfloat16))
        swap(m, k).start()

    def second(m, k):
        pair(m, k, 1).wait_recv()
        swap(m, k).wait_recv()
        whole = added(m, k, 1) + slot(x_wide, x_tall, m, k)[...].astype(jnp.float32)
        put(t_wide, t_tall, m, k, whole.astype(jnp.bfloat16))
        mine = kb * c + k == z

        @pl.when(mine)
        def _():
            keep(m, k).start()
            spread(m, k, slot(t_wide, t_tall, m, k)).start()

        @pl.when(jnp.logical_not(mine))
        def _():
            deliver(m, k).start()

    def third(m, k):
        @pl.when(kb * c + k != z)
        def _():
            delivered(m, k).wait_recv()
            spread(m, k, place(m, k, r)).start()

    def own_share(band):
        over(band).wait_recv()
        own = x_full[band_rows(band), side_columns(y)].astype(jnp.float32)
        return own + y_buf[band].astype(jnp.float32)

    def line_target(i):
        if i == n_fs - 1:
            return jnp.where(low, z - 1, z + 1)
        return line_band(i)

    def normed_outer(i):
        @pl.when(jnp.logical_not(inner))
        def _():
            d_buf[i] = own_share(line_band(i)).astype(jnp.bfloat16)
            line_send(i, jnp.where(low, z + 1, z - 1)).start()

    def normed_inner(i):
        @pl.when(inner)
        def _():
            band = line_band(i)
            value = own_share(band)
            if i < n_fs - 1:
                line_arrival(line_slot, band).wait_recv()
                value = value + z_buf[line_slot, band].astype(jnp.float32)
            d_buf[i] = value.astype(jnp.bfloat16)
            line_send(i, line_target(i)).start()

    def normed_sent():
        for i in range(n_fs):
            if i < n_fs - 1:

                @pl.when(jnp.logical_not(inner))
                def _():
                    line_send(i, jnp.where(low, z + 1, z - 1)).wait_send()

            if i != n_fs - 2:

                @pl.when(inner)
                def _():
                    line_send(i, line_target(i)).wait_send()

    def normed_last():
        value = own_share(z)
        for which in range(2):
            line_arrival(which, z).wait_recv()
            value = value + z_buf[which, z].astype(jnp.float32)
        total[...] = value

        for core in range(CORES):

            @pl.when(c == core)
            def _():
                mine = slice(core * local, (core + 1) * local)
                theirs = slice((1 - core) * local, (2 - core) * local)
                v_normed[core * half : (core + 1) * half, :] = total[:, mine].astype(jnp.bfloat16)
                n_buf[...] = total[:, theirs].astype(jnp.bfloat16)

        last_send().start()

    def fold(value):
        out = value[:, :LANES]
        for i in range(1, value.shape[1] // LANES):
            out = out + value[:, i * LANES : (i + 1) * LANES]
        return out

    def row_of(value):
        return jnp.sum(value.T, axis=0, keepdims=True)

    def lane_peer(j):
        return {"tp": lax.rem(t + j, n_tp)}

    def group_peer(j):
        at = lax.rem(r * n_fs + z + j, 2 * n_fs)
        return {"rep": lax.div(at, n_fs), "fs": lax.rem(at, n_fs)}

    def fan(buffer, count_of, mine, send, recv, peer):
        def start():
            for j in range(1, count_of):
                place = buffer.at[mine]
                remote(place, place, send.at[0], recv.at[0], peer(j)).start()

        def others():
            place = buffer.at[pl.ds(0, count_of - 1)]
            return remote(place, place, send.at[0], recv.at[0], partner)

        return start, others

    row_fan = fan(row_all, n_tp, t, row_send, row_recv, lane_peer)
    wide_fan = fan(wide_all, n_tp, t, wide_send, wide_recv, lane_peer)
    gain_fan = fan(gain_all, 2 * n_fs, r * n_fs + z, gain_send, gain_recv, group_peer)
    tall_fan = fan(tall_all, 2 * n_fs, r * n_fs + z, tall_send, tall_recv, group_peer)

    def gain_here():
        return gain[:, pl.ds(pl.multiple_of(t * local, local), local)]

    def token_sums():
        last_arrival().wait_recv()
        inv_arrival().wait_recv()
        for i in range(2):
            own_loaded(i).wait()
        gain_l = gain_here()
        gain_sum[...] = jnp.zeros_like(gain_sum)

        @pl.loop(0, CORES * half // LANES)
        def _(i):
            at = tile(i, LANES)
            d_tokens = v_normed[at, :].astype(jnp.float32) * v_tokens[at, :].astype(jnp.float32)
            row_all[t, :, at] = row_of(fold(d_tokens * gain_l))
            inv = v_inv[at, :1]
            gain_sum[...] += jnp.sum(d_tokens * inv, axis=0, keepdims=True)

        gain_all[r * n_fs + z] = gain_sum[...]
        row_fan[0]()
        gain_fan[0]()

    def token_grads():
        row_fan[1]().wait_recv()
        gain_l = gain_here()

        @pl.loop(0, CORES * half // LANES)
        def _(i):
            at = tile(i, LANES)
            dots = row_all[0, :, at]
            for j in range(1, n_tp):
                dots = dots + row_all[j, :, at]
            rowdot = jnp.broadcast_to(dots, (LANES, LANES)).T[:, :1]
            inv = v_inv[at, :1]
            value = v_cot[at, :].astype(jnp.float32)
            value = value + inv * (v_normed[at, :].astype(jnp.float32) * gain_l)
            scale = inv**3 * rowdot / model
            value = value - v_tokens[at, :].astype(jnp.float32) * scale
            v_out[at, :] = value.astype(jnp.bfloat16)

        pltpu.make_async_copy(v_out, o_tokens, out_sem.at[3]).start()

    def own_loaded(i):
        source, target = ((tokens, v_tokens), (cot, v_cot))[i]
        return pltpu.make_async_copy(source, target, load_sem.at[5 + i])

    def block_out(m, k):
        at = pl.ds(k * width, width)
        if m == 2:
            return pltpu.make_async_copy(v_down.at[at, :], o_down.at[at, :], out_sem.at[m])
        return pltpu.make_async_copy(
            outs[m].at[:, at], (o_gate, o_up)[m].at[:, at], out_sem.at[m]
        )

    def strip_squares(m, k):
        @pl.when(kb * c + k == z)
        def _():
            keep(m, k).wait()

        if m == 2:
            columns = pl.ds(pl.multiple_of(r * strip, strip), strip)

            @pl.loop(0, width // LANES)
            def _(i):
                at = pl.ds(pl.multiple_of(k * width + i * LANES, LANES), LANES)
                value = v_down[at, columns].astype(jnp.float32)
                tall_all[r * n_fs + z, :, at] = row_of(fold(value * value))
        else:

            @pl.loop(0, strip // LANES)
            def _(i):
                at = tile(i, LANES)
                from_row = pl.ds(pl.multiple_of(r * strip + i * LANES, LANES), LANES)
                value = outs[m][from_row, k * width : (k + 1) * width].astype(jnp.float32)
                part = fold(value * value)
                if k > 0:
                    part = part + lane_sq[m, at, :]
                if k < kb - 1:
                    lane_sq[m, at, :] = part
                else:
                    wide_all[t, m : m + 1, at] = row_of(part)

    def wide_cross():
        strips = pl.ds(pl.multiple_of(r * strip, strip), strip)
        return remote(v_half, v_wide.at[:, strips], n_send.at[2], n_recv.at[2], across)

    def wide_cross_arrival():
        place = v_wide.at[:, pl.ds(pl.multiple_of((1 - r) * strip, strip), strip)]
        return remote(place, place, n_send.at[2], n_recv.at[2], across)

    def summed(buffer, count_of):
        value = buffer[0]
        for j in range(1, count_of):
            value = value + buffer[j]
        return value

    def whole_block(m, k):
        spread_arrival(m, k).wait_recv()
        block_out(m, k).start()

    gain_copy = pltpu.make_async_copy(gain_in, gain_load, out_sem.at[4])
    gain_copy.start()
    for a in range(2):
        loaded(a).start()

    @pl.when(c == owner)
    def _():
        for m in range(3):
            block_loaded(m).start()

    act_start(0)
    own_start(0)
    own_start(1)
    for i in range(2):
        own_loaded(i).start()
    act_round(0, 1)
    greet_far()
    act_round(0, 2)
    weight_start(0)
    weight_start(1)
    act_start(1)
    own_start(2)
    for d in range(3, n_fs):
        act_round(0, d)
    weight_all(0)
    act_round(1, 1)
    weight_all(1)
    across_all(0)
    gain_copy.wait()
    for i in range(model // LANES):
        gain[:, i * LANES : (i + 1) * LANES] = gain_load[i : i + 1, :].astype(jnp.float32)
    act_ready(0)
    pl.loop(0, count // LANES)(normalize)
    inv_send().start()
    v_inv[own_rows(c), :] = inv_all[band_rows(z), :]
    weight_start(2)
    across_all(1)
    act_round(1, 2)
    weight_ready((0, 1))
    pl.loop(0, count // TILE)(forward)
    weight_all(2)
    for d in range(3, n_fs):
        act_round(1, d)
    across_all(2)
    act_ready(1)
    for k in range(kb):
        gradient(2, False, 0, k)
        pair(2, k, 0).start()
        if k:
            first(2, k - 1)
        gradient(2, True, 0, k)
    first(2, kb - 1)
    gradients(2, 1)
    weight_ready((2,))
    pl.loop(0, count // TILE)(backward)
    act_sent(0, True)

    gradients(0, 0)
    for k in range(kb):
        first(0, k)

    @pl.loop(0, n_fs)
    def _(i):
        band = line_band(y_turn(i))
        pull_back(band, 1 - y)
        over(band).start()

    gradients(1, 0)
    for k in range(kb):
        first(1, k)
    gradients(0, 1)
    for k in range(kb):
        second(2, k)

    @pl.loop(0, n_fs)
    def _(i):
        pull_back(i, y)

    gradients(1, 1)
    second(0, 0)
    normed_outer(0)
    second(0, 1)
    third(2, 0)
    third(2, 1)
    normed_outer(1)
    second(1, 0)
    normed_inner(n_fs - 1)
    normed_inner(0)
    second(1, 1)
    normed_outer(2)
    third(0, 0)
    third(0, 1)
    normed_inner(1)
    for k in range(kb):
        strip_squares(2, k)
    tall_fan[0]()
    for k in range(kb):
        strip_squares(0, k)
    third(1, 0)
    strip_squares(1, 0)
    third(1, 1)
    strip_squares(1, 1)
    wide_fan[0]()
    normed_last()
    whole_block(2, 0)
    whole_block(2, 1)
    token_sums()
    wide_fan[1]().wait_recv()
    v_half[...] = summed(wide_all, n_tp)
    wide_cross().start()
    v_wide[:, pl.ds(pl.multiple_of(r * strip, strip), strip)] = v_half[...]
    tall_fan[1]().wait_recv()
    v_tall[...] = summed(tall_all, 2 * n_fs)
    tall_out = pltpu.make_async_copy(v_tall, o_tall_sq, out_sem.at[6])
    tall_out.start()
    token_grads()
    whole_block(0, 0)
    whole_block(0, 1)
    act_sent(0, False)
    act_sent(1, True)
    for m in range(3):
        weight_sent(m)
    over_sent()
    normed_sent()
    inv_send().wait_send()
    last_send().wait_send()
    row_fan[1]().wait_send()
    wide_fan[1]().wait_send()
    for m in range(3):
        pairs_sent(m)
        swaps_sent(m)
        for k in range(kb):

            @pl.when(kb * c + k != z)
            def _():
                deliver(m, k).wait_send()

    whole_block(1, 0)
    gain_fan[1]().wait_recv()
    gain_sum[...] = summed(gain_all, 2 * n_fs)
    gain_out = pltpu.make_async_copy(gain_sum, o_gain, out_sem.at[5])
    gain_out.start()
    wide_cross_arrival().wait_recv()
    wide_out = pltpu.make_async_copy(v_wide, o_wide_sq, out_sem.at[7])
    wide_out.start()
    whole_block(1, 1)
    wide_cross().wait_send()
    gain_fan[1]().wait_send()
    tall_fan[1]().wait_send()
    gain_out.wait()
    tall_out.wait()
    wide_out.wait()
    pltpu.make_async_copy(v_out, o_tokens, out_sem.at[3]).wait()
    for m in range(3):
        spreads_sent(m)
        pltpu.make_async_copy(outs[m], (o_gate, o_up, o_down)[m], out_sem.at[m]).wait()


def layer(n_fs, n_tp, tokens, cot, w_gate, w_up, w_down, gain):
    half, local = tokens.shape[0] // CORES, tokens.shape[1]
    rows, hidden = w_gate.shape
    width = hidden * CORES // n_fs
    model = rows * n_fs
    count = half * n_fs
    dtype = tokens.dtype
    kb = n_fs // CORES
    strip = rows // 2
    reach = model // 2
    wide, tall = (strip, width), (width, strip)
    dma = pltpu.SemaphoreType.DMA
    hbm = pl.BlockSpec(memory_space=pl.ANY)
    pairs, singles = dma((3, kb, 2)), dma((3, kb))

    def bf(*shape):
        return pltpu.VMEM(shape, dtype)

    def f32(*shape):
        return pltpu.VMEM(shape, jnp.float32)

    hidden = kb * width
    shapes = [(rows, hidden)] * 2 + [(hidden, rows)]
    return pl.pallas_call(
        functools.partial(layer_kernel, n_fs, n_tp),
        out_shape=[jax.ShapeDtypeStruct(s, dtype) for s in shapes]
        + [jax.ShapeDtypeStruct((CORES * half, local), dtype)]
        + [jax.ShapeDtypeStruct(s, jnp.float32) for s in ((1, local), (2, rows), (1, hidden))],
        in_specs=[hbm] * 6,
        out_specs=[hbm] * 7,
        scratch_shapes=[
            bf(count, model),
            bf(count, model),
            bf(model, width),
            bf(model, width),
            bf(width, model),
            bf(count, model),
            bf(model, count),
            bf(width, count),
            f32(count, width),
            f32(count, width),
            bf(count, width),
            bf(count, width),
            f32(count, LANES),
            bf(model, width),
            bf(model, width),
            bf(width, model),
            bf(2, kb, 2, *wide),
            bf(kb, 2, *tall),
            bf(2, kb, *wide),
            bf(kb, *tall),
            bf(2, kb, *wide),
            bf(kb, *tall),
            bf(2, kb, *wide),
            bf(kb, *tall),
            bf(n_fs, half, reach),
            bf(n_fs, half, reach),
            bf(2, n_fs, half, reach),
            bf(half, local),
            bf(rows, hidden),
            bf(rows, hidden),
            bf(hidden, rows),
            bf(CORES * half, local),
            bf(CORES * half, local),
            bf(CORES * half, local),
            f32(CORES * half, LANES),
            bf(CORES * half, local),
            f32(2, strip, LANES),
            f32(n_tp, 1, CORES * half),
            f32(2 * n_fs, 1, local),
            f32(n_tp, 2, strip),
            f32(2 * n_fs, 1, hidden),
            dma((7,)),
            dma((2, 2)),
            dma((2,)),
            dma((2, n_fs - 1, CORES, PARTS)),
            dma((2,)),
            dma((2,)),
            dma((2,)),
            dma((2,)),
            dma((2,)),
            dma((3, kb)),
            dma((3, n_fs)),
            dma((3,)),
            dma((3, n_fs)),
            dma((3,)),
            dma((3,)),
            dma((3,)),
            dma((3,)),
            dma((3,)),
            pairs,
            dma((3,)),
            singles,
            singles,
            singles,
            dma((3,)),
            singles,
            dma((1,)),
            dma((n_fs,)),
            dma((n_fs,)),
            dma((2, n_fs)),
            dma((3,)),
            dma((3,)),
            dma((3, kb)),
            dma((1,)),
            dma((1,)),
            dma((1,)),
            dma((1,)),
            dma((1,)),
            dma((1,)),
            dma((1,)),
            dma((1,)),
            dma((8,)),
            f32(half, reach),
            f32(1, local),
            bf(model // LANES, LANES),
            f32(1, model),
            f32(2, rows),
            f32(1, hidden),
            f32(2, strip),
            pltpu.SemaphoreType.REGULAR((2,)),
        ],
        compiler_params=pltpu.CompilerParams(
            collective_id=4, has_side_effects=True, vmem_limit_bytes=67043328
        ),
        name="layer",
    )(tokens, cot, w_gate, w_up, w_down, gain)


def widen_kernel(n, *refs):
    sources, targets = refs[:n], refs[n : 2 * n]
    narrow, wide = refs[2 * n : 3 * n], refs[3 * n : 3 * n + 3]
    flat, load_sem, store_sem = refs[3 * n + 3 : -2], *refs[-2:]

    def rows_of(i, step):
        size = sources[i].shape[0] // STEPS
        return pl.ds(step * size, size)

    def load(i, step):
        at = rows_of(i, step)
        return pltpu.make_async_copy(sources[i].at[at], narrow[i].at[at], load_sem.at[i, step])

    def store(i, step):
        at = rows_of(i, step)
        return pltpu.make_async_copy(wide[i].at[at], targets[i].at[at], store_sem.at[i, step])

    def load_whole(i):
        return pltpu.make_async_copy(sources[i], narrow[i], load_sem.at[i, 0])

    def store_whole(i):
        source = {4: flat[0], 6: flat[1]}.get(i, narrow[i])
        return pltpu.make_async_copy(source, targets[i], store_sem.at[i, 0])

    for i in range(3, n):
        load_whole(i).start()
    for step in range(STEPS):
        for i in range(3):
            load(i, step).start()
    for i in range(3, n):
        load_whole(i).wait()
        if i in (4, 6):
            flat[(i - 4) // 2][...] = narrow[i][0, :]
        store_whole(i).start()
    for step in range(STEPS):
        for i in range(3):
            load(i, step).wait()
            at = rows_of(i, step)
            wide[i][at] = narrow[i][at].astype(jnp.float32)
            store(i, step).start()
    for step in range(STEPS):
        for i in range(3):
            store(i, step).wait()
    for i in range(3, n):
        store_whole(i).wait()


def widen(*arrays):
    n = len(arrays)
    hbm = pl.BlockSpec(memory_space=pl.ANY)
    shapes = [a.shape[1:] if a.shape[0] == 1 else a.shape for a in arrays]
    kinds = [jnp.float32] * 3 + [a.dtype for a in arrays[3:]]
    dma = pltpu.SemaphoreType.DMA
    return pl.pallas_call(
        functools.partial(widen_kernel, n),
        out_shape=[jax.ShapeDtypeStruct(s, k) for s, k in zip(shapes, kinds)],
        in_specs=[hbm] * n,
        out_specs=[hbm] * n,
        scratch_shapes=[pltpu.VMEM(a.shape, a.dtype) for a in arrays]
        + [pltpu.VMEM(a.shape, jnp.float32) for a in arrays[:3]]
        + [pltpu.VMEM(s, jnp.float32) for s in (shapes[4], shapes[6])]
        + [dma((n, STEPS)), dma((n, STEPS))],
        name="widen",
    )(*arrays)


def by_chip(tokens, norm_gain, w_gate, w_up, w_down, cotangent):
    found = layer(
        lax.axis_size("fs"),
        lax.axis_size("tp"),
        tokens,
        cotangent,
        w_gate,
        w_up,
        w_down,
        norm_gain.reshape(-1, LANES),
    )
    grad_gate, grad_up, grad_down, grad_tokens, grad_gain, gate_up_sq, down_sq = widen(*found)
    return (grad_tokens, grad_gain, grad_gate, grad_up, grad_down, gate_up_sq, down_sq)


def fits_chips(mesh):
    n_rep, n_fs, n_tp = mesh.shape["rep"], mesh.shape["fs"], mesh.shape["tp"]
    return n_rep == 2 and n_tp == 2 * CORES and n_fs == 2 * CORES


def solution(mesh):
    placed = (
        P(("rep", "fs"), "tp"),
        P(),
        P("fs", "tp"),
        P("fs", "tp"),
        P("tp", "fs"),
        P(("rep", "fs"), "tp"),
    )
    return jax.shard_map(
        by_chip if fits_chips(mesh) else on_device,
        mesh=mesh,
        in_specs=placed,
        out_specs=(
            P(("rep", "fs"), "tp"),
            P("tp"),
            P("fs", "tp"),
            P("fs", "tp"),
            P("tp", "fs"),
            P(None, "fs"),
            P("tp"),
        ),
        check_vma=False,
    )
```

```python
import functools

import jax
import jax.numpy as jnp
from jax import lax
from jax.experimental import pallas as pl
from jax.experimental.pallas import tpu as pltpu
from jax.sharding import PartitionSpec as P

MESH = pl.DeviceIdType.MESH


def contract_last(left, right):
    return lax.dot_general(
        left, right, (((1,), (1,)), ((), ())), preferred_element_type=jnp.float32
    )


def contract_first(left, right):
    return lax.dot_general(
        left, right, (((0,), (0,)), ((), ())), preferred_element_type=jnp.float32
    )


def remote(source, target, send_sem, recv_sem, where):
    return pltpu.make_async_remote_copy(
        src_ref=source,
        dst_ref=target,
        send_sem=send_sem,
        recv_sem=recv_sem,
        device_id=where,
        device_id_type=MESH,
    )


def line_sends(z, n_fs, side, d):
    if side == 0:
        return jnp.logical_and(z >= d - 1, z <= n_fs - 2)
    return jnp.logical_and(z + d <= n_fs, z >= 1)


def line_receives(z, n_fs, side, d):
    return z >= d if side == 0 else z + d <= n_fs - 1


def greet(peers):
    barrier = pltpu.get_barrier_semaphore()
    for peer in peers:
        pl.semaphore_signal(barrier, inc=1, device_id=peer, device_id_type=MESH)
    pl.semaphore_wait(barrier, len(peers))


def keep_own(sources, holders, targets, sems):
    count = len(sources)
    loads = [
        pltpu.make_async_copy(sources[i], holders[i], sems.at[0, i]) for i in range(count)
    ]
    stores = [
        pltpu.make_async_copy(holders[i], targets[i], sems.at[1, i]) for i in range(count)
    ]
    for load in loads:
        load.start()

    def finish():
        for load, store in zip(loads, stores):
            load.wait()
            store.start()
        for store in stores:
            store.wait()

    return finish


def weights_kernel(n_fs, n_tp, *refs):
    tokens, cot, w_gate, w_up, w_down = refs[:5]
    whole_x, whole_dy, full_gate, full_up, full_down = refs[5:10]
    holders = refs[10:15]
    own_sem, ring_send, ring_recv, rep_send, rep_recv, tp_send, tp_recv = refs[15:]
    r, z, t = lax.axis_index("rep"), lax.axis_index("fs"), lax.axis_index("tp")
    right, left = lax.rem(z + 1, n_fs), lax.rem(z + n_fs - 1, n_fs)
    partner = {"rep": 1 - r}
    sources = (w_gate, w_up, w_down)
    targets = (full_gate, full_up, full_down)
    rows = w_gate.shape[0]
    hidden = w_down.shape[0]
    local = tokens.shape[1]

    def own_piece(m, half):
        size = (hidden if m == 2 else rows) // 2
        return sources[m].at[pl.ds(pl.multiple_of(half * size, size), size), :]

    def piece(m, owner, half):
        if m == 2:
            size = hidden // 2
            return targets[m].at[
                pl.ds(pl.multiple_of(half * size, size), size),
                pl.ds(pl.multiple_of(owner * rows, rows), rows),
            ]
        size = rows // 2
        return targets[m].at[
            pl.ds(pl.multiple_of(owner * rows + half * size, size), size), :
        ]

    peers = [{"fs": right}, {"fs": left}, partner]
    peers += [{"tp": lax.rem(t + j, n_tp)} for j in range(1, n_tp)]
    greet(peers)

    def owner_of(side, back):
        return lax.rem(z + (n_fs - back if side == 0 else back), n_fs)

    def hop(m, side, d):
        place = piece(m, owner_of(side, d - 1), r)
        return remote(
            own_piece(m, r) if d == 1 else place,
            place,
            ring_send.at[m, side, d - 1],
            ring_recv.at[m, side, d - 1],
            {"fs": right if side == 0 else left},
        )

    def arrival(m, side, d):
        place = piece(m, owner_of(side, d), r)
        return remote(
            place,
            place,
            ring_send.at[m, side, d - 1],
            ring_recv.at[m, side, d - 1],
            {"fs": right if side == 0 else left},
        )

    def across(m, side, d):
        place = piece(m, owner_of(side, d), r)
        return remote(
            place, place, rep_send.at[m, side, d - 1], rep_recv.at[m, side, d - 1], partner
        )

    for m in range(3):
        for side in range(2):

            @pl.when(line_sends(z, n_fs, side, 1))
            def _():
                hop(m, side, 1).start()

    ends = []
    for a, (source, target) in enumerate(((tokens, whole_x), (cot, whole_dy))):
        place = target.at[:, pl.ds(pl.multiple_of(t * local, local), local)]
        for j in range(1, n_tp):
            copy = remote(
                source,
                place,
                tp_send.at[a, j - 1],
                tp_recv.at[a, j - 1],
                {"tp": lax.rem(t + j, n_tp)},
            )
            copy.start()
            ends.append(copy)
    mine = pl.ds(pl.multiple_of(t * local, local), local)
    band = pl.ds(pl.multiple_of(z * rows, rows), rows)
    finish = keep_own(
        (tokens, cot, w_gate, w_up, w_down),
        holders,
        (
            whole_x.at[:, mine],
            whole_dy.at[:, mine],
            full_gate.at[band, :],
            full_up.at[band, :],
            full_down.at[:, band],
        ),
        own_sem,
    )
    finish()
    for d in range(1, n_fs):
        for m in range(3):
            for side in range(2):

                @pl.when(line_receives(z, n_fs, side, d))
                def _():
                    arrival(m, side, d).wait_recv()
                    if d < n_fs - 1:

                        @pl.when(line_sends(z, n_fs, side, d + 1))
                        def _():
                            hop(m, side, d + 1).start()

                    across(m, side, d).start()

    for d in range(1, n_fs):
        for m in range(3):
            for side in range(2):

                @pl.when(line_sends(z, n_fs, side, d))
                def _():
                    hop(m, side, d).wait_send()

                @pl.when(line_receives(z, n_fs, side, d))
                def _():
                    across(m, side, d).wait()

    for copy in ends:
        copy.wait()


def gather_weights(n_fs, n_tp, tokens, cot, w_gate, w_up, w_down):
    count, local = tokens.shape
    rows, hidden = w_gate.shape
    width = rows * n_fs
    dtype = tokens.dtype
    shapes = [
        (count, width),
        (count, width),
        (width, hidden),
        (width, hidden),
        (hidden, width),
    ]
    held = (tokens, cot, w_gate, w_up, w_down)
    moved = sum(2 * a * b for a, b in shapes)
    dma = pltpu.SemaphoreType.DMA
    return pl.pallas_call(
        functools.partial(weights_kernel, n_fs, n_tp),
        out_shape=[jax.ShapeDtypeStruct(s, dtype) for s in shapes],
        in_specs=[pl.BlockSpec(memory_space=pl.ANY)] * 5,
        out_specs=[pl.BlockSpec(memory_space=pl.ANY)] * 5,
        scratch_shapes=[pltpu.VMEM(a.shape, a.dtype) for a in held]
        + [
            dma((2, 5)),
            dma((3, 2, n_fs - 1)),
            dma((3, 2, n_fs - 1)),
            dma((3, 2, n_fs - 1)),
            dma((3, 2, n_fs - 1)),
            dma((2, n_tp - 1)),
            dma((2, n_tp - 1)),
        ],
        compiler_params=pltpu.CompilerParams(collective_id=0, has_side_effects=True),
        cost_estimate=pl.CostEstimate(flops=0, bytes_accessed=16 * moved, transcendentals=0),
        name="gather_weights",
    )(*held)


def tokens_kernel(n_fs, n_tp, n_act, n_swap, *refs):
    total = n_act + n_swap
    acts, swaps = refs[:n_act], refs[n_act:total]
    act_outs, swap_outs = refs[total : total + n_act], refs[total + n_act : 2 * total]
    holders = refs[2 * total : 3 * total]
    own_sem, ring_send, ring_recv = refs[3 * total : 3 * total + 3]
    swap_send, swap_recv, relay_send, relay_recv = refs[3 * total + 3 :]
    z, t = lax.axis_index("fs"), lax.axis_index("tp")
    right, left = lax.rem(z + 1, n_fs), lax.rem(z + n_fs - 1, n_fs)
    count = acts[0].shape[0]
    peers = [{"fs": lax.rem(z + j, n_fs)} for j in range(1, n_fs)]
    if n_swap:
        peers += [{"tp": lax.rem(t + j, n_tp)} for j in range(1, n_tp)]
    greet(peers)

    def rows_of(owner):
        return pl.ds(pl.multiple_of(owner * count, count), count)

    def owner_of(side, back):
        return lax.rem(z + (n_fs - back if side == 0 else back), n_fs)

    def hop(m, side, d):
        place = act_outs[m].at[rows_of(owner_of(side, d - 1)), :]
        return remote(
            acts[m] if d == 1 else place,
            place,
            ring_send.at[m, side, d - 1],
            ring_recv.at[m, side, d - 1],
            {"fs": right if side == 0 else left},
        )

    def arrival(m, side, d):
        place = act_outs[m].at[rows_of(owner_of(side, d)), :]
        return remote(
            place,
            place,
            ring_send.at[m, side, d - 1],
            ring_recv.at[m, side, d - 1],
            {"fs": right if side == 0 else left},
        )

    def swap(a, j):
        peer = lax.rem(z + j, n_fs)
        cut = swap_outs[a].shape[1]
        return remote(
            swaps[a].at[:, pl.ds(pl.multiple_of(peer * cut, cut), cut)],
            swap_outs[a].at[rows_of(z), :],
            swap_send.at[a, j - 1],
            swap_recv.at[a, j - 1],
            {"fs": peer},
        )

    def swapped(a, j):
        place = swap_outs[a].at[rows_of(owner_of(0, j)), :]
        return remote(
            place,
            place,
            swap_send.at[a, j - 1],
            swap_recv.at[a, j - 1],
            {"fs": lax.rem(z + j, n_fs)},
        )

    def relay(a, j, k):
        place = swap_outs[a].at[rows_of(owner_of(0, j)), :]
        return remote(
            place,
            place,
            relay_send.at[a, j - 1, k - 1],
            relay_recv.at[a, j - 1],
            {"tp": lax.rem(t + k, n_tp)},
        )

    hub = lax.rem(z, n_tp) == t

    def feeds(j):
        return lax.rem(lax.rem(z + j, n_fs), n_tp) == t

    for a in range(n_swap):
        for j in range(1, n_fs):

            @pl.when(feeds(j))
            def _():
                swap(a, j).start()

    for m in range(n_act):
        for side in range(2):

            @pl.when(line_sends(z, n_fs, side, 1))
            def _():
                hop(m, side, 1).start()

    sources = list(acts)
    for a in range(n_swap):
        cut = swap_outs[a].shape[1]
        sources.append(swaps[a].at[:, pl.ds(pl.multiple_of(z * cut, cut), cut)])
    finish = keep_own(
        sources, holders, [out.at[rows_of(z), :] for out in act_outs + swap_outs], own_sem
    )
    finish()
    if n_swap:

        @pl.when(hub)
        def _():
            for a in range(n_swap):
                for j in range(1, n_fs):
                    swapped(a, j).wait_recv()
                    for k in range(1, n_tp):
                        relay(a, j, k).start()

    for d in range(1, n_fs):
        for m in range(n_act):
            for side in range(2):

                @pl.when(line_receives(z, n_fs, side, d))
                def _():
                    arrival(m, side, d).wait_recv()
                    if d < n_fs - 1:

                        @pl.when(line_sends(z, n_fs, side, d + 1))
                        def _():
                            hop(m, side, d + 1).start()

    for d in range(1, n_fs):
        for m in range(n_act):
            for side in range(2):

                @pl.when(line_sends(z, n_fs, side, d))
                def _():
                    hop(m, side, d).wait_send()

    for a in range(n_swap):
        for j in range(1, n_fs):

            @pl.when(feeds(j))
            def _():
                swap(a, j).wait_send()

            @pl.when(hub)
            def _():
                for k in range(1, n_tp):
                    relay(a, j, k).wait_send()

            @pl.when(jnp.logical_not(hub))
            def _():
                relay(a, j, 1).wait_recv()


def gather_tokens(n_fs, n_tp, collective_id, acts, swaps):
    count = acts[0].shape[0]
    outs = [jax.ShapeDtypeStruct((n_fs * count, a.shape[1]), a.dtype) for a in acts]
    outs += [jax.ShapeDtypeStruct((n_fs * count, a.shape[1] // n_fs), a.dtype) for a in swaps]
    dma = pltpu.SemaphoreType.DMA
    total = len(outs)
    n_swap = max(len(swaps), 1)
    moved = sum(2 * o.shape[0] * o.shape[1] for o in outs)
    return pl.pallas_call(
        functools.partial(tokens_kernel, n_fs, n_tp, len(acts), len(swaps)),
        out_shape=outs,
        in_specs=[pl.BlockSpec(memory_space=pl.ANY)] * total,
        out_specs=[pl.BlockSpec(memory_space=pl.ANY)] * total,
        scratch_shapes=[pltpu.VMEM((count, o.shape[1]), o.dtype) for o in outs]
        + [
            dma((2, total)),
            dma((len(acts), 2, n_fs - 1)),
            dma((len(acts), 2, n_fs - 1)),
            dma((n_swap, n_fs - 1)),
            dma((n_swap, n_fs - 1)),
            dma((n_swap, n_fs - 1, n_tp - 1)),
            dma((n_swap, n_fs - 1)),
        ],
        compiler_params=pltpu.CompilerParams(
            collective_id=collective_id, has_side_effects=True
        ),
        cost_estimate=pl.CostEstimate(flops=0, bytes_accessed=16 * moved, transcendentals=0),
        name=f"gather_tokens_{collective_id}",
    )(*acts, *swaps)


def over_rep(part):
    part = part.astype(jnp.bfloat16)
    n_rep = lax.axis_size("rep")
    other = lax.ppermute(part, "rep", [(i, (i + 1) % n_rep) for i in range(n_rep)])
    return part, other


def added(pair):
    return pair[0].astype(jnp.float32) + pair[1].astype(jnp.float32)


def on_device(tokens, norm_gain, w_gate, w_up, w_down, cotangent):
    n_fs, n_tp = lax.axis_size("fs"), lax.axis_size("tp")
    whole_x, whole_dy, full_gate, full_up, full_down = gather_weights(
        n_fs, n_tp, tokens, cotangent, w_gate, w_up, w_down
    )
    width = whole_x.shape[1]
    wide_tokens = whole_x.astype(jnp.float32)
    gain_f = norm_gain.astype(jnp.float32)
    inverse = lax.rsqrt(jnp.mean(wide_tokens * wide_tokens, axis=-1, keepdims=True) + 1e-06)
    normed = (wide_tokens * inverse * gain_f).astype(jnp.bfloat16)
    gate = jnp.dot(normed, full_gate, preferred_element_type=jnp.float32)
    up_proj = jnp.dot(normed, full_up, preferred_element_type=jnp.float32)
    sigma = jax.nn.sigmoid(gate)
    active = gate * sigma
    hidden = (active * up_proj).astype(jnp.bfloat16)
    back = 0.5 * contract_last(whole_dy, full_down)
    d_up = (back * active).astype(jnp.bfloat16)
    d_gate = (back * up_proj * sigma * (1.0 + gate * (1.0 - sigma))).astype(jnp.bfloat16)

    all_hidden, rows_dy = gather_tokens(n_fs, n_tp, 1, [hidden], [whole_dy])
    down_pair = over_rep(0.5 * contract_first(all_hidden, rows_dy))

    partial_normed = contract_last(d_gate, full_gate) + contract_last(d_up, full_up)
    d_normed = lax.psum_scatter(
        partial_normed.astype(jnp.bfloat16), "tp", scatter_dimension=1, tiled=True
    ).astype(jnp.float32)

    all_gate, rows_normed = gather_tokens(n_fs, n_tp, 2, [d_gate], [normed])
    gate_pair = over_rep(contract_first(rows_normed, all_gate))
    (all_up,) = gather_tokens(n_fs, n_tp, 3, [d_up], [])
    up_pair = over_rep(contract_first(rows_normed, all_up))

    local_width = d_normed.shape[1]
    local_gain = lax.dynamic_slice_in_dim(
        gain_f, lax.axis_index("tp") * local_width, local_width, 0
    )
    local_tokens = tokens.astype(jnp.float32)
    scaled_grad = d_normed * local_gain
    rowdot = lax.psum(jnp.sum(scaled_grad * local_tokens, axis=-1), "tp")
    grad_tokens = (
        cotangent.astype(jnp.float32)
        + inverse * scaled_grad
        - local_tokens * inverse**3 * rowdot[:, None] / width
    ).astype(jnp.bfloat16)
    grad_gain = lax.psum(jnp.sum(d_normed * local_tokens * inverse, axis=0), ("rep", "fs"))

    grad_down = added(down_pair)
    down_sq = lax.psum(jnp.sum(grad_down * grad_down, axis=1), "fs")
    grad_gate = added(gate_pair)
    grad_up = added(up_pair)
    gate_up_sq = lax.psum(
        jnp.stack([jnp.sum(grad_gate * grad_gate, axis=1), jnp.sum(grad_up * grad_up, axis=1)]),
        "tp",
    )
    return (grad_tokens, grad_gain, grad_gate, grad_up, grad_down, gate_up_sq, down_sq)


CORES = 2
LANES = 128
TILE = 256
PARTS = 4
STEPS = 4


def line_next(z, n_fs, side):
    return z <= n_fs - 2 if side == 0 else z >= 1


def layer_kernel(n_fs, n_tp, *refs):
    tokens, cot, w_gate, w_up, w_down, gain_in = refs[:6]
    o_gate, o_up, o_down, o_tokens, o_gain, o_wide_sq, o_tall_sq = refs[6:13]
    full = refs[13:18]
    x_full, dy_full, f_gate, f_up, f_down = full
    normed, normed_t, hidden_t, act_f, slope_f, d_gate, d_up, inv_all = refs[18:26]
    g_gate, g_up, g_down = refs[26:29]
    pair_wide, pair_tall, sum_wide, sum_tall, x_wide, x_tall, t_wide, t_tall = refs[29:37]
    y_buf, d_buf, z_buf, n_buf = refs[37:41]
    v_gate, v_up, v_down, v_tokens, v_cot, v_normed, v_inv, v_out = refs[41:49]
    lane_sq, row_all, gain_all, wide_all, tall_all = refs[49:54]
    (load_sem, az_own, az_fwd, az_recv, ay_own, ay_fwd, ay_recv, ap_send, ap_recv) = refs[54:63]
    (w_send, w_recv, wx_send, wx_recv, wp_send, wp_recv, wo_send, wo_recv) = refs[63:71]
    (p_send, p_recv, x_send, x_recv, z_send, z_recv, f_send, f_recv) = refs[71:79]
    (y_send, y_recv, d_send, d_recv, n_send, n_recv, own_sem) = refs[79:86]
    (row_send, row_recv, gain_send, gain_recv) = refs[86:90]
    (wide_send, wide_recv, tall_send, tall_recv, out_sem, total, gain_sum) = refs[90:97]
    gain_load, gain, v_wide, v_tall, v_half, relay_sem = refs[97:]
    r, z, t = lax.axis_index("rep"), lax.axis_index("fs"), lax.axis_index("tp")
    y, c = lax.div(t, CORES), lax.rem(t, CORES)
    acts, weights = (tokens, cot), (w_gate, w_up, w_down)
    grads, outs = (g_gate, g_up, g_down), (v_gate, v_up, v_down)
    half, local = tokens.shape[0] // CORES, tokens.shape[1]
    count, model = x_full.shape
    rows = w_gate.shape[0]
    kb = n_fs // CORES
    width = w_gate.shape[1] // kb
    strip = rows // 2
    reach = model // 2
    partner = {"tp": y * CORES + 1 - c}
    across = {"rep": 1 - r}
    beside = {"tp": (1 - y) * CORES + c}
    owner = lax.div(z, kb)

    ends = jnp.logical_or(z == 0, z == n_fs - 1)

    def beyond(side):
        return {"fs": z + 1 if side == 0 else z - 1}

    barrier = pltpu.get_barrier_semaphore()
    close = [partner, across] + [{"tp": (1 - y) * CORES + h} for h in range(CORES)]
    for peer in close:
        pl.semaphore_signal(barrier, inc=1, device_id=peer, device_id_type=MESH)
    for side in range(2):

        @pl.when(line_next(z, n_fs, side))
        def _():
            for h in range(CORES):
                peer = {**beyond(side), "tp": y * CORES + h}
                pl.semaphore_signal(barrier, inc=1, device_id=peer, device_id_type=MESH)

    pl.semaphore_wait(barrier, jnp.where(ends, len(close) + CORES, len(close) + 2 * CORES))

    def tell(side):
        pl.semaphore_signal(
            relay_sem.at[side], inc=1, device_id=beyond(side), device_id_type=MESH
        )

    for side in range(2):

        @pl.when(z == 0 if side == 0 else z == n_fs - 1)
        def _():
            tell(side)

    def greet_far():
        for side in range(2):

            @pl.when(line_next(z, n_fs, 1 - side))
            def _():
                pl.semaphore_wait(relay_sem.at[side], 1)

                @pl.when(line_next(z, n_fs, side))
                def _():
                    tell(side)

    def own_act(a, h):
        return acts[a].at[pl.ds(pl.multiple_of(h * half, half), half), :]

    def act_place(a, source, column):
        return full[a].at[
            pl.ds(pl.multiple_of(source * half, half), half),
            pl.ds(pl.multiple_of(column * local, local), local),
        ]

    sub = half // PARTS

    def own_part(a, h, q):
        start = h * half + q * sub
        return acts[a].at[pl.ds(start, sub), :]

    def act_part(a, source, column, q):
        return full[a].at[
            pl.ds(pl.multiple_of(source * half + q * sub, sub), sub),
            pl.ds(pl.multiple_of(column * local, local), local),
        ]

    def source_of(side, d):
        return z - d if side == 0 else z + d

    def next_of(side):
        return z + 1 if side == 0 else z - 1

    def line_turn(source, at):
        return lax.rem(source - at + n_fs, n_fs) - 1

    def act_first(a, side, h, q):
        return remote(
            own_part(a, h, q),
            act_part(a, z, t, q),
            az_own.at[a, side],
            az_recv.at[a, line_turn(z, next_of(side)), c, q],
            {"fs": next_of(side), "tp": y * CORES + h},
        )

    def act_arrival(a, side, d, core, q):
        place = act_part(a, source_of(side, d), y * CORES + core, q)
        return remote(
            place,
            place,
            az_fwd.at[a],
            az_recv.at[a, line_turn(source_of(side, d), z), core, q],
            partner,
        )

    def act_forward(a, side, d, core, q):
        place = act_part(a, source_of(side, d), y * CORES + core, q)
        return remote(
            place,
            place,
            az_fwd.at[a],
            az_recv.at[a, line_turn(source_of(side, d), next_of(side)), core, q],
            {"fs": next_of(side)},
        )

    def act_over(a, side, d, core, q):
        source = source_of(side, d)
        place = act_part(a, source, y * CORES + core, q)
        return remote(
            place,
            place,
            ay_fwd.at[a],
            ay_recv.at[a],
            {"tp": (1 - y) * CORES + c},
        )

    def act_over_own(a, h):
        return remote(
            own_act(a, h),
            act_place(a, z, t),
            ay_own.at[a],
            ay_recv.at[a],
            {"tp": (1 - y) * CORES + h},
        )

    def act_over_arrivals(a):
        place = full[a].at[:, side_columns(1 - y)]
        return remote(place, place, ay_own.at[a], ay_recv.at[a], partner)

    def act_partner(a):
        return remote(own_act(a, 1 - c), act_place(a, z, t), ap_send.at[a], ap_recv.at[a], partner)

    def act_partner_arrival(a):
        place = act_place(a, z, y * CORES + 1 - c)
        return remote(place, place, ap_send.at[a], ap_recv.at[a], partner)

    def block_of(m, k):
        if m == 2:
            return weights[m].at[pl.ds(pl.multiple_of(k * width, width), width), :]
        return weights[m].at[:, pl.ds(pl.multiple_of(k * width, width), width)]

    def band_of(m, source):
        band = pl.ds(pl.multiple_of(source * rows, rows), rows)
        return full[2 + m].at[:, band] if m == 2 else full[2 + m].at[band, :]

    def quarter(m, source, rep, core):
        if m == 2:
            size = width // (2 * CORES)
            return full[4].at[
                pl.ds(pl.multiple_of((rep * CORES + core) * size, size), size),
                pl.ds(pl.multiple_of(source * rows, rows), rows),
            ]
        size = rows // (2 * CORES)
        start = source * rows + (rep * CORES + core) * size
        return full[2 + m].at[pl.ds(pl.multiple_of(start, size), size), :]

    def own_quarter(m, k, core):
        if m == 2:
            size = width // (2 * CORES)
            start = k * width + (r * CORES + core) * size
            return weights[m].at[pl.ds(pl.multiple_of(start, size), size), :]
        size = rows // (2 * CORES)
        return weights[m].at[
            pl.ds(pl.multiple_of((r * CORES + core) * size, size), size),
            pl.ds(k * width, width),
        ]

    def weight_send(m, k, core):
        return remote(
            own_quarter(m, k, core),
            quarter(m, z, r, core),
            w_send.at[m, k],
            w_recv.at[m, z],
            {"fs": kb * c + k, "tp": y * CORES + core},
        )

    def weight_arrival(m, source):
        place = quarter(m, source, r, c)
        return remote(place, place, wx_send.at[m], w_recv.at[m, source], partner)

    def weight_across(m, source):
        place = quarter(m, source, r, c)
        return remote(place, place, wx_send.at[m], wx_recv.at[m, source], across)

    def weight_across_arrival(m, source):
        place = quarter(m, source, 1 - r, c)
        return remote(place, place, wx_send.at[m], wx_recv.at[m, source], across)

    def weight_beside(m, source, which):
        place = quarter(m, source, r if which == 0 else 1 - r, c)
        return remote(
            place, place, wp_send.at[m], wp_recv.at[m], partner
        )

    def weight_beside_arrivals(m):
        part = (width if m == 2 else rows) // (2 * CORES)
        if m == 2:
            place = full[4].at[pl.ds(0, 2 * part), pl.ds(0, model - rows)]
        else:
            place = full[2 + m].at[pl.ds(0, 2 * (n_fs - 1) * part), :]
        return remote(place, place, wp_send.at[m], wp_recv.at[m], partner)

    def own_beside(m):
        return remote(
            block_of(m, z - kb * owner), band_of(m, z), wo_send.at[m], wo_recv.at[m], partner
        )

    def own_beside_arrival(m):
        return remote(band_of(m, z), band_of(m, z), wo_send.at[m], wo_recv.at[m], partner)

    def slot(wide, tall, m, *where):
        return tall.at[where] if m == 2 else wide.at[(m,) + where]

    def strip_of(band, rep):
        return pl.ds(pl.multiple_of(band * rows + rep * strip, strip), strip)

    def grad_piece(m, band, rep):
        if m == 2:
            return grads[m].at[:, strip_of(band, rep)]
        return grads[m].at[strip_of(band, rep), :]

    def rep_of(j):
        return 1 - r if j == 0 else r

    def pair(m, k, j):
        return remote(
            grad_piece(m, kb * (1 - c) + k, rep_of(j)),
            slot(pair_wide, pair_tall, m, k, j),
            p_send.at[m],
            p_recv.at[m, k, j],
            partner,
        )

    def swap(m, k):
        return remote(
            slot(sum_wide, sum_tall, m, k),
            slot(x_wide, x_tall, m, k),
            x_send.at[m],
            x_recv.at[m, k],
            across,
        )

    def place(m, block, rep):
        strips = pl.ds(pl.multiple_of(rep * strip, strip), strip)
        blocks = pl.ds(pl.multiple_of(block * width, width), width)
        return outs[m].at[blocks, strips] if m == 2 else outs[m].at[strips, blocks]

    def deliver(m, k):
        block = lax.rem(z, kb)
        return remote(
            slot(t_wide, t_tall, m, k),
            place(m, block, r),
            z_send.at[m, k],
            z_recv.at[m, block],
            {"fs": kb * c + k, "tp": y * CORES + owner},
        )

    def delivered(m, k):
        return remote(place(m, k, r), place(m, k, r), z_send.at[m, k], z_recv.at[m, k], partner)

    def keep(m, k):
        return pltpu.make_async_copy(slot(t_wide, t_tall, m, k), place(m, k, r), own_sem.at[m, k])

    def spread(m, k, source):
        return remote(source, place(m, k, r), f_send.at[m], f_recv.at[m, k], across)

    def spread_arrival(m, k):
        return remote(
            place(m, k, 1 - r), place(m, k, 1 - r), f_send.at[m], f_recv.at[m, k], across
        )

    def band_rows(band):
        return pl.ds(pl.multiple_of(band * half, half), half)

    def side_columns(which):
        return pl.ds(pl.multiple_of(which * reach, reach), reach)

    def over(band):
        return remote(
            x_full.at[band_rows(band), side_columns(1 - y)],
            y_buf.at[band],
            y_send.at[0],
            y_recv.at[band],
            beside,
        )

    low = z < n_fs // 2
    inner = jnp.logical_and(z > 0, z < n_fs - 1)
    line_slot = jnp.where(low, 0, 1)

    def line_band(i):
        return jnp.where(low, n_fs - 1 - i, i)

    def y_turn(i):
        return jnp.where(jnp.logical_and(inner, i >= 2), n_fs + 1 - i, i)

    def line_send(i, target):
        band = line_band(i)
        return remote(
            d_buf.at[i],
            z_buf.at[line_slot, band],
            d_send.at[i],
            d_recv.at[line_slot, band],
            {"fs": target},
        )

    def line_arrival(which, band):
        place = z_buf.at[which, band]
        return remote(place, place, d_send.at[0], d_recv.at[which, band], partner)

    def own_rows(core):
        return pl.ds(pl.multiple_of(core * half, half), half)

    def inv_send():
        return remote(inv_all.at[band_rows(z), :], v_inv.at[own_rows(c), :], n_send.at[0], n_recv.at[0], partner)

    def inv_arrival():
        at = v_inv.at[own_rows(1 - c), :]
        return remote(at, at, n_send.at[0], n_recv.at[0], partner)

    def last_send():
        return remote(n_buf, v_normed.at[own_rows(c), :], n_send.at[1], n_recv.at[1], partner)

    def last_arrival():
        at = v_normed.at[own_rows(1 - c), :]
        return remote(at, at, n_send.at[1], n_recv.at[1], partner)

    def loaded(a):
        return pltpu.make_async_copy(own_act(a, c), act_place(a, z, t), load_sem.at[a])

    def block_loaded(m):
        return pltpu.make_async_copy(
            block_of(m, z - kb * owner), band_of(m, z), load_sem.at[2 + m]
        )

    def act_start(a):
        for h in range(CORES):
            for side in range(2):

                @pl.when(line_next(z, n_fs, side))
                def _():
                    for q in range(PARTS):
                        act_first(a, side, h, q).start()

            act_over_own(a, h).start()
        act_partner(a).start()

    def own_start(m):
        @pl.when(c == owner)
        def _():
            own_beside(m).start()

    def act_round(a, d):
        for core in range(CORES):
            for q in range(PARTS):
                for side in range(2):

                    @pl.when(line_receives(z, n_fs, side, d))
                    def _():
                        act_arrival(a, side, d, core, q).wait_recv()
                        if d < n_fs - 1:

                            @pl.when(line_next(z, n_fs, side))
                            def _():
                                act_forward(a, side, d, core, q).start()

                        act_over(a, side, d, core, q).start()

    def weight_start(m):
        for k in range(kb):

            @pl.when(kb * c + k != z)
            def _():
                for core in range(CORES):
                    weight_send(m, k, core).start()

    def weight_round(ms, d):
        for m in ms:
            for side in range(2):

                @pl.when(line_receives(z, n_fs, side, d))
                def _():
                    source = source_of(side, d)
                    weight_arrival(m, source).wait_recv()
                    weight_across(m, source).start()
                    weight_beside(m, source, 0).start()

    def across_round(ms, d):
        for m in ms:
            for side in range(2):

                @pl.when(line_receives(z, n_fs, side, d))
                def _():
                    source = source_of(side, d)
                    weight_across_arrival(m, source).wait_recv()
                    weight_beside(m, source, 1).start()

    def weight_all(m):
        for d in range(1, n_fs):
            weight_round((m,), d)

    def across_all(m):
        for d in range(1, n_fs):
            across_round((m,), d)

    def act_ready(a):
        act_over_arrivals(a).wait_recv()
        act_partner_arrival(a).wait_recv()
        loaded(a).wait()

    def sent(ref, sem):
        remote(ref, ref, sem, sem, partner).wait_send()

    def act_sent(a, landed):
        others = full[a].at[pl.ds(0, count - half), pl.ds(0, CORES * local)]
        if landed:
            sent(others, ay_fwd.at[a])

            @pl.when(inner)
            def _():
                sent(others, az_fwd.at[a])

        if a == 1 or not landed:
            act_partner(a).wait_send()
            sent(acts[a], ay_own.at[a])
            for side in range(2):

                @pl.when(line_next(z, n_fs, side))
                def _():
                    sent(acts[a], az_own.at[a, side])

    def weight_ready(ms):
        for m in ms:
            weight_beside_arrivals(m).wait_recv()

            @pl.when(c == owner)
            def _():
                block_loaded(m).wait()

            @pl.when(c != owner)
            def _():
                own_beside_arrival(m).wait_recv()

    def weight_sent(m):
        size = full[2 + m].shape[0 if m < 2 else 1] - rows
        part = (rows if m < 2 else width) // (2 * CORES)
        if m < 2:
            sent(full[2 + m].at[pl.ds(0, (n_fs - 1) * part), :], wx_send.at[m])
            sent(full[2 + m].at[pl.ds(0, 2 * (n_fs - 1) * part), :], wp_send.at[m])
            half_block = weights[m].at[pl.ds(0, CORES * part), pl.ds(0, width)]
        else:
            sent(full[4].at[pl.ds(0, part), pl.ds(0, size)], wx_send.at[m])
            sent(full[4].at[pl.ds(0, 2 * part), pl.ds(0, size)], wp_send.at[m])
            half_block = weights[m].at[pl.ds(0, CORES * part), :]
        for k in range(kb):

            @pl.when(kb * c + k != z)
            def _():
                sent(half_block, w_send.at[m, k])

        @pl.when(c == owner)
        def _():
            own_beside(m).wait_send()

    def pairs_sent(m):
        span = pl.ds(0, kb * rows)
        sent(g_down.at[:, span] if m == 2 else grads[m].at[span, :], p_send.at[m])

    def swaps_sent(m):
        sent(sum_tall if m == 2 else sum_wide.at[m], x_send.at[m])

    def spreads_sent(m):
        sent(sum_tall if m == 2 else sum_wide.at[m], f_send.at[m])

    def over_sent():
        sent(x_full.at[:, side_columns(1 - y)], y_send.at[0])

    def tile(i, size):
        return pl.ds(pl.multiple_of(i * size, size), size)

    def normalize(i):
        at = tile(i, LANES)
        wide = x_full[at, :].astype(jnp.float32)
        inv = lax.rsqrt(jnp.mean(wide * wide, axis=-1, keepdims=True) + 1e-06)
        value = wide * inv * gain[...]
        normed[at, :] = value.astype(jnp.bfloat16)
        normed_t[:, at] = value.T.astype(jnp.bfloat16)
        inv_all[at, :] = jnp.broadcast_to(inv, (LANES, LANES))

    def forward(i):
        at = tile(i, TILE)
        gate = jnp.dot(normed[at, :], f_gate[...], preferred_element_type=jnp.float32)
        up = jnp.dot(normed[at, :], f_up[...], preferred_element_type=jnp.float32)
        sigma = jax.nn.sigmoid(gate)
        active = gate * sigma
        act_f[at, :] = active
        slope_f[at, :] = up * sigma * (1.0 + gate * (1.0 - sigma))
        hidden_t[:, at] = (active * up).T.astype(jnp.bfloat16)

    def backward(i):
        at = tile(i, TILE)
        back = 0.5 * contract_last(dy_full[at, :], f_down[...])
        d_up[at, :] = (back * act_f[at, :]).astype(jnp.bfloat16)
        d_gate[at, :] = (back * slope_f[at, :]).astype(jnp.bfloat16)

    def gradient(m, own, j, k):
        band = kb * (c if own else 1 - c) + k
        at = strip_of(band, 1 - r if j == 0 else r)
        if m == 2:
            value = 0.5 * jnp.dot(
                hidden_t[...], dy_full[:, at], preferred_element_type=jnp.float32
            )
            g_down[:, at] = value.astype(jnp.bfloat16)
        else:
            right = d_gate if m == 0 else d_up
            value = jnp.dot(normed_t[at, :], right[...], preferred_element_type=jnp.float32)
            grads[m][at, :] = value.astype(jnp.bfloat16)

    def gradients(m, j):
        @pl.loop(0, kb)
        def _(k):
            gradient(m, False, j, k)
            pair(m, k, j).start()

        @pl.loop(0, kb)
        def _(k):
            gradient(m, True, j, k)

    def pull_back(band, which):
        at, columns = band_rows(band), side_columns(which)
        value = contract_last(d_gate[at, :], f_gate[columns, :])
        value = value + contract_last(d_up[at, :], f_up[columns, :])
        x_full[at, columns] = value.astype(jnp.bfloat16)

    def added(m, k, j):
        own = grad_piece(m, kb * c + k, rep_of(j))[...].astype(jnp.float32)
        return own + slot(pair_wide, pair_tall, m, k, j)[...].astype(jnp.float32)

    def put(wide, tall, m, k, value):
        if m == 2:
            tall[k] = value
        else:
            wide[m, k] = value

    def first(m, k):
        pair(m, k, 0).wait_recv()
        put(sum_wide, sum_tall, m, k, added(m, k, 0).astype(jnp.bfloat16))
        swap(m, k).start()

    def second(m, k):
        pair(m, k, 1).wait_recv()
        swap(m, k).wait_recv()
        whole = added(m, k, 1) + slot(x_wide, x_tall, m, k)[...].astype(jnp.float32)
        put(t_wide, t_tall, m, k, whole.astype(jnp.bfloat16))
        mine = kb * c + k == z

        @pl.when(mine)
        def _():
            keep(m, k).start()
            spread(m, k, slot(t_wide, t_tall, m, k)).start()

        @pl.when(jnp.logical_not(mine))
        def _():
            deliver(m, k).start()

    def third(m, k):
        @pl.when(kb * c + k != z)
        def _():
            delivered(m, k).wait_recv()
            spread(m, k, place(m, k, r)).start()

    def own_share(band):
        over(band).wait_recv()
        own = x_full[band_rows(band), side_columns(y)].astype(jnp.float32)
        return own + y_buf[band].astype(jnp.float32)

    def line_target(i):
        if i == n_fs - 1:
            return jnp.where(low, z - 1, z + 1)
        return line_band(i)

    def normed_outer(i):
        @pl.when(jnp.logical_not(inner))
        def _():
            d_buf[i] = own_share(line_band(i)).astype(jnp.bfloat16)
            line_send(i, jnp.where(low, z + 1, z - 1)).start()

    def normed_inner(i):
        @pl.when(inner)
        def _():
            band = line_band(i)
            value = own_share(band)
            if i < n_fs - 1:
                line_arrival(line_slot, band).wait_recv()
                value = value + z_buf[line_slot, band].astype(jnp.float32)
            d_buf[i] = value.astype(jnp.bfloat16)
            line_send(i, line_target(i)).start()

    def normed_sent():
        for i in range(n_fs):
            if i < n_fs - 1:

                @pl.when(jnp.logical_not(inner))
                def _():
                    line_send(i, jnp.where(low, z + 1, z - 1)).wait_send()

            if i != n_fs - 2:

                @pl.when(inner)
                def _():
                    line_send(i, line_target(i)).wait_send()

    def normed_last():
        value = own_share(z)
        for which in range(2):
            line_arrival(which, z).wait_recv()
            value = value + z_buf[which, z].astype(jnp.float32)
        total[...] = value

        for core in range(CORES):

            @pl.when(c == core)
            def _():
                mine = slice(core * local, (core + 1) * local)
                theirs = slice((1 - core) * local, (2 - core) * local)
                v_normed[core * half : (core + 1) * half, :] = total[:, mine].astype(jnp.bfloat16)
                n_buf[...] = total[:, theirs].astype(jnp.bfloat16)

        last_send().start()

    def fold(value):
        out = value[:, :LANES]
        for i in range(1, value.shape[1] // LANES):
            out = out + value[:, i * LANES : (i + 1) * LANES]
        return out

    def row_of(value):
        return jnp.sum(value.T, axis=0, keepdims=True)

    def lane_peer(j):
        return {"tp": lax.rem(t + j, n_tp)}

    def group_peer(j):
        at = lax.rem(r * n_fs + z + j, 2 * n_fs)
        return {"rep": lax.div(at, n_fs), "fs": lax.rem(at, n_fs)}

    def fan(buffer, count_of, mine, send, recv, peer):
        def start():
            for j in range(1, count_of):
                place = buffer.at[mine]
                remote(place, place, send.at[0], recv.at[0], peer(j)).start()

        def others():
            place = buffer.at[pl.ds(0, count_of - 1)]
            return remote(place, place, send.at[0], recv.at[0], partner)

        return start, others

    row_fan = fan(row_all, n_tp, t, row_send, row_recv, lane_peer)
    wide_fan = fan(wide_all, n_tp, t, wide_send, wide_recv, lane_peer)
    gain_fan = fan(gain_all, 2 * n_fs, r * n_fs + z, gain_send, gain_recv, group_peer)
    tall_fan = fan(tall_all, 2 * n_fs, r * n_fs + z, tall_send, tall_recv, group_peer)

    def gain_here():
        return gain[:, pl.ds(pl.multiple_of(t * local, local), local)]

    def token_sums():
        last_arrival().wait_recv()
        inv_arrival().wait_recv()
        for i in range(2):
            own_loaded(i).wait()
        gain_l = gain_here()
        gain_sum[...] = jnp.zeros_like(gain_sum)

        @pl.loop(0, CORES * half // LANES)
        def _(i):
            at = tile(i, LANES)
            d_tokens = v_normed[at, :].astype(jnp.float32) * v_tokens[at, :].astype(jnp.float32)
            row_all[t, :, at] = row_of(fold(d_tokens * gain_l))
            inv = v_inv[at, :1]
            gain_sum[...] += jnp.sum(d_tokens * inv, axis=0, keepdims=True)

        gain_all[r * n_fs + z] = gain_sum[...]
        row_fan[0]()
        gain_fan[0]()

    def token_grads():
        row_fan[1]().wait_recv()
        gain_l = gain_here()

        @pl.loop(0, CORES * half // LANES)
        def _(i):
            at = tile(i, LANES)
            dots = row_all[0, :, at]
            for j in range(1, n_tp):
                dots = dots + row_all[j, :, at]
            rowdot = jnp.broadcast_to(dots, (LANES, LANES)).T[:, :1]
            inv = v_inv[at, :1]
            value = v_cot[at, :].astype(jnp.float32)
            value = value + inv * (v_normed[at, :].astype(jnp.float32) * gain_l)
            scale = inv**3 * rowdot / model
            value = value - v_tokens[at, :].astype(jnp.float32) * scale
            v_out[at, :] = value.astype(jnp.bfloat16)

        pltpu.make_async_copy(v_out, o_tokens, out_sem.at[3]).start()

    def own_loaded(i):
        source, target = ((tokens, v_tokens), (cot, v_cot))[i]
        return pltpu.make_async_copy(source, target, load_sem.at[5 + i])

    def block_out(m, k):
        at = pl.ds(k * width, width)
        if m == 2:
            return pltpu.make_async_copy(v_down.at[at, :], o_down.at[at, :], out_sem.at[m])
        return pltpu.make_async_copy(
            outs[m].at[:, at], (o_gate, o_up)[m].at[:, at], out_sem.at[m]
        )

    def strip_squares(m, k):
        @pl.when(kb * c + k == z)
        def _():
            keep(m, k).wait()

        if m == 2:
            columns = pl.ds(pl.multiple_of(r * strip, strip), strip)

            @pl.loop(0, width // LANES)
            def _(i):
                at = pl.ds(pl.multiple_of(k * width + i * LANES, LANES), LANES)
                value = v_down[at, columns].astype(jnp.float32)
                tall_all[r * n_fs + z, :, at] = row_of(fold(value * value))
        else:

            @pl.loop(0, strip // LANES)
            def _(i):
                at = tile(i, LANES)
                from_row = pl.ds(pl.multiple_of(r * strip + i * LANES, LANES), LANES)
                value = outs[m][from_row, k * width : (k + 1) * width].astype(jnp.float32)
                part = fold(value * value)
                if k > 0:
                    part = part + lane_sq[m, at, :]
                if k < kb - 1:
                    lane_sq[m, at, :] = part
                else:
                    wide_all[t, m : m + 1, at] = row_of(part)

    def wide_cross():
        strips = pl.ds(pl.multiple_of(r * strip, strip), strip)
        return remote(v_half, v_wide.at[:, strips], n_send.at[2], n_recv.at[2], across)

    def wide_cross_arrival():
        place = v_wide.at[:, pl.ds(pl.multiple_of((1 - r) * strip, strip), strip)]
        return remote(place, place, n_send.at[2], n_recv.at[2], across)

    def summed(buffer, count_of):
        value = buffer[0]
        for j in range(1, count_of):
            value = value + buffer[j]
        return value

    def whole_block(m, k):
        spread_arrival(m, k).wait_recv()
        block_out(m, k).start()

    gain_copy = pltpu.make_async_copy(gain_in, gain_load, out_sem.at[4])
    gain_copy.start()
    for a in range(2):
        loaded(a).start()

    @pl.when(c == owner)
    def _():
        for m in range(3):
            block_loaded(m).start()

    act_start(0)
    own_start(0)
    own_start(1)
    for i in range(2):
        own_loaded(i).start()
    act_round(0, 1)
    greet_far()
    act_round(0, 2)
    weight_start(0)
    weight_start(1)
    act_start(1)
    own_start(2)
    for d in range(3, n_fs):
        act_round(0, d)
    weight_all(0)
    act_round(1, 1)
    weight_all(1)
    across_all(0)
    weight_start(2)
    gain_copy.wait()
    for i in range(model // LANES):
        gain[:, i * LANES : (i + 1) * LANES] = gain_load[i : i + 1, :].astype(jnp.float32)
    act_ready(0)
    pl.loop(0, count // LANES)(normalize)
    inv_send().start()
    v_inv[own_rows(c), :] = inv_all[band_rows(z), :]
    across_all(1)
    act_round(1, 2)
    weight_ready((0, 1))
    pl.loop(0, count // TILE)(forward)
    weight_all(2)
    for d in range(3, n_fs):
        act_round(1, d)
    across_all(2)
    act_ready(1)
    for k in range(kb):
        gradient(2, False, 0, k)
        pair(2, k, 0).start()
        if k:
            first(2, k - 1)
        gradient(2, True, 0, k)
    first(2, kb - 1)
    gradients(2, 1)
    weight_ready((2,))
    pl.loop(0, count // TILE)(backward)
    act_sent(0, True)

    gradients(0, 0)
    for k in range(kb):
        first(0, k)

    @pl.loop(0, n_fs)
    def _(i):
        band = line_band(y_turn(i))
        pull_back(band, 1 - y)
        over(band).start()

    gradients(1, 0)
    for k in range(kb):
        first(1, k)
    gradients(0, 1)
    for k in range(kb):
        second(2, k)

    @pl.loop(0, n_fs)
    def _(i):
        pull_back(i, y)

    gradients(1, 1)
    second(0, 0)
    normed_outer(0)
    second(0, 1)
    third(2, 0)
    third(2, 1)
    normed_outer(1)
    second(1, 0)
    normed_inner(n_fs - 1)
    normed_inner(0)
    second(1, 1)
    normed_outer(2)
    third(0, 0)
    third(0, 1)
    normed_inner(1)
    for k in range(kb):
        strip_squares(2, k)
    tall_fan[0]()
    for k in range(kb):
        strip_squares(0, k)
    third(1, 0)
    strip_squares(1, 0)
    third(1, 1)
    strip_squares(1, 1)
    wide_fan[0]()
    normed_last()
    whole_block(2, 0)
    whole_block(2, 1)
    token_sums()
    wide_fan[1]().wait_recv()
    v_half[...] = summed(wide_all, n_tp)
    wide_cross().start()
    v_wide[:, pl.ds(pl.multiple_of(r * strip, strip), strip)] = v_half[...]
    tall_fan[1]().wait_recv()
    v_tall[...] = summed(tall_all, 2 * n_fs)
    tall_out = pltpu.make_async_copy(v_tall, o_tall_sq, out_sem.at[6])
    tall_out.start()
    token_grads()
    whole_block(0, 0)
    whole_block(0, 1)
    act_sent(0, False)
    act_sent(1, True)
    for m in range(3):
        weight_sent(m)
    over_sent()
    normed_sent()
    inv_send().wait_send()
    last_send().wait_send()
    row_fan[1]().wait_send()
    wide_fan[1]().wait_send()
    for m in range(3):
        pairs_sent(m)
        swaps_sent(m)
        for k in range(kb):

            @pl.when(kb * c + k != z)
            def _():
                deliver(m, k).wait_send()

    whole_block(1, 0)
    gain_fan[1]().wait_recv()
    gain_sum[...] = summed(gain_all, 2 * n_fs)
    gain_out = pltpu.make_async_copy(gain_sum, o_gain, out_sem.at[5])
    gain_out.start()
    wide_cross_arrival().wait_recv()
    wide_out = pltpu.make_async_copy(v_wide, o_wide_sq, out_sem.at[7])
    wide_out.start()
    whole_block(1, 1)
    wide_cross().wait_send()
    gain_fan[1]().wait_send()
    tall_fan[1]().wait_send()
    gain_out.wait()
    tall_out.wait()
    wide_out.wait()
    pltpu.make_async_copy(v_out, o_tokens, out_sem.at[3]).wait()
    for m in range(3):
        spreads_sent(m)
        pltpu.make_async_copy(outs[m], (o_gate, o_up, o_down)[m], out_sem.at[m]).wait()


def layer(n_fs, n_tp, tokens, cot, w_gate, w_up, w_down, gain):
    half, local = tokens.shape[0] // CORES, tokens.shape[1]
    rows, hidden = w_gate.shape
    width = hidden * CORES // n_fs
    model = rows * n_fs
    count = half * n_fs
    dtype = tokens.dtype
    kb = n_fs // CORES
    strip = rows // 2
    reach = model // 2
    wide, tall = (strip, width), (width, strip)
    dma = pltpu.SemaphoreType.DMA
    hbm = pl.BlockSpec(memory_space=pl.ANY)
    pairs, singles = dma((3, kb, 2)), dma((3, kb))

    def bf(*shape):
        return pltpu.VMEM(shape, dtype)

    def f32(*shape):
        return pltpu.VMEM(shape, jnp.float32)

    hidden = kb * width
    shapes = [(rows, hidden)] * 2 + [(hidden, rows)]
    return pl.pallas_call(
        functools.partial(layer_kernel, n_fs, n_tp),
        out_shape=[jax.ShapeDtypeStruct(s, dtype) for s in shapes]
        + [jax.ShapeDtypeStruct((CORES * half, local), dtype)]
        + [jax.ShapeDtypeStruct(s, jnp.float32) for s in ((1, local), (2, rows), (1, hidden))],
        in_specs=[hbm] * 6,
        out_specs=[hbm] * 7,
        scratch_shapes=[
            bf(count, model),
            bf(count, model),
            bf(model, width),
            bf(model, width),
            bf(width, model),
            bf(count, model),
            bf(model, count),
            bf(width, count),
            f32(count, width),
            f32(count, width),
            bf(count, width),
            bf(count, width),
            f32(count, LANES),
            bf(model, width),
            bf(model, width),
            bf(width, model),
            bf(2, kb, 2, *wide),
            bf(kb, 2, *tall),
            bf(2, kb, *wide),
            bf(kb, *tall),
            bf(2, kb, *wide),
            bf(kb, *tall),
            bf(2, kb, *wide),
            bf(kb, *tall),
            bf(n_fs, half, reach),
            bf(n_fs, half, reach),
            bf(2, n_fs, half, reach),
            bf(half, local),
            bf(rows, hidden),
            bf(rows, hidden),
            bf(hidden, rows),
            bf(CORES * half, local),
            bf(CORES * half, local),
            bf(CORES * half, local),
            f32(CORES * half, LANES),
            bf(CORES * half, local),
            f32(2, strip, LANES),
            f32(n_tp, 1, CORES * half),
            f32(2 * n_fs, 1, local),
            f32(n_tp, 2, strip),
            f32(2 * n_fs, 1, hidden),
            dma((7,)),
            dma((2, 2)),
            dma((2,)),
            dma((2, n_fs - 1, CORES, PARTS)),
            dma((2,)),
            dma((2,)),
            dma((2,)),
            dma((2,)),
            dma((2,)),
            dma((3, kb)),
            dma((3, n_fs)),
            dma((3,)),
            dma((3, n_fs)),
            dma((3,)),
            dma((3,)),
            dma((3,)),
            dma((3,)),
            dma((3,)),
            pairs,
            dma((3,)),
            singles,
            singles,
            singles,
            dma((3,)),
            singles,
            dma((1,)),
            dma((n_fs,)),
            dma((n_fs,)),
            dma((2, n_fs)),
            dma((3,)),
            dma((3,)),
            dma((3, kb)),
            dma((1,)),
            dma((1,)),
            dma((1,)),
            dma((1,)),
            dma((1,)),
            dma((1,)),
            dma((1,)),
            dma((1,)),
            dma((8,)),
            f32(half, reach),
            f32(1, local),
            bf(model // LANES, LANES),
            f32(1, model),
            f32(2, rows),
            f32(1, hidden),
            f32(2, strip),
            pltpu.SemaphoreType.REGULAR((2,)),
        ],
        compiler_params=pltpu.CompilerParams(
            collective_id=4, has_side_effects=True, vmem_limit_bytes=67043328
        ),
        name="layer",
    )(tokens, cot, w_gate, w_up, w_down, gain)


def widen_kernel(n, *refs):
    sources, targets = refs[:n], refs[n : 2 * n]
    narrow, wide = refs[2 * n : 3 * n], refs[3 * n : 3 * n + 3]
    flat, load_sem, store_sem = refs[3 * n + 3 : -2], *refs[-2:]

    def rows_of(i, step):
        size = sources[i].shape[0] // STEPS
        return pl.ds(step * size, size)

    def load(i, step):
        at = rows_of(i, step)
        return pltpu.make_async_copy(sources[i].at[at], narrow[i].at[at], load_sem.at[i, step])

    def store(i, step):
        at = rows_of(i, step)
        return pltpu.make_async_copy(wide[i].at[at], targets[i].at[at], store_sem.at[i, step])

    def load_whole(i):
        return pltpu.make_async_copy(sources[i], narrow[i], load_sem.at[i, 0])

    def store_whole(i):
        source = {4: flat[0], 6: flat[1]}.get(i, narrow[i])
        return pltpu.make_async_copy(source, targets[i], store_sem.at[i, 0])

    for i in range(3, n):
        load_whole(i).start()
    for step in range(STEPS):
        for i in range(3):
            load(i, step).start()
    for i in range(3, n):
        load_whole(i).wait()
        if i in (4, 6):
            flat[(i - 4) // 2][...] = narrow[i][0, :]
        store_whole(i).start()
    for step in range(STEPS):
        for i in range(3):
            load(i, step).wait()
            at = rows_of(i, step)
            wide[i][at] = narrow[i][at].astype(jnp.float32)
            store(i, step).start()
    for step in range(STEPS):
        for i in range(3):
            store(i, step).wait()
    for i in range(3, n):
        store_whole(i).wait()


def widen(*arrays):
    n = len(arrays)
    hbm = pl.BlockSpec(memory_space=pl.ANY)
    shapes = [a.shape[1:] if a.shape[0] == 1 else a.shape for a in arrays]
    kinds = [jnp.float32] * 3 + [a.dtype for a in arrays[3:]]
    dma = pltpu.SemaphoreType.DMA
    return pl.pallas_call(
        functools.partial(widen_kernel, n),
        out_shape=[jax.ShapeDtypeStruct(s, k) for s, k in zip(shapes, kinds)],
        in_specs=[hbm] * n,
        out_specs=[hbm] * n,
        scratch_shapes=[pltpu.VMEM(a.shape, a.dtype) for a in arrays]
        + [pltpu.VMEM(a.shape, jnp.float32) for a in arrays[:3]]
        + [pltpu.VMEM(s, jnp.float32) for s in (shapes[4], shapes[6])]
        + [dma((n, STEPS)), dma((n, STEPS))],
        name="widen",
    )(*arrays)


def by_chip(tokens, norm_gain, w_gate, w_up, w_down, cotangent):
    found = layer(
        lax.axis_size("fs"),
        lax.axis_size("tp"),
        tokens,
        cotangent,
        w_gate,
        w_up,
        w_down,
        norm_gain.reshape(-1, LANES),
    )
    grad_gate, grad_up, grad_down, grad_tokens, grad_gain, gate_up_sq, down_sq = widen(*found)
    return (grad_tokens, grad_gain, grad_gate, grad_up, grad_down, gate_up_sq, down_sq)


def fits_chips(mesh):
    n_rep, n_fs, n_tp = mesh.shape["rep"], mesh.shape["fs"], mesh.shape["tp"]
    return n_rep == 2 and n_tp == 2 * CORES and n_fs == 2 * CORES


def solution(mesh):
    placed = (
        P(("rep", "fs"), "tp"),
        P(),
        P("fs", "tp"),
        P("fs", "tp"),
        P("tp", "fs"),
        P(("rep", "fs"), "tp"),
    )
    return jax.shard_map(
        by_chip if fits_chips(mesh) else on_device,
        mesh=mesh,
        in_specs=placed,
        out_specs=(
            P(("rep", "fs"), "tp"),
            P("tp"),
            P("fs", "tp"),
            P("fs", "tp"),
            P("tp", "fs"),
            P(None, "fs"),
            P("tp"),
        ),
        check_vma=False,
    )
```
